256 devices in a mesh: rep: 2 (over z_hi), fs: 16 (over z_lo, x), tp: 8 (over y, core).
Axes of the slice: x: 4, y: 4, z: 8 (z_hi: 2, z_lo: 4; z = z_hi * 4 + z_lo), core: 2. Of those that a mesh axis runs over, the one named last changes fastest.
Arguments:
- tokens: bfloat16 [4096, 4096], P(('rep', 'fs'), 'tp'), may hold values from -6 to 6
- mixer_gain: float32 [4096], replicated, may hold values from 0.75 to 1.25
- gate_proj: bfloat16 [4096, 2048], P('fs', 'tp'), may hold values from -0.09375 to 0.09375
- value_proj: bfloat16 [4096, 2048], P('fs', 'tp'), may hold values from -0.09375 to 0.09375
- value_gain: float32 [16, 128], P('tp'), may hold values from 0.75 to 1.25
- spatial_mix: bfloat16 [16, 128, 128], P('tp', 'fs'), may hold values from -0.5 to 0.5
- spatial_bias: float32 [16, 128], P('tp'), may hold values from 0.5 to 1.5
- head_gain: float32 [16, 128], P('tp'), may hold values from 0.75 to 1.25
- merge_proj: bfloat16 [2048, 4096], P('tp', 'fs'), may hold values from -0.125 to 0.125
- ffn_gain: float32 [4096], replicated, may hold values from 0.25 to 1.75
- gate_up: bfloat16 [4096, 11008], P('fs', 'tp'), may hold values from -0.09375 to 0.09375
- value_up: bfloat16 [4096, 11008], P('fs', 'tp'), may hold values from -0.09375 to 0.09375
- gate_kernel: float32 [3, 11008], P(None, 'tp'), may hold values from -3.5 to 3.5
- value_kernel: float32 [3, 11008], P(None, 'tp'), may hold values from -3.5 to 3.5
- gate_offset: float32 [11008], P('tp'), may hold values from -0.6 to 0.6
- value_offset: float32 [11008], P('tp'), may hold values from -1.8 to 1.8
- down_proj: bfloat16 [11008, 4096], P('tp', 'fs'), may hold values from -0.0546875 to 0.0546875
Outputs:
- layer_out: bfloat16 [4096, 4096], P(('rep', 'fs'), 'tp')
The draws below stay inside these ranges and needn't reach their ends.
All inputs are finite; a program needn't handle non-finite values.
Results may differ from the reference program's by a relative error of at most 0.02.
Values may be sent and summed in bfloat16 or wider, within the bound.
A program may use at most 128 MiB of HBM per device.

```python
import jax
import jax.numpy as jnp
from jax import lax

D = 4096
HEADS = 16
HEAD_DIM = 128
SEQ_LEN = 128
FF = 11008
DG = 2048
TOKENS = 4096


def shard_levels(own_key, extent, shards, smallest, top_value):
    level = 1.0
    for axis_at, blocks in shards:
        steps = jax.random.uniform(jax.random.fold_in(jax.random.fold_in(own_key, 6), axis_at), (blocks,), jnp.float32, smallest / len(shards), top_value / len(shards))
        level = level * jnp.repeat(jnp.exp(steps), extent[axis_at] // blocks).reshape((-1,) + (1,) * (len(extent) - 1 - axis_at))
    return level


def scatter_about(own_key, shape, deviation, bound, cuts=(), dtype=jnp.bfloat16):
    drawn = deviation * jax.random.normal(own_key, shape, jnp.float32)
    if cuts:
        drawn = drawn * shard_levels(own_key, shape, cuts, -0.22, 0.18)
    return jnp.clip(drawn, -bound, bound).astype(dtype)


def setup_inputs(seed: int = 0) -> dict:
    keys = jax.random.split(jax.random.key(seed), 18)
    tokens = scatter_about(keys[0], (TOKENS, D), 1.0, 6.0, ((0, 32), (1, 8)))
    mixer_gain = jnp.clip(1.0 + 0.05 * jax.random.normal(keys[1], (D,), jnp.float32), 0.75, 1.25)
    gate_proj = scatter_about(keys[2], (D, DG), D ** -0.5, 0.09375, ((0, 16), (1, 8)))
    value_proj = scatter_about(keys[3], (D, DG), D ** -0.5, 0.09375, ((0, 16), (1, 8)))
    value_gain = jnp.clip(1.0 + 0.05 * jax.random.normal(keys[4], (HEADS, HEAD_DIM), jnp.float32), 0.75, 1.25)
    spatial_mix = scatter_about(keys[5], (HEADS, SEQ_LEN, SEQ_LEN), SEQ_LEN ** -0.5, 0.5, ((0, 8), (1, 16)))
    spatial_bias = jnp.clip(1.0 + 0.1 * jax.random.normal(keys[6], (HEADS, SEQ_LEN), jnp.float32), 0.5, 1.5)
    head_gain = jnp.clip(1.0 + 0.05 * jax.random.normal(keys[7], (HEADS, HEAD_DIM), jnp.float32), 0.75, 1.25)
    merge_proj = scatter_about(keys[8], (DG, D), DG ** -0.5, 0.125, ((0, 8), (1, 16)))
    ffn_gain = jnp.clip(1.0 + 0.15 * jax.random.normal(keys[9], (D,), jnp.float32), 0.25, 1.75)
    gate_up = scatter_about(keys[10], (D, FF), D ** -0.5, 0.09375, ((0, 16), (1, 8)))
    value_up = scatter_about(keys[11], (D, FF), D ** -0.5, 0.09375, ((0, 16), (1, 8)))
    gate_kernel = scatter_about(keys[12], (3, FF), 3 ** -0.5, 3.5, ((1, 8),), jnp.float32)
    value_kernel = scatter_about(keys[13], (3, FF), 3 ** -0.5, 3.5, ((1, 8),), jnp.float32)
    gate_offset = scatter_about(keys[14], (FF,), 0.1, 0.6, ((0, 8),), jnp.float32)
    value_offset = scatter_about(keys[15], (FF,), 0.3, 1.8, ((0, 8),), jnp.float32)
    down_proj = scatter_about(keys[16], (FF, D), FF ** -0.5, 0.0546875, ((0, 8), (1, 16)))
    return {"tokens": tokens, "mixer_gain": mixer_gain, "gate_proj": gate_proj, "value_proj": value_proj, "value_gain": value_gain, "spatial_mix": spatial_mix, "spatial_bias": spatial_bias, "head_gain": head_gain, "merge_proj": merge_proj, "ffn_gain": ffn_gain, "gate_up": gate_up, "value_up": value_up, "gate_kernel": gate_kernel, "value_kernel": value_kernel, "gate_offset": gate_offset, "value_offset": value_offset, "down_proj": down_proj}


epsilon = 1e-06

def normalize(values, gain):
    values = values.astype(jnp.float32)
    scaled = values * lax.rsqrt(lax.optimization_barrier(jnp.mean(values * values, axis=-1, keepdims=True)) + epsilon)
    return scaled * gain

def rounded(values):
    return lax.optimization_barrier(values.astype(jnp.bfloat16)).astype(jnp.float32)

def gelu_exact(values):
    return jax.nn.gelu(values, approximate=False)

def convolve(values, kernel, offset, length):
    total_rows, width = values.shape
    blocks = values.reshape(total_rows // length, length, width)
    padded = jnp.pad(blocks, ((0, 0), (1, 1), (0, 0)))
    result = offset + padded[:, 0:length] * kernel[0] + padded[:, 1:length + 1] * kernel[1] + padded[:, 2:] * kernel[2]
    return result.reshape(total_rows, width)

def reference(tokens, mixer_gain, gate_proj, value_proj, value_gain, spatial_mix, spatial_bias, head_gain, merge_proj, ffn_gain, gate_up, value_up, gate_kernel, value_kernel, gate_offset, value_offset, down_proj):
    total_rows = tokens.shape[0]
    seqs = total_rows // SEQ_LEN
    normed = normalize(tokens, mixer_gain).astype(jnp.bfloat16)
    gated = gelu_exact(rounded(jnp.dot(normed, gate_proj, preferred_element_type=jnp.float32)))
    spread = gelu_exact(rounded(jnp.dot(normed, value_proj, preferred_element_type=jnp.float32)))
    spread = normalize(spread.reshape(seqs, SEQ_LEN, HEADS, HEAD_DIM), value_gain).astype(jnp.bfloat16)
    mixed = jnp.einsum('hij,njhd->nihd', spatial_mix.astype(jnp.float32), spread.astype(jnp.float32), precision=lax.Precision.HIGHEST)
    mixed = mixed + spatial_bias.T[None, :, :, None]
    joined = gated.reshape(seqs, SEQ_LEN, HEADS, HEAD_DIM) * mixed
    merged = normalize(joined, head_gain).astype(jnp.bfloat16).reshape(total_rows, DG)
    branch = jnp.dot(merged, merge_proj, preferred_element_type=jnp.float32)
    hidden = (tokens.astype(jnp.float32) + branch).astype(jnp.bfloat16)
    normed_ffn = normalize(hidden, ffn_gain).astype(jnp.bfloat16)
    upper_gate = rounded(jnp.dot(normed_ffn, gate_up, preferred_element_type=jnp.float32))
    upper_value = rounded(jnp.dot(normed_ffn, value_up, preferred_element_type=jnp.float32))
    conv_gate = convolve(upper_gate, gate_kernel, gate_offset, SEQ_LEN)
    conv_value = convolve(upper_value, value_kernel, value_offset, SEQ_LEN)
    active = (gelu_exact(conv_gate) * conv_value).astype(jnp.bfloat16)
    change = jnp.dot(active, down_proj, preferred_element_type=jnp.float32)
    return (hidden.astype(jnp.float32) + change).astype(jnp.bfloat16)
```

```python
import jax
import jax.numpy as jnp
from jax import lax
from jax.experimental import pallas as pl
from jax.experimental.pallas import tpu as pltpu
from jax.sharding import Mesh
from jax.sharding import PartitionSpec as P

TP = ("tp_0", "tp_1")
FS = ("fs_0", "fs_1")
REP_FS = ("rep", "fs_0", "fs_1")
MESH = pl.DeviceIdType.MESH
EPS = 1e-06
F32 = jnp.float32
BF16 = jnp.bfloat16
SEMS = 160


def gelu(v):
    return 0.5 * v * (1.0 + lax.erf(v * 0.7071067811865476))


def lanes_of(n):
    return lax.broadcasted_iota(jnp.int32, (n, 128), 1)


def kernel(
    tok, gains, gp, vp, vgain, smix, sbias, hgain, mp, gu, vu, cv, dn,
    out,
    XG, HG, XS, WGP, WVP, WMP, WGU, WVU, WDN, SM, SQ, MG, ACT, OP,
    P1, A1, B1, C1, HL1, HR1, FL1, FR1,
    P2, A2, B2, C2, HL2, HR2, FL2, FR2,
    P3, A3, B3, C3, HL3, HR3, FL3, FR3,
    T, CS4, CR4, YA4, YB4, YC4, YHL4, YHR4, YFL4, YFR4,
    CS5, CR5, YA5, YB5, YC5, YHL5, YHR5, YFL5, YFR5,
    ssem, rsem, lsem,
):
    r, z, x, y, c = (lax.axis_index(a) for a in ("rep", "fs_0", "fs_1", "tp_0", "tp_1"))
    other = 1 - c
    f = 4 * z + x
    inner = gu.shape[1]
    depth = gains.shape[1] * gains.shape[2]

    def at(z_=None, x_=None, y_=None, c_=None, r_=None):
        pick = lambda new, old: old if new is None else new
        return (pick(r_, r), pick(z_, z), pick(x_, x), pick(y_, y), pick(c_, c))

    up = lambda v: lax.rem(v + 1, 4)
    down = lambda v: lax.rem(v + 3, 4)
    far = lambda v: lax.rem(v + 2, 4)

    zr = 4 * r + z
    zu, zd = lax.rem(zr + 1, 8), lax.rem(zr + 7, 8)
    z_up = at(r_=zu // 4, z_=lax.rem(zu, 4))
    z_dn = at(r_=zd // 4, z_=lax.rem(zd, 4))
    x_up, x_dn = at(x_=up(x)), at(x_=down(x))
    y_up, y_dn = at(y_=up(y)), at(y_=down(y))
    mate = at(c_=other)
    fs_peers = []
    for i in range(1, 16):
        g = lax.rem(f + i, 16)
        fs_peers.append(at(z_=g // 4, x_=lax.rem(g, 4)))

    barrier = pltpu.get_barrier_semaphore()
    greet = fs_peers + [at(x_=jnp.int32(k), c_=other) for k in range(4)]
    greet += [y_up, y_dn, z_up, z_dn]
    for peer in greet:
        pl.semaphore_signal(barrier, inc=1, device_id=peer, device_id_type=MESH)
    pl.semaphore_wait(barrier, len(greet))

    started = []
    count = [0]

    def take(n=1):
        first = count[0]
        count[0] += n
        return first

    def remote(src, dst, s, k, peer):
        return pltpu.make_async_remote_copy(
            src_ref=src, dst_ref=dst, send_sem=ssem.at[s], recv_sem=rsem.at[k],
            device_id=peer, device_id_type=MESH,
        )

    def send(src, dst, k, peer):
        copy = remote(src, dst, k, k, peer)
        copy.start()
        started.append(copy)

    def recv(dst, k):
        remote(dst, dst, 0, k, mate).wait_recv()

    half = dn.shape[0] // 2
    chunks = [
        (gp, WGP, 0, 256, 128), (vp, WVP, 0, 256, 128), (mp, WMP, 0, 256, 128),
        (gu, WGU, 0, 128, 64), (gu, WGU, 128, 128, 64),
        (vu, WVU, 0, 128, 64), (vu, WVU, 128, 128, 64),
        (dn, WDN, 0, half, 352), (dn, WDN, half, half, 352),
    ]
    zk = [take(4) for _ in chunks]

    def z_own(i):
        src, buf, at0, n, _ = chunks[i]
        rows = pl.ds(at0, n)
        send(src.at[rows], buf.at[z, rows], zk[i], z_up)
        send(src.at[rows], buf.at[z, rows], zk[i] + 1, z_dn)
        pltpu.make_async_copy(src.at[rows], buf.at[z, rows], lsem.at[i]).start()

    def z_fwd(i):
        _, buf, at0, n, cut = chunks[i]
        lo, hi = down(z), up(z)
        recv(buf.at[lo, pl.ds(at0, n)], zk[i])
        a = pl.ds(at0, cut)
        send(buf.at[lo, a], buf.at[lo, a], zk[i] + 2, z_up)
        recv(buf.at[hi, pl.ds(at0, n)], zk[i] + 1)
        b = pl.ds(at0 + cut, n - cut)
        send(buf.at[hi, b], buf.at[hi, b], zk[i] + 3, z_dn)

    def z_fin(i):
        src, buf, at0, n, cut = chunks[i]
        rows = pl.ds(at0, n)
        recv(buf.at[far(z), pl.ds(at0, cut)], zk[i] + 2)
        recv(buf.at[far(z), pl.ds(at0 + cut, n - cut)], zk[i] + 3)
        pltpu.make_async_copy(src.at[rows], buf.at[z, rows], lsem.at[i]).wait()

    for k in range(4):
        WDN[k, dn.shape[0] :, :] = jnp.zeros((inner - dn.shape[0], 256), BF16)

    swaps = []
    kx = take(4)
    me = 2 * y + c
    to_me = x // 2 == c
    for j in range(2):
        for h in range(2):
            xt = 2 * c + j
            mine = jnp.logical_and(xt == x, c == h)
            cols = slice(j * 256 + h * 128, j * 256 + h * 128 + 128)
            copy = remote(
                tok.at[:, cols], XG.at[2 * y + h, x], kx + 2 * j + h, kx + x,
                at(x_=xt, c_=jnp.int32(h)),
            )

            swaps.append((mine, copy))

            @pl.when(jnp.logical_not(mine))
            def _():
                copy.start()

            @pl.when(mine)
            def _():
                XG[2 * y + h, x] = tok[:, cols]

    z_own(0)
    z_own(1)
    z_own(2)
    km = take(15)
    for i in range(15):
        send(smix, SM.at[f], km + i, fs_peers[i])
    SM[f] = smix[...]

    for j in range(4):

        @pl.when(jnp.logical_not(jnp.logical_and(x == j, to_me)))
        def _():
            recv(XG.at[me, j], kx + j)

    def y_start(buf, k):
        send(buf.at[me], buf.at[me], k, y_up)
        send(buf.at[me], buf.at[me], k + 1, y_dn)
        send(buf.at[me], buf.at[me], k + 2, mate)

    lo_y, hi_y, far_y = 2 * down(y) + c, 2 * up(y) + c, 2 * far(y) + c
    a2, b2 = pl.ds(0, 2), pl.ds(2, 2)

    def y_mid(buf, k):
        recv(buf.at[lo_y], k)
        send(buf.at[lo_y, a2], buf.at[lo_y, a2], k + 3, y_up)
        recv(buf.at[hi_y], k + 1)
        send(buf.at[hi_y, b2], buf.at[hi_y, b2], k + 4, y_dn)
        send(buf.at[lo_y], buf.at[lo_y], k + 5, mate)
        send(buf.at[hi_y], buf.at[hi_y], k + 6, mate)

    def y_end(buf, k):
        recv(buf.at[far_y, a2], k + 3)
        send(buf.at[far_y, a2], buf.at[far_y, a2], k + 7, mate)
        recv(buf.at[far_y, b2], k + 4)
        send(buf.at[far_y, b2], buf.at[far_y, b2], k + 8, mate)

    def y_last(buf, k):
        recv(buf.at[2 * y + other], k + 2)
        recv(buf.at[2 * down(y) + other], k + 5)
        recv(buf.at[2 * up(y) + other], k + 6)
        recv(buf.at[2 * far(y) + other, a2], k + 7)
        recv(buf.at[2 * far(y) + other, b2], k + 8)

    def scaled(buf, which):
        gain = jnp.concatenate([gains[which, pl.ds(4 * k + x, 1), :] for k in range(4)], axis=1)

        def block(b, _):
            rows = jnp.concatenate([buf[i, b] for i in range(8)], axis=1).astype(F32)
            SQ[b] = jnp.broadcast_to(jnp.sum(rows * rows, axis=-1, keepdims=True), (128, 128))
            XS[pl.ds(pl.multiple_of(b * 128, 128), 128), :] = (rows * gain).astype(BF16)
            return 0

        lax.fori_loop(0, 4, block, 0)

    ky = take(9)
    y_start(XG, ky)
    z_fwd(0)
    y_mid(XG, ky)
    z_fwd(1)
    y_end(XG, ky)
    z_fwd(2)
    z_own(3)
    z_own(4)
    y_last(XG, ky)

    scaled(XG, 0)
    z_fin(0)
    z_fin(1)
    for w, W in ((0, WGP), (1, WVP)):
        prod = jnp.dot(XS[...], W[...].reshape(1024, 256), preferred_element_type=F32)
        P1[:, :, w * 256 : w * 256 + 256] = prod.reshape(4, 128, 256)
    P1[:, :, 512:640] = SQ[...]

    def enc(v, edge):
        if edge is None:
            return v.astype(BF16)
        m = v.shape[1] - 128
        last = v[:, m:]
        low = last - last.astype(BF16).astype(F32)
        last = jnp.where(lanes_of(v.shape[0]) >= (edge + 128) // 2, low, last)
        return jnp.concatenate([v[:, :m].astype(BF16), last.astype(BF16)], axis=1)

    def dec(v, edge):
        v = v.astype(F32)
        if edge is None:
            return v
        m = v.shape[1] - 128
        last, lane = v[:, m:], lanes_of(v.shape[0])
        keep = jnp.logical_or(lane == edge, lane == (edge + 128) // 2)
        total = jnp.sum(jnp.where(keep, last, 0.0), axis=-1, keepdims=True)
        last = jnp.where(lane < edge, last, total)
        return jnp.concatenate([v[:, :m], last], axis=1) if m else last

    def row_loop(n, fn):
        def step(i, _):
            fn(pl.ds(pl.multiple_of(i * 16, 16), 16))
            return 0

        lax.fori_loop(0, n // 16, step, 0)

    def shifted(rows, by):
        return pl.ds(pl.multiple_of(rows.start + by, 16), 16)

    def rs_first(p, A, HL, HR, k, edge):
        def conv(rows):
            A[rows, :] = enc(p[far(x), rows, :], edge)

        row_loop(128, conv)
        send(A.at[pl.ds(0, 64)], HL, k, x_up)
        send(A.at[pl.ds(64, 64)], HR, k + 1, x_dn)

    def rs_second(p, B, C, HL, HR, FL, FR, k, edge):
        u, d = up(x), down(x)
        recv(HL, k)

        def left(rows):
            low = shifted(rows, 64)
            B[rows, :] = enc(p[u, rows, :] + dec(HL[rows, :], edge), edge)
            B[low, :] = enc(p[u, low, :], edge)

        row_loop(64, left)
        send(B, FL, k + 2, x_up)
        recv(HR, k + 1)

        def right(rows):
            low = shifted(rows, 64)
            C[low, :] = enc(p[d, low, :] + dec(HR[rows, :], edge), edge)
            C[rows, :] = enc(p[d, rows, :], edge)

        row_loop(64, right)
        send(C, FR, k + 3, x_dn)

    def rs_wait(FL, FR, k):
        recv(FL, k + 2)
        recv(FR, k + 3)

    k1 = take(4)
    rs_first(P1, A1, HL1, HR1, k1, 0)
    z_fwd(3)
    z_own(5)
    rs_second(P1, B1, C1, HL1, HR1, FL1, FR1, k1, 0)
    for i in range(15):
        recv(SM.at[lax.rem(f + 15 - i, 16)], km + i)
    rs_wait(FL1, FR1, k1)

    total = P1[x] + dec(FL1[...], 0) + dec(FR1[...], 0)
    rs = lax.rsqrt(total[:, 512:513] / depth + EPS)
    eye = lax.broadcasted_iota(jnp.int32, (128, 128), 0) == lanes_of(128)
    for h in range(2):
        cols = slice(h * 128, h * 128 + 128)
        gated = gelu((rs * total[:, cols]).astype(BF16).astype(F32))
        spread = gelu((rs * total[:, 256 + h * 128 : 384 + h * 128]).astype(BF16).astype(F32))
        spread = spread * lax.rsqrt(jnp.mean(spread * spread, axis=-1, keepdims=True) + EPS)
        spread = (spread * vgain[h : h + 1, :]).astype(BF16)
        matrix = SM[:, h].astype(F32).reshape(128, 128).astype(BF16)
        mixed = jnp.dot(matrix, spread, preferred_element_type=F32)
        bias = jnp.broadcast_to(sbias[h : h + 1, :], (128, 128))
        mixed = mixed + jnp.sum(jnp.where(eye, bias, 0.0), axis=-1, keepdims=True)
        joined = gated * mixed
        joined = joined * lax.rsqrt(jnp.mean(joined * joined, axis=-1, keepdims=True) + EPS)
        MG[x, :, cols] = (joined * hgain[h : h + 1, :]).astype(BF16)

    ra, rb = pl.ds(0, 64), pl.ds(64, 64)

    def x_start(buf, k):
        send(buf.at[x], buf.at[x], k, x_up)
        send(buf.at[x], buf.at[x], k + 1, x_dn)

    def x_mid(buf, k):
        recv(buf.at[down(x)], k)
        send(buf.at[down(x), ra], buf.at[down(x), ra], k + 2, x_up)
        recv(buf.at[up(x)], k + 1)
        send(buf.at[up(x), rb], buf.at[up(x), rb], k + 3, x_dn)

    def x_last(buf, k):
        recv(buf.at[far(x), ra], k + 2)
        recv(buf.at[far(x), rb], k + 3)

    k2 = take(4)
    x_start(MG, k2)
    x_mid(MG, k2)
    z_fwd(4)
    z_own(6)
    z_fin(2)
    x_last(MG, k2)

    def cy_first(lhs, W, CS, CR, k):
        for n, yt in enumerate((far(y), up(y), down(y), y)):
            prod = jnp.dot(lhs(), W[yt], preferred_element_type=F32)
            T[n] = jnp.where(c == 0, prod[:, :128], prod[:, 128:])
            CS[n] = jnp.where(c == 0, prod[:, 128:], prod[:, :128]).astype(BF16)
            send(CS.at[n], CR.at[n], k + n, mate)

    def cy_second(CR, YA, YHL, YHR, k):
        recv(CR.at[0], k)
        YA[...] = (T[0] + CR[0].astype(F32)).astype(BF16)
        send(YA.at[pl.ds(0, 256)], YHL, k + 4, y_up)
        send(YA.at[pl.ds(256, 256)], YHR, k + 5, y_dn)
        for n in (1, 2, 3):
            recv(CR.at[n], k + n)
            T[n] = T[n] + CR[n].astype(F32)

    def cy_third(YB, YC, YHL, YHR, YFL, YFR, k):
        recv(YHL, k + 4)
        YB[0:256, :] = (T[1, 0:256, :] + YHL[...].astype(F32)).astype(BF16)
        YB[256:512, :] = T[1, 256:512, :].astype(BF16)
        send(YB, YFL, k + 6, y_up)
        recv(YHR, k + 5)
        YC[256:512, :] = (T[2, 256:512, :] + YHR[...].astype(F32)).astype(BF16)
        YC[0:256, :] = T[2, 0:256, :].astype(BF16)
        send(YC, YFR, k + 7, y_dn)

    def cy_last(YFL, YFR, k):
        recv(YFL, k + 6)
        recv(YFR, k + 7)
        return T[3] + YFL[...].astype(F32) + YFR[...].astype(F32)

    k3 = take(8)
    cy_first(lambda: MG[...].reshape(512, 256), WMP, CS4, CR4, k3)
    cy_second(CR4, YA4, YHL4, YHR4, k3)
    cy_third(YB4, YC4, YHL4, YHR4, YFL4, YFR4, k3)
    z_fwd(5)
    z_own(7)
    branch = cy_last(YFL4, YFR4, k3)
    hidden = (XG[me].reshape(512, 128).astype(F32) + branch).astype(BF16)
    HG[me] = hidden.reshape(4, 128, 128)

    kh = take(9)
    y_start(HG, kh)
    y_mid(HG, kh)
    y_end(HG, kh)
    z_fin(3)
    z_fin(4)
    y_last(HG, kh)
    scaled(HG, 1)

    def project(W, p):
        def cut(cols, n):
            w = W[:, :, cols].reshape(1024, n)
            prod = jnp.dot(XS[...], w, preferred_element_type=F32)
            p[:, :, cols] = prod.reshape(4, 128, n)

        def step(i, _):
            cut(pl.ds(pl.multiple_of(i * 256, 256), 256), 256)
            return 0

        lax.fori_loop(0, inner // 256, step, 0)
        if inner % 256:
            cut(pl.ds(inner - inner % 256, inner % 256), inner % 256)

    project(WGU, P2)
    edge = 128 - (inner - dn.shape[0])
    last = P2[:, :, inner - 128 : inner]
    lane = lax.broadcasted_iota(jnp.int32, (4, 128, 128), 2)
    P2[:, :, inner - 128 : inner] = jnp.where(lane < edge, last, SQ[...])
    k4, k5 = take(4), take(4)
    rs_first(P2, A2, HL2, HR2, k4, edge)
    z_fwd(6)
    z_own(8)
    z_fin(5)
    z_fin(6)
    project(WVU, P3)
    rs_second(P2, B2, C2, HL2, HR2, FL2, FR2, k4, edge)
    rs_first(P3, A3, HL3, HR3, k5, None)
    z_fwd(7)
    rs_wait(FL2, FR2, k4)
    rs_second(P3, B3, C3, HL3, HR3, FL3, FR3, k5, None)
    z_fwd(8)
    rs_wait(FL3, FR3, k5)

    at_end = slice(inner - 128, inner)
    sq = P2[x, :, at_end] + dec(FL2[:, at_end], edge) + dec(FR2[:, at_end], edge)
    rs2 = lax.rsqrt(sq[:, 127:128] / depth + EPS)
    row = lax.broadcasted_iota(jnp.int32, (128, 128), 0)

    def conv_tile(i, _):
        cols = pl.ds(pl.multiple_of(i * 128, 128), 128)

        def one(p, FL, FR, w):
            v = p[x, :, cols] + FL[:, cols].astype(F32) + FR[:, cols].astype(F32)
            v = (rs2 * v).astype(BF16).astype(F32)
            prev = jnp.where(row == 0, 0.0, pltpu.roll(v, 1, axis=0))
            after = jnp.where(row == 127, 0.0, pltpu.roll(v, 127, axis=0))
            k = cv[w, :, cols]
            return k[3:4] + prev * k[0:1] + v * k[1:2] + after * k[2:3]

        active = gelu(one(P2, FL2, FR2, 0)) * one(P3, FL3, FR3, 1)
        ACT[x, :, cols] = active.astype(BF16)
        return 0

    lax.fori_loop(0, inner // 128, conv_tile, 0)

    k6 = take(4)
    x_start(ACT, k6)
    x_mid(ACT, k6)
    z_fin(7)
    z_fin(8)
    x_last(ACT, k6)

    k7 = take(8)
    cy_first(lambda: ACT[...].reshape(512, inner), WDN, CS5, CR5, k7)
    cy_second(CR5, YA5, YHL5, YHR5, k7)
    cy_third(YB5, YC5, YHL5, YHR5, YFL5, YFR5, k7)
    change = cy_last(YFL5, YFR5, k7)
    result = (HG[me].reshape(512, 128).astype(F32) + change).astype(BF16)
    OP[...] = result.reshape(4, 128, 128)

    ko = take(4)
    place = lax.rem(x, 2)
    to_cols = pl.ds(pl.multiple_of(place * 256 + c * 128, 128), 128)
    for j in range(4):
        mine = jnp.logical_and(x == j, to_me)
        copy = remote(
            OP.at[j], out.at[:, to_cols], ko + j, ko + 2 * place + c,
            at(x_=jnp.int32(j), c_=x // 2),
        )
        swaps.append((mine, copy))

        @pl.when(jnp.logical_not(mine))
        def _():
            copy.start()

        @pl.when(mine)
        def _():
            out[:, to_cols] = OP[j]

    for j in range(2):
        for h in range(2):

            @pl.when(jnp.logical_not(jnp.logical_and(2 * c + j == x, c == h)))
            def _():
                recv(out.at[:, pl.ds(j * 256 + h * 128, 128)], ko + 2 * j + h)

    for copy in started:
        copy.wait_send()
    for mine, copy in swaps:

        @pl.when(jnp.logical_not(mine))
        def _():
            copy.wait_send()


def body(
    tokens, mixer_gain, gate_proj, value_proj, value_gain, spatial_mix, spatial_bias,
    head_gain, merge_proj, ffn_gain, gate_up, value_up, gate_kernel, value_kernel,
    gate_offset, value_offset, down_proj,
):
    inner = gate_up.shape[1]
    wide = -(-inner // 128) * 128
    extra = ((0, 0), (0, wide - inner))
    gains = jnp.stack([mixer_gain, ffn_gain]).reshape(2, 16, 256)
    conv = jnp.stack([
        jnp.concatenate([gate_kernel, gate_offset[None]]),
        jnp.concatenate([value_kernel, value_offset[None]]),
    ])
    conv = jnp.pad(conv, ((0, 0), *extra))
    gate_up, value_up = jnp.pad(gate_up, extra), jnp.pad(value_up, extra)
    vm = lambda shape, dtype=BF16: pltpu.VMEM(shape, dtype)

    def rs_x(n):
        return [
            vm((4, 128, n), F32), *[vm((128, n))] * 3, *[vm((64, n))] * 2, *[vm((128, n))] * 2,
        ]

    def rs_y():
        return [
            *[vm((4, 512, 128))] * 2, *[vm((512, 128))] * 3, *[vm((256, 128))] * 2,
            *[vm((512, 128))] * 2,
        ]

    in_vmem = pl.BlockSpec(memory_space=pltpu.VMEM)
    left = pl.BlockSpec(memory_space=pl.ANY)
    call = pl.pallas_call(
        kernel,
        out_shape=jax.ShapeDtypeStruct(tokens.shape, tokens.dtype),
        in_specs=[
            in_vmem, in_vmem, left, left, in_vmem, in_vmem, in_vmem, in_vmem, left,
            left, left, in_vmem, left,
        ],
        out_specs=in_vmem,
        scratch_shapes=[
            vm((8, 4, 128, 128)), vm((8, 4, 128, 128)), vm((512, 1024)),
            vm((4, 256, 256)), vm((4, 256, 256)), vm((4, 256, 256)),
            vm((4, 256, wide)), vm((4, 256, wide)), vm((4, wide, 256)),
            vm((16, 2, 8, 128)), vm((4, 128, 128), F32), vm((4, 128, 256)),
            vm((4, 128, wide)), vm((4, 128, 128)),
            *rs_x(640), *rs_x(wide), *rs_x(wide),
            vm((4, 512, 128), F32), *rs_y(), *rs_y(),
            pltpu.SemaphoreType.DMA((SEMS,)), pltpu.SemaphoreType.DMA((SEMS,)),
            pltpu.SemaphoreType.DMA((9,)),
        ],
        compiler_params=pltpu.CompilerParams(
            collective_id=0, has_side_effects=True, vmem_limit_bytes=58 << 20
        ),
        name="layer",
    )
    return call(
        tokens, gains, gate_proj, value_proj, value_gain, spatial_mix, spatial_bias,
        head_gain, merge_proj, gate_up, value_up, conv, down_proj,
    )


def solution(mesh):
    finer = Mesh(
        mesh.devices.reshape(mesh.shape["rep"], 4, 4, 4, 2), ("rep", "fs_0", "fs_1", "tp_0", "tp_1")
    )
    return jax.shard_map(
        body,
        mesh=finer,
        in_specs=(
            P(REP_FS, TP), P(), P(FS, TP), P(FS, TP), P(TP, None), P(TP, FS, None),
            P(TP, None), P(TP, None), P(TP, FS), P(), P(FS, TP), P(FS, TP), P(None, TP),
            P(None, TP), P(TP), P(TP), P(TP, FS),
        ),
        out_specs=P(REP_FS, TP),
        check_vma=False,
    )
```

```python
import jax
import jax.numpy as jnp
from jax import lax
from jax.experimental import pallas as pl
from jax.experimental.pallas import tpu as pltpu
from jax.sharding import Mesh
from jax.sharding import PartitionSpec as P

TP = ("tp_0", "tp_1")
FS = ("fs_0", "fs_1")
REP_FS = ("rep", "fs_0", "fs_1")
MESH = pl.DeviceIdType.MESH
EPS = 1e-06
F32 = jnp.float32
BF16 = jnp.bfloat16
SEMS = 160


def gelu(v):
    return 0.5 * v * (1.0 + lax.erf(v * 0.7071067811865476))


def lanes_of(n):
    return lax.broadcasted_iota(jnp.int32, (n, 128), 1)


def kernel(
    tok, mgain, fgain, gp, vp, vgain, smix, sbias, hgain, mp, gu, vu, gk, vk, go, vo, dn,
    out,
    cv, XG, HG, XS, WGP, WVP, WMP, WGU, WVU, WDN, SM, SQ, MG, ACT, OP,
    P1, A1, B1, C1, HL1, HR1, FL1, FR1,
    P2, A2, B2, C2, HL2, HR2, FL2, FR2,
    P3, A3, B3, C3, HL3, HR3, FL3, FR3,
    T, CS4, CR4, YA4, YB4, YC4, YHL4, YHR4, YFL4, YFR4,
    CS5, CR5, YA5, YB5, YC5, YHL5, YHR5, YFL5, YFR5,
    ssem, rsem, lsem,
):
    r, z, x, y, c = (lax.axis_index(a) for a in ("rep", "fs_0", "fs_1", "tp_0", "tp_1"))
    other = 1 - c
    f = 4 * z + x
    units = dn.shape[0]
    inner = cv.shape[2]
    depth = mgain.shape[0]

    def at(z_=None, x_=None, y_=None, c_=None, r_=None):
        pick = lambda new, old: old if new is None else new
        return (pick(r_, r), pick(z_, z), pick(x_, x), pick(y_, y), pick(c_, c))

    up = lambda v: lax.rem(v + 1, 4)
    down = lambda v: lax.rem(v + 3, 4)
    far = lambda v: lax.rem(v + 2, 4)

    zr = 4 * r + z
    zu, zd = lax.rem(zr + 1, 8), lax.rem(zr + 7, 8)
    z_up = at(r_=zu // 4, z_=lax.rem(zu, 4))
    z_dn = at(r_=zd // 4, z_=lax.rem(zd, 4))
    x_up, x_dn = at(x_=up(x)), at(x_=down(x))
    y_up, y_dn = at(y_=up(y)), at(y_=down(y))
    mate = at(c_=other)
    fs_peers = []
    for i in range(1, 16):
        g = lax.rem(f + i, 16)
        fs_peers.append(at(z_=g // 4, x_=lax.rem(g, 4)))

    barrier = pltpu.get_barrier_semaphore()
    greet = fs_peers + [at(x_=jnp.int32(k), c_=other) for k in range(4)]
    greet += [y_up, y_dn, z_up, z_dn]
    for peer in greet:
        pl.semaphore_signal(barrier, inc=1, device_id=peer, device_id_type=MESH)
    pl.semaphore_wait(barrier, len(greet))

    started = []
    count = [0]

    def take(n=1):
        first = count[0]
        count[0] += n
        return first

    def remote(src, dst, s, k, peer):
        return pltpu.make_async_remote_copy(
            src_ref=src, dst_ref=dst, send_sem=ssem.at[s], recv_sem=rsem.at[k],
            device_id=peer, device_id_type=MESH,
        )

    def send(src, dst, k, peer):
        copy = remote(src, dst, k, k, peer)
        copy.start()
        started.append(copy)

    def recv(dst, k):
        remote(dst, dst, 0, k, mate).wait_recv()

    half = units // 2
    chunks = [
        (gp, WGP, 0, 256, 128), (vp, WVP, 0, 256, 128), (mp, WMP, 0, 256, 128),
        (gu, WGU, 0, half, 352), (gu, WGU, half, half, 352),
        (vu, WVU, 0, half, 352), (vu, WVU, half, half, 352),
        (dn, WDN, 0, half, 352), (dn, WDN, half, half, 352),
    ]
    zk = [take(4) for _ in chunks]

    def z_own(i):
        src, buf, at0, n, _ = chunks[i]
        rows = pl.ds(at0, n)
        send(src.at[rows], buf.at[z, rows], zk[i], z_up)
        send(src.at[rows], buf.at[z, rows], zk[i] + 1, z_dn)
        pltpu.make_async_copy(src.at[rows], buf.at[z, rows], lsem.at[i]).start()

    def z_fwd(i):
        _, buf, at0, n, cut = chunks[i]
        lo, hi = down(z), up(z)
        recv(buf.at[lo, pl.ds(at0, n)], zk[i])
        a = pl.ds(at0, cut)
        send(buf.at[lo, a], buf.at[lo, a], zk[i] + 2, z_up)
        recv(buf.at[hi, pl.ds(at0, n)], zk[i] + 1)
        b = pl.ds(at0 + cut, n - cut)
        send(buf.at[hi, b], buf.at[hi, b], zk[i] + 3, z_dn)

    def z_fin(i):
        src, buf, at0, n, cut = chunks[i]
        rows = pl.ds(at0, n)
        recv(buf.at[far(z), pl.ds(at0, cut)], zk[i] + 2)
        recv(buf.at[far(z), pl.ds(at0 + cut, n - cut)], zk[i] + 3)
        pltpu.make_async_copy(src.at[rows], buf.at[z, rows], lsem.at[i]).wait()

    for W in (WGU, WVU, WDN):
        for k in range(4):
            W[k, units:, :] = jnp.zeros((inner - units, 256), BF16)
    for w, kern, off in ((0, gk, go), (1, vk, vo)):
        cv[w, :, inner - 128 :] = jnp.zeros((4, 128), F32)
        cv[w, 0:3, 0:units] = kern[...]
        cv[w, 3:4, 0:units] = off[...].reshape(1, units)

    swaps = []
    kx = take(4)
    me = 2 * y + c
    to_me = x // 2 == c
    for j in range(2):
        for h in range(2):
            xt = 2 * c + j
            mine = jnp.logical_and(xt == x, c == h)
            cols = slice(j * 256 + h * 128, j * 256 + h * 128 + 128)
            copy = remote(
                tok.at[:, cols], XG.at[2 * y + h, x], kx + 2 * j + h, kx + x,
                at(x_=xt, c_=jnp.int32(h)),
            )

            swaps.append((mine, copy))

            @pl.when(jnp.logical_not(mine))
            def _():
                copy.start()

            @pl.when(mine)
            def _():
                XG[2 * y + h, x] = tok[:, cols]

    z_own(0)
    z_own(1)
    z_own(2)
    km = take(15)
    for i in range(15):
        send(smix, SM.at[f], km + i, fs_peers[i])
    SM[f] = smix[...]

    for j in range(4):

        @pl.when(jnp.logical_not(jnp.logical_and(x == j, to_me)))
        def _():
            recv(XG.at[me, j], kx + j)

    def y_start(buf, k):
        send(buf.at[me], buf.at[me], k, y_up)
        send(buf.at[me], buf.at[me], k + 1, y_dn)
        send(buf.at[me], buf.at[me], k + 2, mate)

    lo_y, hi_y, far_y = 2 * down(y) + c, 2 * up(y) + c, 2 * far(y) + c
    a2, b2 = pl.ds(0, 2), pl.ds(2, 2)

    def y_mid(buf, k):
        recv(buf.at[lo_y], k)
        send(buf.at[lo_y, a2], buf.at[lo_y, a2], k + 3, y_up)
        recv(buf.at[hi_y], k + 1)
        send(buf.at[hi_y, b2], buf.at[hi_y, b2], k + 4, y_dn)
        send(buf.at[lo_y], buf.at[lo_y], k + 5, mate)
        send(buf.at[hi_y], buf.at[hi_y], k + 6, mate)

    def y_end(buf, k):
        recv(buf.at[far_y, a2], k + 3)
        send(buf.at[far_y, a2], buf.at[far_y, a2], k + 7, mate)
        recv(buf.at[far_y, b2], k + 4)
        send(buf.at[far_y, b2], buf.at[far_y, b2], k + 8, mate)

    def y_last(buf, k):
        recv(buf.at[2 * y + other], k + 2)
        recv(buf.at[2 * down(y) + other], k + 5)
        recv(buf.at[2 * up(y) + other], k + 6)
        recv(buf.at[2 * far(y) + other, a2], k + 7)
        recv(buf.at[2 * far(y) + other, b2], k + 8)

    def scaled(buf, gains):
        parts = [gains[pl.ds(pl.multiple_of((4 * k + x) * 256, 256), 256)] for k in range(4)]
        gain = jnp.concatenate([part.reshape(1, 256) for part in parts], axis=1)

        def block(b, _):
            rows = jnp.concatenate([buf[i, b] for i in range(8)], axis=1).astype(F32)
            SQ[b] = jnp.broadcast_to(jnp.sum(rows * rows, axis=-1, keepdims=True), (128, 128))
            XS[pl.ds(pl.multiple_of(b * 128, 128), 128), :] = (rows * gain).astype(BF16)
            return 0

        lax.fori_loop(0, 4, block, 0)

    ky = take(9)
    y_start(XG, ky)
    z_fwd(0)
    y_mid(XG, ky)
    z_fwd(1)
    y_end(XG, ky)
    z_fwd(2)
    z_own(3)
    z_own(4)
    y_last(XG, ky)

    scaled(XG, mgain)
    z_fin(0)
    z_fin(1)
    for w, W in ((0, WGP), (1, WVP)):
        prod = jnp.dot(XS[...], W[...].reshape(1024, 256), preferred_element_type=F32)
        P1[:, :, w * 256 : w * 256 + 256] = prod.reshape(4, 128, 256)
    P1[:, :, 512:640] = SQ[...]

    def enc(v, edge):
        if edge is None:
            return v.astype(BF16)
        m = v.shape[1] - 128
        last = v[:, m:]
        low = last - last.astype(BF16).astype(F32)
        last = jnp.where(lanes_of(v.shape[0]) >= (edge + 128) // 2, low, last)
        return jnp.concatenate([v[:, :m].astype(BF16), last.astype(BF16)], axis=1)

    def dec(v, edge):
        v = v.astype(F32)
        if edge is None:
            return v
        m = v.shape[1] - 128
        last, lane = v[:, m:], lanes_of(v.shape[0])
        keep = jnp.logical_or(lane == edge, lane == (edge + 128) // 2)
        total = jnp.sum(jnp.where(keep, last, 0.0), axis=-1, keepdims=True)
        last = jnp.where(lane < edge, last, total)
        return jnp.concatenate([v[:, :m], last], axis=1) if m else last

    def row_loop(n, fn):
        def step(i, _):
            fn(pl.ds(pl.multiple_of(i * 16, 16), 16))
            return 0

        lax.fori_loop(0, n // 16, step, 0)

    def shifted(rows, by):
        return pl.ds(pl.multiple_of(rows.start + by, 16), 16)

    def rs_first(p, A, HL, HR, k, edge):
        def conv(rows):
            A[rows, :] = enc(p[far(x), rows, :], edge)

        row_loop(128, conv)
        send(A.at[pl.ds(0, 64)], HL, k, x_up)
        send(A.at[pl.ds(64, 64)], HR, k + 1, x_dn)

    def rs_second(p, B, C, HL, HR, FL, FR, k, edge):
        u, d = up(x), down(x)
        recv(HL, k)

        def left(rows):
            low = shifted(rows, 64)
            B[rows, :] = enc(p[u, rows, :] + dec(HL[rows, :], edge), edge)
            B[low, :] = enc(p[u, low, :], edge)

        row_loop(64, left)
        send(B, FL, k + 2, x_up)
        recv(HR, k + 1)

        def right(rows):
            low = shifted(rows, 64)
            C[low, :] = enc(p[d, low, :] + dec(HR[rows, :], edge), edge)
            C[rows, :] = enc(p[d, rows, :], edge)

        row_loop(64, right)
        send(C, FR, k + 3, x_dn)

    def rs_wait(FL, FR, k):
        recv(FL, k + 2)
        recv(FR, k + 3)

    k1 = take(4)
    rs_first(P1, A1, HL1, HR1, k1, 0)
    z_fwd(3)
    z_own(5)
    rs_second(P1, B1, C1, HL1, HR1, FL1, FR1, k1, 0)
    for i in range(15):
        recv(SM.at[lax.rem(f + 15 - i, 16)], km + i)
    rs_wait(FL1, FR1, k1)

    total = P1[x] + dec(FL1[...], 0) + dec(FR1[...], 0)
    rs = lax.rsqrt(total[:, 512:513] / depth + EPS)
    eye = lax.broadcasted_iota(jnp.int32, (128, 128), 0) == lanes_of(128)
    for h in range(2):
        cols = slice(h * 128, h * 128 + 128)
        gated = gelu((rs * total[:, cols]).astype(BF16).astype(F32))
        spread = gelu((rs * total[:, 256 + h * 128 : 384 + h * 128]).astype(BF16).astype(F32))
        spread = spread * lax.rsqrt(jnp.mean(spread * spread, axis=-1, keepdims=True) + EPS)
        spread = (spread * vgain[h : h + 1, :]).astype(BF16)
        matrix = SM[:, h].astype(F32).reshape(128, 128).astype(BF16)
        mixed = jnp.dot(matrix, spread, preferred_element_type=F32)
        bias = jnp.broadcast_to(sbias[h : h + 1, :], (128, 128))
        mixed = mixed + jnp.sum(jnp.where(eye, bias, 0.0), axis=-1, keepdims=True)
        joined = gated * mixed
        joined = joined * lax.rsqrt(jnp.mean(joined * joined, axis=-1, keepdims=True) + EPS)
        MG[x, :, cols] = (joined * hgain[h : h + 1, :]).astype(BF16)

    ra, rb = pl.ds(0, 64), pl.ds(64, 64)

    def x_start(buf, k):
        send(buf.at[x], buf.at[x], k, x_up)
        send(buf.at[x], buf.at[x], k + 1, x_dn)

    def x_mid(buf, k):
        recv(buf.at[down(x)], k)
        send(buf.at[down(x), ra], buf.at[down(x), ra], k + 2, x_up)
        recv(buf.at[up(x)], k + 1)
        send(buf.at[up(x), rb], buf.at[up(x), rb], k + 3, x_dn)

    def x_last(buf, k):
        recv(buf.at[far(x), ra], k + 2)
        recv(buf.at[far(x), rb], k + 3)

    k2 = take(4)
    x_start(MG, k2)
    x_mid(MG, k2)
    z_fwd(4)
    z_own(6)
    z_fin(2)
    x_last(MG, k2)

    def cy_first(lhs, W, CS, CR, k):
        for n, yt in enumerate((far(y), up(y), down(y), y)):
            prod = jnp.dot(lhs(), W[yt], preferred_element_type=F32)
            T[n] = jnp.where(c == 0, prod[:, :128], prod[:, 128:])
            CS[n] = jnp.where(c == 0, prod[:, 128:], prod[:, :128]).astype(BF16)
            send(CS.at[n], CR.at[n], k + n, mate)

    def cy_second(CR, YA, YHL, YHR, k):
        recv(CR.at[0], k)
        YA[...] = (T[0] + CR[0].astype(F32)).astype(BF16)
        send(YA.at[pl.ds(0, 256)], YHL, k + 4, y_up)
        send(YA.at[pl.ds(256, 256)], YHR, k + 5, y_dn)
        for n in (1, 2, 3):
            recv(CR.at[n], k + n)
            T[n] = T[n] + CR[n].astype(F32)

    def cy_third(YB, YC, YHL, YHR, YFL, YFR, k):
        recv(YHL, k + 4)
        YB[0:256, :] = (T[1, 0:256, :] + YHL[...].astype(F32)).astype(BF16)
        YB[256:512, :] = T[1, 256:512, :].astype(BF16)
        send(YB, YFL, k + 6, y_up)
        recv(YHR, k + 5)
        YC[256:512, :] = (T[2, 256:512, :] + YHR[...].astype(F32)).astype(BF16)
        YC[0:256, :] = T[2, 0:256, :].astype(BF16)
        send(YC, YFR, k + 7, y_dn)

    def cy_last(YFL, YFR, k):
        recv(YFL, k + 6)
        recv(YFR, k + 7)
        return T[3] + YFL[...].astype(F32) + YFR[...].astype(F32)

    k3 = take(8)
    cy_first(lambda: MG[...].reshape(512, 256), WMP, CS4, CR4, k3)
    cy_second(CR4, YA4, YHL4, YHR4, k3)
    cy_third(YB4, YC4, YHL4, YHR4, YFL4, YFR4, k3)
    z_fwd(5)
    z_own(7)
    branch = cy_last(YFL4, YFR4, k3)
    hidden = (XG[me].reshape(512, 128).astype(F32) + branch).astype(BF16)
    HG[me] = hidden.reshape(4, 128, 128)

    kh = take(9)
    y_start(HG, kh)
    y_mid(HG, kh)
    y_end(HG, kh)
    z_fin(3)
    z_fin(4)
    y_last(HG, kh)
    scaled(HG, fgain)

    def project(W, p):
        def cut(cols, n):
            w = jnp.concatenate([W[k, cols, :] for k in range(4)], axis=1)
            prod = lax.dot_general(
                XS[...], w, (((1,), (1,)), ((), ())), preferred_element_type=F32
            )
            p[:, :, cols] = prod.reshape(4, 128, n)

        def step(i, _):
            cut(pl.ds(pl.multiple_of(i * 256, 256), 256), 256)
            return 0

        lax.fori_loop(0, inner // 256, step, 0)
        if inner % 256:
            cut(pl.ds(inner - inner % 256, inner % 256), inner % 256)

    project(WGU, P2)
    edge = 128 - (inner - units)
    last = P2[:, :, inner - 128 : inner]
    lane = lax.broadcasted_iota(jnp.int32, (4, 128, 128), 2)
    P2[:, :, inner - 128 : inner] = jnp.where(lane < edge, last, SQ[...])
    k4, k5 = take(4), take(4)
    rs_first(P2, A2, HL2, HR2, k4, edge)
    z_fwd(6)
    z_own(8)
    z_fin(5)
    z_fin(6)
    project(WVU, P3)
    rs_second(P2, B2, C2, HL2, HR2, FL2, FR2, k4, edge)
    rs_first(P3, A3, HL3, HR3, k5, None)
    z_fwd(7)
    rs_wait(FL2, FR2, k4)
    rs_second(P3, B3, C3, HL3, HR3, FL3, FR3, k5, None)
    z_fwd(8)
    rs_wait(FL3, FR3, k5)

    at_end = slice(inner - 128, inner)
    sq = P2[x, :, at_end] + dec(FL2[:, at_end], edge) + dec(FR2[:, at_end], edge)
    rs2 = lax.rsqrt(sq[:, 127:128] / depth + EPS)
    row = lax.broadcasted_iota(jnp.int32, (128, 128), 0)

    def conv_tile(i, _):
        cols = pl.ds(pl.multiple_of(i * 128, 128), 128)

        def one(p, FL, FR, w):
            v = p[x, :, cols] + FL[:, cols].astype(F32) + FR[:, cols].astype(F32)
            v = (rs2 * v).astype(BF16).astype(F32)
            prev = jnp.where(row == 0, 0.0, pltpu.roll(v, 1, axis=0))
            after = jnp.where(row == 127, 0.0, pltpu.roll(v, 127, axis=0))
            k = cv[w, :, cols]
            return k[3:4] + prev * k[0:1] + v * k[1:2] + after * k[2:3]

        active = gelu(one(P2, FL2, FR2, 0)) * one(P3, FL3, FR3, 1)
        ACT[x, :, cols] = active.astype(BF16)
        return 0

    lax.fori_loop(0, inner // 128, conv_tile, 0)

    k6 = take(4)
    x_start(ACT, k6)
    x_mid(ACT, k6)
    z_fin(7)
    z_fin(8)
    x_last(ACT, k6)

    k7 = take(8)
    cy_first(lambda: ACT[...].reshape(512, inner), WDN, CS5, CR5, k7)
    cy_second(CR5, YA5, YHL5, YHR5, k7)
    cy_third(YB5, YC5, YHL5, YHR5, YFL5, YFR5, k7)
    change = cy_last(YFL5, YFR5, k7)
    result = (HG[me].reshape(512, 128).astype(F32) + change).astype(BF16)
    OP[...] = result.reshape(4, 128, 128)

    ko = take(4)
    place = lax.rem(x, 2)
    to_cols = pl.ds(pl.multiple_of(place * 256 + c * 128, 128), 128)
    for j in range(4):
        mine = jnp.logical_and(x == j, to_me)
        copy = remote(
            OP.at[j], out.at[:, to_cols], ko + j, ko + 2 * place + c,
            at(x_=jnp.int32(j), c_=x // 2),
        )
        swaps.append((mine, copy))

        @pl.when(jnp.logical_not(mine))
        def _():
            copy.start()

        @pl.when(mine)
        def _():
            out[:, to_cols] = OP[j]

    for j in range(2):
        for h in range(2):

            @pl.when(jnp.logical_not(jnp.logical_and(2 * c + j == x, c == h)))
            def _():
                recv(out.at[:, pl.ds(j * 256 + h * 128, 128)], ko + 2 * j + h)

    for copy in started:
        copy.wait_send()
    for mine, copy in swaps:

        @pl.when(jnp.logical_not(mine))
        def _():
            copy.wait_send()


def body(
    tokens, mixer_gain, gate_proj, value_proj, value_gain, spatial_mix, spatial_bias,
    head_gain, merge_proj, ffn_gain, gate_up, value_up, gate_kernel, value_kernel,
    gate_offset, value_offset, down_proj,
):
    wide = -(-gate_up.shape[1] // 128) * 128
    vm = lambda shape, dtype=BF16: pltpu.VMEM(shape, dtype)

    def rs_x(n):
        return [
            vm((4, 128, n), F32), *[vm((128, n))] * 3, *[vm((64, n))] * 2, *[vm((128, n))] * 2,
        ]

    def rs_y():
        return [
            *[vm((4, 512, 128))] * 2, *[vm((512, 128))] * 3, *[vm((256, 128))] * 2,
            *[vm((512, 128))] * 2,
        ]

    in_vmem = pl.BlockSpec(memory_space=pltpu.VMEM)
    left = pl.BlockSpec(memory_space=pl.ANY)
    call = pl.pallas_call(
        kernel,
        out_shape=jax.ShapeDtypeStruct(tokens.shape, tokens.dtype),
        in_specs=[
            in_vmem, in_vmem, in_vmem, left, left, in_vmem, in_vmem, in_vmem, in_vmem, left,
            left, left, in_vmem, in_vmem, in_vmem, in_vmem, left,
        ],
        out_specs=in_vmem,
        scratch_shapes=[
            vm((2, 4, wide), F32),
            vm((8, 4, 128, 128)), vm((8, 4, 128, 128)), vm((512, 1024)),
            vm((4, 256, 256)), vm((4, 256, 256)), vm((4, 256, 256)),
            vm((4, wide, 256)), vm((4, wide, 256)), vm((4, wide, 256)),
            vm((16, 2, 8, 128)), vm((4, 128, 128), F32), vm((4, 128, 256)),
            vm((4, 128, wide)), vm((4, 128, 128)),
            *rs_x(640), *rs_x(wide), *rs_x(wide),
            vm((4, 512, 128), F32), *rs_y(), *rs_y(),
            pltpu.SemaphoreType.DMA((SEMS,)), pltpu.SemaphoreType.DMA((SEMS,)),
            pltpu.SemaphoreType.DMA((9,)),
        ],
        compiler_params=pltpu.CompilerParams(
            collective_id=0, has_side_effects=True, vmem_limit_bytes=58 << 20
        ),
        name="layer",
    )
    return call(
        tokens, mixer_gain, ffn_gain, gate_proj, value_proj, value_gain, spatial_mix,
        spatial_bias, head_gain, merge_proj, gate_up.T, value_up.T, gate_kernel, value_kernel,
        gate_offset, value_offset, down_proj,
    )


def solution(mesh):
    finer = Mesh(
        mesh.devices.reshape(mesh.shape["rep"], 4, 4, 4, 2), ("rep", "fs_0", "fs_1", "tp_0", "tp_1")
    )
    return jax.shard_map(
        body,
        mesh=finer,
        in_specs=(
            P(REP_FS, TP), P(), P(FS, TP), P(FS, TP), P(TP, None), P(TP, FS, None),
            P(TP, None), P(TP, None), P(TP, FS), P(), P(FS, TP), P(FS, TP), P(None, TP),
            P(None, TP), P(TP), P(TP), P(TP, FS),
        ),
        out_specs=P(REP_FS, TP),
        check_vma=False,
    )
```

```python
import jax
import jax.numpy as jnp
from jax import lax
from jax.experimental import pallas as pl
from jax.experimental.pallas import tpu as pltpu
from jax.sharding import Mesh
from jax.sharding import PartitionSpec as P

TP = ("tp_0", "tp_1")
FS = ("fs_0", "fs_1")
REP_FS = ("rep", "fs_0", "fs_1")
MESH = pl.DeviceIdType.MESH
EPS = 1e-06
F32 = jnp.float32
BF16 = jnp.bfloat16
SEMS = 192


def gelu(v):
    return 0.5 * v * (1.0 + lax.erf(v * 0.7071067811865476))


def lanes_of(n):
    return lax.broadcasted_iota(jnp.int32, (n, 128), 1)


def kernel(
    tok, mgain, fgain, gp, vp, vgain, smix, sbias, hgain, mp, gu, vu, gk, vk, go, vo, dn,
    out,
    CV0, CV1, XG, HG, XS, SQ, RS, SM, MG, OP,
    WGP, WVP, WMP, WGU0, WVU0, WGU1, WVU1, WDN0, WDN1,
    ACT0, ACT1, T, ACC,
    P1, A1, B1, C1, HL1, HR1, FL1, FR1,
    P2, A2, B2, C2, HL2, HR2, FL2, FR2,
    P3, A3, B3, C3, HL3, HR3, FL3, FR3,
    CS4, CR4, YA4, YB4, YC4, YHL4, YHR4, YFL4, YFR4,
    CS5, CR5, YA5, YB5, YC5, YHL5, YHR5, YFL5, YFR5,
    ssem, rsem, lsem,
):
    r, z, x, y, c = (lax.axis_index(a) for a in ("rep", "fs_0", "fs_1", "tp_0", "tp_1"))
    other = 1 - c
    f = 4 * z + x
    units = dn.shape[0]
    n1 = CV1.shape[2]
    n0 = CV0.shape[2]
    real0 = units - n1
    edge = 128 - (n0 - real0)
    depth = mgain.shape[0]

    def at(z_=None, x_=None, y_=None, c_=None, r_=None):
        pick = lambda new, old: old if new is None else new
        return (pick(r_, r), pick(z_, z), pick(x_, x), pick(y_, y), pick(c_, c))

    up = lambda v: lax.rem(v + 1, 4)
    down = lambda v: lax.rem(v + 3, 4)
    far = lambda v: lax.rem(v + 2, 4)

    zr = 4 * r + z
    zu, zd = lax.rem(zr + 1, 8), lax.rem(zr + 7, 8)
    z_up = at(r_=zu // 4, z_=lax.rem(zu, 4))
    z_dn = at(r_=zd // 4, z_=lax.rem(zd, 4))
    x_up, x_dn = at(x_=up(x)), at(x_=down(x))
    y_up, y_dn = at(y_=up(y)), at(y_=down(y))
    mate = at(c_=other)
    fs_peers = []
    for i in range(1, 16):
        g = lax.rem(f + i, 16)
        fs_peers.append(at(z_=g // 4, x_=lax.rem(g, 4)))

    barrier = pltpu.get_barrier_semaphore()
    greet = fs_peers + [at(x_=jnp.int32(k), c_=other) for k in range(4)]
    greet += [y_up, y_dn, z_up, z_dn]
    for peer in greet:
        pl.semaphore_signal(barrier, inc=1, device_id=peer, device_id_type=MESH)
    pl.semaphore_wait(barrier, len(greet))

    started = []
    count = [0]

    def take(n=1):
        first = count[0]
        count[0] += n
        return first

    def remote(src, dst, s, k, peer):
        return pltpu.make_async_remote_copy(
            src_ref=src, dst_ref=dst, send_sem=ssem.at[s], recv_sem=rsem.at[k],
            device_id=peer, device_id_type=MESH,
        )

    def send(src, dst, k, peer):
        copy = remote(src, dst, k, k, peer)
        copy.start()
        started.append(copy)

    def push(ref, k, peer):
        send(ref, ref, k, peer)

    def recv(dst, k):
        remote(dst, dst, 0, k, mate).wait_recv()

    chunks = [
        (gp, WGP, 0, 256), (vp, WVP, 0, 256), (mp, WMP, 0, 256),
        (gu, WGU0, 0, real0), (vu, WVU0, 0, real0),
        (gu, WGU1, real0, n1), (vu, WVU1, real0, n1),
        (dn, WDN0, 0, real0), (dn, WDN1, real0, n1),
    ]
    zk = [take(6) for _ in chunks]

    def z_parts(i):
        _, _, at0, n = chunks[i]
        return (at0, pl.ds(0, n // 2)), (at0 + n // 2, pl.ds(n // 2, n // 2))

    def z_own(i):
        src, buf, at0, n = chunks[i]
        (sa, a), (sb, b) = z_parts(i)
        from_a, from_b = src.at[pl.ds(sa, n // 2)], src.at[pl.ds(sb, n // 2)]
        send(from_a, buf.at[z, a], zk[i], z_up)
        send(from_b, buf.at[z, b], zk[i] + 1, z_dn)
        send(from_b, buf.at[z, b], zk[i] + 2, z_up)
        send(from_a, buf.at[z, a], zk[i] + 3, z_dn)
        z_local(i).start()

    def z_local(i):
        src, buf, at0, n = chunks[i]
        return pltpu.make_async_copy(src.at[pl.ds(at0, n)], buf.at[z, pl.ds(0, n)], lsem.at[i])

    def z_fwd(i):
        buf = chunks[i][1]
        (_, a), (_, b) = z_parts(i)
        recv(buf.at[down(z), a], zk[i])
        push(buf.at[down(z), a], zk[i] + 4, z_up)
        recv(buf.at[up(z), b], zk[i] + 1)
        push(buf.at[up(z), b], zk[i] + 5, z_dn)

    def z_fin(i):
        buf = chunks[i][1]
        (_, a), (_, b) = z_parts(i)
        recv(buf.at[down(z), b], zk[i] + 2)
        recv(buf.at[up(z), a], zk[i] + 3)
        recv(buf.at[far(z), a], zk[i] + 4)
        recv(buf.at[far(z), b], zk[i] + 5)
        z_local(i).wait()

    swaps = []
    kx = take(4)
    me = 2 * y + c
    to_me = x // 2 == c
    for j in range(2):
        for h in range(2):
            xt = 2 * c + j
            mine = jnp.logical_and(xt == x, c == h)
            cols = slice(j * 256 + h * 128, j * 256 + h * 128 + 128)
            copy = remote(
                tok.at[:, cols], XG.at[2 * y + h, x], kx + 2 * j + h, kx + x,
                at(x_=xt, c_=jnp.int32(h)),
            )
            swaps.append((mine, copy))

            @pl.when(jnp.logical_not(mine))
            def _():
                copy.start()

            @pl.when(mine)
            def _():
                XG[2 * y + h, x] = tok[:, cols]

    z_own(0)
    z_own(1)
    z_own(2)

    for j in range(4):

        @pl.when(jnp.logical_not(jnp.logical_and(x == j, to_me)))
        def _():
            recv(XG.at[me, j], kx + j)

    lo_y, hi_y, far_y = 2 * down(y) + c, 2 * up(y) + c, 2 * far(y) + c
    a2, b2 = pl.ds(0, 2), pl.ds(2, 2)

    def y_start(buf, k):
        push(buf.at[me, a2], k, y_up)
        push(buf.at[me, b2], k + 1, y_dn)
        push(buf.at[me, b2], k + 2, y_up)
        push(buf.at[me, a2], k + 3, y_dn)
        push(buf.at[me], k + 6, mate)

    def y_mid(buf, k):
        recv(buf.at[lo_y, a2], k)
        push(buf.at[lo_y, a2], k + 4, y_up)
        push(buf.at[lo_y, a2], k + 7, mate)
        recv(buf.at[hi_y, b2], k + 1)
        push(buf.at[hi_y, b2], k + 5, y_dn)
        push(buf.at[hi_y, b2], k + 8, mate)

    def y_end(buf, k):
        recv(buf.at[lo_y, b2], k + 2)
        push(buf.at[lo_y, b2], k + 9, mate)
        recv(buf.at[hi_y, a2], k + 3)
        push(buf.at[hi_y, a2], k + 10, mate)
        recv(buf.at[far_y, a2], k + 4)
        push(buf.at[far_y, a2], k + 11, mate)
        recv(buf.at[far_y, b2], k + 5)
        push(buf.at[far_y, b2], k + 12, mate)

    def y_last(buf, k):
        recv(buf.at[2 * y + other], k + 6)
        recv(buf.at[2 * down(y) + other, a2], k + 7)
        recv(buf.at[2 * up(y) + other, b2], k + 8)
        recv(buf.at[2 * down(y) + other, b2], k + 9)
        recv(buf.at[2 * up(y) + other, a2], k + 10)
        recv(buf.at[2 * far(y) + other, a2], k + 11)
        recv(buf.at[2 * far(y) + other, b2], k + 12)

    def scaled(buf, gains):
        parts = [gains[pl.ds(pl.multiple_of((4 * k + x) * 256, 256), 256)] for k in range(4)]
        gain = jnp.concatenate([part.reshape(1, 256) for part in parts], axis=1)

        def block(b, _):
            rows = jnp.concatenate([buf[i, b] for i in range(8)], axis=1).astype(F32)
            SQ[b] = jnp.broadcast_to(jnp.sum(rows * rows, axis=-1, keepdims=True), (128, 128))
            XS[pl.ds(pl.multiple_of(b * 128, 128), 128), :] = (rows * gain).astype(BF16)
            return 0

        lax.fori_loop(0, 4, block, 0)

    ky = take(13)
    y_start(XG, ky)
    km = take(15)
    for i in range(15):
        send(smix, SM.at[f], km + i, fs_peers[i])
    SM[f] = smix[...]
    for W in (WGU0, WVU0, WDN0):
        for k in range(4):
            W[k, real0:, :] = jnp.zeros((n0 - real0, 256), BF16)
    for w, kern, off in ((0, gk, go), (1, vk, vo)):
        CV0[w, :, n0 - 128 :] = jnp.zeros((4, 128), F32)
        CV0[w, 0:3, 0:real0] = kern[:, 0:real0]
        CV1[w, 0:3, :] = kern[:, real0:]
        bias = off[...].reshape(1, units)
        CV0[w, 3:4, 0:real0] = bias[:, 0:real0]
        CV1[w, 3:4, :] = bias[:, real0:]
    y_mid(XG, ky)
    z_fwd(0)
    z_fwd(1)
    y_end(XG, ky)
    z_fwd(2)
    z_own(3)
    z_own(4)
    y_last(XG, ky)

    scaled(XG, mgain)
    z_fin(0)
    z_fin(1)
    for w, W in ((0, WGP), (1, WVP)):
        prod = jnp.dot(XS[...], W[...].reshape(1024, 256), preferred_element_type=F32)
        P1[:, :, w * 256 : w * 256 + 256] = prod.reshape(4, 128, 256)
    P1[:, :, 512:640] = SQ[...]

    def enc(v, edge):
        if edge is None:
            return v.astype(BF16)
        m = v.shape[1] - 128
        last = v[:, m:]
        low = last - last.astype(BF16).astype(F32)
        last = jnp.where(lanes_of(v.shape[0]) >= (edge + 128) // 2, low, last)
        return jnp.concatenate([v[:, :m].astype(BF16), last.astype(BF16)], axis=1)

    def dec(v, edge):
        v = v.astype(F32)
        if edge is None:
            return v
        m = v.shape[1] - 128
        last, lane = v[:, m:], lanes_of(v.shape[0])
        keep = jnp.logical_or(lane == edge, lane == (edge + 128) // 2)
        total = jnp.sum(jnp.where(keep, last, 0.0), axis=-1, keepdims=True)
        last = jnp.where(lane < edge, last, total)
        return jnp.concatenate([v[:, :m], last], axis=1) if m else last

    def row_loop(first, n, fn):
        def step(i, _):
            fn(pl.ds(pl.multiple_of(first + i * 16, 16), 16))
            return 0

        lax.fori_loop(0, n // 16, step, 0)

    ra, rb = pl.ds(0, 64), pl.ds(64, 64)

    def rs_first(p, A, B, C, HL, HR, FL, FR, k, edge):
        u, d = up(x), down(x)

        def far_rows(rows):
            A[rows, :] = enc(p[far(x), rows, :], edge)

        def up_rows(rows):
            B[rows, :] = enc(p[u, rows, :], edge)

        def down_rows(rows):
            C[rows, :] = enc(p[d, rows, :], edge)

        row_loop(0, 128, far_rows)
        send(A.at[ra], HL, k, x_up)
        send(A.at[rb], HR, k + 1, x_dn)
        row_loop(64, 64, up_rows)
        send(B.at[rb], FL.at[rb], k + 2, x_up)
        row_loop(0, 64, down_rows)
        send(C.at[ra], FR.at[ra], k + 3, x_dn)

    def rs_second(p, A, B, C, HL, HR, FL, FR, k, edge):
        u, d = up(x), down(x)

        def left(rows):
            B[rows, :] = enc(p[u, rows, :] + dec(HL[rows, :], edge), edge)

        def right(rows):
            low = pl.ds(pl.multiple_of(rows.start + 64, 16), 16)
            C[low, :] = enc(p[d, low, :] + dec(HR[rows, :], edge), edge)

        recv(HL, k)
        row_loop(0, 64, left)
        send(B.at[ra], FL.at[ra], k + 4, x_up)
        recv(HR, k + 1)
        row_loop(0, 64, right)
        send(C.at[rb], FR.at[rb], k + 5, x_dn)

    def rs_wait(FL, FR, k):
        recv(FL.at[rb], k + 2)
        recv(FR.at[ra], k + 3)
        recv(FL.at[ra], k + 4)
        recv(FR.at[rb], k + 5)

    k1 = take(6)
    set1 = (P1, A1, B1, C1, HL1, HR1, FL1, FR1, k1, 0)
    rs_first(*set1)
    rs_second(*set1)
    for i in range(15):
        recv(SM.at[lax.rem(f + 15 - i, 16)], km + i)
    rs_wait(FL1, FR1, k1)

    total = P1[x] + dec(FL1[...], 0) + dec(FR1[...], 0)
    rs = lax.rsqrt(total[:, 512:513] / depth + EPS)
    eye = lax.broadcasted_iota(jnp.int32, (128, 128), 0) == lanes_of(128)
    for h in range(2):
        cols = slice(h * 128, h * 128 + 128)
        gated = gelu((rs * total[:, cols]).astype(BF16).astype(F32))
        spread = gelu((rs * total[:, 256 + h * 128 : 384 + h * 128]).astype(BF16).astype(F32))
        spread = spread * lax.rsqrt(jnp.mean(spread * spread, axis=-1, keepdims=True) + EPS)
        spread = (spread * vgain[h : h + 1, :]).astype(BF16)
        matrix = SM[:, h].astype(F32).reshape(128, 128).astype(BF16)
        mixed = jnp.dot(matrix, spread, preferred_element_type=F32)
        bias = jnp.broadcast_to(sbias[h : h + 1, :], (128, 128))
        mixed = mixed + jnp.sum(jnp.where(eye, bias, 0.0), axis=-1, keepdims=True)
        joined = gated * mixed
        joined = joined * lax.rsqrt(jnp.mean(joined * joined, axis=-1, keepdims=True) + EPS)
        MG[x, :, cols] = (joined * hgain[h : h + 1, :]).astype(BF16)

    def x_start(buf, k):
        push(buf.at[x, ra], k, x_up)
        push(buf.at[x, rb], k + 1, x_dn)
        push(buf.at[x, rb], k + 2, x_up)
        push(buf.at[x, ra], k + 3, x_dn)

    def x_mid(buf, k):
        recv(buf.at[down(x), ra], k)
        push(buf.at[down(x), ra], k + 4, x_up)
        recv(buf.at[up(x), rb], k + 1)
        push(buf.at[up(x), rb], k + 5, x_dn)

    def x_last(buf, k):
        recv(buf.at[down(x), rb], k + 2)
        recv(buf.at[up(x), ra], k + 3)
        recv(buf.at[far(x), ra], k + 4)
        recv(buf.at[far(x), rb], k + 5)

    k2 = take(6)
    x_start(MG, k2)
    z_fwd(3)
    z_own(5)
    x_mid(MG, k2)
    z_fin(2)
    x_last(MG, k2)

    ya, yb = pl.ds(0, 256), pl.ds(256, 256)

    def cy_first(product, CS, CR, k):
        for n, yt in enumerate((far(y), up(y), down(y), y)):
            prod = product(yt)
            T[n] = jnp.where(c == 0, prod[:, :128], prod[:, 128:])
            CS[n] = jnp.where(c == 0, prod[:, 128:], prod[:, :128]).astype(BF16)
            send(CS.at[n], CR.at[n], k + n, mate)

    def cy_second(CR, YA, YB, YC, YHL, YHR, YFL, YFR, k):
        recv(CR.at[0], k)
        YA[...] = (T[0] + CR[0].astype(F32)).astype(BF16)
        send(YA.at[ya], YHL, k + 4, y_up)
        send(YA.at[yb], YHR, k + 5, y_dn)
        recv(CR.at[1], k + 1)
        YB[yb, :] = (T[1, yb, :] + CR[1, yb, :].astype(F32)).astype(BF16)
        send(YB.at[yb], YFL.at[yb], k + 6, y_up)
        recv(CR.at[2], k + 2)
        YC[ya, :] = (T[2, ya, :] + CR[2, ya, :].astype(F32)).astype(BF16)
        send(YC.at[ya], YFR.at[ya], k + 7, y_dn)

    def cy_third(CR, YB, YC, YHL, YHR, YFL, YFR, k):
        recv(YHL, k + 4)
        mixed = T[1, ya, :] + CR[1, ya, :].astype(F32) + YHL[...].astype(F32)
        YB[ya, :] = mixed.astype(BF16)
        send(YB.at[ya], YFL.at[ya], k + 8, y_up)
        recv(YHR, k + 5)
        mixed = T[2, yb, :] + CR[2, yb, :].astype(F32) + YHR[...].astype(F32)
        YC[yb, :] = mixed.astype(BF16)
        send(YC.at[yb], YFR.at[yb], k + 9, y_dn)
        recv(CR.at[3], k + 3)

    def cy_last(CR, YFL, YFR, k):
        recv(YFL.at[yb], k + 6)
        recv(YFR.at[ya], k + 7)
        recv(YFL.at[ya], k + 8)
        recv(YFR.at[yb], k + 9)
        both = YFL[...].astype(F32) + YFR[...].astype(F32)
        return T[3] + CR[3].astype(F32) + both

    def merge(yt):
        return jnp.dot(MG[...].reshape(512, 256), WMP[yt], preferred_element_type=F32)

    k3 = take(10)
    cy_first(merge, CS4, CR4, k3)
    cy_second(CR4, YA4, YB4, YC4, YHL4, YHR4, YFL4, YFR4, k3)
    cy_third(CR4, YB4, YC4, YHL4, YHR4, YFL4, YFR4, k3)
    z_fwd(4)
    z_own(6)
    branch = cy_last(CR4, YFL4, YFR4, k3)
    hidden = (XG[me].reshape(512, 128).astype(F32) + branch).astype(BF16)
    HG[me] = hidden.reshape(4, 128, 128)

    kh = take(13)
    y_start(HG, kh)
    y_mid(HG, kh)
    z_fwd(5)
    y_end(HG, kh)
    z_fin(3)
    z_fin(4)
    y_last(HG, kh)
    scaled(HG, fgain)

    def project(W, p, n, first):
        def cut(cols, to, size):
            w = jnp.concatenate([W[k, cols, :] for k in range(4)], axis=1)
            prod = lax.dot_general(
                XS[...], w, (((1,), (1,)), ((), ())), preferred_element_type=F32
            )
            p[:, :, to] = prod.reshape(4, 128, size)

        def step(i, _):
            cut(
                pl.ds(pl.multiple_of(i * 256, 256), 256),
                pl.ds(pl.multiple_of(first + i * 256, 128), 256), 256,
            )
            return 0

        lax.fori_loop(0, n // 256, step, 0)
        rest = n % 256
        if rest:
            cut(pl.ds(n - rest, rest), pl.ds(first + n - rest, rest), rest)

    project(WVU0, P2, n0, 0)
    project(WGU0, P2, n0, n0)
    ends = slice(2 * n0 - 128, 2 * n0)
    lane = lax.broadcasted_iota(jnp.int32, (4, 128, 128), 2)
    P2[:, :, ends] = jnp.where(lane < edge, P2[:, :, ends], SQ[...])
    k4, k5 = take(6), take(6)
    set2 = (P2, A2, B2, C2, HL2, HR2, FL2, FR2, k4, edge)
    set3 = (P3, A3, B3, C3, HL3, HR3, FL3, FR3, k5, None)
    rs_first(*set2)
    z_fwd(6)
    z_own(7)
    z_own(8)
    rs_second(*set2)
    z_fin(5)
    z_fin(6)
    project(WVU1, P3, n1, 0)
    project(WGU1, P3, n1, n1)
    rs_first(*set3)

    row = lax.broadcasted_iota(jnp.int32, (128, 128), 0)

    def activate(p, FL, FR, cv, act, n):
        def conv_tile(i, _):
            cols = pl.ds(pl.multiple_of(i * 128, 128), 128)

            def one(first, w):
                at_ = pl.ds(pl.multiple_of(first + i * 128, 128), 128)
                v = p[x, :, at_] + FL[:, at_].astype(F32) + FR[:, at_].astype(F32)
                v = (RS[...] * v).astype(BF16).astype(F32)
                prev = jnp.where(row == 0, 0.0, pltpu.roll(v, 1, axis=0))
                after = jnp.where(row == 127, 0.0, pltpu.roll(v, 127, axis=0))
                k = cv[w, :, cols]
                return k[3:4] + prev * k[0:1] + v * k[1:2] + after * k[2:3]

            act[x, :, cols] = (gelu(one(n, 0)) * one(0, 1)).astype(BF16)
            return 0

        lax.fori_loop(0, n // 128, conv_tile, 0)

    rs_wait(FL2, FR2, k4)
    sq = P2[x, :, ends] + dec(FL2[:, ends], edge) + dec(FR2[:, ends], edge)
    rs2 = lax.rsqrt(sq[:, 127:128] / depth + EPS)
    RS[...] = jnp.broadcast_to(rs2, (128, 128))
    rs_second(*set3)
    activate(P2, FL2, FR2, CV0, ACT0, n0)
    k6, k8 = take(6), take(6)
    x_start(ACT0, k6)
    z_fwd(7)
    rs_wait(FL3, FR3, k5)
    activate(P3, FL3, FR3, CV1, ACT1, n1)
    x_start(ACT1, k8)
    x_mid(ACT0, k6)
    z_fwd(8)
    x_last(ACT0, k6)
    z_fin(7)

    def early(n, _):
        ACC[n] = jnp.dot(ACT0[...].reshape(512, n0), WDN0[n], preferred_element_type=F32)
        return 0

    lax.fori_loop(0, 4, early, 0)
    x_mid(ACT1, k8)
    z_fin(8)
    x_last(ACT1, k8)

    def late(yt):
        prod = jnp.dot(ACT1[...].reshape(512, n1), WDN1[yt], preferred_element_type=F32)
        return prod + ACC[yt]

    k7 = take(10)
    cy_first(late, CS5, CR5, k7)
    cy_second(CR5, YA5, YB5, YC5, YHL5, YHR5, YFL5, YFR5, k7)
    cy_third(CR5, YB5, YC5, YHL5, YHR5, YFL5, YFR5, k7)
    change = cy_last(CR5, YFL5, YFR5, k7)
    result = (HG[me].reshape(512, 128).astype(F32) + change).astype(BF16)
    OP[...] = result.reshape(4, 128, 128)

    ko = take(8)
    place = lax.rem(x, 2)
    to_cols = pl.ds(pl.multiple_of(place * 256 + c * 128, 128), 128)
    for j in range(4):
        mine = jnp.logical_and(x == j, to_me)
        copy = remote(
            OP.at[j], out.at[:, to_cols], ko + 4 + j, ko + 2 * place + c,
            at(x_=jnp.int32(j), c_=x // 2),
        )
        swaps.append((mine, copy))

        @pl.when(jnp.logical_not(mine))
        def _():
            copy.start()

        @pl.when(mine)
        def _():
            out[:, to_cols] = OP[j]

    for j in range(2):
        for h in range(2):

            @pl.when(jnp.logical_not(jnp.logical_and(2 * c + j == x, c == h)))
            def _():
                recv(out.at[:, pl.ds(j * 256 + h * 128, 128)], ko + 2 * j + h)

    for copy in started:
        copy.wait_send()
    for mine, copy in swaps:

        @pl.when(jnp.logical_not(mine))
        def _():
            copy.wait_send()


def body(
    tokens, mixer_gain, gate_proj, value_proj, value_gain, spatial_mix, spatial_bias,
    head_gain, merge_proj, ffn_gain, gate_up, value_up, gate_kernel, value_kernel,
    gate_offset, value_offset, down_proj,
):
    units = gate_up.shape[1]
    n1 = units // 2 // 128 * 128 + 128
    n0 = -(-(units - n1) // 128) * 128
    vm = lambda shape, dtype=BF16: pltpu.VMEM(shape, dtype)

    def rs_x(n):
        return [
            vm((4, 128, n), F32), *[vm((128, n))] * 3, *[vm((64, n))] * 2, *[vm((128, n))] * 2,
        ]

    def rs_y():
        return [
            *[vm((4, 512, 128))] * 2, *[vm((512, 128))] * 3, *[vm((256, 128))] * 2,
            *[vm((512, 128))] * 2,
        ]

    in_vmem = pl.BlockSpec(memory_space=pltpu.VMEM)
    left = pl.BlockSpec(memory_space=pl.ANY)
    call = pl.pallas_call(
        kernel,
        out_shape=jax.ShapeDtypeStruct(tokens.shape, tokens.dtype),
        in_specs=[
            in_vmem, in_vmem, in_vmem, left, left, in_vmem, in_vmem, in_vmem, in_vmem, left,
            left, left, in_vmem, in_vmem, in_vmem, in_vmem, left,
        ],
        out_specs=in_vmem,
        scratch_shapes=[
            vm((2, 4, n0), F32), vm((2, 4, n1), F32),
            vm((8, 4, 128, 128)), vm((8, 4, 128, 128)), vm((512, 1024)),
            vm((4, 128, 128), F32), vm((128, 128), F32), vm((16, 2, 8, 128)),
            vm((4, 128, 256)), vm((4, 128, 128)),
            *[vm((4, 256, 256))] * 3, *[vm((4, n0, 256))] * 2, *[vm((4, n1, 256))] * 2,
            vm((4, n0, 256)), vm((4, n1, 256)),
            vm((4, 128, n0)), vm((4, 128, n1)), vm((4, 512, 128), F32), vm((4, 512, 256), F32),
            *rs_x(640), *rs_x(2 * n0), *rs_x(2 * n1),
            *rs_y(), *rs_y(),
            pltpu.SemaphoreType.DMA((SEMS,)), pltpu.SemaphoreType.DMA((SEMS,)),
            pltpu.SemaphoreType.DMA((9,)),
        ],
        compiler_params=pltpu.CompilerParams(
            collective_id=0, has_side_effects=True, vmem_limit_bytes=58 << 20
        ),
        name="layer",
    )
    return call(
        tokens, mixer_gain, ffn_gain, gate_proj, value_proj, value_gain, spatial_mix,
        spatial_bias, head_gain, merge_proj, gate_up.T, value_up.T, gate_kernel, value_kernel,
        gate_offset, value_offset, down_proj,
    )


def solution(mesh):
    finer = Mesh(
        mesh.devices.reshape(mesh.shape["rep"], 4, 4, 4, 2), ("rep", "fs_0", "fs_1", "tp_0", "tp_1")
    )
    return jax.shard_map(
        body,
        mesh=finer,
        in_specs=(
            P(REP_FS, TP), P(), P(FS, TP), P(FS, TP), P(TP, None), P(TP, FS, None),
            P(TP, None), P(TP, None), P(TP, FS), P(), P(FS, TP), P(FS, TP), P(None, TP),
            P(None, TP), P(TP), P(TP), P(TP, FS),
        ),
        out_specs=P(REP_FS, TP),
        check_vma=False,
    )
```

```python
import jax
import jax.numpy as jnp
from jax import lax
from jax.experimental import pallas as pl
from jax.experimental.pallas import tpu as pltpu
from jax.sharding import Mesh
from jax.sharding import PartitionSpec as P

TP = ("tp_0", "tp_1")
FS = ("fs_0", "fs_1")
REP_FS = ("rep", "fs_0", "fs_1")
MESH = pl.DeviceIdType.MESH
EPS = 1e-06
F32 = jnp.float32
BF16 = jnp.bfloat16
SEMS = 224


def gelu(v):
    return 0.5 * v * (1.0 + lax.erf(v * 0.7071067811865476))


def lanes_of(n):
    return lax.broadcasted_iota(jnp.int32, (n, 128), 1)


def kernel(
    tok, mgain, fgain, gp, vp, vgain, smix, sbias, hgain, mp, gu, vu, gk, vk, go, vo, dn,
    out,
    CV0, CV1, XG, HG, XS, SQ, RS, SM, MG, SSB, HRES, TB, TI,
    WGP, WVP, WMP, WGU0, WVU0, WGU1, WVU1, WDN0, WDN1,
    ACT0, ACT1, T, ACC,
    P1, A1, B1, C1, HL1, HR1, FL1, FR1,
    P2, A2, B2, C2, HL2, HR2, FL2, FR2,
    P3, A3, B3, C3, HL3, HR3, FL3, FR3,
    CS4, CR4, YA4, YB4, YC4, YHL4, YHR4, YFL4, YFR4,
    CS5, CR5,
    ssem, rsem, lsem,
):
    r, z, x, y, c = (lax.axis_index(a) for a in ("rep", "fs_0", "fs_1", "tp_0", "tp_1"))
    other = 1 - c
    f = 4 * z + x
    units = dn.shape[0]
    n1 = CV1.shape[2]
    n0 = CV0.shape[2]
    real0 = units - n1
    edge = 128 - (n0 - real0)
    depth = mgain.shape[0]

    def at(z_=None, x_=None, y_=None, c_=None, r_=None):
        pick = lambda new, old: old if new is None else new
        return (pick(r_, r), pick(z_, z), pick(x_, x), pick(y_, y), pick(c_, c))

    up = lambda v: lax.rem(v + 1, 4)
    down = lambda v: lax.rem(v + 3, 4)
    far = lambda v: lax.rem(v + 2, 4)

    zr = 4 * r + z
    zu, zd = lax.rem(zr + 1, 8), lax.rem(zr + 7, 8)
    z_up = at(r_=zu // 4, z_=lax.rem(zu, 4))
    z_dn = at(r_=zd // 4, z_=lax.rem(zd, 4))
    x_up, x_dn = at(x_=up(x)), at(x_=down(x))
    y_up, y_dn = at(y_=up(y)), at(y_=down(y))
    mate = at(c_=other)
    fs_peers = []
    for i in range(1, 16):
        g = lax.rem(f + i, 16)
        fs_peers.append(at(z_=g // 4, x_=lax.rem(g, 4)))

    barrier = pltpu.get_barrier_semaphore()
    near = []
    for i in range(1, 16):
        g = lax.rem(4 * y + x + i, 16)
        near += [at(y_=g // 4, x_=lax.rem(g, 4), c_=jnp.int32(k)) for k in range(2)]
    greet = [mate, z_up, z_dn] + near + [fs_peers[i - 1] for i in range(1, 16)]
    for peer in greet:
        pl.semaphore_signal(barrier, inc=1, device_id=peer, device_id_type=MESH)
    pl.semaphore_wait(barrier, len(greet))

    started = []
    count = [0]

    def take(n=1):
        first = count[0]
        count[0] += n
        return first

    def remote(src, dst, s, k, peer):
        return pltpu.make_async_remote_copy(
            src_ref=src, dst_ref=dst, send_sem=ssem.at[s], recv_sem=rsem.at[k],
            device_id=peer, device_id_type=MESH,
        )

    def send(src, dst, k, peer):
        copy = remote(src, dst, k, k, peer)
        copy.start()
        started.append(copy)

    def push(ref, k, peer):
        send(ref, ref, k, peer)

    def recv(dst, k):
        remote(dst, dst, 0, k, mate).wait_recv()

    chunks = [
        (gp, WGP, 0, 256), (vp, WVP, 0, 256), (mp, WMP, 0, 256),
        (gu, WGU0, 0, real0), (vu, WVU0, 0, real0),
        (gu, WGU1, real0, n1), (vu, WVU1, real0, n1),
        (dn, WDN0, 0, real0), (dn, WDN1, real0, n1),
    ]
    zk = [take(6) for _ in chunks]

    def z_parts(i):
        _, _, at0, n = chunks[i]
        return (at0, pl.ds(0, n // 2)), (at0 + n // 2, pl.ds(n // 2, n // 2))

    def z_own(i):
        src, buf, at0, n = chunks[i]
        (sa, a), (sb, b) = z_parts(i)
        from_a, from_b = src.at[pl.ds(sa, n // 2)], src.at[pl.ds(sb, n // 2)]
        send(from_a, buf.at[z, a], zk[i], z_up)
        send(from_b, buf.at[z, b], zk[i] + 1, z_dn)
        send(from_b, buf.at[z, b], zk[i] + 2, z_up)
        send(from_a, buf.at[z, a], zk[i] + 3, z_dn)
        z_local(i).start()

    def z_local(i):
        src, buf, at0, n = chunks[i]
        return pltpu.make_async_copy(src.at[pl.ds(at0, n)], buf.at[z, pl.ds(0, n)], lsem.at[i])

    def z_fwd(i):
        buf = chunks[i][1]
        (_, a), (_, b) = z_parts(i)
        recv(buf.at[down(z), a], zk[i])
        push(buf.at[down(z), a], zk[i] + 4, z_up)
        recv(buf.at[up(z), b], zk[i] + 1)
        push(buf.at[up(z), b], zk[i] + 5, z_dn)

    def z_fin(i):
        buf = chunks[i][1]
        (_, a), (_, b) = z_parts(i)
        recv(buf.at[down(z), b], zk[i] + 2)
        recv(buf.at[up(z), a], zk[i] + 3)
        recv(buf.at[far(z), a], zk[i] + 4)
        recv(buf.at[far(z), b], zk[i] + 5)
        z_local(i).wait()

    swaps = []
    kx = take(4)
    me = 2 * y + c
    to_me = x // 2 == c
    for j in range(2):
        for h in range(2):
            xt = 2 * c + j
            mine = jnp.logical_and(xt == x, c == h)
            cols = slice(j * 256 + h * 128, j * 256 + h * 128 + 128)
            copy = remote(
                tok.at[:, cols], XG.at[2 * y + h, x], kx + 2 * j + h, kx + x,
                at(x_=xt, c_=jnp.int32(h)),
            )
            swaps.append((mine, copy))

            @pl.when(jnp.logical_not(mine))
            def _():
                copy.start()

            @pl.when(mine)
            def _():
                XG[2 * y + h, x] = tok[:, cols]

    z_own(0)
    z_own(1)
    z_own(2)

    me = 2 * y + c
    square = tok[...].astype(F32)
    square = jnp.sum(square * square, axis=-1, keepdims=True)
    SSB[me] = jnp.broadcast_to(square, (128, 128)).T[0:8, :]
    ks = take(7)
    for i in range(1, 8):
        t = lax.rem(me + i, 8)
        send(SSB.at[me], SSB.at[me], ks + i - 1, at(y_=t // 2, c_=lax.rem(t, 2)))

    for j in range(4):

        @pl.when(jnp.logical_not(jnp.logical_and(x == j, to_me)))
        def _():
            recv(XG.at[me, j], kx + j)

    lo_y, hi_y, far_y = 2 * down(y) + c, 2 * up(y) + c, 2 * far(y) + c
    a2, b2 = pl.ds(0, 2), pl.ds(2, 2)

    def y_start(buf, k):
        push(buf.at[me, a2], k, y_up)
        push(buf.at[me, b2], k + 1, y_dn)
        push(buf.at[me, b2], k + 2, y_up)
        push(buf.at[me, a2], k + 3, y_dn)
        push(buf.at[me], k + 6, mate)

    def y_mid(buf, k):
        recv(buf.at[lo_y, a2], k)
        push(buf.at[lo_y, a2], k + 4, y_up)
        push(buf.at[lo_y, a2], k + 7, mate)
        recv(buf.at[hi_y, b2], k + 1)
        push(buf.at[hi_y, b2], k + 5, y_dn)
        push(buf.at[hi_y, b2], k + 8, mate)

    def y_end(buf, k):
        recv(buf.at[lo_y, b2], k + 2)
        push(buf.at[lo_y, b2], k + 9, mate)
        recv(buf.at[hi_y, a2], k + 3)
        push(buf.at[hi_y, a2], k + 10, mate)
        recv(buf.at[far_y, a2], k + 4)
        push(buf.at[far_y, a2], k + 11, mate)
        recv(buf.at[far_y, b2], k + 5)
        push(buf.at[far_y, b2], k + 12, mate)

    def y_last(buf, k):
        recv(buf.at[2 * y + other], k + 6)
        recv(buf.at[2 * down(y) + other, a2], k + 7)
        recv(buf.at[2 * up(y) + other, b2], k + 8)
        recv(buf.at[2 * down(y) + other, b2], k + 9)
        recv(buf.at[2 * up(y) + other, a2], k + 10)
        recv(buf.at[2 * far(y) + other, a2], k + 11)
        recv(buf.at[2 * far(y) + other, b2], k + 12)

    def scaled(buf, gains):
        parts = [gains[pl.ds(pl.multiple_of((4 * k + x) * 256, 256), 256)] for k in range(4)]
        gain = jnp.concatenate([part.reshape(1, 256) for part in parts], axis=1)

        def block(b, _):
            rows = jnp.concatenate([buf[i, b] for i in range(8)], axis=1).astype(F32)
            SQ[b] = jnp.broadcast_to(jnp.sum(rows * rows, axis=-1, keepdims=True), (128, 128))
            XS[pl.ds(pl.multiple_of(b * 128, 128), 128), :] = (rows * gain).astype(BF16)
            return 0

        lax.fori_loop(0, 4, block, 0)

    ky = take(13)
    y_start(XG, ky)
    km = take(15)
    for i in range(15):
        send(smix, SM.at[f], km + i, fs_peers[i])
    SM[f] = smix[...]
    for W in (WGU0, WVU0, WDN0):
        for k in range(4):
            W[k, real0:, :] = jnp.zeros((n0 - real0, 256), BF16)
    for w, kern, off in ((0, gk, go), (1, vk, vo)):
        CV0[w, :, n0 - 128 :] = jnp.zeros((4, 128), F32)
        CV0[w, 0:3, 0:real0] = kern[:, 0:real0]
        CV1[w, 0:3, :] = kern[:, real0:]
        bias = off[...].reshape(1, units)
        CV0[w, 3:4, 0:real0] = bias[:, 0:real0]
        CV1[w, 3:4, :] = bias[:, real0:]
    y_mid(XG, ky)
    z_fwd(0)
    z_fwd(1)
    y_end(XG, ky)
    z_fwd(2)
    z_own(3)
    z_own(4)
    y_last(XG, ky)

    scaled(XG, mgain)
    z_fin(0)
    z_fin(1)
    for w, W in ((0, WGP), (1, WVP)):
        prod = jnp.dot(XS[...], W[...].reshape(1024, 256), preferred_element_type=F32)
        P1[:, :, w * 256 : w * 256 + 256] = prod.reshape(4, 128, 256)

    def enc(v, edge):
        if edge is None:
            return v.astype(BF16)
        m = v.shape[1] - 128
        last = v[:, m:]
        low = last - last.astype(BF16).astype(F32)
        last = jnp.where(lanes_of(v.shape[0]) >= (edge + 128) // 2, low, last)
        return jnp.concatenate([v[:, :m].astype(BF16), last.astype(BF16)], axis=1)

    def dec(v, edge):
        v = v.astype(F32)
        if edge is None:
            return v
        m = v.shape[1] - 128
        last, lane = v[:, m:], lanes_of(v.shape[0])
        keep = jnp.logical_or(lane == edge, lane == (edge + 128) // 2)
        total = jnp.sum(jnp.where(keep, last, 0.0), axis=-1, keepdims=True)
        last = jnp.where(lane < edge, last, total)
        return jnp.concatenate([v[:, :m], last], axis=1) if m else last

    def row_loop(first, n, fn):
        def step(i, _):
            fn(pl.ds(pl.multiple_of(first + i * 16, 16), 16))
            return 0

        lax.fori_loop(0, n // 16, step, 0)

    ra, rb = pl.ds(0, 64), pl.ds(64, 64)

    def rs_far(p, A, B, C, HL, HR, FL, FR, k, edge):
        def far_rows(rows):
            A[rows, :] = enc(p[far(x), rows, :], edge)

        row_loop(0, 128, far_rows)
        send(A.at[ra], HL, k, x_up)
        send(A.at[rb], HR, k + 1, x_dn)

    def rs_first(p, A, B, C, HL, HR, FL, FR, k, edge):
        u, d = up(x), down(x)

        def up_rows(rows):
            B[rows, :] = enc(p[u, rows, :], edge)

        def down_rows(rows):
            C[rows, :] = enc(p[d, rows, :], edge)

        row_loop(64, 64, up_rows)
        send(B.at[rb], FL.at[rb], k + 2, x_up)
        row_loop(0, 64, down_rows)
        send(C.at[ra], FR.at[ra], k + 3, x_dn)

    def rs_second(p, A, B, C, HL, HR, FL, FR, k, edge):
        u, d = up(x), down(x)

        def left(rows):
            B[rows, :] = enc(p[u, rows, :] + dec(HL[rows, :], edge), edge)

        def right(rows):
            low = pl.ds(pl.multiple_of(rows.start + 64, 16), 16)
            C[low, :] = enc(p[d, low, :] + dec(HR[rows, :], edge), edge)

        recv(HL, k)
        row_loop(0, 64, left)
        send(B.at[ra], FL.at[ra], k + 4, x_up)
        recv(HR, k + 1)
        row_loop(0, 64, right)
        send(C.at[rb], FR.at[rb], k + 5, x_dn)

    def rs_wait(FL, FR, k):
        recv(FL.at[rb], k + 2)
        recv(FR.at[ra], k + 3)
        recv(FL.at[ra], k + 4)
        recv(FR.at[rb], k + 5)

    k1 = take(6)
    set1 = (P1, A1, B1, C1, HL1, HR1, FL1, FR1, k1, None)
    rs_far(*set1)
    rs_first(*set1)
    rs_second(*set1)
    for i in range(15):
        recv(SM.at[lax.rem(f + 15 - i, 16)], km + i)
    rs_wait(FL1, FR1, k1)

    total = P1[x] + FL1[...].astype(F32) + FR1[...].astype(F32)
    for i in range(1, 8):
        recv(SSB.at[lax.rem(me + 8 - i, 8)], ks + i - 1)
    square = jnp.sum(SSB[...], axis=0)[0:1, :]
    rs = lax.rsqrt(jnp.broadcast_to(square, (128, 128)).T / depth + EPS)
    eye = lax.broadcasted_iota(jnp.int32, (128, 128), 0) == lanes_of(128)
    for h in range(2):
        cols = slice(h * 128, h * 128 + 128)
        gated = gelu((rs * total[:, cols]).astype(BF16).astype(F32))
        spread = gelu((rs * total[:, 256 + h * 128 : 384 + h * 128]).astype(BF16).astype(F32))
        spread = spread * lax.rsqrt(jnp.mean(spread * spread, axis=-1, keepdims=True) + EPS)
        spread = (spread * vgain[h : h + 1, :]).astype(BF16)
        matrix = SM[:, h].astype(F32).reshape(128, 128).astype(BF16)
        mixed = jnp.dot(matrix, spread, preferred_element_type=F32)
        bias = jnp.broadcast_to(sbias[h : h + 1, :], (128, 128))
        mixed = mixed + jnp.sum(jnp.where(eye, bias, 0.0), axis=-1, keepdims=True)
        joined = gated * mixed
        joined = joined * lax.rsqrt(jnp.mean(joined * joined, axis=-1, keepdims=True) + EPS)
        MG[x, :, cols] = (joined * hgain[h : h + 1, :]).astype(BF16)

    def x_start(buf, k):
        push(buf.at[x, ra], k, x_up)
        push(buf.at[x, rb], k + 1, x_dn)
        push(buf.at[x, rb], k + 2, x_up)
        push(buf.at[x, ra], k + 3, x_dn)

    def x_mid(buf, k):
        recv(buf.at[down(x), ra], k)
        push(buf.at[down(x), ra], k + 4, x_up)
        recv(buf.at[up(x), rb], k + 1)
        push(buf.at[up(x), rb], k + 5, x_dn)

    def x_last(buf, k):
        recv(buf.at[down(x), rb], k + 2)
        recv(buf.at[up(x), ra], k + 3)
        recv(buf.at[far(x), ra], k + 4)
        recv(buf.at[far(x), rb], k + 5)

    k2 = take(6)
    x_start(MG, k2)
    z_fwd(3)
    z_own(5)
    x_mid(MG, k2)
    z_fin(2)
    x_last(MG, k2)

    ya, yb = pl.ds(0, 256), pl.ds(256, 256)

    def cy_first(product, CS, CR, k):
        for n, yt in enumerate((far(y), up(y), down(y), y)):
            prod = product(yt)
            T[n] = jnp.where(c == 0, prod[:, :128], prod[:, 128:])
            CS[n] = jnp.where(c == 0, prod[:, 128:], prod[:, :128]).astype(BF16)
            send(CS.at[n], CR.at[n], k + n, mate)

    def cy_second(CR, YA, YB, YC, YHL, YHR, YFL, YFR, k):
        recv(CR.at[0], k)
        YA[...] = (T[0] + CR[0].astype(F32)).astype(BF16)
        send(YA.at[ya], YHL, k + 4, y_up)
        send(YA.at[yb], YHR, k + 5, y_dn)
        recv(CR.at[1], k + 1)
        YB[yb, :] = (T[1, yb, :] + CR[1, yb, :].astype(F32)).astype(BF16)
        send(YB.at[yb], YFL.at[yb], k + 6, y_up)
        recv(CR.at[2], k + 2)
        YC[ya, :] = (T[2, ya, :] + CR[2, ya, :].astype(F32)).astype(BF16)
        send(YC.at[ya], YFR.at[ya], k + 7, y_dn)

    def cy_third(CR, YB, YC, YHL, YHR, YFL, YFR, k):
        recv(YHL, k + 4)
        mixed = T[1, ya, :] + CR[1, ya, :].astype(F32) + YHL[...].astype(F32)
        YB[ya, :] = mixed.astype(BF16)
        send(YB.at[ya], YFL.at[ya], k + 8, y_up)
        recv(YHR, k + 5)
        mixed = T[2, yb, :] + CR[2, yb, :].astype(F32) + YHR[...].astype(F32)
        YC[yb, :] = mixed.astype(BF16)
        send(YC.at[yb], YFR.at[yb], k + 9, y_dn)
        recv(CR.at[3], k + 3)

    def cy_last(CR, YFL, YFR, k):
        recv(YFL.at[yb], k + 6)
        recv(YFR.at[ya], k + 7)
        recv(YFL.at[ya], k + 8)
        recv(YFR.at[yb], k + 9)
        both = YFL[...].astype(F32) + YFR[...].astype(F32)
        return T[3] + CR[3].astype(F32) + both

    def merge(yt):
        return jnp.dot(MG[...].reshape(512, 256), WMP[yt], preferred_element_type=F32)

    k3 = take(10)
    cy_first(merge, CS4, CR4, k3)
    cy_second(CR4, YA4, YB4, YC4, YHL4, YHR4, YFL4, YFR4, k3)
    cy_third(CR4, YB4, YC4, YHL4, YHR4, YFL4, YFR4, k3)
    z_fwd(4)
    z_own(6)
    branch = cy_last(CR4, YFL4, YFR4, k3)
    hidden = (XG[me].reshape(512, 128).astype(F32) + branch).astype(BF16)
    HG[me] = hidden.reshape(4, 128, 128)

    kh, ko = take(13), take(8)
    y_start(HG, kh)
    spot = 2 * lax.rem(x, 2) + c
    for j in range(4):
        mine = jnp.logical_and(x == j, to_me)
        copy = remote(
            HG.at[me, j], HRES.at[spot], ko + 4 + j, ko + spot, at(x_=jnp.int32(j), c_=x // 2)
        )
        swaps.append((mine, copy))

        @pl.when(jnp.logical_not(mine))
        def _():
            copy.start()

        @pl.when(mine)
        def _():
            HRES[spot] = HG[me, j]

    y_mid(HG, kh)
    z_fwd(5)
    y_end(HG, kh)
    z_fin(3)
    z_fin(4)
    y_last(HG, kh)
    scaled(HG, fgain)

    def project(W, p, n, first, block=None):
        def cut(cols, to, size):
            w = jnp.concatenate([W[k, cols, :] for k in range(4)], axis=1)
            rows = XS[...]
            if block is not None:
                rows = XS[pl.ds(pl.multiple_of(block * 128, 128), 128), :]
            prod = lax.dot_general(
                rows, w, (((1,), (1,)), ((), ())), preferred_element_type=F32
            )
            if block is None:
                p[:, :, to] = prod.reshape(4, 128, size)
            else:
                p[block, :, to] = prod

        def step(i, _):
            cut(
                pl.ds(pl.multiple_of(i * 256, 256), 256),
                pl.ds(pl.multiple_of(first + i * 256, 128), 256), 256,
            )
            return 0

        lax.fori_loop(0, n // 256, step, 0)
        rest = n % 256
        if rest:
            cut(pl.ds(n - rest, rest), pl.ds(first + n - rest, rest), rest)

    k4, k5 = take(6), take(6)
    set2 = (P2, A2, B2, C2, HL2, HR2, FL2, FR2, k4, edge)
    set3 = (P3, A3, B3, C3, HL3, HR3, FL3, FR3, k5, None)
    ends = slice(2 * n0 - 128, 2 * n0)
    lane = lax.broadcasted_iota(jnp.int32, (4, 128, 128), 2)
    project(WVU0, P2, n0, 0, far(x))
    project(WGU0, P2, n0, n0, far(x))
    P2[far(x), :, ends] = jnp.where(lane[0] < edge, P2[far(x), :, ends], SQ[far(x)])
    rs_far(*set2)
    project(WVU0, P2, n0, 0)
    project(WGU0, P2, n0, n0)
    P2[:, :, ends] = jnp.where(lane < edge, P2[:, :, ends], SQ[...])
    rs_first(*set2)
    z_fwd(6)
    z_own(7)
    z_own(8)
    rs_second(*set2)
    z_fin(5)
    z_fin(6)
    project(WVU1, P3, n1, 0)
    project(WGU1, P3, n1, n1)
    rs_far(*set3)
    rs_first(*set3)

    row = lax.broadcasted_iota(jnp.int32, (128, 128), 0)

    def activate(p, FL, FR, cv, act, n):
        def conv_tile(i, _):
            cols = pl.ds(pl.multiple_of(i * 128, 128), 128)

            def one(first, w):
                at_ = pl.ds(pl.multiple_of(first + i * 128, 128), 128)
                v = p[x, :, at_] + FL[:, at_].astype(F32) + FR[:, at_].astype(F32)
                v = (RS[...] * v).astype(BF16).astype(F32)
                prev = jnp.where(row == 0, 0.0, pltpu.roll(v, 1, axis=0))
                after = jnp.where(row == 127, 0.0, pltpu.roll(v, 127, axis=0))
                k = cv[w, :, cols]
                return k[3:4] + prev * k[0:1] + v * k[1:2] + after * k[2:3]

            act[x, :, cols] = (gelu(one(n, 0)) * one(0, 1)).astype(BF16)
            return 0

        lax.fori_loop(0, n // 128, conv_tile, 0)

    rs_wait(FL2, FR2, k4)
    sq = P2[x, :, ends] + dec(FL2[:, ends], edge) + dec(FR2[:, ends], edge)
    rs2 = lax.rsqrt(sq[:, 127:128] / depth + EPS)
    RS[...] = jnp.broadcast_to(rs2, (128, 128))
    rs_second(*set3)
    activate(P2, FL2, FR2, CV0, ACT0, n0)
    k6, k8 = take(6), take(6)
    x_start(ACT0, k6)
    z_fwd(7)
    rs_wait(FL3, FR3, k5)
    activate(P3, FL3, FR3, CV1, ACT1, n1)
    x_start(ACT1, k8)
    x_mid(ACT0, k6)
    z_fwd(8)
    x_mid(ACT1, k8)
    x_last(ACT0, k6)
    z_fin(7)

    def early(n, _):
        ACC[n] = jnp.dot(ACT0[...].reshape(512, n0), WDN0[n], preferred_element_type=F32)
        return 0

    lax.fori_loop(0, 4, early, 0)
    z_fin(8)
    x_last(ACT1, k8)

    def late(yt):
        prod = jnp.dot(ACT1[...].reshape(512, n1), WDN1[yt], preferred_element_type=F32)
        return prod + ACC[yt]

    k7 = take(4)
    kt, kn = take(16), take(16)
    cy_first(late, CS5, CR5, k7)

    for n, yt in enumerate((far(y), up(y), down(y), y)):
        recv(CR5.at[n], k7 + n)
        term = T[n] + CR5[n].astype(F32)
        TB[n] = term.astype(BF16).reshape(4, 128, 128)
        for j in range(4):
            copy = remote(
                TB.at[n, j], TI.at[y, spot], kn + 4 * n + j, kt + 4 * y + spot,
                at(x_=jnp.int32(j), y_=yt, c_=x // 2),
            )
            if n < 3:
                copy.start()
                started.append(copy)
                continue
            mine = jnp.logical_and(x == j, to_me)
            swaps.append((mine, copy))

            @pl.when(jnp.logical_not(mine))
            def _():
                copy.start()

            @pl.when(mine)
            def _():
                TI[y, spot] = TB[n, j]

    for j in range(2):
        for h in range(2):
            q = 2 * j + h
            mine = jnp.logical_and(2 * c + j == x, c == h)

            @pl.when(jnp.logical_not(mine))
            def _():
                recv(HRES.at[q], ko + q)

            for n in range(4):

                @pl.when(jnp.logical_not(jnp.logical_and(mine, y == n)))
                def _():
                    recv(TI.at[n, q], kt + 4 * n + q)

            change = jnp.sum(TI[:, q].astype(F32), axis=0)
            result = (HRES[q].astype(F32) + change).astype(BF16)
            out[:, q * 128 : q * 128 + 128] = result

    for copy in started:
        copy.wait_send()
    for mine, copy in swaps:

        @pl.when(jnp.logical_not(mine))
        def _():
            copy.wait_send()


def body(
    tokens, mixer_gain, gate_proj, value_proj, value_gain, spatial_mix, spatial_bias,
    head_gain, merge_proj, ffn_gain, gate_up, value_up, gate_kernel, value_kernel,
    gate_offset, value_offset, down_proj,
):
    units = gate_up.shape[1]
    n1 = units // 2 // 128 * 128 + 128
    n0 = -(-(units - n1) // 128) * 128
    vm = lambda shape, dtype=BF16: pltpu.VMEM(shape, dtype)

    def rs_x(n):
        return [
            vm((4, 128, n), F32), *[vm((128, n))] * 3, *[vm((64, n))] * 2, *[vm((128, n))] * 2,
        ]

    def rs_y():
        return [
            *[vm((4, 512, 128))] * 2, *[vm((512, 128))] * 3, *[vm((256, 128))] * 2,
            *[vm((512, 128))] * 2,
        ]

    in_vmem = pl.BlockSpec(memory_space=pltpu.VMEM)
    left = pl.BlockSpec(memory_space=pl.ANY)
    call = pl.pallas_call(
        kernel,
        out_shape=jax.ShapeDtypeStruct(tokens.shape, tokens.dtype),
        in_specs=[
            in_vmem, in_vmem, in_vmem, left, left, in_vmem, in_vmem, in_vmem, in_vmem, left,
            left, left, in_vmem, in_vmem, in_vmem, in_vmem, left,
        ],
        out_specs=in_vmem,
        scratch_shapes=[
            vm((2, 4, n0), F32), vm((2, 4, n1), F32),
            vm((8, 4, 128, 128)), vm((8, 4, 128, 128)), vm((512, 1024)),
            vm((4, 128, 128), F32), vm((128, 128), F32), vm((16, 2, 8, 128)),
            vm((4, 128, 256)), vm((8, 8, 128), F32), vm((4, 128, 128)),
            vm((4, 4, 128, 128)), vm((4, 4, 128, 128)),
            *[vm((4, 256, 256))] * 3, *[vm((4, n0, 256))] * 2, *[vm((4, n1, 256))] * 2,
            vm((4, n0, 256)), vm((4, n1, 256)),
            vm((4, 128, n0)), vm((4, 128, n1)), vm((4, 512, 128), F32), vm((4, 512, 256), F32),
            *rs_x(512), *rs_x(2 * n0), *rs_x(2 * n1),
            *rs_y(), vm((4, 512, 128)), vm((4, 512, 128)),
            pltpu.SemaphoreType.DMA((SEMS,)), pltpu.SemaphoreType.DMA((SEMS,)),
            pltpu.SemaphoreType.DMA((9,)),
        ],
        compiler_params=pltpu.CompilerParams(
            collective_id=0, has_side_effects=True, vmem_limit_bytes=58 << 20
        ),
        name="layer",
    )
    return call(
        tokens, mixer_gain, ffn_gain, gate_proj, value_proj, value_gain, spatial_mix,
        spatial_bias, head_gain, merge_proj, gate_up.T, value_up.T, gate_kernel, value_kernel,
        gate_offset, value_offset, down_proj,
    )


def solution(mesh):
    finer = Mesh(
        mesh.devices.reshape(mesh.shape["rep"], 4, 4, 4, 2), ("rep", "fs_0", "fs_1", "tp_0", "tp_1")
    )
    return jax.shard_map(
        body,
        mesh=finer,
        in_specs=(
            P(REP_FS, TP), P(), P(FS, TP), P(FS, TP), P(TP, None), P(TP, FS, None),
            P(TP, None), P(TP, None), P(TP, FS), P(), P(FS, TP), P(FS, TP), P(None, TP),
            P(None, TP), P(TP), P(TP), P(TP, FS),
        ),
        out_specs=P(REP_FS, TP),
        check_vma=False,
    )
```

```python
import functools

import jax
import jax.numpy as jnp
from jax import lax
from jax.experimental import pallas as pl
from jax.experimental.pallas import tpu as pltpu
from jax.sharding import Mesh
from jax.sharding import PartitionSpec as P

TP = ("tp_0", "tp_1")
FS = ("fs_0", "fs_1")
REP_FS = ("rep", "fs_0", "fs_1")
MESH = pl.DeviceIdType.MESH
EPS = 1e-06
SENDS, RECVS = 33, 96
CHUNK = 512
F32 = jnp.float32
BF16 = jnp.bfloat16


def gelu(v):
    return 0.5 * v * (1.0 + lax.erf(v * 0.7071067811865476))


def lanes_of(n):
    return lax.broadcasted_iota(jnp.int32, (n, 128), 1)


def kernel(layout, tok, mgain, fgain, gp, vp, vgain, smix, sbias, hgain, mp, gu, vu, gk, vk, go, vo,
           dn, out, tokv, gkv, vkv, CV, XG, HG, XS, SQR, RS, SM, MG, SSB, SSF, HRES, TB, TI,
           WGP, WVP, WMP, T, ACC, P1, S1, H1, F1, CS4, CR4, YS4, YH4, YF4, CS5, CR5, *rest):
    chunks = len(layout)
    WGU, WVU, WDN, ACT, PC, SC, HC, FC = (rest[i * chunks : (i + 1) * chunks] for i in range(8))
    ssem, rsem, lsem = rest[8 * chunks :]
    r, z, x, y, c = (lax.axis_index(a) for a in ("rep", "fs_0", "fs_1", "tp_0", "tp_1"))
    other = 1 - c
    f = 4 * z + x
    units = dn.shape[0]
    depth = mgain.shape[0]

    def at(z_=None, x_=None, y_=None, c_=None, r_=None):
        pick = lambda new, old: old if new is None else new
        return (pick(r_, r), pick(z_, z), pick(x_, x), pick(y_, y), pick(c_, c))

    up = lambda v: lax.rem(v + 1, 4)
    down = lambda v: lax.rem(v + 3, 4)
    far = lambda v: lax.rem(v + 2, 4)

    zr = 4 * r + z
    zu, zd = lax.rem(zr + 1, 8), lax.rem(zr + 7, 8)
    z_up = at(r_=zu // 4, z_=lax.rem(zu, 4))
    z_dn = at(r_=zd // 4, z_=lax.rem(zd, 4))
    x_up, x_dn, x_far = at(x_=up(x)), at(x_=down(x)), at(x_=far(x))
    y_up, y_dn = at(y_=up(y)), at(y_=down(y))
    mate = at(c_=other)
    fs_peers = []
    for i in range(1, 16):
        g = lax.rem(f + i, 16)
        fs_peers.append(at(z_=g // 4, x_=lax.rem(g, 4)))
    near = []
    for i in range(1, 16):
        g = lax.rem(4 * y + x + i, 16)
        near += [at(y_=g // 4, x_=lax.rem(g, 4), c_=jnp.int32(k)) for k in range(2)]

    barrier = pltpu.get_barrier_semaphore()
    greet = [mate, z_up, z_dn] + near + fs_peers
    for peer in greet:
        pl.semaphore_signal(barrier, inc=1, device_id=peer, device_id_type=MESH)
    loads = [
        pltpu.make_async_copy(src, dst, lsem.at[i])
        for i, (src, dst) in enumerate(((tok, tokv), (gk, gkv), (vk, vkv)))
    ]
    for copy in loads:
        copy.start()
    pl.semaphore_wait(barrier, len(greet))

    sends, recvs, ends = [0], [0], []

    def new(counter, n=1):
        counter[0] += n
        return counter[0] - n

    def remote(src, dst, s, k, peer):
        return pltpu.make_async_remote_copy(
            src_ref=src, dst_ref=dst, send_sem=ssem.at[s], recv_sem=rsem.at[k],
            device_id=peer, device_id_type=MESH,
        )

    def send(src, dst, s, k, peer):
        remote(src, dst, s, k, peer).start()

    def recv(dst, k):
        remote(dst, dst, 0, k, mate).wait_recv()

    def sender(ref):
        s = new(sends)
        ends.append(lambda: remote(ref, ref, s, 0, mate).wait_send())
        return s

    pieces = [(gp, WGP, 0, 256), (vp, WVP, 0, 256), (mp, WMP, 0, 256)]
    for (at0, n, _), G, V in zip(layout, WGU, WVU):
        pieces += [(gu, G, at0, n), (vu, V, at0, n)]
    for (at0, n, _), W in zip(layout, WDN):
        pieces.append((dn, W, at0, n))
    zk = [new(recvs, 3) for _ in pieces]
    zs = [sender(buf.at[pl.ds(0, 3), pl.ds(0, n)]) for _, buf, _, n in pieces]

    def z_local(i):
        src, buf, at0, n = pieces[i]
        return pltpu.make_async_copy(src.at[pl.ds(at0, n)], buf.at[z, pl.ds(0, n)], lsem.at[3 + i])

    def z_own(i):
        src, buf, at0, n = pieces[i]
        a, b = pl.ds(0, n // 2), pl.ds(n // 2, n // 2)
        from_a, from_b = src.at[pl.ds(at0, n // 2)], src.at[pl.ds(at0 + n // 2, n // 2)]
        send(from_a, buf.at[z, a], zs[i], zk[i], z_up)
        send(from_b, buf.at[z, b], zs[i], zk[i] + 1, z_dn)
        send(from_b, buf.at[z, b], zs[i], zk[i] + 2, z_up)
        send(from_a, buf.at[z, a], zs[i], zk[i] + 2, z_dn)
        z_local(i).start()

    def z_fwd(i):
        _, buf, _, n = pieces[i]
        a, b = buf.at[down(z), pl.ds(0, n // 2)], buf.at[up(z), pl.ds(n // 2, n // 2)]
        recv(a, zk[i])
        send(a, a, zs[i], zk[i] + 2, z_up)
        recv(b, zk[i] + 1)
        send(b, b, zs[i], zk[i] + 2, z_dn)

    def z_fin(i):
        _, buf, _, n = pieces[i]
        recv(buf.at[pl.ds(0, 2), pl.ds(0, n)], zk[i] + 2)
        z_local(i).wait()

    def weight(kind, j):
        return {"g": 3 + 2 * j, "v": 4 + 2 * j, "d": 3 + 2 * chunks + j}[kind]

    me = 2 * y + c
    to_me = x // 2 == c
    loads[0].wait()
    kx = new(recvs, 2)
    sx = new(sends)
    for j in range(2):
        for h in range(2):
            xt = 2 * c + j
            ahead = lax.rem(x - xt + 4, 4)
            place = jnp.where(ahead >= 2, 5 - ahead, ahead)
            mine = jnp.logical_and(xt == x, c == h)
            block = tokv.at[:, j * 256 + h * 128 : j * 256 + h * 128 + 128]

            @pl.when(jnp.logical_not(mine))
            def _():
                dst = XG.at[2 * y + h, place]
                send(block, dst, sx, kx + place // 2, at(x_=xt, c_=jnp.int32(h)))

            @pl.when(mine)
            def _():
                XG[2 * y + h, 0] = block[...]

    def fewer(ref_of, n, wait):
        @pl.when(to_me)
        def _():
            wait(ref_of(n - 1))

        @pl.when(jnp.logical_not(to_me))
        def _():
            wait(ref_of(n))

    stay = lambda s: lambda ref: remote(ref, ref, s, 0, mate).wait_send()
    ends.append(lambda: fewer(lambda n: XG.at[0, pl.ds(0, n)], 4, stay(sx)))
    z_own(0)
    z_own(1)
    square = tokv[...].astype(F32)
    square = jnp.sum(square * square, axis=-1, keepdims=True)
    SSB[me] = jnp.broadcast_to(square, (128, 128)).T[0:8, :]
    kss = new(recvs)
    sss = sender(SSB.at[pl.ds(0, 7)])
    for i in range(1, 8):
        t = lax.rem(me + i, 8)
        send(SSB.at[me], SSB.at[me], sss, kss, at(y_=t // 2, c_=lax.rem(t, 2)))

    lo_y, hi_y, far_y = 2 * down(y) + c, 2 * up(y) + c, 2 * far(y) + c

    def y_start(buf, k, s, g):
        a, b = buf.at[me, 2 * g], buf.at[me, 2 * g + 1]
        send(a, a, s, k, y_up)
        send(b, b, s, k + 1, y_dn)
        send(b, b, s, k + 2, y_up)
        send(a, a, s, k + 3, y_dn)
        both = buf.at[me, pl.ds(2 * g, 2)]
        send(both, both, s, k + 6, mate)

    def y_mid(buf, k, s, g):
        a, b = buf.at[lo_y, 2 * g], buf.at[hi_y, 2 * g + 1]
        recv(a, k)
        send(a, a, s, k + 4, y_up)
        send(a, a, s, k + 6, mate)
        recv(b, k + 1)
        send(b, b, s, k + 5, y_dn)
        send(b, b, s, k + 6, mate)

    def y_end(buf, k, s, g):
        rows = (buf.at[lo_y, 2 * g + 1], buf.at[hi_y, 2 * g], buf.at[far_y, 2 * g], buf.at[far_y, 2 * g + 1])
        for i, ref in enumerate(rows):
            recv(ref, k + 2 + i)
            send(ref, ref, s, k + 6, mate)

    def y_last(buf, k):
        recv(buf.at[pl.ds(0, 4), pl.ds(0, 2)], k + 6)

    def scaled(buf, gains, squares):
        parts = [gains[pl.ds(pl.multiple_of((4 * k + x) * 256, 256), 256)] for k in range(4)]
        gain = jnp.concatenate([part.reshape(1, 256) for part in parts], axis=1)

        def block(b, _):
            rows = jnp.concatenate([buf[i, b] for i in range(8)], axis=1).astype(F32)
            if squares:
                total = jnp.sum(rows * rows, axis=-1, keepdims=True)
                SQR[b] = jnp.broadcast_to(total, (128, 128)).T[0:8, :]
            XS[pl.ds(pl.multiple_of(b * 128, 128), 128), :] = (rows * gain).astype(BF16)
            return 0

        lax.fori_loop(0, 4, block, 0)

    def scale_of(rows):
        return lax.rsqrt(jnp.broadcast_to(rows, (128, 128)).T / depth + EPS)

    ky = [new(recvs, 7) for _ in range(2)]
    sy = [sender(buf.at[pl.ds(0, 7), pl.ds(0, 2)]) for buf in (XG, XG)]
    fewer(lambda n: XG.at[me, pl.ds(0, n)], 2, lambda ref: recv(ref, kx))
    y_start(XG, ky[0], sy[0], 0)
    recv(XG.at[me, pl.ds(2, 2)], kx + 1)
    y_start(XG, ky[1], sy[1], 1)
    km = new(recvs)
    sm = sender(SM.at[pl.ds(0, 15)])
    for i in range(15):
        send(smix, SM.at[f], sm, km, fs_peers[i])
    SM[f] = smix[...]
    last0, lastn, wide = layout[-1]
    for W in (WGU[-1], WVU[-1], WDN[-1]):
        for k in range(4):
            W[k, lastn:, :] = jnp.zeros((wide - lastn, 256), BF16)
    z_fwd(0)
    z_fwd(1)
    z_own(2)
    z_own(3)
    y_mid(XG, ky[0], sy[0], 0)
    y_mid(XG, ky[1], sy[1], 1)
    loads[1].wait()
    loads[2].wait()
    for w, kern, off in ((0, gkv, go), (1, vkv, vo)):
        CV[w, :, last0:] = jnp.zeros((4, wide), F32)
        CV[w, 0:3, 0:units] = kern[...]
        CV[w, 3:4, 0:units] = off[...].reshape(1, units)
    y_end(XG, ky[0], sy[0], 0)
    y_end(XG, ky[1], sy[1], 1)
    y_last(XG, ky[0])
    y_last(XG, ky[1])
    scaled(XG, mgain, False)
    z_fin(0)
    z_fin(1)
    for w, W in ((0, WGP), (1, WVP)):
        prod = jnp.dot(XS[...], W[...].reshape(1024, 256), preferred_element_type=F32)
        P1[:, :, w * 256 : w * 256 + 256] = prod.reshape(4, 128, 256)

    def row_loop(first, n, fn):
        def step(i, _):
            fn(pl.ds(pl.multiple_of(first + i * 16, 16), 16))
            return 0

        lax.fori_loop(0, n // 16, step, 0)

    ra, rb = pl.ds(0, 64), pl.ds(64, 64)

    def rounded_rows(p, S, i, first, n):
        def fn(rows):
            S[i % 3, rows, :] = p[i, rows, :].astype(BF16)

        row_loop(first, n, fn)

    def rs_far(p, S, H, F, k, s):
        rounded_rows(p, S, 3, 0, 128)
        send(S.at[0, ra], H.at[0], s, k, x_up)
        send(S.at[0, rb], H.at[1], s, k + 1, x_dn)

    def rs_first(p, S, H, F, k, s):
        rounded_rows(p, S, 1, 64, 64)
        send(S.at[1, rb], F.at[0, rb], s, k + 2, x_up)
        rounded_rows(p, S, 2, 0, 64)
        send(S.at[2, ra], F.at[1, ra], s, k + 2, x_dn)

    def rs_second(p, S, H, F, k, s):
        def left(rows):
            S[1, rows, :] = (p[1, rows, :] + H[0, rows, :].astype(F32)).astype(BF16)

        def right(rows):
            low = pl.ds(pl.multiple_of(rows.start + 64, 16), 16)
            S[2, low, :] = (p[2, low, :] + H[1, rows, :].astype(F32)).astype(BF16)

        recv(H.at[0], k)
        row_loop(0, 64, left)
        send(S.at[1, ra], F.at[0, ra], s, k + 2, x_up)
        recv(H.at[1], k + 1)
        row_loop(0, 64, right)
        send(S.at[2, rb], F.at[1, rb], s, k + 2, x_dn)

    def rs_wait(F, k):
        recv(F, k + 2)

    kr = [new(recvs, 3) for _ in layout]
    set1 = (P1, S1, H1, F1, kr[0], sender(S1))
    rs_far(*set1)
    rs_first(*set1)
    z_fwd(2)
    z_own(4)
    rs_second(*set1)
    z_fwd(3)
    z_own(5)
    recv(SM.at[pl.ds(0, 15)], km)
    recv(SSB.at[pl.ds(0, 7)], kss)
    rs_wait(F1, kr[0])

    total = P1[0] + F1[0].astype(F32) + F1[1].astype(F32)
    rs = scale_of(jnp.sum(SSB[...], axis=0)[0:1, :])
    eye = lax.broadcasted_iota(jnp.int32, (128, 128), 0) == lanes_of(128)
    for h in range(2):
        cols = slice(h * 128, h * 128 + 128)
        gated = gelu((rs * total[:, cols]).astype(BF16).astype(F32))
        spread = gelu((rs * total[:, 256 + h * 128 : 384 + h * 128]).astype(BF16).astype(F32))
        spread = spread * lax.rsqrt(jnp.mean(spread * spread, axis=-1, keepdims=True) + EPS)
        spread = (spread * vgain[h : h + 1, :]).astype(BF16)
        matrix = SM[:, h].astype(F32).reshape(128, 128).astype(BF16)
        mixed = jnp.dot(matrix, spread, preferred_element_type=F32)
        bias = jnp.broadcast_to(sbias[h : h + 1, :], (128, 128))
        mixed = mixed + jnp.sum(jnp.where(eye, bias, 0.0), axis=-1, keepdims=True)
        joined = gated * mixed
        joined = joined * lax.rsqrt(jnp.mean(joined * joined, axis=-1, keepdims=True) + EPS)
        MG[0, :, cols] = (joined * hgain[h : h + 1, :]).astype(BF16)

    k2 = new(recvs, 3)
    s2 = sender(MG.at[pl.ds(0, 3)])
    send(MG.at[0], MG.at[2], s2, k2 + 2, x_up)
    send(MG.at[0], MG.at[1], s2, k2 + 1, x_dn)
    send(MG.at[0], MG.at[3], s2, k2, x_far)
    z_fin(2)

    y_order = (far(y), up(y), down(y), y)

    def cy_first(g, product, CS, CR, k, s):
        for n, yt in enumerate(y_order):
            prod = product(yt)
            size = prod.shape[0] // 128
            rows = pl.ds(2 * g, size)
            T[n, rows] = jnp.where(c == 0, prod[:, :128], prod[:, 128:]).reshape(size, 128, 128)
            give = jnp.where(c == 0, prod[:, 128:], prod[:, :128]).astype(BF16)
            CS[n, rows] = give.reshape(size, 128, 128)
            send(CS.at[n, rows], CR.at[n, rows], s, k + n, mate)

    def joined_at(n, b, CR):
        return T[n, b] + CR[n, b].astype(F32)

    def cy_second(g, CR, YS, YH, YF, k, kc, s):
        a, b = 2 * g, 2 * g + 1
        recv(CR.at[0, pl.ds(a, 2)], kc)
        YS[0, a] = joined_at(0, a, CR).astype(BF16)
        YS[0, b] = joined_at(0, b, CR).astype(BF16)
        send(YS.at[0, a], YH.at[a], s, k, y_up)
        send(YS.at[0, b], YH.at[b], s, k + 1, y_dn)
        recv(CR.at[1, pl.ds(a, 2)], kc + 1)
        YS[1, b] = joined_at(1, b, CR).astype(BF16)
        send(YS.at[1, b], YF.at[g, 0, 1], s, k + 2, y_up)
        recv(CR.at[2, pl.ds(a, 2)], kc + 2)
        YS[2, a] = joined_at(2, a, CR).astype(BF16)
        send(YS.at[2, a], YF.at[g, 1, 0], s, k + 2, y_dn)

    def cy_third(g, CR, YS, YH, YF, k, kc, s):
        a, b = 2 * g, 2 * g + 1
        recv(YH.at[a], k)
        YS[1, a] = (joined_at(1, a, CR) + YH[a].astype(F32)).astype(BF16)
        send(YS.at[1, a], YF.at[g, 0, 0], s, k + 2, y_up)
        recv(YH.at[b], k + 1)
        YS[2, b] = (joined_at(2, b, CR) + YH[b].astype(F32)).astype(BF16)
        send(YS.at[2, b], YF.at[g, 1, 1], s, k + 2, y_dn)
        recv(CR.at[3, pl.ds(a, 2)], kc + 3)

    def cy_last(g, CR, YF, k):
        recv(YF.at[g], k + 2)
        return [
            joined_at(3, 2 * g + i, CR) + YF[g, 0, i].astype(F32) + YF[g, 1, i].astype(F32)
            for i in range(2)
        ]

    def merge(g):
        rows = MG[2 * g : 2 * g + 2].reshape(256, 256)
        return lambda yt: jnp.dot(rows, WMP[yt], preferred_element_type=F32)

    kc = [new(recvs, 4) for _ in range(2)]
    k3 = [new(recvs, 3) for _ in range(2)]
    sc, s3 = sender(CS4), sender(YS4)
    recv(MG.at[1], k2 + 1)
    cy_first(0, merge(0), CS4, CR4, kc[0], sc)
    cy_second(0, CR4, YS4, YH4, YF4, k3[0], kc[0], s3)
    recv(MG.at[2], k2 + 2)
    recv(MG.at[3], k2)
    cy_first(1, merge(1), CS4, CR4, kc[1], sc)
    cy_second(1, CR4, YS4, YH4, YF4, k3[1], kc[1], s3)
    z_fwd(4)
    z_own(6)
    cy_third(0, CR4, YS4, YH4, YF4, k3[0], kc[0], s3)
    cy_third(1, CR4, YS4, YH4, YF4, k3[1], kc[1], s3)

    ko = new(recvs)
    so = new(sends)
    ends.append(lambda: fewer(lambda n: HG.at[0, pl.ds(0, n)], 4, stay(so)))
    spot = 2 * lax.rem(x, 2) + c
    blocks = (x, up(x), down(x), far(x))
    sh = [sender(buf.at[pl.ds(0, 7), pl.ds(0, 2)]) for buf in (HG, HG)]
    for g in range(2):
        branch = cy_last(g, CR4, YF4, k3[g])
        for i in range(2):
            b = 2 * g + i
            HG[me, b] = (XG[me, b].astype(F32) + branch[i]).astype(BF16)
        y_start(HG, ky[g], sh[g], g)
    for b in range(4):
        if b:
            dst = HRES.at[spot]
            send(HG.at[me, b], dst, so, ko, at(x_=blocks[b], c_=x // 2))
            continue

        @pl.when(to_me)
        def _():
            HRES[spot] = HG[me, 0]

        @pl.when(jnp.logical_not(to_me))
        def _():
            send(HG.at[me, 0], HRES.at[spot], so, ko, mate)

    z_fwd(5)
    z_own(7)
    y_mid(HG, ky[0], sh[0], 0)
    y_mid(HG, ky[1], sh[1], 1)
    y_end(HG, ky[0], sh[0], 0)
    y_end(HG, ky[1], sh[1], 1)
    z_fwd(6)
    z_own(8)
    z_fin(weight("g", 0))
    z_fin(weight("v", 0))
    y_last(HG, ky[0])
    y_last(HG, ky[1])
    scaled(HG, fgain, True)
    kf = new(recvs)
    sf = sender(SSF.at[pl.ds(0, 3)])
    SSF[0] = SQR[0]
    send(SQR.at[1], SSF.at[2], sf, kf, x_up)
    send(SQR.at[2], SSF.at[1], sf, kf, x_dn)
    send(SQR.at[3], SSF.at[3], sf, kf, x_far)

    def project(W, p, n, first, only_far=False):
        def cut(cols, to, size):
            w = jnp.concatenate([W[k, cols, :] for k in range(4)], axis=1)
            rows = XS[384:512, :] if only_far else XS[...]
            prod = lax.dot_general(
                rows, w, (((1,), (1,)), ((), ())), preferred_element_type=F32
            )
            if only_far:
                p[3, :, to] = prod
            else:
                p[:, :, to] = prod.reshape(4, 128, size)

        def step(i, _):
            cut(
                pl.ds(pl.multiple_of(i * 256, 256), 256),
                pl.ds(pl.multiple_of(first + i * 256, 128), 256), 256,
            )
            return 0

        lax.fori_loop(0, n // 256, step, 0)
        left = n % 256
        if left:
            cut(pl.ds(n - left, left), pl.ds(first + n - left, left), left)

    def both(j, only_far=False):
        n = layout[j][2]
        project(WGU[j], PC[j], n, 0, only_far)
        project(WVU[j], PC[j], n, n, only_far)

    row = lax.broadcasted_iota(jnp.int32, (128, 128), 0)

    def activate(j):
        p, F, act = PC[j], FC[j], ACT[j]
        at0, _, n = layout[j]

        def conv_tile(i, _):
            def one(first, w):
                at_ = pl.ds(pl.multiple_of(first + i * 128, 128), 128)
                v = p[0, :, at_] + F[0, :, at_].astype(F32) + F[1, :, at_].astype(F32)
                v = (RS[...] * v).astype(BF16).astype(F32)
                prev = jnp.where(row == 0, 0.0, pltpu.roll(v, 1, axis=0))
                after = jnp.where(row == 127, 0.0, pltpu.roll(v, 127, axis=0))
                k = CV[w, :, pl.ds(pl.multiple_of(at0 + i * 128, 128), 128)]
                return k[3:4] + prev * k[0:1] + v * k[1:2] + after * k[2:3]

            cols = pl.ds(pl.multiple_of(i * 128, 128), 128)
            act[0, :, cols] = (gelu(one(0, 0)) * one(n, 1)).astype(BF16)
            return 0

        lax.fori_loop(0, n // 128, conv_tile, 0)

    sets = [
        (PC[j], SC[j], HC[j], FC[j], kr[j], sender(SC[j])) for j in range(chunks)
    ]
    kg = [new(recvs, 3) for _ in layout]
    sg = [sender(ACT[j].at[pl.ds(0, 3)]) for j in range(chunks)]

    def x_start(j):
        buf, k, s = ACT[j], kg[j], sg[j]
        send(buf.at[0, ra], buf.at[2, ra], s, k, x_up)
        send(buf.at[0, rb], buf.at[1, rb], s, k + 1, x_dn)
        send(buf.at[0, rb], buf.at[2, rb], s, k + 2, x_up)
        send(buf.at[0, ra], buf.at[1, ra], s, k + 2, x_dn)

    def x_mid(j):
        buf, k, s = ACT[j], kg[j], sg[j]
        recv(buf.at[2, ra], k)
        send(buf.at[2, ra], buf.at[3, ra], s, k + 2, x_up)
        recv(buf.at[1, rb], k + 1)
        send(buf.at[1, rb], buf.at[3, rb], s, k + 2, x_dn)

    def x_last(j):
        recv(ACT[j].at[pl.ds(0, 2)], kg[j] + 2)

    def down_early(j):
        def step(n, _):
            rows = ACT[j][...].reshape(512, layout[j][2])
            prod = jnp.dot(rows, WDN[j][n], preferred_element_type=F32)
            ACC[n] = prod if j == 0 else ACC[n] + prod
            return 0

        lax.fori_loop(0, 4, step, 0)

    both(0, True)
    rs_far(*sets[0])
    both(0)
    rs_first(*sets[0])
    z_fwd(7)
    rs_second(*sets[0])
    z_fin(weight("g", 1))
    z_fin(weight("v", 1))
    both(1)
    rs_far(*sets[1])
    rs_first(*sets[1])
    z_fwd(8)
    z_own(9)
    z_own(10)
    z_own(11)
    rs_second(*sets[1])
    z_fin(weight("g", 2))
    z_fin(weight("v", 2))
    both(2)
    rs_far(*sets[2])
    rs_first(*sets[2])
    recv(SSF.at[pl.ds(0, 3)], kf)
    RS[...] = scale_of(jnp.sum(SSF[...], axis=0)[0:1, :])
    rs_wait(FC[0], kr[0])
    activate(0)
    x_start(0)
    rs_second(*sets[2])
    rs_wait(FC[1], kr[1])
    activate(1)
    x_start(1)
    x_mid(0)
    z_fwd(9)
    rs_wait(FC[2], kr[2])
    activate(2)
    x_start(2)
    x_mid(1)
    z_fwd(10)
    z_fwd(11)
    x_mid(2)
    x_last(0)
    z_fin(9)
    down_early(0)
    x_last(1)
    z_fin(10)
    down_early(1)
    z_fin(11)
    x_last(2)

    final = ACT[2][...].reshape(512, layout[2][2])
    k7 = new(recvs, 4)
    s7 = sender(CS5)
    cy_first(
        0, lambda yt: jnp.dot(final, WDN[2][yt], preferred_element_type=F32) + ACC[yt],
        CS5, CR5, k7, s7,
    )
    kt = new(recvs)
    st = new(sends)
    ends.append(lambda: fewer(lambda n: TB.at[pl.ds(0, n)], 16, stay(st)))
    for n, yt in enumerate(y_order):
        recv(CR5.at[n], k7 + n)
        for b in range(4):
            i = 4 * n + b
            TB[i] = (T[n, b] + CR5[n, b].astype(F32)).astype(BF16)
            if i != 12:
                peer = at(x_=blocks[b], y_=yt, c_=x // 2)
                send(TB.at[i], TI.at[4 * y + spot], st, kt, peer)
                continue

            @pl.when(to_me)
            def _():
                TI[4 * y + spot] = TB[12]

            @pl.when(jnp.logical_not(to_me))
            def _():
                send(TB.at[12], TI.at[4 * y + spot], st, kt, mate)

    fewer(lambda n: HRES.at[pl.ds(0, n)], 4, lambda ref: recv(ref, ko))
    fewer(lambda n: TI.at[pl.ds(0, n)], 16, lambda ref: recv(ref, kt))
    for q in range(4):
        change = sum(TI[4 * n + q].astype(F32) for n in range(4))
        out[:, q * 128 : q * 128 + 128] = (HRES[q].astype(F32) + change).astype(BF16)
    for wait in ends:
        wait()
    assert sends[0] <= ssem.shape[0] and recvs[0] <= rsem.shape[0], (sends[0], recvs[0])


def body(
    tokens, mixer_gain, gate_proj, value_proj, value_gain, spatial_mix, spatial_bias,
    head_gain, merge_proj, ffn_gain, gate_up, value_up, gate_kernel, value_kernel,
    gate_offset, value_offset, down_proj,
):
    units = gate_up.shape[1]
    layout = []
    for first in range(0, units, CHUNK):
        n = min(CHUNK, units - first)
        layout.append((first, n, -(-n // 128) * 128))
    wide = sum(n for _, _, n in layout)
    widths = [n for _, _, n in layout]
    vm = lambda shape, dtype=BF16: pltpu.VMEM(shape, dtype)
    in_vmem = pl.BlockSpec(memory_space=pltpu.VMEM)
    left = pl.BlockSpec(memory_space=pl.ANY)
    call = pl.pallas_call(
        functools.partial(kernel, layout),
        out_shape=jax.ShapeDtypeStruct(tokens.shape, tokens.dtype),
        in_specs=[
            left, in_vmem, in_vmem, left, left, in_vmem, in_vmem, in_vmem, in_vmem, left,
            left, left, left, left, in_vmem, in_vmem, left,
        ],
        out_specs=in_vmem,
        scratch_shapes=[
            vm(tokens.shape), vm(gate_kernel.shape, F32), vm(gate_kernel.shape, F32),
            vm((2, 4, wide), F32),
            vm((8, 4, 128, 128)), vm((8, 4, 128, 128)), vm((512, 1024)),
            vm((4, 8, 128), F32), vm((128, 128), F32), vm((16, 2, 8, 128)),
            vm((4, 128, 256)), vm((8, 8, 128), F32), vm((4, 8, 128), F32), vm((4, 128, 128)),
            vm((16, 128, 128)), vm((16, 128, 128)),
            *[vm((4, 256, 256))] * 3, vm((4, 4, 128, 128), F32), vm((4, 512, 256), F32),
            vm((4, 128, 512), F32), vm((3, 128, 512)), vm((2, 64, 512)), vm((2, 128, 512)),
            vm((4, 4, 128, 128)), vm((4, 4, 128, 128)), vm((3, 4, 128, 128)),
            vm((4, 128, 128)), vm((2, 2, 2, 128, 128)),
            vm((4, 4, 128, 128)), vm((4, 4, 128, 128)),
            *[vm((4, n, 256)) for _ in range(3) for n in widths],
            *[vm((4, 128, n)) for n in widths],
            *[vm((4, 128, 2 * n), F32) for n in widths],
            *[vm((3, 128, 2 * n)) for n in widths],
            *[vm((2, 64, 2 * n)) for n in widths],
            *[vm((2, 128, 2 * n)) for n in widths],
            pltpu.SemaphoreType.DMA((SENDS,)), pltpu.SemaphoreType.DMA((RECVS,)),
            pltpu.SemaphoreType.DMA((6 + 3 * len(layout),)),
        ],
        compiler_params=pltpu.CompilerParams(
            collective_id=0, has_side_effects=True, vmem_limit_bytes=58 << 20
        ),
        name="layer",
    )
    return call(
        tokens, mixer_gain, ffn_gain, gate_proj, value_proj, value_gain, spatial_mix,
        spatial_bias, head_gain, merge_proj, gate_up.T, value_up.T, gate_kernel, value_kernel,
        gate_offset, value_offset, down_proj,
    )


def solution(mesh):
    finer = Mesh(
        mesh.devices.reshape(mesh.shape["rep"], 4, 4, 4, 2), ("rep", "fs_0", "fs_1", "tp_0", "tp_1")
    )
    return jax.shard_map(
        body,
        mesh=finer,
        in_specs=(
            P(REP_FS, TP), P(), P(FS, TP), P(FS, TP), P(TP, None), P(TP, FS, None),
            P(TP, None), P(TP, None), P(TP, FS), P(), P(FS, TP), P(FS, TP), P(None, TP),
            P(None, TP), P(TP), P(TP), P(TP, FS),
        ),
        out_specs=P(REP_FS, TP),
        check_vma=False,
    )
```

```python
import functools

import jax
import jax.numpy as jnp
from jax import lax
from jax.experimental import pallas as pl
from jax.experimental.pallas import tpu as pltpu
from jax.sharding import Mesh
from jax.sharding import PartitionSpec as P

TP = ("tp_0", "tp_1")
FS = ("fs_0", "fs_1")
REP_FS = ("rep", "fs_0", "fs_1")
MESH = pl.DeviceIdType.MESH
EPS = 1e-06
SENDS, RECVS = 33, 103
CHUNK = 512
F32 = jnp.float32
BF16 = jnp.bfloat16


def gelu(v):
    return 0.5 * v * (1.0 + lax.erf(v * 0.7071067811865476))


def lanes_of(n):
    return lax.broadcasted_iota(jnp.int32, (n, 128), 1)


def kernel(layout, tok, mgain, fgain, gp, vp, vgain, smix, sbias, hgain, mp, gu, vu, gk, vk, go, vo,
           dn, out, tokv, gkv, vkv, CV, XG, HG, XS, SQR, RS, SM, MG, SSB, SSF, HRES, TB, TI,
           WGP, WVP, WMP, T, ACC, P1, S1, H1, F1, CS4, CR4, YS4, YH4, YF4, CS5, CR5, *rest):
    chunks = len(layout)
    WGU, WVU, WDN, ACT, PC, SC, HC, FC = (rest[i * chunks : (i + 1) * chunks] for i in range(8))
    ssem, rsem, lsem = rest[8 * chunks :]
    r, z, x, y, c = (lax.axis_index(a) for a in ("rep", "fs_0", "fs_1", "tp_0", "tp_1"))
    other = 1 - c
    f = 4 * z + x
    units = dn.shape[0]
    depth = mgain.shape[0]

    def at(z_=None, x_=None, y_=None, c_=None, r_=None):
        pick = lambda new, old: old if new is None else new
        return (pick(r_, r), pick(z_, z), pick(x_, x), pick(y_, y), pick(c_, c))

    up = lambda v: lax.rem(v + 1, 4)
    down = lambda v: lax.rem(v + 3, 4)
    far = lambda v: lax.rem(v + 2, 4)

    zr = 4 * r + z
    zu, zd = lax.rem(zr + 1, 8), lax.rem(zr + 7, 8)
    z_up = at(r_=zu // 4, z_=lax.rem(zu, 4))
    z_dn = at(r_=zd // 4, z_=lax.rem(zd, 4))
    x_up, x_dn, x_far = at(x_=up(x)), at(x_=down(x)), at(x_=far(x))
    y_up, y_dn = at(y_=up(y)), at(y_=down(y))
    mate = at(c_=other)
    fs_peers = []
    for i in range(1, 16):
        g = lax.rem(f + i, 16)
        fs_peers.append(at(z_=g // 4, x_=lax.rem(g, 4)))
    near = []
    for i in range(1, 16):
        g = lax.rem(4 * y + x + i, 16)
        near += [at(y_=g // 4, x_=lax.rem(g, 4), c_=jnp.int32(k)) for k in range(2)]

    barrier = pltpu.get_barrier_semaphore()
    greet = [mate, z_up, z_dn] + near + fs_peers
    for peer in greet:
        pl.semaphore_signal(barrier, inc=1, device_id=peer, device_id_type=MESH)
    loads = [
        pltpu.make_async_copy(src, dst, lsem.at[i])
        for i, (src, dst) in enumerate(((tok, tokv), (gk, gkv), (vk, vkv)))
    ]
    for copy in loads:
        copy.start()
    pl.semaphore_wait(barrier, len(greet))

    sends, recvs, ends = [0], [0], []

    def new(counter, n=1):
        counter[0] += n
        return counter[0] - n

    def remote(src, dst, s, k, peer):
        return pltpu.make_async_remote_copy(
            src_ref=src, dst_ref=dst, send_sem=ssem.at[s], recv_sem=rsem.at[k],
            device_id=peer, device_id_type=MESH,
        )

    def send(src, dst, s, k, peer):
        remote(src, dst, s, k, peer).start()

    def recv(dst, k):
        remote(dst, dst, 0, k, mate).wait_recv()

    def sender(ref):
        s = new(sends)
        ends.append(lambda: remote(ref, ref, s, 0, mate).wait_send())
        return s

    pieces = [(gp, WGP, 0, 256), (vp, WVP, 0, 256), (mp, WMP, 0, 256)]
    for (at0, n, _), G, V in zip(layout, WGU, WVU):
        pieces += [(gu, G, at0, n), (vu, V, at0, n)]
    for (at0, n, _), W in zip(layout, WDN):
        pieces.append((dn, W, at0, n))
    zk = [new(recvs, 3) for _ in pieces]
    zs = [sender(buf.at[pl.ds(0, 3), pl.ds(0, n)]) for _, buf, _, n in pieces]

    def z_local(i):
        src, buf, at0, n = pieces[i]
        return pltpu.make_async_copy(src.at[pl.ds(at0, n)], buf.at[z, pl.ds(0, n)], lsem.at[3 + i])

    def z_own(i):
        src, buf, at0, n = pieces[i]
        a, b = pl.ds(0, n // 2), pl.ds(n // 2, n // 2)
        from_a, from_b = src.at[pl.ds(at0, n // 2)], src.at[pl.ds(at0 + n // 2, n // 2)]
        send(from_a, buf.at[z, a], zs[i], zk[i], z_up)
        send(from_b, buf.at[z, b], zs[i], zk[i] + 1, z_dn)
        send(from_b, buf.at[z, b], zs[i], zk[i] + 2, z_up)
        send(from_a, buf.at[z, a], zs[i], zk[i] + 2, z_dn)
        z_local(i).start()

    def z_fwd(i):
        _, buf, _, n = pieces[i]
        a, b = buf.at[down(z), pl.ds(0, n // 2)], buf.at[up(z), pl.ds(n // 2, n // 2)]
        recv(a, zk[i])
        send(a, a, zs[i], zk[i] + 2, z_up)
        recv(b, zk[i] + 1)
        send(b, b, zs[i], zk[i] + 2, z_dn)

    def z_fin(i):
        _, buf, _, n = pieces[i]
        recv(buf.at[pl.ds(0, 2), pl.ds(0, n)], zk[i] + 2)
        z_local(i).wait()

    def weight(kind, j):
        return {"g": 3 + 2 * j, "v": 4 + 2 * j, "d": 3 + 2 * chunks + j}[kind]

    me = 2 * y + c
    to_me = x // 2 == c
    loads[0].wait()
    kx = new(recvs, 2)
    sx = new(sends)
    for j in range(2):
        for h in range(2):
            xt = 2 * c + j
            ahead = lax.rem(x - xt + 4, 4)
            place = jnp.where(ahead == 0, 3, jnp.where(ahead == 2, 2, ahead // 2))
            mine = jnp.logical_and(xt == x, c == h)
            block = tokv.at[:, j * 256 + h * 128 : j * 256 + h * 128 + 128]

            @pl.when(jnp.logical_not(mine))
            def _():
                dst = XG.at[2 * y + h, place]
                send(block, dst, sx, kx + place // 2, at(x_=xt, c_=jnp.int32(h)))

            @pl.when(mine)
            def _():
                XG[2 * y + h, 3] = block[...]

    def fewer(ref_of, n, wait):
        @pl.when(to_me)
        def _():
            wait(ref_of(n - 1))

        @pl.when(jnp.logical_not(to_me))
        def _():
            wait(ref_of(n))

    stay = lambda s: lambda ref: remote(ref, ref, s, 0, mate).wait_send()
    ends.append(lambda: fewer(lambda n: XG.at[0, pl.ds(0, n)], 4, stay(sx)))
    z_own(0)
    z_own(1)
    square = tokv[...].astype(F32)
    square = jnp.sum(square * square, axis=-1, keepdims=True)
    SSB[me] = jnp.broadcast_to(square, (128, 128)).T[0:8, :]
    kss = new(recvs)
    sss = sender(SSB.at[pl.ds(0, 7)])
    for i in range(1, 8):
        t = lax.rem(me + i, 8)
        send(SSB.at[me], SSB.at[me], sss, kss, at(y_=t // 2, c_=lax.rem(t, 2)))

    lo_y, hi_y, far_y = 2 * down(y) + c, 2 * up(y) + c, 2 * far(y) + c

    def y_start(buf, k, s, g):
        a, b = buf.at[me, 2 * g], buf.at[me, 2 * g + 1]
        send(a, a, s, k, y_up)
        send(b, b, s, k + 1, y_dn)
        send(b, b, s, k + 2, y_up)
        send(a, a, s, k + 3, y_dn)
        both = buf.at[me, pl.ds(2 * g, 2)]
        send(both, both, s, k + 6, mate)

    def y_mid(buf, k, s, g):
        a, b = buf.at[lo_y, 2 * g], buf.at[hi_y, 2 * g + 1]
        recv(a, k)
        send(a, a, s, k + 4, y_up)
        send(a, a, s, k + 6, mate)
        recv(b, k + 1)
        send(b, b, s, k + 5, y_dn)
        send(b, b, s, k + 6, mate)

    def y_end(buf, k, s, g):
        rows = (buf.at[lo_y, 2 * g + 1], buf.at[hi_y, 2 * g], buf.at[far_y, 2 * g], buf.at[far_y, 2 * g + 1])
        for i, ref in enumerate(rows):
            recv(ref, k + 2 + i)
            send(ref, ref, s, k + 6, mate)

    def y_last(buf, k):
        recv(buf.at[pl.ds(0, 4), pl.ds(0, 2)], k + 6)

    def scaled(buf, gains, squares, first, n):
        parts = [gains[pl.ds(pl.multiple_of((4 * k + x) * 256, 256), 256)] for k in range(4)]
        gain = jnp.concatenate([part.reshape(1, 256) for part in parts], axis=1)

        def block(b, _):
            rows = jnp.concatenate([buf[i, b] for i in range(8)], axis=1).astype(F32)
            if squares:
                total = jnp.sum(rows * rows, axis=-1, keepdims=True)
                SQR[b] = jnp.broadcast_to(total, (128, 128)).T[0:8, :]
            XS[pl.ds(pl.multiple_of(b * 128, 128), 128), :] = (rows * gain).astype(BF16)
            return 0

        lax.fori_loop(first, first + n, block, 0)

    def scale_of(rows):
        return lax.rsqrt(jnp.broadcast_to(rows, (128, 128)).T / depth + EPS)

    ky = [new(recvs, 7) for _ in range(2)]
    sy = [sender(buf.at[pl.ds(0, 7), pl.ds(0, 2)]) for buf in (XG, XG)]
    recv(XG.at[me, pl.ds(0, 2)], kx)
    y_start(XG, ky[0], sy[0], 0)
    fewer(lambda n: XG.at[me, pl.ds(0, n)], 2, lambda ref: recv(ref, kx + 1))
    y_start(XG, ky[1], sy[1], 1)
    km = new(recvs)
    sm = sender(SM.at[pl.ds(0, 15)])
    for i in range(15):
        send(smix, SM.at[f], sm, km, fs_peers[i])
    SM[f] = smix[...]
    last0, lastn, wide = layout[-1]
    for W in (WGU[-1], WVU[-1], WDN[-1]):
        for k in range(4):
            W[k, lastn:, :] = jnp.zeros((wide - lastn, 256), BF16)
    z_fwd(0)
    z_fwd(1)
    z_own(2)
    z_own(3)
    y_mid(XG, ky[0], sy[0], 0)
    y_mid(XG, ky[1], sy[1], 1)
    loads[1].wait()
    loads[2].wait()
    for w, kern, off in ((0, gkv, go), (1, vkv, vo)):
        CV[w, :, last0:] = jnp.zeros((4, wide), F32)
        CV[w, 0:3, 0:units] = kern[...]
        CV[w, 3:4, 0:units] = off[...].reshape(1, units)
    y_end(XG, ky[0], sy[0], 0)
    y_end(XG, ky[1], sy[1], 1)
    y_last(XG, ky[0])
    y_last(XG, ky[1])
    scaled(XG, mgain, False, 0, 4)
    z_fin(0)
    z_fin(1)
    for w, W in ((0, WGP), (1, WVP)):
        prod = jnp.dot(XS[...], W[...].reshape(1024, 256), preferred_element_type=F32)
        P1[:, :, w * 256 : w * 256 + 256] = prod.reshape(4, 128, 256)

    def row_loop(first, n, fn):
        def step(i, _):
            fn(pl.ds(pl.multiple_of(first + i * 16, 16), 16))
            return 0

        lax.fori_loop(0, n // 16, step, 0)

    ra, rb = pl.ds(0, 64), pl.ds(64, 64)

    def rounded_rows(p, i, S, k, first, n):
        def fn(rows):
            S[k, rows, :] = p[i, rows, :].astype(BF16)

        row_loop(first, n, fn)

    def rs_far(p, S, H, F, k, s):
        rounded_rows(p, 2, S, 0, 0, 128)
        send(S.at[0, ra], H.at[0], s, k, x_up)
        send(S.at[0, rb], H.at[1], s, k + 1, x_dn)

    def rs_first(p, S, H, F, k, s):
        rounded_rows(p, 0, S, 1, 64, 64)
        send(S.at[1, rb], F.at[0, rb], s, k + 2, x_up)
        rounded_rows(p, 1, S, 2, 0, 64)
        send(S.at[2, ra], F.at[1, ra], s, k + 2, x_dn)

    def rs_second(p, S, H, F, k, s):
        def left(rows):
            S[1, rows, :] = (p[0, rows, :] + H[0, rows, :].astype(F32)).astype(BF16)

        def right(rows):
            low = pl.ds(pl.multiple_of(rows.start + 64, 16), 16)
            S[2, low, :] = (p[1, low, :] + H[1, rows, :].astype(F32)).astype(BF16)

        recv(H.at[0], k)
        row_loop(0, 64, left)
        send(S.at[1, ra], F.at[0, ra], s, k + 2, x_up)
        recv(H.at[1], k + 1)
        row_loop(0, 64, right)
        send(S.at[2, rb], F.at[1, rb], s, k + 2, x_dn)

    def rs_wait(F, k):
        recv(F, k + 2)

    kr = [new(recvs, 3) for _ in layout]
    set1 = (P1, S1, H1, F1, kr[0], sender(S1))
    rs_far(*set1)
    rs_first(*set1)
    z_fwd(2)
    z_own(4)
    rs_second(*set1)
    z_fwd(3)
    z_own(5)
    recv(SM.at[pl.ds(0, 15)], km)
    recv(SSB.at[pl.ds(0, 7)], kss)
    rs_wait(F1, kr[0])

    total = P1[3] + F1[0].astype(F32) + F1[1].astype(F32)
    rs = scale_of(jnp.sum(SSB[...], axis=0)[0:1, :])
    eye = lax.broadcasted_iota(jnp.int32, (128, 128), 0) == lanes_of(128)
    for h in range(2):
        cols = slice(h * 128, h * 128 + 128)
        gated = gelu((rs * total[:, cols]).astype(BF16).astype(F32))
        spread = gelu((rs * total[:, 256 + h * 128 : 384 + h * 128]).astype(BF16).astype(F32))
        spread = spread * lax.rsqrt(jnp.mean(spread * spread, axis=-1, keepdims=True) + EPS)
        spread = (spread * vgain[h : h + 1, :]).astype(BF16)
        matrix = SM[:, h].astype(F32).reshape(128, 128).astype(BF16)
        mixed = jnp.dot(matrix, spread, preferred_element_type=F32)
        bias = jnp.broadcast_to(sbias[h : h + 1, :], (128, 128))
        mixed = mixed + jnp.sum(jnp.where(eye, bias, 0.0), axis=-1, keepdims=True)
        joined = gated * mixed
        joined = joined * lax.rsqrt(jnp.mean(joined * joined, axis=-1, keepdims=True) + EPS)
        MG[3, :, cols] = (joined * hgain[h : h + 1, :]).astype(BF16)

    k2 = new(recvs, 3)
    s2 = sender(MG.at[pl.ds(0, 3)])
    send(MG.at[3], MG.at[1], s2, k2 + 1, x_up)
    send(MG.at[3], MG.at[0], s2, k2 + 2, x_dn)
    send(MG.at[3], MG.at[2], s2, k2, x_far)
    z_fin(2)

    y_order = (far(y), up(y), down(y), y)

    def cy_first(g, product, CS, CR, k, s):
        for n, yt in enumerate(y_order):
            prod = product(yt)
            size = prod.shape[0] // 128
            rows = pl.ds(2 * g, size)
            T[n, rows] = jnp.where(c == 0, prod[:, :128], prod[:, 128:]).reshape(size, 128, 128)
            give = jnp.where(c == 0, prod[:, 128:], prod[:, :128]).astype(BF16)
            CS[n, rows] = give.reshape(size, 128, 128)
            send(CS.at[n, rows], CR.at[n, rows], s, k + n, mate)

    def joined_at(n, b, CR):
        return T[n, b] + CR[n, b].astype(F32)

    def cy_second(g, CR, YS, YH, YF, k, kc, s):
        a, b = 2 * g, 2 * g + 1
        recv(CR.at[0, pl.ds(a, 2)], kc)
        YS[0, a] = joined_at(0, a, CR).astype(BF16)
        YS[0, b] = joined_at(0, b, CR).astype(BF16)
        send(YS.at[0, a], YH.at[a], s, k, y_up)
        send(YS.at[0, b], YH.at[b], s, k + 1, y_dn)
        recv(CR.at[1, pl.ds(a, 2)], kc + 1)
        YS[1, b] = joined_at(1, b, CR).astype(BF16)
        send(YS.at[1, b], YF.at[g, 0, 1], s, k + 2, y_up)
        recv(CR.at[2, pl.ds(a, 2)], kc + 2)
        YS[2, a] = joined_at(2, a, CR).astype(BF16)
        send(YS.at[2, a], YF.at[g, 1, 0], s, k + 2, y_dn)

    def cy_third(g, CR, YS, YH, YF, k, kc, s):
        a, b = 2 * g, 2 * g + 1
        recv(YH.at[a], k)
        YS[1, a] = (joined_at(1, a, CR) + YH[a].astype(F32)).astype(BF16)
        send(YS.at[1, a], YF.at[g, 0, 0], s, k + 2, y_up)
        recv(YH.at[b], k + 1)
        YS[2, b] = (joined_at(2, b, CR) + YH[b].astype(F32)).astype(BF16)
        send(YS.at[2, b], YF.at[g, 1, 1], s, k + 2, y_dn)
        recv(CR.at[3, pl.ds(a, 2)], kc + 3)

    def cy_last(g, CR, YF, k):
        recv(YF.at[g], k + 2)
        return [
            joined_at(3, 2 * g + i, CR) + YF[g, 0, i].astype(F32) + YF[g, 1, i].astype(F32)
            for i in range(2)
        ]

    def merge(g):
        rows = MG[2 * g : 2 * g + 2].reshape(256, 256)
        return lambda yt: jnp.dot(rows, WMP[yt], preferred_element_type=F32)

    kc = [new(recvs, 4) for _ in range(2)]
    k3 = [new(recvs, 3) for _ in range(2)]
    sc, s3 = sender(CS4), sender(YS4)
    recv(MG.at[0], k2 + 2)
    recv(MG.at[1], k2 + 1)
    cy_first(0, merge(0), CS4, CR4, kc[0], sc)
    cy_second(0, CR4, YS4, YH4, YF4, k3[0], kc[0], s3)
    recv(MG.at[2], k2)
    cy_first(1, merge(1), CS4, CR4, kc[1], sc)
    cy_second(1, CR4, YS4, YH4, YF4, k3[1], kc[1], s3)
    z_fwd(4)
    z_own(6)
    cy_third(0, CR4, YS4, YH4, YF4, k3[0], kc[0], s3)
    cy_third(1, CR4, YS4, YH4, YF4, k3[1], kc[1], s3)

    ko = new(recvs)
    so = new(sends)
    ends.append(lambda: fewer(lambda n: HG.at[0, pl.ds(0, n)], 4, stay(so)))
    spot = 2 * lax.rem(x, 2) + c
    blocks = (up(x), down(x), far(x), x)
    sh = [sender(buf.at[pl.ds(0, 7), pl.ds(0, 2)]) for buf in (HG, HG)]
    for g in range(2):
        branch = cy_last(g, CR4, YF4, k3[g])
        for i in range(2):
            b = 2 * g + i
            HG[me, b] = (XG[me, b].astype(F32) + branch[i]).astype(BF16)
        y_start(HG, ky[g], sh[g], g)
    for b in range(4):
        if b < 3:
            dst = HRES.at[spot]
            send(HG.at[me, b], dst, so, ko, at(x_=blocks[b], c_=x // 2))
            continue

        @pl.when(to_me)
        def _():
            HRES[spot] = HG[me, 3]

        @pl.when(jnp.logical_not(to_me))
        def _():
            send(HG.at[me, 3], HRES.at[spot], so, ko, mate)

    z_fwd(5)
    y_mid(HG, ky[0], sh[0], 0)
    y_mid(HG, ky[1], sh[1], 1)
    y_end(HG, ky[0], sh[0], 0)
    z_fwd(6)
    z_own(7)
    z_own(8)
    y_end(HG, ky[1], sh[1], 1)
    z_fin(weight("g", 0))
    z_fin(weight("v", 0))
    y_last(HG, ky[0])
    scaled(HG, fgain, True, 0, 2)

    def project(W, p, n, first, b0, b1):
        def cut(cols, to, size):
            w = jnp.concatenate([W[k, cols, :] for k in range(4)], axis=1)
            prod = lax.dot_general(
                XS[b0 * 128 : b1 * 128, :], w, (((1,), (1,)), ((), ())),
                preferred_element_type=F32,
            )
            p[b0:b1, :, to] = prod.reshape(b1 - b0, 128, size)

        def step(i, _):
            cut(
                pl.ds(pl.multiple_of(i * 256, 256), 256),
                pl.ds(pl.multiple_of(first + i * 256, 128), 256), 256,
            )
            return 0

        lax.fori_loop(0, n // 256, step, 0)
        left = n % 256
        if left:
            cut(pl.ds(n - left, left), pl.ds(first + n - left, left), left)

    def both(j, b0=0, b1=4):
        n = layout[j][2]
        project(WGU[j], PC[j], n, 0, b0, b1)
        project(WVU[j], PC[j], n, n, b0, b1)

    row = lax.broadcasted_iota(jnp.int32, (128, 128), 0)

    def activate(j):
        p, F, act = PC[j], FC[j], ACT[j]
        at0, _, n = layout[j]

        def conv_tile(i, _):
            def one(first, w):
                at_ = pl.ds(pl.multiple_of(first + i * 128, 128), 128)
                v = p[3, :, at_] + F[0, :, at_].astype(F32) + F[1, :, at_].astype(F32)
                v = (RS[...] * v).astype(BF16).astype(F32)
                prev = jnp.where(row == 0, 0.0, pltpu.roll(v, 1, axis=0))
                after = jnp.where(row == 127, 0.0, pltpu.roll(v, 127, axis=0))
                k = CV[w, :, pl.ds(pl.multiple_of(at0 + i * 128, 128), 128)]
                return k[3:4] + prev * k[0:1] + v * k[1:2] + after * k[2:3]

            cols = pl.ds(pl.multiple_of(i * 128, 128), 128)
            act[3, :, cols] = (gelu(one(0, 0)) * one(n, 1)).astype(BF16)
            return 0

        lax.fori_loop(0, n // 128, conv_tile, 0)

    sets = [
        (PC[j], SC[j], HC[j], FC[j], kr[j], sender(SC[j])) for j in range(chunks)
    ]
    kg = [new(recvs, 4) for _ in layout]
    sg = [sender(ACT[j].at[pl.ds(0, 3)]) for j in range(chunks)]

    def x_start(j):
        buf, k, s = ACT[j], kg[j], sg[j]
        send(buf.at[3, ra], buf.at[1, ra], s, k, x_up)
        send(buf.at[3, rb], buf.at[0, rb], s, k + 1, x_dn)
        send(buf.at[3, rb], buf.at[1, rb], s, k + 2, x_up)
        send(buf.at[3, ra], buf.at[0, ra], s, k + 2, x_dn)

    def x_mid(j):
        buf, k, s = ACT[j], kg[j], sg[j]
        recv(buf.at[1, ra], k)
        send(buf.at[1, ra], buf.at[2, ra], s, k + 3, x_up)
        recv(buf.at[0, rb], k + 1)
        send(buf.at[0, rb], buf.at[2, rb], s, k + 3, x_dn)

    def x_near(j):
        recv(ACT[j].at[0], kg[j] + 2)

    def x_last(j):
        recv(ACT[j].at[2], kg[j] + 3)

    def down_rows(j, g):
        n = layout[j][2]
        rows = ACT[j][2 * g : 2 * g + 2].reshape(256, n)
        return lambda k: jnp.dot(rows, WDN[j][k], preferred_element_type=F32)

    def down_early(j, g):
        product = down_rows(j, g)

        def step(k, _):
            prod = product(k)
            ACC[k, g] = prod if j == 0 else ACC[k, g] + prod
            return 0

        lax.fori_loop(0, 4, step, 0)

    both(0, 0, 2)
    rs_first(*sets[0])
    y_last(HG, ky[1])
    scaled(HG, fgain, True, 2, 2)
    both(0, 2, 4)
    rs_far(*sets[0])
    kf = new(recvs)
    sf = sender(SSF.at[pl.ds(0, 3)])
    SSF[3] = SQR[3]
    send(SQR.at[0], SSF.at[1], sf, kf, x_up)
    send(SQR.at[1], SSF.at[0], sf, kf, x_dn)
    send(SQR.at[2], SSF.at[2], sf, kf, x_far)
    z_fin(weight("g", 1))
    z_fin(weight("v", 1))
    both(1)
    rs_second(*sets[0])
    rs_far(*sets[1])
    rs_first(*sets[1])
    z_fwd(7)
    z_fwd(8)
    z_own(9)
    z_own(10)
    z_own(11)
    rs_second(*sets[1])
    recv(SSF.at[pl.ds(0, 3)], kf)
    RS[...] = scale_of(jnp.sum(SSF[...], axis=0)[0:1, :])
    rs_wait(FC[0], kr[0])
    activate(0)
    x_start(0)
    z_fin(weight("g", 2))
    z_fin(weight("v", 2))
    both(2)
    rs_far(*sets[2])
    rs_first(*sets[2])
    rs_wait(FC[1], kr[1])
    activate(1)
    rs_second(*sets[2])
    x_start(1)
    x_mid(0)
    z_fwd(9)
    x_near(0)
    z_fin(9)
    down_early(0, 0)
    rs_wait(FC[2], kr[2])
    activate(2)
    x_start(2)
    x_mid(1)
    z_fwd(10)
    z_fwd(11)
    x_near(1)
    z_fin(10)
    down_early(1, 0)
    x_mid(2)
    x_near(2)
    z_fin(11)

    k7 = [new(recvs, 4) for _ in range(2)]
    s7 = sender(CS5)
    kt = new(recvs)
    st = new(sends)
    ends.append(lambda: fewer(lambda n: TB.at[pl.ds(0, n)], 16, stay(st)))

    def give(n, yt, b):
        i = 4 * n + b
        TB[i] = (T[n, b] + CR5[n, b].astype(F32)).astype(BF16)
        dst = TI.at[4 * y + spot]
        if i != 15:
            send(TB.at[i], dst, st, kt, at(x_=blocks[b], y_=yt, c_=x // 2))
            return

        @pl.when(to_me)
        def _():
            TI[4 * y + spot] = TB[15]

        @pl.when(jnp.logical_not(to_me))
        def _():
            send(TB.at[15], dst, st, kt, mate)

    for g in range(2):
        if g:
            x_last(0)
            down_early(0, 1)
            x_last(1)
            down_early(1, 1)
            x_last(2)
        product = down_rows(2, g)
        cy_first(g, lambda yt: product(yt) + ACC[yt, g], CS5, CR5, k7[g], s7)
        for n, yt in enumerate(y_order):
            recv(CR5.at[n, pl.ds(2 * g, 2)], k7[g] + n)
            for b in (2 * g, 2 * g + 1):
                give(n, yt, b)

    fewer(lambda n: HRES.at[pl.ds(0, n)], 4, lambda ref: recv(ref, ko))
    fewer(lambda n: TI.at[pl.ds(0, n)], 16, lambda ref: recv(ref, kt))
    for q in range(4):
        change = sum(TI[4 * n + q].astype(F32) for n in range(4))
        out[:, q * 128 : q * 128 + 128] = (HRES[q].astype(F32) + change).astype(BF16)
    for wait in ends:
        wait()
    assert sends[0] <= ssem.shape[0] and recvs[0] <= rsem.shape[0], (sends[0], recvs[0])


def body(
    tokens, mixer_gain, gate_proj, value_proj, value_gain, spatial_mix, spatial_bias,
    head_gain, merge_proj, ffn_gain, gate_up, value_up, gate_kernel, value_kernel,
    gate_offset, value_offset, down_proj,
):
    units = gate_up.shape[1]
    layout = []
    for first in range(0, units, CHUNK):
        n = min(CHUNK, units - first)
        layout.append((first, n, -(-n // 128) * 128))
    wide = sum(n for _, _, n in layout)
    widths = [n for _, _, n in layout]
    vm = lambda shape, dtype=BF16: pltpu.VMEM(shape, dtype)
    in_vmem = pl.BlockSpec(memory_space=pltpu.VMEM)
    left = pl.BlockSpec(memory_space=pl.ANY)
    call = pl.pallas_call(
        functools.partial(kernel, layout),
        out_shape=jax.ShapeDtypeStruct(tokens.shape, tokens.dtype),
        in_specs=[
            left, in_vmem, in_vmem, left, left, in_vmem, in_vmem, in_vmem, in_vmem, left,
            left, left, left, left, in_vmem, in_vmem, left,
        ],
        out_specs=in_vmem,
        scratch_shapes=[
            vm(tokens.shape), vm(gate_kernel.shape, F32), vm(gate_kernel.shape, F32),
            vm((2, 4, wide), F32),
            vm((8, 4, 128, 128)), vm((8, 4, 128, 128)), vm((512, 1024)),
            vm((4, 8, 128), F32), vm((128, 128), F32), vm((16, 2, 8, 128)),
            vm((4, 128, 256)), vm((8, 8, 128), F32), vm((4, 8, 128), F32), vm((4, 128, 128)),
            vm((16, 128, 128)), vm((16, 128, 128)),
            *[vm((4, 256, 256))] * 3, vm((4, 4, 128, 128), F32), vm((4, 2, 256, 256), F32),
            vm((4, 128, 512), F32), vm((3, 128, 512)), vm((2, 64, 512)), vm((2, 128, 512)),
            vm((4, 4, 128, 128)), vm((4, 4, 128, 128)), vm((3, 4, 128, 128)),
            vm((4, 128, 128)), vm((2, 2, 2, 128, 128)),
            vm((4, 4, 128, 128)), vm((4, 4, 128, 128)),
            *[vm((4, n, 256)) for _ in range(3) for n in widths],
            *[vm((4, 128, n)) for n in widths],
            *[vm((4, 128, 2 * n), F32) for n in widths],
            *[vm((3, 128, 2 * n)) for n in widths],
            *[vm((2, 64, 2 * n)) for n in widths],
            *[vm((2, 128, 2 * n)) for n in widths],
            pltpu.SemaphoreType.DMA((SENDS,)), pltpu.SemaphoreType.DMA((RECVS,)),
            pltpu.SemaphoreType.DMA((6 + 3 * len(layout),)),
        ],
        compiler_params=pltpu.CompilerParams(
            collective_id=0, has_side_effects=True, vmem_limit_bytes=58 << 20
        ),
        name="layer",
    )
    return call(
        tokens, mixer_gain, ffn_gain, gate_proj, value_proj, value_gain, spatial_mix,
        spatial_bias, head_gain, merge_proj, gate_up.T, value_up.T, gate_kernel, value_kernel,
        gate_offset, value_offset, down_proj,
    )


def solution(mesh):
    finer = Mesh(
        mesh.devices.reshape(mesh.shape["rep"], 4, 4, 4, 2), ("rep", "fs_0", "fs_1", "tp_0", "tp_1")
    )
    return jax.shard_map(
        body,
        mesh=finer,
        in_specs=(
            P(REP_FS, TP), P(), P(FS, TP), P(FS, TP), P(TP, None), P(TP, FS, None),
            P(TP, None), P(TP, None), P(TP, FS), P(), P(FS, TP), P(FS, TP), P(None, TP),
            P(None, TP), P(TP), P(TP), P(TP, FS),
        ),
        out_specs=P(REP_FS, TP),
        check_vma=False,
    )
```

```python
import functools

import jax
import jax.numpy as jnp
from jax import lax
from jax.experimental import pallas as pl
from jax.experimental.pallas import tpu as pltpu
from jax.sharding import Mesh
from jax.sharding import PartitionSpec as P

TP = ("tp_0", "tp_1")
FS = ("fs_0", "fs_1")
REP_FS = ("rep", "fs_0", "fs_1")
MESH = pl.DeviceIdType.MESH
EPS = 1e-06
SENDS, RECVS = 33, 103
CHUNK = 512
F32 = jnp.float32
BF16 = jnp.bfloat16


def gelu(v):
    return 0.5 * v * (1.0 + lax.erf(v * 0.7071067811865476))


def lanes_of(n):
    return lax.broadcasted_iota(jnp.int32, (n, 128), 1)


def kernel(layout, tok, mgain, fgain, gp, vp, vgain, smix, sbias, hgain, mp, gu, vu, gk, vk, go, vo,
           dn, out, tokv, gkv, vkv, CV, XG, HG, XS, SQR, RS, SM, MG, SSB, SSF, HRES, TB, TI,
           WGP, WVP, WMP, T, ACC, P1, S1, H1, F1, CS4, CR4, YS4, YH4, YF4, CS5, CR5, *rest):
    chunks = len(layout)
    WGU, WVU, WDN, ACT, PC, SC, HC, FC = (rest[i * chunks : (i + 1) * chunks] for i in range(8))
    ssem, rsem, lsem = rest[8 * chunks :]
    r, z, x, y, c = (lax.axis_index(a) for a in ("rep", "fs_0", "fs_1", "tp_0", "tp_1"))
    other = 1 - c
    f = 4 * z + x
    units = dn.shape[0]
    depth = mgain.shape[0]

    def at(z_=None, x_=None, y_=None, c_=None, r_=None):
        pick = lambda new, old: old if new is None else new
        return (pick(r_, r), pick(z_, z), pick(x_, x), pick(y_, y), pick(c_, c))

    up = lambda v: lax.rem(v + 1, 4)
    down = lambda v: lax.rem(v + 3, 4)
    far = lambda v: lax.rem(v + 2, 4)

    zr = 4 * r + z
    zu, zd = lax.rem(zr + 1, 8), lax.rem(zr + 7, 8)
    z_up = at(r_=zu // 4, z_=lax.rem(zu, 4))
    z_dn = at(r_=zd // 4, z_=lax.rem(zd, 4))
    x_up, x_dn, x_far = at(x_=up(x)), at(x_=down(x)), at(x_=far(x))
    y_up, y_dn = at(y_=up(y)), at(y_=down(y))
    mate = at(c_=other)
    fs_peers = []
    for i in range(1, 16):
        g = lax.rem(f + i, 16)
        fs_peers.append(at(z_=g // 4, x_=lax.rem(g, 4)))
    near = []
    for i in range(1, 16):
        g = lax.rem(4 * y + x + i, 16)
        near += [at(y_=g // 4, x_=lax.rem(g, 4), c_=jnp.int32(k)) for k in range(2)]

    barrier = pltpu.get_barrier_semaphore()
    greet = [mate, z_up, z_dn] + near + fs_peers
    for peer in greet:
        pl.semaphore_signal(barrier, inc=1, device_id=peer, device_id_type=MESH)
    loads = [
        pltpu.make_async_copy(src, dst, lsem.at[i])
        for i, (src, dst) in enumerate(((tok, tokv), (gk, gkv), (vk, vkv)))
    ]
    for copy in loads:
        copy.start()
    pl.semaphore_wait(barrier, len(greet))

    sends, recvs, ends = [0], [0], []

    def new(counter, n=1):
        counter[0] += n
        return counter[0] - n

    def remote(src, dst, s, k, peer):
        return pltpu.make_async_remote_copy(
            src_ref=src, dst_ref=dst, send_sem=ssem.at[s], recv_sem=rsem.at[k],
            device_id=peer, device_id_type=MESH,
        )

    def send(src, dst, s, k, peer):
        remote(src, dst, s, k, peer).start()

    def recv(dst, k):
        remote(dst, dst, 0, k, mate).wait_recv()

    def sender(ref):
        s = new(sends)
        ends.append(lambda: remote(ref, ref, s, 0, mate).wait_send())
        return s

    pieces = [(gp, WGP, 0, 256), (vp, WVP, 0, 256), (mp, WMP, 0, 256)]
    for (at0, n, _), G, V in zip(layout, WGU, WVU):
        pieces += [(gu, G, at0, n), (vu, V, at0, n)]
    for (at0, n, _), W in zip(layout, WDN):
        pieces.append((dn, W, at0, n))
    zk = [new(recvs, 3) for _ in pieces]
    zs = [sender(buf.at[pl.ds(0, 3), pl.ds(0, n)]) for _, buf, _, n in pieces]

    def z_local(i):
        src, buf, at0, n = pieces[i]
        return pltpu.make_async_copy(src.at[pl.ds(at0, n)], buf.at[z, pl.ds(0, n)], lsem.at[3 + i])

    def z_own(i):
        src, buf, at0, n = pieces[i]
        a, b = pl.ds(0, n // 2), pl.ds(n // 2, n // 2)
        from_a, from_b = src.at[pl.ds(at0, n // 2)], src.at[pl.ds(at0 + n // 2, n // 2)]
        send(from_a, buf.at[z, a], zs[i], zk[i], z_up)
        send(from_b, buf.at[z, b], zs[i], zk[i] + 1, z_dn)
        send(from_b, buf.at[z, b], zs[i], zk[i] + 2, z_up)
        send(from_a, buf.at[z, a], zs[i], zk[i] + 2, z_dn)
        z_local(i).start()

    def z_fwd(i):
        _, buf, _, n = pieces[i]
        a, b = buf.at[down(z), pl.ds(0, n // 2)], buf.at[up(z), pl.ds(n // 2, n // 2)]
        recv(a, zk[i])
        send(a, a, zs[i], zk[i] + 2, z_up)
        recv(b, zk[i] + 1)
        send(b, b, zs[i], zk[i] + 2, z_dn)

    def z_fin(i):
        _, buf, _, n = pieces[i]
        recv(buf.at[pl.ds(0, 2), pl.ds(0, n)], zk[i] + 2)
        z_local(i).wait()

    def weight(kind, j):
        return {"g": 3 + 2 * j, "v": 4 + 2 * j, "d": 3 + 2 * chunks + j}[kind]

    me = 2 * y + c
    to_me = x // 2 == c
    loads[0].wait()
    kx = new(recvs, 2)
    sx = new(sends)
    for j in range(2):
        for h in range(2):
            xt = 2 * c + j
            ahead = lax.rem(x - xt + 4, 4)
            place = jnp.where(ahead == 0, 3, jnp.where(ahead == 2, 2, ahead // 2))
            mine = jnp.logical_and(xt == x, c == h)
            block = tokv.at[:, j * 256 + h * 128 : j * 256 + h * 128 + 128]

            @pl.when(jnp.logical_not(mine))
            def _():
                dst = XG.at[2 * y + h, place]
                send(block, dst, sx, kx + place // 2, at(x_=xt, c_=jnp.int32(h)))

            @pl.when(mine)
            def _():
                XG[2 * y + h, 3] = block[...]

    def fewer(ref_of, n, wait):
        @pl.when(to_me)
        def _():
            wait(ref_of(n - 1))

        @pl.when(jnp.logical_not(to_me))
        def _():
            wait(ref_of(n))

    stay = lambda s: lambda ref: remote(ref, ref, s, 0, mate).wait_send()
    ends.append(lambda: fewer(lambda n: XG.at[0, pl.ds(0, n)], 4, stay(sx)))
    z_own(0)
    z_own(1)
    square = tokv[...].astype(F32)
    square = jnp.sum(square * square, axis=-1, keepdims=True)
    SSB[me] = jnp.broadcast_to(square, (128, 128)).T[0:8, :]
    kss = new(recvs)
    sss = sender(SSB.at[pl.ds(0, 7)])
    for i in range(1, 8):
        t = lax.rem(me + i, 8)
        send(SSB.at[me], SSB.at[me], sss, kss, at(y_=t // 2, c_=lax.rem(t, 2)))

    lo_y, hi_y, far_y = 2 * down(y) + c, 2 * up(y) + c, 2 * far(y) + c

    def y_start(buf, k, s, g):
        a, b = buf.at[me, 2 * g], buf.at[me, 2 * g + 1]
        send(a, a, s, k, y_up)
        send(b, b, s, k + 1, y_dn)
        send(b, b, s, k + 2, y_up)
        send(a, a, s, k + 3, y_dn)
        both = buf.at[me, pl.ds(2 * g, 2)]
        send(both, both, s, k + 6, mate)

    def y_mid(buf, k, s, g):
        a, b = buf.at[lo_y, 2 * g], buf.at[hi_y, 2 * g + 1]
        recv(a, k)
        send(a, a, s, k + 4, y_up)
        send(a, a, s, k + 6, mate)
        recv(b, k + 1)
        send(b, b, s, k + 5, y_dn)
        send(b, b, s, k + 6, mate)

    def y_end(buf, k, s, g):
        rows = (buf.at[lo_y, 2 * g + 1], buf.at[hi_y, 2 * g], buf.at[far_y, 2 * g], buf.at[far_y, 2 * g + 1])
        for i, ref in enumerate(rows):
            recv(ref, k + 2 + i)
            send(ref, ref, s, k + 6, mate)

    def y_last(buf, k):
        recv(buf.at[pl.ds(0, 4), pl.ds(0, 2)], k + 6)

    def scaled(buf, gains, squares, first, n):
        parts = [gains[pl.ds(pl.multiple_of((4 * k + x) * 256, 256), 256)] for k in range(4)]
        gain = jnp.concatenate([part.reshape(1, 256) for part in parts], axis=1)

        def block(b, _):
            rows = jnp.concatenate([buf[i, b] for i in range(8)], axis=1).astype(F32)
            if squares:
                total = jnp.sum(rows * rows, axis=-1, keepdims=True)
                SQR[b] = jnp.broadcast_to(total, (128, 128)).T[0:8, :]
            XS[pl.ds(pl.multiple_of(b * 128, 128), 128), :] = (rows * gain).astype(BF16)
            return 0

        lax.fori_loop(first, first + n, block, 0)

    def scale_of(rows):
        return lax.rsqrt(jnp.broadcast_to(rows, (128, 128)).T / depth + EPS)

    ky = [new(recvs, 7) for _ in range(2)]
    sy = [sender(buf.at[pl.ds(0, 7), pl.ds(0, 2)]) for buf in (XG, XG)]
    recv(XG.at[me, pl.ds(0, 2)], kx)
    y_start(XG, ky[0], sy[0], 0)
    fewer(lambda n: XG.at[me, pl.ds(0, n)], 2, lambda ref: recv(ref, kx + 1))
    y_start(XG, ky[1], sy[1], 1)
    km = new(recvs)
    sm = sender(SM.at[pl.ds(0, 15)])
    for i in range(15):
        send(smix, SM.at[f], sm, km, fs_peers[i])
    SM[f] = smix[...]
    last0, lastn, wide = layout[-1]
    for W in (WGU[-1], WVU[-1], WDN[-1]):
        for k in range(4):
            W[k, lastn:, :] = jnp.zeros((wide - lastn, 256), BF16)
    z_fwd(0)
    z_fwd(1)
    z_own(2)
    z_own(3)
    y_mid(XG, ky[0], sy[0], 0)
    y_mid(XG, ky[1], sy[1], 1)
    loads[1].wait()
    loads[2].wait()
    for w, kern, off in ((0, gkv, go), (1, vkv, vo)):
        CV[w, :, last0:] = jnp.zeros((4, wide), F32)
        CV[w, 0:3, 0:units] = kern[...]
        CV[w, 3:4, 0:units] = off[...].reshape(1, units)
    y_end(XG, ky[0], sy[0], 0)
    y_end(XG, ky[1], sy[1], 1)
    y_last(XG, ky[0])
    y_last(XG, ky[1])
    scaled(XG, mgain, False, 0, 4)
    z_fin(0)
    z_fin(1)
    for w, W in ((0, WGP), (1, WVP)):
        prod = jnp.dot(XS[...], W[...].reshape(1024, 256), preferred_element_type=F32)
        P1[:, :, w * 256 : w * 256 + 256] = prod.reshape(4, 128, 256)

    def row_loop(first, n, fn):
        def step(i, _):
            fn(pl.ds(pl.multiple_of(first + i * 16, 16), 16))
            return 0

        lax.fori_loop(0, n // 16, step, 0)

    ra, rb = pl.ds(0, 64), pl.ds(64, 64)

    def rounded_rows(p, i, S, k, first, n):
        def fn(rows):
            S[k, rows, :] = p[i, rows, :].astype(BF16)

        row_loop(first, n, fn)

    def rs_far(p, S, H, F, k, s):
        rounded_rows(p, 2, S, 0, 0, 128)
        send(S.at[0, ra], H.at[0], s, k, x_up)
        send(S.at[0, rb], H.at[1], s, k + 1, x_dn)

    def rs_first(p, S, H, F, k, s):
        rounded_rows(p, 0, S, 1, 64, 64)
        send(S.at[1, rb], F.at[0, rb], s, k + 2, x_up)
        rounded_rows(p, 1, S, 2, 0, 64)
        send(S.at[2, ra], F.at[1, ra], s, k + 2, x_dn)

    def rs_second(p, S, H, F, k, s):
        def left(rows):
            S[1, rows, :] = (p[0, rows, :] + H[0, rows, :].astype(F32)).astype(BF16)

        def right(rows):
            low = pl.ds(pl.multiple_of(rows.start + 64, 16), 16)
            S[2, low, :] = (p[1, low, :] + H[1, rows, :].astype(F32)).astype(BF16)

        recv(H.at[0], k)
        row_loop(0, 64, left)
        send(S.at[1, ra], F.at[0, ra], s, k + 2, x_up)
        recv(H.at[1], k + 1)
        row_loop(0, 64, right)
        send(S.at[2, rb], F.at[1, rb], s, k + 2, x_dn)

    def rs_wait(F, k):
        recv(F, k + 2)

    kr = [new(recvs, 3) for _ in layout]
    set1 = (P1, S1, H1, F1, kr[0], sender(S1))
    rs_far(*set1)
    rs_first(*set1)
    z_fwd(2)
    z_own(4)
    rs_second(*set1)
    z_fwd(3)
    z_own(5)
    recv(SM.at[pl.ds(0, 15)], km)
    recv(SSB.at[pl.ds(0, 7)], kss)
    rs_wait(F1, kr[0])

    total = P1[3] + F1[0].astype(F32) + F1[1].astype(F32)
    rs = scale_of(jnp.sum(SSB[...], axis=0)[0:1, :])
    eye = lax.broadcasted_iota(jnp.int32, (128, 128), 0) == lanes_of(128)
    for h in range(2):
        cols = slice(h * 128, h * 128 + 128)
        gated = gelu((rs * total[:, cols]).astype(BF16).astype(F32))
        spread = gelu((rs * total[:, 256 + h * 128 : 384 + h * 128]).astype(BF16).astype(F32))
        spread = spread * lax.rsqrt(jnp.mean(spread * spread, axis=-1, keepdims=True) + EPS)
        spread = (spread * vgain[h : h + 1, :]).astype(BF16)
        matrix = SM[:, h].astype(F32).reshape(128, 128).astype(BF16)
        mixed = jnp.dot(matrix, spread, preferred_element_type=F32)
        bias = jnp.broadcast_to(sbias[h : h + 1, :], (128, 128))
        mixed = mixed + jnp.sum(jnp.where(eye, bias, 0.0), axis=-1, keepdims=True)
        joined = gated * mixed
        joined = joined * lax.rsqrt(jnp.mean(joined * joined, axis=-1, keepdims=True) + EPS)
        MG[3, :, cols] = (joined * hgain[h : h + 1, :]).astype(BF16)

    k2 = new(recvs, 3)
    s2 = sender(MG.at[pl.ds(0, 3)])
    send(MG.at[3], MG.at[1], s2, k2 + 1, x_up)
    send(MG.at[3], MG.at[0], s2, k2 + 2, x_dn)
    send(MG.at[3], MG.at[2], s2, k2, x_far)
    z_fin(2)

    y_order = (far(y), up(y), down(y), y)

    def cy_first(g, product, CS, CR, k, s):
        for n, yt in enumerate(y_order):
            prod = product(yt)
            size = prod.shape[0] // 128
            rows = pl.ds(2 * g, size)
            T[n, rows] = jnp.where(c == 0, prod[:, :128], prod[:, 128:]).reshape(size, 128, 128)
            give = jnp.where(c == 0, prod[:, 128:], prod[:, :128]).astype(BF16)
            CS[n, rows] = give.reshape(size, 128, 128)
            send(CS.at[n, rows], CR.at[n, rows], s, k + n, mate)

    def joined_at(n, b, CR):
        return T[n, b] + CR[n, b].astype(F32)

    def cy_second(g, CR, YS, YH, YF, k, kc, s):
        a, b = 2 * g, 2 * g + 1
        recv(CR.at[0, pl.ds(a, 2)], kc)
        YS[0, a] = joined_at(0, a, CR).astype(BF16)
        YS[0, b] = joined_at(0, b, CR).astype(BF16)
        send(YS.at[0, a], YH.at[a], s, k, y_up)
        send(YS.at[0, b], YH.at[b], s, k + 1, y_dn)
        recv(CR.at[1, pl.ds(a, 2)], kc + 1)
        YS[1, b] = joined_at(1, b, CR).astype(BF16)
        send(YS.at[1, b], YF.at[g, 0, 1], s, k + 2, y_up)
        recv(CR.at[2, pl.ds(a, 2)], kc + 2)
        YS[2, a] = joined_at(2, a, CR).astype(BF16)
        send(YS.at[2, a], YF.at[g, 1, 0], s, k + 2, y_dn)

    def cy_third(g, CR, YS, YH, YF, k, kc, s):
        a, b = 2 * g, 2 * g + 1
        recv(YH.at[a], k)
        YS[1, a] = (joined_at(1, a, CR) + YH[a].astype(F32)).astype(BF16)
        send(YS.at[1, a], YF.at[g, 0, 0], s, k + 2, y_up)
        recv(YH.at[b], k + 1)
        YS[2, b] = (joined_at(2, b, CR) + YH[b].astype(F32)).astype(BF16)
        send(YS.at[2, b], YF.at[g, 1, 1], s, k + 2, y_dn)
        recv(CR.at[3, pl.ds(a, 2)], kc + 3)

    def cy_last(g, CR, YF, k):
        recv(YF.at[g], k + 2)
        return [
            joined_at(3, 2 * g + i, CR) + YF[g, 0, i].astype(F32) + YF[g, 1, i].astype(F32)
            for i in range(2)
        ]

    def merge(g):
        rows = MG[2 * g : 2 * g + 2].reshape(256, 256)
        return lambda yt: jnp.dot(rows, WMP[yt], preferred_element_type=F32)

    kc = [new(recvs, 4) for _ in range(2)]
    k3 = [new(recvs, 3) for _ in range(2)]
    sc, s3 = sender(CS4), sender(YS4)
    recv(MG.at[0], k2 + 2)
    recv(MG.at[1], k2 + 1)
    cy_first(0, merge(0), CS4, CR4, kc[0], sc)
    cy_second(0, CR4, YS4, YH4, YF4, k3[0], kc[0], s3)
    recv(MG.at[2], k2)
    cy_first(1, merge(1), CS4, CR4, kc[1], sc)
    cy_second(1, CR4, YS4, YH4, YF4, k3[1], kc[1], s3)
    z_fwd(4)
    z_own(6)
    cy_third(0, CR4, YS4, YH4, YF4, k3[0], kc[0], s3)
    cy_third(1, CR4, YS4, YH4, YF4, k3[1], kc[1], s3)

    ko = new(recvs)
    so = new(sends)
    ends.append(lambda: fewer(lambda n: HG.at[0, pl.ds(0, n)], 4, stay(so)))
    spot = 2 * lax.rem(x, 2) + c
    blocks = (up(x), down(x), far(x), x)
    sh = [sender(buf.at[pl.ds(0, 7), pl.ds(0, 2)]) for buf in (HG, HG)]
    for g in range(2):
        branch = cy_last(g, CR4, YF4, k3[g])
        for i in range(2):
            b = 2 * g + i
            HG[me, b] = (XG[me, b].astype(F32) + branch[i]).astype(BF16)
        y_start(HG, ky[g], sh[g], g)
    for b in range(4):
        if b < 3:
            dst = HRES.at[spot]
            send(HG.at[me, b], dst, so, ko, at(x_=blocks[b], c_=x // 2))
            continue

        @pl.when(to_me)
        def _():
            HRES[spot] = HG[me, 3]

        @pl.when(jnp.logical_not(to_me))
        def _():
            send(HG.at[me, 3], HRES.at[spot], so, ko, mate)

    z_fwd(5)
    y_mid(HG, ky[0], sh[0], 0)
    y_mid(HG, ky[1], sh[1], 1)
    y_end(HG, ky[0], sh[0], 0)
    z_fwd(6)
    z_own(7)
    z_own(8)
    y_end(HG, ky[1], sh[1], 1)
    z_fin(weight("g", 0))
    z_fin(weight("v", 0))
    y_last(HG, ky[0])
    scaled(HG, fgain, True, 0, 2)

    def project(W, p, n, first, b0, b1):
        def cut(cols, to, size):
            w = jnp.concatenate([W[k, cols, :] for k in range(4)], axis=1)
            prod = lax.dot_general(
                XS[b0 * 128 : b1 * 128, :], w, (((1,), (1,)), ((), ())),
                preferred_element_type=F32,
            )
            p[b0:b1, :, to] = prod.reshape(b1 - b0, 128, size)

        def step(i, _):
            cut(
                pl.ds(pl.multiple_of(i * 256, 256), 256),
                pl.ds(pl.multiple_of(first + i * 256, 128), 256), 256,
            )
            return 0

        lax.fori_loop(0, n // 256, step, 0)
        left = n % 256
        if left:
            cut(pl.ds(n - left, left), pl.ds(first + n - left, left), left)

    def both(j, b0=0, b1=4):
        n = layout[j][2]
        project(WGU[j], PC[j], n, 0, b0, b1)
        project(WVU[j], PC[j], n, n, b0, b1)

    row = lax.broadcasted_iota(jnp.int32, (128, 128), 0)

    def activate(j):
        p, F, act = PC[j], FC[j], ACT[j]
        at0, _, n = layout[j]

        def conv_tile(i, _):
            def one(first, w):
                at_ = pl.ds(pl.multiple_of(first + i * 128, 128), 128)
                v = p[3, :, at_] + F[0, :, at_].astype(F32) + F[1, :, at_].astype(F32)
                v = (RS[...] * v).astype(BF16).astype(F32)
                prev = jnp.where(row == 0, 0.0, pltpu.roll(v, 1, axis=0))
                after = jnp.where(row == 127, 0.0, pltpu.roll(v, 127, axis=0))
                k = CV[w, :, pl.ds(pl.multiple_of(at0 + i * 128, 128), 128)]
                return k[3:4] + prev * k[0:1] + v * k[1:2] + after * k[2:3]

            cols = pl.ds(pl.multiple_of(i * 128, 128), 128)
            act[3, :, cols] = (gelu(one(0, 0)) * one(n, 1)).astype(BF16)
            return 0

        lax.fori_loop(0, n // 128, conv_tile, 0)

    sets = [
        (PC[j], SC[j], HC[j], FC[j], kr[j], sender(SC[j])) for j in range(chunks)
    ]
    kg = [new(recvs, 4) for _ in layout]
    sg = [sender(ACT[j].at[pl.ds(0, 3)]) for j in range(chunks)]

    def x_start(j):
        buf, k, s = ACT[j], kg[j], sg[j]
        send(buf.at[3, ra], buf.at[1, ra], s, k, x_up)
        send(buf.at[3, rb], buf.at[0, rb], s, k + 1, x_dn)
        send(buf.at[3, rb], buf.at[1, rb], s, k + 2, x_up)
        send(buf.at[3, ra], buf.at[0, ra], s, k + 2, x_dn)

    def x_mid(j):
        buf, k, s = ACT[j], kg[j], sg[j]
        recv(buf.at[1, ra], k)
        send(buf.at[1, ra], buf.at[2, ra], s, k + 3, x_up)
        recv(buf.at[0, rb], k + 1)
        send(buf.at[0, rb], buf.at[2, rb], s, k + 3, x_dn)

    def x_near(j):
        recv(ACT[j].at[0], kg[j] + 2)

    def x_last(j):
        recv(ACT[j].at[2], kg[j] + 3)

    def down_rows(j, g):
        n = layout[j][2]
        rows = ACT[j][2 * g : 2 * g + 2].reshape(256, n)
        return lambda k: jnp.dot(rows, WDN[j][k], preferred_element_type=F32)

    def down_early(j, g):
        product = down_rows(j, g)

        def step(k, _):
            prod = product(k)
            ACC[k, g] = prod if j == 0 else ACC[k, g] + prod
            return 0

        lax.fori_loop(0, 4, step, 0)

    both(0, 0, 2)
    rs_first(*sets[0])
    y_last(HG, ky[1])
    scaled(HG, fgain, True, 2, 2)
    both(0, 2, 4)
    rs_far(*sets[0])
    kf = new(recvs)
    sf = sender(SSF.at[pl.ds(0, 3)])
    SSF[3] = SQR[3]
    send(SQR.at[0], SSF.at[1], sf, kf, x_up)
    send(SQR.at[1], SSF.at[0], sf, kf, x_dn)
    send(SQR.at[2], SSF.at[2], sf, kf, x_far)
    z_fin(weight("g", 1))
    z_fin(weight("v", 1))
    both(1)
    rs_second(*sets[0])
    rs_far(*sets[1])
    rs_first(*sets[1])
    z_fwd(7)
    z_fwd(8)
    z_own(9)
    z_own(10)
    rs_second(*sets[1])
    recv(SSF.at[pl.ds(0, 3)], kf)
    RS[...] = scale_of(jnp.sum(SSF[...], axis=0)[0:1, :])
    rs_wait(FC[0], kr[0])
    activate(0)
    x_start(0)
    z_fin(weight("g", 2))
    z_fin(weight("v", 2))
    both(2)
    rs_far(*sets[2])
    rs_first(*sets[2])
    z_fwd(9)
    z_own(11)
    rs_wait(FC[1], kr[1])
    activate(1)
    rs_second(*sets[2])
    x_start(1)
    x_mid(0)
    z_fwd(10)
    rs_wait(FC[2], kr[2])
    activate(2)
    x_start(2)
    x_mid(1)
    z_fin(9)
    x_near(0)
    down_early(0, 0)
    z_fwd(11)
    x_mid(2)
    z_fin(10)
    x_near(1)
    down_early(1, 0)
    x_near(2)
    z_fin(11)

    k7 = [new(recvs, 4) for _ in range(2)]
    s7 = sender(CS5)
    kt = new(recvs)
    st = new(sends)
    ends.append(lambda: fewer(lambda n: TB.at[pl.ds(0, n)], 16, stay(st)))

    def give(n, yt, b):
        i = 4 * n + b
        TB[i] = (T[n, b] + CR5[n, b].astype(F32)).astype(BF16)
        dst = TI.at[4 * y + spot]
        if i != 15:
            send(TB.at[i], dst, st, kt, at(x_=blocks[b], y_=yt, c_=x // 2))
            return

        @pl.when(to_me)
        def _():
            TI[4 * y + spot] = TB[15]

        @pl.when(jnp.logical_not(to_me))
        def _():
            send(TB.at[15], dst, st, kt, mate)

    for g in range(2):
        if g:
            x_last(0)
            down_early(0, 1)
            x_last(1)
            down_early(1, 1)
            x_last(2)
        product = down_rows(2, g)
        cy_first(g, lambda yt: product(yt) + ACC[yt, g], CS5, CR5, k7[g], s7)
        for n, yt in enumerate(y_order):
            recv(CR5.at[n, pl.ds(2 * g, 2)], k7[g] + n)
            for b in (2 * g, 2 * g + 1):
                give(n, yt, b)

    fewer(lambda n: HRES.at[pl.ds(0, n)], 4, lambda ref: recv(ref, ko))
    fewer(lambda n: TI.at[pl.ds(0, n)], 16, lambda ref: recv(ref, kt))
    for q in range(4):
        change = sum(TI[4 * n + q].astype(F32) for n in range(4))
        out[:, q * 128 : q * 128 + 128] = (HRES[q].astype(F32) + change).astype(BF16)
    for wait in ends:
        wait()
    assert sends[0] <= ssem.shape[0] and recvs[0] <= rsem.shape[0], (sends[0], recvs[0])


def body(
    tokens, mixer_gain, gate_proj, value_proj, value_gain, spatial_mix, spatial_bias,
    head_gain, merge_proj, ffn_gain, gate_up, value_up, gate_kernel, value_kernel,
    gate_offset, value_offset, down_proj,
):
    units = gate_up.shape[1]
    layout = []
    for first in range(0, units, CHUNK):
        n = min(CHUNK, units - first)
        layout.append((first, n, -(-n // 128) * 128))
    wide = sum(n for _, _, n in layout)
    widths = [n for _, _, n in layout]
    vm = lambda shape, dtype=BF16: pltpu.VMEM(shape, dtype)
    in_vmem = pl.BlockSpec(memory_space=pltpu.VMEM)
    left = pl.BlockSpec(memory_space=pl.ANY)
    call = pl.pallas_call(
        functools.partial(kernel, layout),
        out_shape=jax.ShapeDtypeStruct(tokens.shape, tokens.dtype),
        in_specs=[
            left, in_vmem, in_vmem, left, left, in_vmem, in_vmem, in_vmem, in_vmem, left,
            left, left, left, left, in_vmem, in_vmem, left,
        ],
        out_specs=in_vmem,
        scratch_shapes=[
            vm(tokens.shape), vm(gate_kernel.shape, F32), vm(gate_kernel.shape, F32),
            vm((2, 4, wide), F32),
            vm((8, 4, 128, 128)), vm((8, 4, 128, 128)), vm((512, 1024)),
            vm((4, 8, 128), F32), vm((128, 128), F32), vm((16, 2, 8, 128)),
            vm((4, 128, 256)), vm((8, 8, 128), F32), vm((4, 8, 128), F32), vm((4, 128, 128)),
            vm((16, 128, 128)), vm((16, 128, 128)),
            *[vm((4, 256, 256))] * 3, vm((4, 4, 128, 128), F32), vm((4, 2, 256, 256), F32),
            vm((4, 128, 512), F32), vm((3, 128, 512)), vm((2, 64, 512)), vm((2, 128, 512)),
            vm((4, 4, 128, 128)), vm((4, 4, 128, 128)), vm((3, 4, 128, 128)),
            vm((4, 128, 128)), vm((2, 2, 2, 128, 128)),
            vm((4, 4, 128, 128)), vm((4, 4, 128, 128)),
            *[vm((4, n, 256)) for _ in range(3) for n in widths],
            *[vm((4, 128, n)) for n in widths],
            *[vm((4, 128, 2 * n), F32) for n in widths],
            *[vm((3, 128, 2 * n)) for n in widths],
            *[vm((2, 64, 2 * n)) for n in widths],
            *[vm((2, 128, 2 * n)) for n in widths],
            pltpu.SemaphoreType.DMA((SENDS,)), pltpu.SemaphoreType.DMA((RECVS,)),
            pltpu.SemaphoreType.DMA((6 + 3 * len(layout),)),
        ],
        compiler_params=pltpu.CompilerParams(
            collective_id=0, has_side_effects=True, vmem_limit_bytes=58 << 20
        ),
        name="layer",
    )
    return call(
        tokens, mixer_gain, ffn_gain, gate_proj, value_proj, value_gain, spatial_mix,
        spatial_bias, head_gain, merge_proj, gate_up.T, value_up.T, gate_kernel, value_kernel,
        gate_offset, value_offset, down_proj,
    )


def solution(mesh):
    finer = Mesh(
        mesh.devices.reshape(mesh.shape["rep"], 4, 4, 4, 2), ("rep", "fs_0", "fs_1", "tp_0", "tp_1")
    )
    return jax.shard_map(
        body,
        mesh=finer,
        in_specs=(
            P(REP_FS, TP), P(), P(FS, TP), P(FS, TP), P(TP, None), P(TP, FS, None),
            P(TP, None), P(TP, None), P(TP, FS), P(), P(FS, TP), P(FS, TP), P(None, TP),
            P(None, TP), P(TP), P(TP), P(TP, FS),
        ),
        out_specs=P(REP_FS, TP),
        check_vma=False,
    )
```

```python
import functools

import jax
import jax.numpy as jnp
from jax import lax
from jax.experimental import pallas as pl
from jax.experimental.pallas import tpu as pltpu
from jax.sharding import Mesh
from jax.sharding import PartitionSpec as P

TP = ("tp_0", "tp_1")
FS = ("fs_0", "fs_1")
REP_FS = ("rep", "fs_0", "fs_1")
MESH = pl.DeviceIdType.MESH
EPS = 1e-06
SENDS, RECVS = 33, 103
CHUNK = 512
F32 = jnp.float32
BF16 = jnp.bfloat16


def gelu(v):
    return 0.5 * v * (1.0 + lax.erf(v * 0.7071067811865476))


def lanes_of(n):
    return lax.broadcasted_iota(jnp.int32, (n, 128), 1)


def kernel(layout, tok, mgain, fgain, gp, vp, vgain, smix, sbias, hgain, mp, gu, vu, gk, vk, go, vo,
           dn, out, tokv, gkv, vkv, CV, XG, HG, XS, SQR, RS, SM, MG, SSB, SSF, HRES, TB, TI,
           WGP, WVP, WMP, T, ACC, P1, S1, H1, F1, CS4, CR4, YS4, YH4, YF4, CS5, CR5, T5, *rest):
    chunks = len(layout)
    WGU, WVU, WDN, ACT, PC, SC, HC, FC = (rest[i * chunks : (i + 1) * chunks] for i in range(8))
    ssem, rsem, lsem = rest[8 * chunks :]
    r, z, x, y, c = (lax.axis_index(a) for a in ("rep", "fs_0", "fs_1", "tp_0", "tp_1"))
    other = 1 - c
    f = 4 * z + x
    units = dn.shape[0]
    depth = mgain.shape[0]

    def at(z_=None, x_=None, y_=None, c_=None, r_=None):
        pick = lambda new, old: old if new is None else new
        return (pick(r_, r), pick(z_, z), pick(x_, x), pick(y_, y), pick(c_, c))

    up = lambda v: lax.rem(v + 1, 4)
    down = lambda v: lax.rem(v + 3, 4)
    far = lambda v: lax.rem(v + 2, 4)

    zr = 4 * r + z
    zu, zd = lax.rem(zr + 1, 8), lax.rem(zr + 7, 8)
    z_up = at(r_=zu // 4, z_=lax.rem(zu, 4))
    z_dn = at(r_=zd // 4, z_=lax.rem(zd, 4))
    x_up, x_dn, x_far = at(x_=up(x)), at(x_=down(x)), at(x_=far(x))
    y_up, y_dn = at(y_=up(y)), at(y_=down(y))
    mate = at(c_=other)
    fs_peers = []
    for i in range(1, 16):
        g = lax.rem(f + i, 16)
        fs_peers.append(at(z_=g // 4, x_=lax.rem(g, 4)))
    near = []
    for i in range(1, 4):
        near += [at(x_=lax.rem(x + i, 4), c_=k) for k in (c, other)]
        near += [at(y_=lax.rem(y + i, 4), c_=other)]

    def along(d, y_=None):
        there = lax.rem(zr + 8 + d, 8)
        return at(r_=there // 4, z_=lax.rem(there, 4), y_=y_)

    for i in range(4):
        for d in (-2, -1, 0, 1, 2):
            if i or d:
                near.append(along(d, lax.rem(y + i, 4)))

    barrier = pltpu.get_barrier_semaphore()
    greet = [mate] + near + fs_peers
    for peer in greet:
        pl.semaphore_signal(barrier, inc=1, device_id=peer, device_id_type=MESH)
    loads = [
        pltpu.make_async_copy(src, dst, lsem.at[i])
        for i, (src, dst) in enumerate(((tok, tokv), (gk, gkv), (vk, vkv)))
    ]
    for copy in loads:
        copy.start()
    pl.semaphore_wait(barrier, len(greet))

    sends, recvs, ends = [0], [0], []

    def new(counter, n=1):
        counter[0] += n
        return counter[0] - n

    def remote(src, dst, s, k, peer):
        return pltpu.make_async_remote_copy(
            src_ref=src, dst_ref=dst, send_sem=ssem.at[s], recv_sem=rsem.at[k],
            device_id=peer, device_id_type=MESH,
        )

    def send(src, dst, s, k, peer):
        remote(src, dst, s, k, peer).start()

    def recv(dst, k):
        remote(dst, dst, 0, k, mate).wait_recv()

    def sender(ref):
        s = new(sends)
        ends.append(lambda: remote(ref, ref, s, 0, mate).wait_send())
        return s

    pieces = [(gp, WGP, 0, 256), (vp, WVP, 0, 256), (mp, WMP, 0, 256)]
    for (at0, n, _), G, V in zip(layout, WGU, WVU):
        pieces += [(gu, G, at0, n), (vu, V, at0, n)]
    for (at0, n, _), W in zip(layout, WDN):
        pieces.append((dn, W, at0, n))
    zk = [new(recvs, 3) for _ in pieces]
    zs = [sender(buf.at[pl.ds(0, 3), pl.ds(0, n)]) for _, buf, _, n in pieces]

    def z_local(i):
        src, buf, at0, n = pieces[i]
        own = buf.at[ring(i)[0], pl.ds(0, n)]
        return pltpu.make_async_copy(src.at[pl.ds(at0, n)], own, lsem.at[3 + i])

    def ring(i):
        return (x, x_up, x_dn) if pieces[i][0] is dn else (z, z_up, z_dn)

    def z_own(i):
        src, buf, at0, n = pieces[i]
        a, b = pl.ds(0, n // 2), pl.ds(n // 2, n // 2)
        from_a, from_b = src.at[pl.ds(at0, n // 2)], src.at[pl.ds(at0 + n // 2, n // 2)]
        place, above, below = ring(i)
        send(from_a, buf.at[place, a], zs[i], zk[i], above)
        send(from_b, buf.at[place, b], zs[i], zk[i] + 1, below)
        send(from_b, buf.at[place, b], zs[i], zk[i] + 2, above)
        send(from_a, buf.at[place, a], zs[i], zk[i] + 2, below)
        z_local(i).start()

    def z_fwd(i):
        _, buf, _, n = pieces[i]
        place, above, below = ring(i)
        a, b = buf.at[down(place), pl.ds(0, n // 2)], buf.at[up(place), pl.ds(n // 2, n // 2)]
        recv(a, zk[i])
        send(a, a, zs[i], zk[i] + 2, above)
        recv(b, zk[i] + 1)
        send(b, b, zs[i], zk[i] + 2, below)

    def z_fin(i):
        _, buf, _, n = pieces[i]
        recv(buf.at[pl.ds(0, 2), pl.ds(0, n)], zk[i] + 2)
        z_local(i).wait()

    def weight(kind, j):
        return {"g": 3 + 2 * j, "v": 4 + 2 * j, "d": 3 + 2 * chunks + j}[kind]

    me = 2 * y + c
    to_me = x // 2 == c
    loads[0].wait()
    kx = new(recvs, 2)
    sx = new(sends)
    for j in range(2):
        for h in range(2):
            xt = 2 * c + j
            ahead = lax.rem(x - xt + 4, 4)
            place = jnp.where(ahead == 0, 3, jnp.where(ahead == 2, 2, ahead // 2))
            mine = jnp.logical_and(xt == x, c == h)
            block = tokv.at[:, j * 256 + h * 128 : j * 256 + h * 128 + 128]

            @pl.when(jnp.logical_not(mine))
            def _():
                dst = XG.at[2 * y + h, place]
                send(block, dst, sx, kx + place // 2, at(x_=xt, c_=jnp.int32(h)))

            @pl.when(mine)
            def _():
                XG[2 * y + h, 3] = block[...]

    def fewer(ref_of, n, wait, stays=to_me):
        @pl.when(stays)
        def _():
            wait(ref_of(n - 1))

        @pl.when(jnp.logical_not(stays))
        def _():
            wait(ref_of(n))

    stay = lambda s: lambda ref: remote(ref, ref, s, 0, mate).wait_send()
    ends.append(lambda: fewer(lambda n: XG.at[0, pl.ds(0, n)], 4, stay(sx)))
    z_own(0)
    z_own(1)
    square = tokv[...].astype(F32)
    square = jnp.sum(square * square, axis=-1, keepdims=True)
    SSB[me] = jnp.broadcast_to(square, (128, 128)).T[0:8, :]
    kss = new(recvs)
    sss = sender(SSB.at[pl.ds(0, 7)])
    for i in range(1, 8):
        t = lax.rem(me + i, 8)
        send(SSB.at[me], SSB.at[me], sss, kss, at(y_=t // 2, c_=lax.rem(t, 2)))

    lo_y, hi_y, far_y = 2 * down(y) + c, 2 * up(y) + c, 2 * far(y) + c

    def y_start(buf, k, s, g):
        a, b = buf.at[me, 2 * g], buf.at[me, 2 * g + 1]
        send(a, a, s, k, y_up)
        send(b, b, s, k + 1, y_dn)
        send(b, b, s, k + 2, y_up)
        send(a, a, s, k + 3, y_dn)
        both = buf.at[me, pl.ds(2 * g, 2)]
        send(both, both, s, k + 6, mate)

    def y_mid(buf, k, s, g):
        a, b = buf.at[lo_y, 2 * g], buf.at[hi_y, 2 * g + 1]
        recv(a, k)
        send(a, a, s, k + 4, y_up)
        send(a, a, s, k + 6, mate)
        recv(b, k + 1)
        send(b, b, s, k + 5, y_dn)
        send(b, b, s, k + 6, mate)

    def y_end(buf, k, s, g):
        rows = (buf.at[lo_y, 2 * g + 1], buf.at[hi_y, 2 * g], buf.at[far_y, 2 * g], buf.at[far_y, 2 * g + 1])
        for i, ref in enumerate(rows):
            recv(ref, k + 2 + i)
            send(ref, ref, s, k + 6, mate)

    def y_last(buf, k):
        recv(buf.at[pl.ds(0, 4), pl.ds(0, 2)], k + 6)

    def scaled(buf, gains, squares, first, n):
        parts = [gains[pl.ds(pl.multiple_of((4 * k + x) * 256, 256), 256)] for k in range(4)]
        gain = jnp.concatenate([part.reshape(1, 256) for part in parts], axis=1)

        def block(b, _):
            rows = jnp.concatenate([buf[i, b] for i in range(8)], axis=1).astype(F32)
            if squares:
                total = jnp.sum(rows * rows, axis=-1, keepdims=True)
                SQR[b] = jnp.broadcast_to(total, (128, 128)).T[0:8, :]
            XS[pl.ds(pl.multiple_of(b * 128, 128), 128), :] = (rows * gain).astype(BF16)
            return 0

        lax.fori_loop(first, first + n, block, 0)

    def scale_of(rows):
        return lax.rsqrt(jnp.broadcast_to(rows, (128, 128)).T / depth + EPS)

    ky = [new(recvs, 7) for _ in range(2)]
    sy = [sender(buf.at[pl.ds(0, 7), pl.ds(0, 2)]) for buf in (XG, XG)]
    recv(XG.at[me, pl.ds(0, 2)], kx)
    y_start(XG, ky[0], sy[0], 0)
    fewer(lambda n: XG.at[me, pl.ds(0, n)], 2, lambda ref: recv(ref, kx + 1))
    y_start(XG, ky[1], sy[1], 1)
    km = new(recvs)
    sm = sender(SM.at[pl.ds(0, 15)])
    for i in range(15):
        send(smix, SM.at[f], sm, km, fs_peers[i])
    SM[f] = smix[...]
    last0, lastn, wide = layout[-1]
    for W in (WGU[-1], WVU[-1], WDN[-1]):
        for k in range(4):
            W[k, lastn:, :] = jnp.zeros((wide - lastn, 256), BF16)
    z_own(9)
    z_own(11)
    z_fwd(0)
    z_fwd(1)
    z_own(2)
    z_own(3)
    y_mid(XG, ky[0], sy[0], 0)
    y_mid(XG, ky[1], sy[1], 1)
    loads[1].wait()
    loads[2].wait()
    for w, kern, off in ((0, gkv, go), (1, vkv, vo)):
        CV[w, :, last0:] = jnp.zeros((4, wide), F32)
        CV[w, 0:3, 0:units] = kern[...]
        CV[w, 3:4, 0:units] = off[...].reshape(1, units)
    y_end(XG, ky[0], sy[0], 0)
    y_end(XG, ky[1], sy[1], 1)
    y_last(XG, ky[0])
    y_last(XG, ky[1])
    scaled(XG, mgain, False, 0, 4)
    z_fin(0)
    z_fin(1)
    for w, W in ((0, WGP), (1, WVP)):
        prod = jnp.dot(XS[...], W[...].reshape(1024, 256), preferred_element_type=F32)
        P1[:, :, w * 256 : w * 256 + 256] = prod.reshape(4, 128, 256)

    def row_loop(first, n, fn):
        def step(i, _):
            fn(pl.ds(pl.multiple_of(first + i * 16, 16), 16))
            return 0

        lax.fori_loop(0, n // 16, step, 0)

    ra, rb = pl.ds(0, 64), pl.ds(64, 64)

    def rounded_rows(p, i, S, k, first, n):
        def fn(rows):
            S[k, rows, :] = p[i, rows, :].astype(BF16)

        row_loop(first, n, fn)

    def rs_far(p, S, H, F, k, s):
        rounded_rows(p, 2, S, 0, 0, 128)
        send(S.at[0, ra], H.at[0], s, k, x_up)
        send(S.at[0, rb], H.at[1], s, k + 1, x_dn)

    def rs_first(p, S, H, F, k, s):
        rounded_rows(p, 0, S, 1, 64, 64)
        send(S.at[1, rb], F.at[0, rb], s, k + 2, x_up)
        rounded_rows(p, 1, S, 2, 0, 64)
        send(S.at[2, ra], F.at[1, ra], s, k + 2, x_dn)

    def rs_second(p, S, H, F, k, s):
        def left(rows):
            S[1, rows, :] = (p[0, rows, :] + H[0, rows, :].astype(F32)).astype(BF16)

        def right(rows):
            low = pl.ds(pl.multiple_of(rows.start + 64, 16), 16)
            S[2, low, :] = (p[1, low, :] + H[1, rows, :].astype(F32)).astype(BF16)

        recv(H.at[0], k)
        row_loop(0, 64, left)
        send(S.at[1, ra], F.at[0, ra], s, k + 2, x_up)
        recv(H.at[1], k + 1)
        row_loop(0, 64, right)
        send(S.at[2, rb], F.at[1, rb], s, k + 2, x_dn)

    def rs_wait(F, k):
        recv(F, k + 2)

    kr = [new(recvs, 3) for _ in layout]
    set1 = (P1, S1, H1, F1, kr[0], sender(S1))
    rs_far(*set1)
    rs_first(*set1)
    z_fwd(2)
    z_own(4)
    rs_second(*set1)
    z_fwd(3)
    z_own(5)
    recv(SM.at[pl.ds(0, 15)], km)
    recv(SSB.at[pl.ds(0, 7)], kss)
    rs_wait(F1, kr[0])

    total = P1[3] + F1[0].astype(F32) + F1[1].astype(F32)
    rs = scale_of(jnp.sum(SSB[...], axis=0)[0:1, :])
    eye = lax.broadcasted_iota(jnp.int32, (128, 128), 0) == lanes_of(128)
    for h in range(2):
        cols = slice(h * 128, h * 128 + 128)
        gated = gelu((rs * total[:, cols]).astype(BF16).astype(F32))
        spread = gelu((rs * total[:, 256 + h * 128 : 384 + h * 128]).astype(BF16).astype(F32))
        spread = spread * lax.rsqrt(jnp.mean(spread * spread, axis=-1, keepdims=True) + EPS)
        spread = (spread * vgain[h : h + 1, :]).astype(BF16)
        matrix = SM[:, h].astype(F32).reshape(128, 128).astype(BF16)
        mixed = jnp.dot(matrix, spread, preferred_element_type=F32)
        bias = jnp.broadcast_to(sbias[h : h + 1, :], (128, 128))
        mixed = mixed + jnp.sum(jnp.where(eye, bias, 0.0), axis=-1, keepdims=True)
        joined = gated * mixed
        joined = joined * lax.rsqrt(jnp.mean(joined * joined, axis=-1, keepdims=True) + EPS)
        MG[3, :, cols] = (joined * hgain[h : h + 1, :]).astype(BF16)

    k2 = new(recvs, 3)
    s2 = sender(MG.at[pl.ds(0, 3)])
    send(MG.at[3], MG.at[1], s2, k2 + 1, x_up)
    send(MG.at[3], MG.at[0], s2, k2 + 2, x_dn)
    send(MG.at[3], MG.at[2], s2, k2, x_far)
    z_fin(2)

    y_order = (far(y), up(y), down(y), y)

    def cy_first(g, product, CS, CR, k, s):
        for n, yt in enumerate(y_order):
            prod = product(yt)
            size = prod.shape[0] // 128
            rows = pl.ds(2 * g, size)
            T[n, rows] = jnp.where(c == 0, prod[:, :128], prod[:, 128:]).reshape(size, 128, 128)
            give = jnp.where(c == 0, prod[:, 128:], prod[:, :128]).astype(BF16)
            CS[n, rows] = give.reshape(size, 128, 128)
            send(CS.at[n, rows], CR.at[n, rows], s, k + n, mate)

    def joined_at(n, b, CR):
        return T[n, b] + CR[n, b].astype(F32)

    def cy_second(g, CR, YS, YH, YF, k, kc, s):
        a, b = 2 * g, 2 * g + 1
        recv(CR.at[0, pl.ds(a, 2)], kc)
        YS[0, a] = joined_at(0, a, CR).astype(BF16)
        YS[0, b] = joined_at(0, b, CR).astype(BF16)
        send(YS.at[0, a], YH.at[a], s, k, y_up)
        send(YS.at[0, b], YH.at[b], s, k + 1, y_dn)
        recv(CR.at[1, pl.ds(a, 2)], kc + 1)
        YS[1, b] = joined_at(1, b, CR).astype(BF16)
        send(YS.at[1, b], YF.at[g, 0, 1], s, k + 2, y_up)
        recv(CR.at[2, pl.ds(a, 2)], kc + 2)
        YS[2, a] = joined_at(2, a, CR).astype(BF16)
        send(YS.at[2, a], YF.at[g, 1, 0], s, k + 2, y_dn)

    def cy_third(g, CR, YS, YH, YF, k, kc, s):
        a, b = 2 * g, 2 * g + 1
        recv(YH.at[a], k)
        YS[1, a] = (joined_at(1, a, CR) + YH[a].astype(F32)).astype(BF16)
        send(YS.at[1, a], YF.at[g, 0, 0], s, k + 2, y_up)
        recv(YH.at[b], k + 1)
        YS[2, b] = (joined_at(2, b, CR) + YH[b].astype(F32)).astype(BF16)
        send(YS.at[2, b], YF.at[g, 1, 1], s, k + 2, y_dn)
        recv(CR.at[3, pl.ds(a, 2)], kc + 3)

    def cy_last(g, CR, YF, k):
        recv(YF.at[g], k + 2)
        return [
            joined_at(3, 2 * g + i, CR) + YF[g, 0, i].astype(F32) + YF[g, 1, i].astype(F32)
            for i in range(2)
        ]

    def merge(g):
        rows = MG[2 * g : 2 * g + 2].reshape(256, 256)
        return lambda yt: jnp.dot(rows, WMP[yt], preferred_element_type=F32)

    kc = [new(recvs, 4) for _ in range(2)]
    k3 = [new(recvs, 3) for _ in range(2)]
    sc, s3 = sender(CS4), sender(YS4)
    recv(MG.at[0], k2 + 2)
    recv(MG.at[1], k2 + 1)
    cy_first(0, merge(0), CS4, CR4, kc[0], sc)
    cy_second(0, CR4, YS4, YH4, YF4, k3[0], kc[0], s3)
    recv(MG.at[2], k2)
    z_own(10)
    z_fwd(9)
    z_fwd(11)
    cy_first(1, merge(1), CS4, CR4, kc[1], sc)
    cy_second(1, CR4, YS4, YH4, YF4, k3[1], kc[1], s3)
    z_fwd(4)
    z_own(6)
    cy_third(0, CR4, YS4, YH4, YF4, k3[0], kc[0], s3)
    cy_third(1, CR4, YS4, YH4, YF4, k3[1], kc[1], s3)

    z_fwd(10)

    ko = new(recvs)
    so = new(sends)
    ends.append(lambda: fewer(lambda n: HG.at[0, pl.ds(0, n)], 4, stay(so)))
    spot = 2 * lax.rem(x, 2) + c
    blocks = (up(x), down(x), far(x), x)
    sh = [sender(buf.at[pl.ds(0, 7), pl.ds(0, 2)]) for buf in (HG, HG)]
    for g in range(2):
        branch = cy_last(g, CR4, YF4, k3[g])
        for i in range(2):
            b = 2 * g + i
            HG[me, b] = (XG[me, b].astype(F32) + branch[i]).astype(BF16)
        y_start(HG, ky[g], sh[g], g)
    for b in range(4):
        if b < 3:
            dst = HRES.at[spot]
            send(HG.at[me, b], dst, so, ko, at(x_=blocks[b], c_=x // 2))
            continue

        @pl.when(to_me)
        def _():
            HRES[spot] = HG[me, 3]

        @pl.when(jnp.logical_not(to_me))
        def _():
            send(HG.at[me, 3], HRES.at[spot], so, ko, mate)

    z_fwd(5)
    y_mid(HG, ky[0], sh[0], 0)
    y_mid(HG, ky[1], sh[1], 1)
    y_end(HG, ky[0], sh[0], 0)
    z_fwd(6)
    z_own(7)
    z_own(8)
    y_end(HG, ky[1], sh[1], 1)
    z_fin(weight("g", 0))
    z_fin(weight("v", 0))
    y_last(HG, ky[0])
    scaled(HG, fgain, True, 0, 2)

    def project(W, p, n, first, b0, b1):
        def cut(cols, to, size):
            w = jnp.concatenate([W[k, cols, :] for k in range(4)], axis=1)
            prod = lax.dot_general(
                XS[b0 * 128 : b1 * 128, :], w, (((1,), (1,)), ((), ())),
                preferred_element_type=F32,
            )
            p[b0:b1, :, to] = prod.reshape(b1 - b0, 128, size)

        def step(i, _):
            cut(
                pl.ds(pl.multiple_of(i * 256, 256), 256),
                pl.ds(pl.multiple_of(first + i * 256, 128), 256), 256,
            )
            return 0

        lax.fori_loop(0, n // 256, step, 0)
        left = n % 256
        if left:
            cut(pl.ds(n - left, left), pl.ds(first + n - left, left), left)

    def both(j, b0=0, b1=4):
        n = layout[j][2]
        project(WGU[j], PC[j], n, 0, b0, b1)
        project(WVU[j], PC[j], n, n, b0, b1)

    row = lax.broadcasted_iota(jnp.int32, (128, 128), 0)

    def activate(j):
        p, F, act = PC[j], FC[j], ACT[j]
        at0, _, n = layout[j]

        def conv_tile(i, _):
            def one(first, w):
                at_ = pl.ds(pl.multiple_of(first + i * 128, 128), 128)
                v = p[3, :, at_] + F[0, :, at_].astype(F32) + F[1, :, at_].astype(F32)
                v = (RS[...] * v).astype(BF16).astype(F32)
                prev = jnp.where(row == 0, 0.0, pltpu.roll(v, 1, axis=0))
                after = jnp.where(row == 127, 0.0, pltpu.roll(v, 127, axis=0))
                k = CV[w, :, pl.ds(pl.multiple_of(at0 + i * 128, 128), 128)]
                return k[3:4] + prev * k[0:1] + v * k[1:2] + after * k[2:3]

            cols = pl.ds(pl.multiple_of(i * 128, 128), 128)
            act[3, :, cols] = (gelu(one(0, 0)) * one(n, 1)).astype(BF16)
            return 0

        lax.fori_loop(0, n // 128, conv_tile, 0)

    sets = [
        (PC[j], SC[j], HC[j], FC[j], kr[j], sender(SC[j])) for j in range(chunks)
    ]
    kg = [new(recvs, 4) for _ in layout]
    sg = [sender(ACT[j].at[pl.ds(0, 3)]) for j in range(chunks)]

    def x_start(j):
        buf, k, s = ACT[j], kg[j], sg[j]
        send(buf.at[3, ra], buf.at[1, ra], s, k, z_up)
        send(buf.at[3, rb], buf.at[0, rb], s, k + 1, z_dn)
        send(buf.at[3, rb], buf.at[1, rb], s, k + 2, z_up)
        send(buf.at[3, ra], buf.at[0, ra], s, k + 2, z_dn)

    def x_mid(j):
        buf, k, s = ACT[j], kg[j], sg[j]
        recv(buf.at[1, ra], k)
        send(buf.at[1, ra], buf.at[2, ra], s, k + 3, z_up)
        recv(buf.at[0, rb], k + 1)
        send(buf.at[0, rb], buf.at[2, rb], s, k + 3, z_dn)

    def x_near(j):
        recv(ACT[j].at[0], kg[j] + 2)

    def x_last(j):
        recv(ACT[j].at[2], kg[j] + 3)

    def down_rows(j, b0, b1):
        n = layout[j][2]
        rows = ACT[j][b0:b1].reshape((b1 - b0) * 128, n)
        return lambda k: jnp.dot(rows, WDN[j][k], preferred_element_type=F32)

    def down_early(j):
        product = down_rows(j, 0, 4)

        def step(k, _):
            prod = product(k).reshape(4, 128, 256)
            ACC[k] = prod if j == 0 else ACC[k] + prod
            return 0

        lax.fori_loop(0, 4, step, 0)

    both(0, 0, 2)
    rs_first(*sets[0])
    y_last(HG, ky[1])
    scaled(HG, fgain, True, 2, 2)
    both(0, 2, 4)
    rs_far(*sets[0])
    kf = new(recvs)
    sf = sender(SSF.at[pl.ds(0, 3)])
    SSF[3] = SQR[3]
    send(SQR.at[0], SSF.at[1], sf, kf, x_up)
    send(SQR.at[1], SSF.at[0], sf, kf, x_dn)
    send(SQR.at[2], SSF.at[2], sf, kf, x_far)
    z_fin(weight("g", 1))
    z_fin(weight("v", 1))
    both(1)
    rs_second(*sets[0])
    rs_far(*sets[1])
    rs_first(*sets[1])
    z_fwd(7)
    z_fwd(8)
    rs_second(*sets[1])
    recv(SSF.at[pl.ds(0, 3)], kf)
    RS[...] = scale_of(jnp.sum(SSF[...], axis=0)[0:1, :])
    rs_wait(FC[0], kr[0])
    activate(0)
    x_start(0)
    z_fin(weight("g", 2))
    z_fin(weight("v", 2))
    both(2)
    rs_far(*sets[2])
    rs_first(*sets[2])
    rs_wait(FC[1], kr[1])
    activate(1)
    x_start(1)
    x_mid(0)
    rs_second(*sets[2])
    x_mid(1)
    x_near(0)
    x_last(0)
    z_fin(9)
    down_early(0)
    rs_wait(FC[2], kr[2])
    activate(2)
    x_start(2)
    x_near(1)
    x_last(1)
    z_fin(10)
    z_fin(11)
    down_early(1)
    x_mid(2)
    x_near(2)

    k7 = [new(recvs, 2) for _ in range(2)]
    s7 = sender(CS5)
    kt = new(recvs)
    st = new(sends)
    stays = y == z
    ends.append(lambda: fewer(lambda n: TB.at[pl.ds(0, n)], 4, stay(st), stays))

    def give(b):
        for i in range(2):
            TB[b, :, i * 256 : i * 256 + 256] = (T5[i, b] + CR5[i, b].astype(F32)).astype(BF16)
        if b < 2:
            send(TB.at[b], TI.at[y], st, kt, along(1 - 2 * b, z))
        elif b == 2:
            send(TB.at[b, ra], TI.at[y, ra], st, kt, along(-2, z))
            send(TB.at[b, rb], TI.at[y, rb], st, kt, along(2, z))
        else:

            @pl.when(stays)
            def _():
                TI[y] = TB[b]

            @pl.when(jnp.logical_not(stays))
            def _():
                send(TB.at[b], TI.at[y], st, kt, at(y_=z))

    for g in range(2):
        if g:
            x_last(2)
        rows = pl.ds(2 * g, 2)
        product = down_rows(2, 2 * g, 2 * g + 2)

        def final(k):
            return product(k).reshape(2, 128, 256) + ACC[k, rows]

        for i in range(2):
            CS5[i, rows] = final(2 * other + i).astype(BF16)
            send(CS5.at[i, rows], CR5.at[i, rows], s7, k7[g] + i, mate)
        for i in range(2):
            T5[i, rows] = final(2 * c + i)
        for i in range(2):
            recv(CR5.at[i, rows], k7[g] + i)
        give(2 * g)
        give(2 * g + 1)

    fewer(lambda n: HRES.at[pl.ds(0, n)], 4, lambda ref: recv(ref, ko))
    fewer(lambda n: TI.at[pl.ds(0, n)], 4, lambda ref: recv(ref, kt), stays)
    for q in range(4):
        cols = slice(q * 128, q * 128 + 128)
        change = sum(TI[n, :, cols].astype(F32) for n in range(4))
        out[:, cols] = (HRES[q].astype(F32) + change).astype(BF16)
    for wait in ends:
        wait()
    assert sends[0] <= ssem.shape[0] and recvs[0] <= rsem.shape[0], (sends[0], recvs[0])


def body(
    tokens, mixer_gain, gate_proj, value_proj, value_gain, spatial_mix, spatial_bias,
    head_gain, merge_proj, ffn_gain, gate_up, value_up, gate_kernel, value_kernel,
    gate_offset, value_offset, down_proj,
):
    units = gate_up.shape[1]
    layout = []
    for first in range(0, units, CHUNK):
        n = min(CHUNK, units - first)
        layout.append((first, n, -(-n // 128) * 128))
    wide = sum(n for _, _, n in layout)
    widths = [n for _, _, n in layout]
    vm = lambda shape, dtype=BF16: pltpu.VMEM(shape, dtype)
    in_vmem = pl.BlockSpec(memory_space=pltpu.VMEM)
    left = pl.BlockSpec(memory_space=pl.ANY)
    call = pl.pallas_call(
        functools.partial(kernel, layout),
        out_shape=jax.ShapeDtypeStruct(tokens.shape, tokens.dtype),
        in_specs=[
            left, in_vmem, in_vmem, left, left, in_vmem, in_vmem, in_vmem, in_vmem, left,
            left, left, left, left, in_vmem, in_vmem, left,
        ],
        out_specs=in_vmem,
        scratch_shapes=[
            vm(tokens.shape), vm(gate_kernel.shape, F32), vm(gate_kernel.shape, F32),
            vm((2, 4, wide), F32),
            vm((8, 4, 128, 128)), vm((8, 4, 128, 128)), vm((512, 1024)),
            vm((4, 8, 128), F32), vm((128, 128), F32), vm((16, 2, 8, 128)),
            vm((4, 128, 256)), vm((8, 8, 128), F32), vm((4, 8, 128), F32), vm((4, 128, 128)),
            vm((4, 128, 512)), vm((4, 128, 512)),
            *[vm((4, 256, 256))] * 3, vm((4, 4, 128, 128), F32), vm((4, 4, 128, 256), F32),
            vm((4, 128, 512), F32), vm((3, 128, 512)), vm((2, 64, 512)), vm((2, 128, 512)),
            vm((4, 4, 128, 128)), vm((4, 4, 128, 128)), vm((3, 4, 128, 128)),
            vm((4, 128, 128)), vm((2, 2, 2, 128, 128)),
            vm((2, 4, 128, 256)), vm((2, 4, 128, 256)), vm((2, 4, 128, 256), F32),
            *[vm((4, n, 256)) for _ in range(3) for n in widths],
            *[vm((4, 128, n)) for n in widths],
            *[vm((4, 128, 2 * n), F32) for n in widths],
            *[vm((3, 128, 2 * n)) for n in widths],
            *[vm((2, 64, 2 * n)) for n in widths],
            *[vm((2, 128, 2 * n)) for n in widths],
            pltpu.SemaphoreType.DMA((SENDS,)), pltpu.SemaphoreType.DMA((RECVS,)),
            pltpu.SemaphoreType.DMA((6 + 3 * len(layout),)),
        ],
        compiler_params=pltpu.CompilerParams(
            collective_id=0, has_side_effects=True, vmem_limit_bytes=58 << 20
        ),
        name="layer",
    )
    return call(
        tokens, mixer_gain, ffn_gain, gate_proj, value_proj, value_gain, spatial_mix,
        spatial_bias, head_gain, merge_proj, gate_up.T, value_up.T, gate_kernel, value_kernel,
        gate_offset, value_offset, down_proj,
    )


def solution(mesh):
    finer = Mesh(
        mesh.devices.reshape(mesh.shape["rep"], 4, 4, 4, 2), ("rep", "fs_0", "fs_1", "tp_0", "tp_1")
    )
    return jax.shard_map(
        body,
        mesh=finer,
        in_specs=(
            P(REP_FS, TP), P(), P(FS, TP), P(FS, TP), P(TP, None), P(TP, FS, None),
            P(TP, None), P(TP, None), P(TP, FS), P(), P(FS, TP), P(FS, TP), P(None, TP),
            P(None, TP), P(TP), P(TP), P(TP, FS),
        ),
        out_specs=P(REP_FS, TP),
        check_vma=False,
    )
```

```python
import functools

import jax
import jax.numpy as jnp
from jax import lax
from jax.experimental import pallas as pl
from jax.experimental.pallas import tpu as pltpu
from jax.sharding import Mesh
from jax.sharding import PartitionSpec as P

TP = ("tp_0", "tp_1")
FS = ("fs_0", "fs_1")
REP_FS = ("rep", "fs_0", "fs_1")
MESH = pl.DeviceIdType.MESH
EPS = 1e-06
SENDS, RECVS = 33, 103
CHUNK = 512
F32 = jnp.float32
BF16 = jnp.bfloat16


def gelu(v):
    return 0.5 * v * (1.0 + lax.erf(v * 0.7071067811865476))


def lanes_of(n):
    return lax.broadcasted_iota(jnp.int32, (n, 128), 1)


def kernel(layout, tok, mgain, fgain, gp, vp, vgain, smix, sbias, hgain, mp, gu, vu, gk, vk, go, vo,
           dn, out, tokv, gkv, vkv, CV, XG, HG, XS, SQR, RS, SM, MG, SSB, SSF, HRES, TB, TI,
           WGP, WVP, WMP, T, ACC, P1, S1, H1, F1, CS4, CR4, YS4, YH4, YF4, CS5, CR5, T5, *rest):
    chunks = len(layout)
    WGU, WVU, WDN, ACT, PC, SC, HC, FC = (rest[i * chunks : (i + 1) * chunks] for i in range(8))
    ssem, rsem, lsem = rest[8 * chunks :]
    r, z, x, y, c = (lax.axis_index(a) for a in ("rep", "fs_0", "fs_1", "tp_0", "tp_1"))
    other = 1 - c
    f = 4 * z + x
    units = dn.shape[0]
    depth = mgain.shape[0]

    def at(z_=None, x_=None, y_=None, c_=None, r_=None):
        pick = lambda new, old: old if new is None else new
        return (pick(r_, r), pick(z_, z), pick(x_, x), pick(y_, y), pick(c_, c))

    up = lambda v: lax.rem(v + 1, 4)
    down = lambda v: lax.rem(v + 3, 4)
    far = lambda v: lax.rem(v + 2, 4)

    zr = 4 * r + z
    zu, zd = lax.rem(zr + 1, 8), lax.rem(zr + 7, 8)
    z_up = at(r_=zu // 4, z_=lax.rem(zu, 4))
    z_dn = at(r_=zd // 4, z_=lax.rem(zd, 4))
    x_up, x_dn, x_far = at(x_=up(x)), at(x_=down(x)), at(x_=far(x))
    y_up, y_dn = at(y_=up(y)), at(y_=down(y))
    mate = at(c_=other)
    fs_peers = []
    for i in range(1, 16):
        g = lax.rem(f + i, 16)
        fs_peers.append(at(z_=g // 4, x_=lax.rem(g, 4)))
    near = []
    for i in range(1, 4):
        near += [at(x_=lax.rem(x + i, 4), c_=k) for k in (c, other)]
        near += [at(y_=lax.rem(y + i, 4), c_=other)]

    def along(d, y_=None):
        there = lax.rem(zr + 8 + d, 8)
        return at(r_=there // 4, z_=lax.rem(there, 4), y_=y_)

    for i in range(4):
        for d in (-2, -1, 0, 1, 2):
            if i or d:
                near.append(along(d, lax.rem(y + i, 4)))

    barrier = pltpu.get_barrier_semaphore()
    greet = [mate] + near + fs_peers
    for peer in greet:
        pl.semaphore_signal(barrier, inc=1, device_id=peer, device_id_type=MESH)
    loads = [
        pltpu.make_async_copy(src, dst, lsem.at[i])
        for i, (src, dst) in enumerate(((tok, tokv), (gk, gkv), (vk, vkv)))
    ]
    for copy in loads:
        copy.start()
    pl.semaphore_wait(barrier, len(greet))

    sends, recvs, ends = [0], [0], []

    def new(counter, n=1):
        counter[0] += n
        return counter[0] - n

    def remote(src, dst, s, k, peer):
        return pltpu.make_async_remote_copy(
            src_ref=src, dst_ref=dst, send_sem=ssem.at[s], recv_sem=rsem.at[k],
            device_id=peer, device_id_type=MESH,
        )

    def send(src, dst, s, k, peer):
        remote(src, dst, s, k, peer).start()

    def recv(dst, k):
        remote(dst, dst, 0, k, mate).wait_recv()

    def sender(ref):
        s = new(sends)
        ends.append(lambda: remote(ref, ref, s, 0, mate).wait_send())
        return s

    pieces = [(gp, WGP, 0, 256), (vp, WVP, 0, 256), (mp, WMP, 0, 256)]
    for (at0, n, _), G, V in zip(layout, WGU, WVU):
        pieces += [(gu, G, at0, n), (vu, V, at0, n)]
    for (at0, n, _), W in zip(layout, WDN):
        pieces.append((dn, W, at0, n))
    zk = [new(recvs, 3) for _ in pieces]
    zs = [sender(buf.at[pl.ds(0, 3), pl.ds(0, n)]) for _, buf, _, n in pieces]

    def z_local(i):
        src, buf, at0, n = pieces[i]
        own = buf.at[ring(i)[0], pl.ds(0, n)]
        return pltpu.make_async_copy(src.at[pl.ds(at0, n)], own, lsem.at[3 + i])

    def ring(i):
        return (x, x_up, x_dn) if pieces[i][0] is dn else (z, z_up, z_dn)

    def z_own(i):
        src, buf, at0, n = pieces[i]
        a, b = pl.ds(0, n // 2), pl.ds(n // 2, n // 2)
        from_a, from_b = src.at[pl.ds(at0, n // 2)], src.at[pl.ds(at0 + n // 2, n // 2)]
        place, above, below = ring(i)
        send(from_a, buf.at[place, a], zs[i], zk[i], above)
        send(from_b, buf.at[place, b], zs[i], zk[i] + 1, below)
        send(from_b, buf.at[place, b], zs[i], zk[i] + 2, above)
        send(from_a, buf.at[place, a], zs[i], zk[i] + 2, below)
        z_local(i).start()

    def z_fwd(i):
        _, buf, _, n = pieces[i]
        place, above, below = ring(i)
        a, b = buf.at[down(place), pl.ds(0, n // 2)], buf.at[up(place), pl.ds(n // 2, n // 2)]
        recv(a, zk[i])
        send(a, a, zs[i], zk[i] + 2, above)
        recv(b, zk[i] + 1)
        send(b, b, zs[i], zk[i] + 2, below)

    def z_fin(i):
        _, buf, _, n = pieces[i]
        recv(buf.at[pl.ds(0, 2), pl.ds(0, n)], zk[i] + 2)
        z_local(i).wait()

    def weight(kind, j):
        return {"g": 3 + 2 * j, "v": 4 + 2 * j, "d": 3 + 2 * chunks + j}[kind]

    me = 2 * y + c
    to_me = x // 2 == c
    loads[0].wait()
    kx = new(recvs, 2)
    sx = new(sends)
    for j in range(2):
        for h in range(2):
            xt = 2 * c + j
            ahead = lax.rem(x - xt + 4, 4)
            place = jnp.where(ahead == 0, 2, jnp.where(ahead == 2, 3, ahead // 2))
            mine = jnp.logical_and(xt == x, c == h)
            block = tokv.at[:, j * 256 + h * 128 : j * 256 + h * 128 + 128]

            @pl.when(jnp.logical_not(mine))
            def _():
                dst = XG.at[2 * y + h, place]
                send(block, dst, sx, kx + place // 2, at(x_=xt, c_=jnp.int32(h)))

            @pl.when(mine)
            def _():
                XG[2 * y + h, 2] = block[...]

    def fewer(ref_of, n, wait, stays=to_me):
        @pl.when(stays)
        def _():
            wait(ref_of(n - 1))

        @pl.when(jnp.logical_not(stays))
        def _():
            wait(ref_of(n))

    stay = lambda s: lambda ref: remote(ref, ref, s, 0, mate).wait_send()
    ends.append(lambda: fewer(lambda n: XG.at[0, pl.ds(0, n)], 4, stay(sx)))
    z_own(0)
    z_own(1)
    square = tokv[...].astype(F32)
    square = jnp.sum(square * square, axis=-1, keepdims=True)
    SSB[me] = jnp.broadcast_to(square, (128, 128)).T[0:8, :]
    kss = new(recvs)
    sss = sender(SSB.at[pl.ds(0, 7)])
    for i in range(1, 8):
        t = lax.rem(me + i, 8)
        send(SSB.at[me], SSB.at[me], sss, kss, at(y_=t // 2, c_=lax.rem(t, 2)))

    lo_y, hi_y, far_y = 2 * down(y) + c, 2 * up(y) + c, 2 * far(y) + c

    def y_start(buf, k, s, g):
        a, b = buf.at[me, 2 * g], buf.at[me, 2 * g + 1]
        send(a, a, s, k, y_up)
        send(b, b, s, k + 1, y_dn)
        send(b, b, s, k + 2, y_up)
        send(a, a, s, k + 3, y_dn)
        both = buf.at[me, pl.ds(2 * g, 2)]
        send(both, both, s, k + 6, mate)

    def y_mid(buf, k, s, g):
        a, b = buf.at[lo_y, 2 * g], buf.at[hi_y, 2 * g + 1]
        recv(a, k)
        send(a, a, s, k + 4, y_up)
        send(a, a, s, k + 6, mate)
        recv(b, k + 1)
        send(b, b, s, k + 5, y_dn)
        send(b, b, s, k + 6, mate)

    def y_end(buf, k, s, g):
        rows = (buf.at[lo_y, 2 * g + 1], buf.at[hi_y, 2 * g], buf.at[far_y, 2 * g], buf.at[far_y, 2 * g + 1])
        for i, ref in enumerate(rows):
            recv(ref, k + 2 + i)
            send(ref, ref, s, k + 6, mate)

    def y_last(buf, k):
        recv(buf.at[pl.ds(0, 4), pl.ds(0, 2)], k + 6)

    def scaled(buf, gains, squares, first, n):
        parts = [gains[pl.ds(pl.multiple_of((4 * k + x) * 256, 256), 256)] for k in range(4)]
        gain = jnp.concatenate([part.reshape(1, 256) for part in parts], axis=1)

        def block(b, _):
            rows = jnp.concatenate([buf[i, b] for i in range(8)], axis=1).astype(F32)
            if squares:
                total = jnp.sum(rows * rows, axis=-1, keepdims=True)
                SQR[b] = jnp.broadcast_to(total, (128, 128)).T[0:8, :]
            XS[pl.ds(pl.multiple_of(b * 128, 128), 128), :] = (rows * gain).astype(BF16)
            return 0

        lax.fori_loop(first, first + n, block, 0)

    def scale_of(rows):
        return lax.rsqrt(jnp.broadcast_to(rows, (128, 128)).T / depth + EPS)

    ky = [new(recvs, 7) for _ in range(2)]
    sy = [sender(buf.at[pl.ds(0, 7), pl.ds(0, 2)]) for buf in (XG, XG)]
    recv(XG.at[me, pl.ds(0, 2)], kx)
    y_start(XG, ky[0], sy[0], 0)
    fewer(lambda n: XG.at[me, pl.ds(0, n)], 2, lambda ref: recv(ref, kx + 1))
    y_start(XG, ky[1], sy[1], 1)
    km = new(recvs)
    sm = sender(SM.at[pl.ds(0, 15)])
    for i in range(15):
        send(smix, SM.at[f], sm, km, fs_peers[i])
    SM[f] = smix[...]
    last0, lastn, wide = layout[-1]
    for W in (WGU[-1], WVU[-1], WDN[-1]):
        for k in range(4):
            W[k, lastn:, :] = jnp.zeros((wide - lastn, 256), BF16)
    z_own(9)
    z_own(11)
    z_fwd(0)
    z_fwd(1)
    z_own(2)
    z_own(3)
    y_mid(XG, ky[0], sy[0], 0)
    y_mid(XG, ky[1], sy[1], 1)
    loads[1].wait()
    loads[2].wait()
    for w, kern, off in ((0, gkv, go), (1, vkv, vo)):
        CV[w, :, last0:] = jnp.zeros((4, wide), F32)
        CV[w, 0:3, 0:units] = kern[...]
        CV[w, 3:4, 0:units] = off[...].reshape(1, units)
    y_end(XG, ky[0], sy[0], 0)
    y_end(XG, ky[1], sy[1], 1)
    y_last(XG, ky[0])
    y_last(XG, ky[1])
    scaled(XG, mgain, False, 0, 4)
    z_fin(0)
    z_fin(1)
    for w, W in ((0, WGP), (1, WVP)):
        prod = jnp.dot(XS[...], W[...].reshape(1024, 256), preferred_element_type=F32)
        P1[:, :, w * 256 : w * 256 + 256] = prod.reshape(4, 128, 256)

    def row_loop(first, n, fn):
        def step(i, _):
            fn(pl.ds(pl.multiple_of(first + i * 16, 16), 16))
            return 0

        lax.fori_loop(0, n // 16, step, 0)

    ra, rb = pl.ds(0, 64), pl.ds(64, 64)

    def rounded_rows(p, i, S, k, first, n):
        def fn(rows):
            S[k, rows, :] = p[i, rows, :].astype(BF16)

        row_loop(first, n, fn)

    def rs_far(p, S, H, F, k, s):
        rounded_rows(p, 3, S, 0, 0, 128)
        send(S.at[0, ra], H.at[0], s, k, x_up)
        send(S.at[0, rb], H.at[1], s, k + 1, x_dn)

    def rs_first(p, S, H, F, k, s):
        rounded_rows(p, 0, S, 1, 64, 64)
        send(S.at[1, rb], F.at[0, rb], s, k + 2, x_up)
        rounded_rows(p, 1, S, 2, 0, 64)
        send(S.at[2, ra], F.at[1, ra], s, k + 2, x_dn)

    def rs_second(p, S, H, F, k, s):
        def left(rows):
            S[1, rows, :] = (p[0, rows, :] + H[0, rows, :].astype(F32)).astype(BF16)

        def right(rows):
            low = pl.ds(pl.multiple_of(rows.start + 64, 16), 16)
            S[2, low, :] = (p[1, low, :] + H[1, rows, :].astype(F32)).astype(BF16)

        recv(H.at[0], k)
        row_loop(0, 64, left)
        send(S.at[1, ra], F.at[0, ra], s, k + 2, x_up)
        recv(H.at[1], k + 1)
        row_loop(0, 64, right)
        send(S.at[2, rb], F.at[1, rb], s, k + 2, x_dn)

    def rs_wait(F, k):
        recv(F, k + 2)

    kr = [new(recvs, 3) for _ in layout]
    set1 = (P1, S1, H1, F1, kr[0], sender(S1))
    rs_far(*set1)
    rs_first(*set1)
    z_fwd(2)
    z_own(4)
    rs_second(*set1)
    z_fwd(3)
    z_own(5)
    recv(SM.at[pl.ds(0, 15)], km)
    recv(SSB.at[pl.ds(0, 7)], kss)
    rs_wait(F1, kr[0])

    total = P1[2] + F1[0].astype(F32) + F1[1].astype(F32)
    rs = scale_of(jnp.sum(SSB[...], axis=0)[0:1, :])
    eye = lax.broadcasted_iota(jnp.int32, (128, 128), 0) == lanes_of(128)
    for h in range(2):
        cols = slice(h * 128, h * 128 + 128)
        gated = gelu((rs * total[:, cols]).astype(BF16).astype(F32))
        spread = gelu((rs * total[:, 256 + h * 128 : 384 + h * 128]).astype(BF16).astype(F32))
        spread = spread * lax.rsqrt(jnp.mean(spread * spread, axis=-1, keepdims=True) + EPS)
        spread = (spread * vgain[h : h + 1, :]).astype(BF16)
        matrix = SM[:, h].astype(F32).reshape(128, 128).astype(BF16)
        mixed = jnp.dot(matrix, spread, preferred_element_type=F32)
        bias = jnp.broadcast_to(sbias[h : h + 1, :], (128, 128))
        mixed = mixed + jnp.sum(jnp.where(eye, bias, 0.0), axis=-1, keepdims=True)
        joined = gated * mixed
        joined = joined * lax.rsqrt(jnp.mean(joined * joined, axis=-1, keepdims=True) + EPS)
        MG[2, :, cols] = (joined * hgain[h : h + 1, :]).astype(BF16)

    k2 = new(recvs, 3)
    s2 = sender(MG.at[pl.ds(0, 3)])
    send(MG.at[2], MG.at[1], s2, k2 + 1, x_up)
    send(MG.at[2], MG.at[0], s2, k2 + 2, x_dn)
    send(MG.at[2], MG.at[3], s2, k2, x_far)
    z_fin(2)

    y_order = (far(y), up(y), down(y), y)

    def cy_first(g, product, CS, CR, k, s):
        for n, yt in enumerate(y_order):
            prod = product(yt)
            size = prod.shape[0] // 128
            rows = pl.ds(2 * g, size)
            T[n, rows] = jnp.where(c == 0, prod[:, :128], prod[:, 128:]).reshape(size, 128, 128)
            give = jnp.where(c == 0, prod[:, 128:], prod[:, :128]).astype(BF16)
            CS[n, rows] = give.reshape(size, 128, 128)
            send(CS.at[n, rows], CR.at[n, rows], s, k + n, mate)

    def joined_at(n, b, CR):
        return T[n, b] + CR[n, b].astype(F32)

    def cy_second(g, CR, YS, YH, YF, k, kc, s):
        a, b = 2 * g, 2 * g + 1
        recv(CR.at[0, pl.ds(a, 2)], kc)
        YS[0, a] = joined_at(0, a, CR).astype(BF16)
        YS[0, b] = joined_at(0, b, CR).astype(BF16)
        send(YS.at[0, a], YH.at[a], s, k, y_up)
        send(YS.at[0, b], YH.at[b], s, k + 1, y_dn)
        recv(CR.at[1, pl.ds(a, 2)], kc + 1)
        YS[1, b] = joined_at(1, b, CR).astype(BF16)
        send(YS.at[1, b], YF.at[g, 0, 1], s, k + 2, y_up)
        recv(CR.at[2, pl.ds(a, 2)], kc + 2)
        YS[2, a] = joined_at(2, a, CR).astype(BF16)
        send(YS.at[2, a], YF.at[g, 1, 0], s, k + 2, y_dn)

    def cy_third(g, CR, YS, YH, YF, k, kc, s):
        a, b = 2 * g, 2 * g + 1
        recv(YH.at[a], k)
        YS[1, a] = (joined_at(1, a, CR) + YH[a].astype(F32)).astype(BF16)
        send(YS.at[1, a], YF.at[g, 0, 0], s, k + 2, y_up)
        recv(YH.at[b], k + 1)
        YS[2, b] = (joined_at(2, b, CR) + YH[b].astype(F32)).astype(BF16)
        send(YS.at[2, b], YF.at[g, 1, 1], s, k + 2, y_dn)
        recv(CR.at[3, pl.ds(a, 2)], kc + 3)

    def cy_last(g, CR, YF, k):
        recv(YF.at[g], k + 2)
        return [
            joined_at(3, 2 * g + i, CR) + YF[g, 0, i].astype(F32) + YF[g, 1, i].astype(F32)
            for i in range(2)
        ]

    def merge(g):
        rows = MG[2 * g : 2 * g + 2].reshape(256, 256)
        return lambda yt: jnp.dot(rows, WMP[yt], preferred_element_type=F32)

    kc = [new(recvs, 4) for _ in range(2)]
    k3 = [new(recvs, 3) for _ in range(2)]
    sc, s3 = sender(CS4), sender(YS4)
    recv(MG.at[0], k2 + 2)
    recv(MG.at[1], k2 + 1)
    cy_first(0, merge(0), CS4, CR4, kc[0], sc)
    cy_second(0, CR4, YS4, YH4, YF4, k3[0], kc[0], s3)
    recv(MG.at[3], k2)
    z_own(10)
    z_fwd(9)
    z_fwd(11)
    cy_first(1, merge(1), CS4, CR4, kc[1], sc)
    cy_second(1, CR4, YS4, YH4, YF4, k3[1], kc[1], s3)
    z_fwd(4)
    z_own(6)
    cy_third(0, CR4, YS4, YH4, YF4, k3[0], kc[0], s3)
    cy_third(1, CR4, YS4, YH4, YF4, k3[1], kc[1], s3)


    ko = new(recvs)
    so = new(sends)
    ends.append(lambda: fewer(lambda n: HG.at[0, pl.ds(0, n)], 4, stay(so)))
    spot = 2 * lax.rem(x, 2) + c
    blocks = (up(x), down(x), x, far(x))
    sh = [sender(buf.at[pl.ds(0, 7), pl.ds(0, 2)]) for buf in (HG, HG)]
    for g in range(2):
        branch = cy_last(g, CR4, YF4, k3[g])
        for i in range(2):
            b = 2 * g + i
            HG[me, b] = (XG[me, b].astype(F32) + branch[i]).astype(BF16)
        y_start(HG, ky[g], sh[g], g)
    for b in range(4):
        if b != 2:
            dst = HRES.at[spot]
            send(HG.at[me, b], dst, so, ko, at(x_=blocks[b], c_=x // 2))
            continue

        @pl.when(to_me)
        def _():
            HRES[spot] = HG[me, 2]

        @pl.when(jnp.logical_not(to_me))
        def _():
            send(HG.at[me, 2], HRES.at[spot], so, ko, mate)

    z_fwd(5)
    y_mid(HG, ky[0], sh[0], 0)
    y_mid(HG, ky[1], sh[1], 1)
    y_end(HG, ky[0], sh[0], 0)
    z_fwd(6)
    z_own(7)
    z_own(8)
    z_fwd(10)
    y_end(HG, ky[1], sh[1], 1)
    z_fin(weight("g", 0))
    z_fin(weight("v", 0))
    y_last(HG, ky[0])
    scaled(HG, fgain, True, 0, 2)

    def project(W, p, n, first, b0, b1):
        def cut(cols, to, size):
            w = jnp.concatenate([W[k, cols, :] for k in range(4)], axis=1)
            prod = lax.dot_general(
                XS[b0 * 128 : b1 * 128, :], w, (((1,), (1,)), ((), ())),
                preferred_element_type=F32,
            )
            p[b0:b1, :, to] = prod.reshape(b1 - b0, 128, size)

        def step(i, _):
            cut(
                pl.ds(pl.multiple_of(i * 256, 256), 256),
                pl.ds(pl.multiple_of(first + i * 256, 128), 256), 256,
            )
            return 0

        lax.fori_loop(0, n // 256, step, 0)
        left = n % 256
        if left:
            cut(pl.ds(n - left, left), pl.ds(first + n - left, left), left)

    def both(j, b0=0, b1=4):
        n = layout[j][2]
        project(WGU[j], PC[j], n, 0, b0, b1)
        project(WVU[j], PC[j], n, n, b0, b1)

    row = lax.broadcasted_iota(jnp.int32, (128, 128), 0)

    def activate(j):
        p, F, act = PC[j], FC[j], ACT[j]
        at0, _, n = layout[j]

        def conv_tile(i, _):
            def one(first, w):
                at_ = pl.ds(pl.multiple_of(first + i * 128, 128), 128)
                v = p[2, :, at_] + F[0, :, at_].astype(F32) + F[1, :, at_].astype(F32)
                v = (RS[...] * v).astype(BF16).astype(F32)
                prev = jnp.where(row == 0, 0.0, pltpu.roll(v, 1, axis=0))
                after = jnp.where(row == 127, 0.0, pltpu.roll(v, 127, axis=0))
                k = CV[w, :, pl.ds(pl.multiple_of(at0 + i * 128, 128), 128)]
                return k[3:4] + prev * k[0:1] + v * k[1:2] + after * k[2:3]

            cols = pl.ds(pl.multiple_of(i * 128, 128), 128)
            act[2, :, cols] = (gelu(one(0, 0)) * one(n, 1)).astype(BF16)
            return 0

        lax.fori_loop(0, n // 128, conv_tile, 0)

    sets = [
        (PC[j], SC[j], HC[j], FC[j], kr[j], sender(SC[j])) for j in range(chunks)
    ]
    kg = [new(recvs, 4) for _ in layout]
    sg = [sender(ACT[j].at[pl.ds(0, 3)]) for j in range(chunks)]

    def x_start(j):
        buf, k, s = ACT[j], kg[j], sg[j]
        send(buf.at[2, ra], buf.at[1, ra], s, k, z_up)
        send(buf.at[2, rb], buf.at[0, rb], s, k + 1, z_dn)
        send(buf.at[2, rb], buf.at[1, rb], s, k + 2, z_up)
        send(buf.at[2, ra], buf.at[0, ra], s, k + 2, z_dn)

    def x_mid(j):
        buf, k, s = ACT[j], kg[j], sg[j]
        recv(buf.at[1, ra], k)
        send(buf.at[1, ra], buf.at[3, ra], s, k + 3, z_up)
        recv(buf.at[0, rb], k + 1)
        send(buf.at[0, rb], buf.at[3, rb], s, k + 3, z_dn)

    def x_near(j):
        recv(ACT[j].at[0], kg[j] + 2)

    def x_last(j):
        recv(ACT[j].at[3], kg[j] + 3)

    def down_rows(j, b0, b1):
        n = layout[j][2]
        rows = ACT[j][b0:b1].reshape((b1 - b0) * 128, n)
        return lambda k: jnp.dot(rows, WDN[j][k], preferred_element_type=F32)

    def down_early(j):
        product = down_rows(j, 0, 4)

        def step(k, _):
            prod = product(k).reshape(4, 128, 256)
            ACC[k] = prod if j == 0 else ACC[k] + prod
            return 0

        lax.fori_loop(0, 4, step, 0)

    both(0, 0, 2)
    rs_first(*sets[0])
    y_last(HG, ky[1])
    scaled(HG, fgain, True, 2, 2)
    both(0, 2, 4)
    rs_far(*sets[0])
    kf = new(recvs)
    sf = sender(SSF.at[pl.ds(0, 3)])
    SSF[2] = SQR[2]
    send(SQR.at[0], SSF.at[1], sf, kf, x_up)
    send(SQR.at[1], SSF.at[0], sf, kf, x_dn)
    send(SQR.at[3], SSF.at[3], sf, kf, x_far)
    z_fin(weight("g", 1))
    z_fin(weight("v", 1))
    both(1)
    rs_far(*sets[1])
    rs_second(*sets[0])
    rs_first(*sets[1])
    z_fwd(7)
    z_fwd(8)
    rs_second(*sets[1])
    recv(SSF.at[pl.ds(0, 3)], kf)
    RS[...] = scale_of(jnp.sum(SSF[...], axis=0)[0:1, :])
    rs_wait(FC[0], kr[0])
    activate(0)
    x_start(0)
    z_fin(weight("g", 2))
    z_fin(weight("v", 2))
    both(2)
    rs_far(*sets[2])
    rs_first(*sets[2])
    rs_wait(FC[1], kr[1])
    activate(1)
    x_start(1)
    x_mid(0)
    rs_second(*sets[2])
    x_mid(1)
    x_near(0)
    x_last(0)
    z_fin(9)
    down_early(0)
    rs_wait(FC[2], kr[2])
    activate(2)
    x_start(2)
    x_near(1)
    x_last(1)
    z_fin(10)
    z_fin(11)
    down_early(1)
    x_mid(2)
    x_near(2)

    k7 = [new(recvs, 2) for _ in range(2)]
    s7 = sender(CS5)
    kt = new(recvs)
    st = new(sends)
    stays = y == z
    ends.append(lambda: fewer(lambda n: TB.at[pl.ds(0, n)], 4, stay(st), stays))

    def give(b):
        for i in range(2):
            TB[b, :, i * 256 : i * 256 + 256] = (T5[i, b] + CR5[i, b].astype(F32)).astype(BF16)
        if b < 2:
            send(TB.at[b], TI.at[y], st, kt, along(1 - 2 * b, z))
        elif b == 3:
            send(TB.at[b, ra], TI.at[y, ra], st, kt, along(-2, z))
            send(TB.at[b, rb], TI.at[y, rb], st, kt, along(2, z))
        else:

            @pl.when(stays)
            def _():
                TI[y] = TB[b]

            @pl.when(jnp.logical_not(stays))
            def _():
                send(TB.at[b], TI.at[y], st, kt, at(y_=z))

    for g, (b0, b1) in enumerate(((0, 3), (3, 4))):
        if g:
            x_last(2)
        rows = pl.ds(b0, b1 - b0)
        product = down_rows(2, b0, b1)

        def final(k):
            return product(k).reshape(b1 - b0, 128, 256) + ACC[k, rows]

        for i in range(2):
            CS5[i, rows] = final(2 * other + i).astype(BF16)
            send(CS5.at[i, rows], CR5.at[i, rows], s7, k7[g] + i, mate)
        for i in range(2):
            T5[i, rows] = final(2 * c + i)
        for i in range(2):
            recv(CR5.at[i, rows], k7[g] + i)
        for b in range(b0, b1):
            give(b)

    fewer(lambda n: HRES.at[pl.ds(0, n)], 4, lambda ref: recv(ref, ko))
    fewer(lambda n: TI.at[pl.ds(0, n)], 4, lambda ref: recv(ref, kt), stays)
    for q in range(4):
        cols = slice(q * 128, q * 128 + 128)
        change = sum(TI[n, :, cols].astype(F32) for n in range(4))
        out[:, cols] = (HRES[q].astype(F32) + change).astype(BF16)
    for wait in ends:
        wait()
    assert sends[0] <= ssem.shape[0] and recvs[0] <= rsem.shape[0], (sends[0], recvs[0])


def body(
    tokens, mixer_gain, gate_proj, value_proj, value_gain, spatial_mix, spatial_bias,
    head_gain, merge_proj, ffn_gain, gate_up, value_up, gate_kernel, value_kernel,
    gate_offset, value_offset, down_proj,
):
    units = gate_up.shape[1]
    layout = []
    for first in range(0, units, CHUNK):
        n = min(CHUNK, units - first)
        layout.append((first, n, -(-n // 128) * 128))
    wide = sum(n for _, _, n in layout)
    widths = [n for _, _, n in layout]
    vm = lambda shape, dtype=BF16: pltpu.VMEM(shape, dtype)
    in_vmem = pl.BlockSpec(memory_space=pltpu.VMEM)
    left = pl.BlockSpec(memory_space=pl.ANY)
    call = pl.pallas_call(
        functools.partial(kernel, layout),
        out_shape=jax.ShapeDtypeStruct(tokens.shape, tokens.dtype),
        in_specs=[
            left, in_vmem, in_vmem, left, left, in_vmem, in_vmem, in_vmem, in_vmem, left,
            left, left, left, left, in_vmem, in_vmem, left,
        ],
        out_specs=in_vmem,
        scratch_shapes=[
            vm(tokens.shape), vm(gate_kernel.shape, F32), vm(gate_kernel.shape, F32),
            vm((2, 4, wide), F32),
            vm((8, 4, 128, 128)), vm((8, 4, 128, 128)), vm((512, 1024)),
            vm((4, 8, 128), F32), vm((128, 128), F32), vm((16, 2, 8, 128)),
            vm((4, 128, 256)), vm((8, 8, 128), F32), vm((4, 8, 128), F32), vm((4, 128, 128)),
            vm((4, 128, 512)), vm((4, 128, 512)),
            *[vm((4, 256, 256))] * 3, vm((4, 4, 128, 128), F32), vm((4, 4, 128, 256), F32),
            vm((4, 128, 512), F32), vm((3, 128, 512)), vm((2, 64, 512)), vm((2, 128, 512)),
            vm((4, 4, 128, 128)), vm((4, 4, 128, 128)), vm((3, 4, 128, 128)),
            vm((4, 128, 128)), vm((2, 2, 2, 128, 128)),
            vm((2, 4, 128, 256)), vm((2, 4, 128, 256)), vm((2, 4, 128, 256), F32),
            *[vm((4, n, 256)) for _ in range(3) for n in widths],
            *[vm((4, 128, n)) for n in widths],
            *[vm((4, 128, 2 * n), F32) for n in widths],
            *[vm((3, 128, 2 * n)) for n in widths],
            *[vm((2, 64, 2 * n)) for n in widths],
            *[vm((2, 128, 2 * n)) for n in widths],
            pltpu.SemaphoreType.DMA((SENDS,)), pltpu.SemaphoreType.DMA((RECVS,)),
            pltpu.SemaphoreType.DMA((6 + 3 * len(layout),)),
        ],
        compiler_params=pltpu.CompilerParams(
            collective_id=0, has_side_effects=True, vmem_limit_bytes=58 << 20
        ),
        name="layer",
    )
    return call(
        tokens, mixer_gain, ffn_gain, gate_proj, value_proj, value_gain, spatial_mix,
        spatial_bias, head_gain, merge_proj, gate_up.T, value_up.T, gate_kernel, value_kernel,
        gate_offset, value_offset, down_proj,
    )


def solution(mesh):
    finer = Mesh(
        mesh.devices.reshape(mesh.shape["rep"], 4, 4, 4, 2), ("rep", "fs_0", "fs_1", "tp_0", "tp_1")
    )
    return jax.shard_map(
        body,
        mesh=finer,
        in_specs=(
            P(REP_FS, TP), P(), P(FS, TP), P(FS, TP), P(TP, None), P(TP, FS, None),
            P(TP, None), P(TP, None), P(TP, FS), P(), P(FS, TP), P(FS, TP), P(None, TP),
            P(None, TP), P(TP), P(TP), P(TP, FS),
        ),
        out_specs=P(REP_FS, TP),
        check_vma=False,
    )
```

```python
import functools

import jax
import jax.numpy as jnp
from jax import lax
from jax.experimental import pallas as pl
from jax.experimental.pallas import tpu as pltpu
from jax.sharding import Mesh
from jax.sharding import PartitionSpec as P

TP = ("tp_0", "tp_1")
FS = ("fs_0", "fs_1")
REP_FS = ("rep", "fs_0", "fs_1")
MESH = pl.DeviceIdType.MESH
EPS = 1e-06
SENDS, RECVS = 33, 105
CHUNK = 512
F32 = jnp.float32
BF16 = jnp.bfloat16


def gelu(v):
    return 0.5 * v * (1.0 + lax.erf(v * 0.7071067811865476))


def lanes_of(n):
    return lax.broadcasted_iota(jnp.int32, (n, 128), 1)


def kernel(layout, tok, mgain, fgain, gp, vp, vgain, smix, sbias, hgain, mp, gu, vu, gk, vk, go, vo,
           dn, out, tokv, gkv, vkv, CV, XG, HG, XS, SQR, RS, SM, MG, SSB, SSF, HRES, TB, TI,
           WGP, WVP, WMP, T, ACC, P1, S1, H1, F1, CS4, CR4, YS4, YH4, YF4, CS5, CR5, T5, *rest):
    chunks = len(layout)
    WGU, WVU, WDN, ACT, PC, SC, HC, FC = (rest[i * chunks : (i + 1) * chunks] for i in range(8))
    ssem, rsem, lsem = rest[8 * chunks :]
    r, z, x, y, c = (lax.axis_index(a) for a in ("rep", "fs_0", "fs_1", "tp_0", "tp_1"))
    other = 1 - c
    f = 4 * z + x
    units = dn.shape[0]
    depth = mgain.shape[0]

    def at(z_=None, x_=None, y_=None, c_=None, r_=None):
        pick = lambda new, old: old if new is None else new
        return (pick(r_, r), pick(z_, z), pick(x_, x), pick(y_, y), pick(c_, c))

    up = lambda v: lax.rem(v + 1, 4)
    down = lambda v: lax.rem(v + 3, 4)
    far = lambda v: lax.rem(v + 2, 4)

    zr = 4 * r + z
    zu, zd = lax.rem(zr + 1, 8), lax.rem(zr + 7, 8)
    z_up = at(r_=zu // 4, z_=lax.rem(zu, 4))
    z_dn = at(r_=zd // 4, z_=lax.rem(zd, 4))
    x_up, x_dn, x_far = at(x_=up(x)), at(x_=down(x)), at(x_=far(x))
    y_up, y_dn = at(y_=up(y)), at(y_=down(y))
    mate = at(c_=other)
    fs_peers = []
    for i in range(1, 16):
        g = lax.rem(f + i, 16)
        fs_peers.append(at(z_=g // 4, x_=lax.rem(g, 4)))
    near = []
    for i in range(1, 4):
        near += [at(x_=lax.rem(x + i, 4), c_=k) for k in (c, other)]
        near += [at(y_=lax.rem(y + i, 4), c_=other)]

    def along(d, y_=None):
        there = lax.rem(zr + 8 + d, 8)
        return at(r_=there // 4, z_=lax.rem(there, 4), y_=y_)

    for i in range(4):
        for d in (-2, -1, 0, 1, 2):
            if i or d:
                near.append(along(d, lax.rem(y + i, 4)))

    barrier = pltpu.get_barrier_semaphore()
    greet = [mate] + near + fs_peers
    for peer in greet:
        pl.semaphore_signal(barrier, inc=1, device_id=peer, device_id_type=MESH)
    loads = [
        pltpu.make_async_copy(src, dst, lsem.at[i])
        for i, (src, dst) in enumerate(((tok, tokv), (gk, gkv), (vk, vkv)))
    ]
    for copy in loads:
        copy.start()
    pl.semaphore_wait(barrier, len(greet))

    sends, recvs, ends = [0], [0], []

    def new(counter, n=1):
        counter[0] += n
        return counter[0] - n

    def remote(src, dst, s, k, peer):
        return pltpu.make_async_remote_copy(
            src_ref=src, dst_ref=dst, send_sem=ssem.at[s], recv_sem=rsem.at[k],
            device_id=peer, device_id_type=MESH,
        )

    def send(src, dst, s, k, peer):
        remote(src, dst, s, k, peer).start()

    def recv(dst, k):
        remote(dst, dst, 0, k, mate).wait_recv()

    def sender(ref):
        s = new(sends)
        ends.append(lambda: remote(ref, ref, s, 0, mate).wait_send())
        return s

    pieces = [(gp, WGP, 0, 256), (vp, WVP, 0, 256), (mp, WMP, 0, 256)]
    for (at0, n, _), G, V in zip(layout, WGU, WVU):
        pieces += [(gu, G, at0, n), (vu, V, at0, n)]
    for (at0, n, _), W in zip(layout, WDN):
        pieces.append((dn, W, at0, n))
    zk = [new(recvs, 3) for _ in pieces]
    zs = [sender(buf.at[pl.ds(0, 3), pl.ds(0, n)]) for _, buf, _, n in pieces]

    def z_local(i):
        src, buf, at0, n = pieces[i]
        own = buf.at[ring(i)[0], pl.ds(0, n)]
        return pltpu.make_async_copy(src.at[pl.ds(at0, n)], own, lsem.at[3 + i])

    def ring(i):
        return (x, x_up, x_dn) if pieces[i][0] is dn else (z, z_up, z_dn)

    def z_own(i):
        src, buf, at0, n = pieces[i]
        a, b = pl.ds(0, n // 2), pl.ds(n // 2, n // 2)
        from_a, from_b = src.at[pl.ds(at0, n // 2)], src.at[pl.ds(at0 + n // 2, n // 2)]
        place, above, below = ring(i)
        send(from_a, buf.at[place, a], zs[i], zk[i], above)
        send(from_b, buf.at[place, b], zs[i], zk[i] + 1, below)
        send(from_b, buf.at[place, b], zs[i], zk[i] + 2, above)
        send(from_a, buf.at[place, a], zs[i], zk[i] + 2, below)
        z_local(i).start()

    def z_fwd(i):
        _, buf, _, n = pieces[i]
        place, above, below = ring(i)
        a, b = buf.at[down(place), pl.ds(0, n // 2)], buf.at[up(place), pl.ds(n // 2, n // 2)]
        recv(a, zk[i])
        send(a, a, zs[i], zk[i] + 2, above)
        recv(b, zk[i] + 1)
        send(b, b, zs[i], zk[i] + 2, below)

    def z_fin(i):
        _, buf, _, n = pieces[i]
        recv(buf.at[pl.ds(0, 2), pl.ds(0, n)], zk[i] + 2)
        z_local(i).wait()

    def weight(kind, j):
        return {"g": 3 + 2 * j, "v": 4 + 2 * j, "d": 3 + 2 * chunks + j}[kind]

    me = 2 * y + c
    to_me = x // 2 == c
    loads[0].wait()
    kx = new(recvs, 2)
    sx = new(sends)
    for j in range(2):
        for h in range(2):
            xt = 2 * c + j
            ahead = lax.rem(x - xt + 4, 4)
            place = jnp.where(ahead == 0, 2, jnp.where(ahead == 2, 3, ahead // 2))
            mine = jnp.logical_and(xt == x, c == h)
            block = tokv.at[:, j * 256 + h * 128 : j * 256 + h * 128 + 128]

            @pl.when(jnp.logical_not(mine))
            def _():
                dst = XG.at[2 * y + h, place]
                send(block, dst, sx, kx + place // 2, at(x_=xt, c_=jnp.int32(h)))

            @pl.when(mine)
            def _():
                XG[2 * y + h, 2] = block[...]

    def fewer(ref_of, n, wait, stays=to_me):
        @pl.when(stays)
        def _():
            wait(ref_of(n - 1))

        @pl.when(jnp.logical_not(stays))
        def _():
            wait(ref_of(n))

    stay = lambda s: lambda ref: remote(ref, ref, s, 0, mate).wait_send()
    ends.append(lambda: fewer(lambda n: XG.at[0, pl.ds(0, n)], 4, stay(sx)))
    z_own(0)
    z_own(1)
    square = tokv[...].astype(F32)
    square = jnp.sum(square * square, axis=-1, keepdims=True)
    SSB[me] = jnp.broadcast_to(square, (128, 128)).T[0:8, :]
    kss = new(recvs)
    sss = sender(SSB.at[pl.ds(0, 7)])
    for i in range(1, 8):
        t = lax.rem(me + i, 8)
        send(SSB.at[me], SSB.at[me], sss, kss, at(y_=t // 2, c_=lax.rem(t, 2)))

    lo_y, hi_y, far_y = 2 * down(y) + c, 2 * up(y) + c, 2 * far(y) + c

    def y_start(buf, k, s, g):
        a, b = buf.at[me, 2 * g], buf.at[me, 2 * g + 1]
        send(a, a, s, k, y_up)
        send(b, b, s, k + 1, y_dn)
        send(b, b, s, k + 2, y_up)
        send(a, a, s, k + 3, y_dn)
        both = buf.at[me, pl.ds(2 * g, 2)]
        send(both, both, s, k + 6, mate)

    def y_mid(buf, k, s, g):
        a, b = buf.at[lo_y, 2 * g], buf.at[hi_y, 2 * g + 1]
        recv(a, k)
        send(a, a, s, k + 4, y_up)
        send(a, a, s, k + 6, mate)
        recv(b, k + 1)
        send(b, b, s, k + 5, y_dn)
        send(b, b, s, k + 6, mate)

    def y_end(buf, k, s, g):
        rows = (buf.at[lo_y, 2 * g + 1], buf.at[hi_y, 2 * g], buf.at[far_y, 2 * g], buf.at[far_y, 2 * g + 1])
        for i, ref in enumerate(rows):
            recv(ref, k + 2 + i)
            send(ref, ref, s, k + 6, mate)

    def y_last(buf, k):
        recv(buf.at[pl.ds(0, 4), pl.ds(0, 2)], k + 6)

    def scaled(buf, gains, squares, first, n):
        parts = [gains[pl.ds(pl.multiple_of((4 * k + x) * 256, 256), 256)] for k in range(4)]
        gain = jnp.concatenate([part.reshape(1, 256) for part in parts], axis=1)

        def block(b, _):
            rows = jnp.concatenate([buf[i, b] for i in range(8)], axis=1).astype(F32)
            if squares:
                total = jnp.sum(rows * rows, axis=-1, keepdims=True)
                SQR[b] = jnp.broadcast_to(total, (128, 128)).T[0:8, :]
            XS[pl.ds(pl.multiple_of(b * 128, 128), 128), :] = (rows * gain).astype(BF16)
            return 0

        lax.fori_loop(first, first + n, block, 0)

    def scale_of(rows):
        return lax.rsqrt(jnp.broadcast_to(rows, (128, 128)).T / depth + EPS)

    ky = [new(recvs, 7) for _ in range(2)]
    sy = [sender(buf.at[pl.ds(0, 7), pl.ds(0, 2)]) for buf in (XG, XG)]
    recv(XG.at[me, pl.ds(0, 2)], kx)
    y_start(XG, ky[0], sy[0], 0)
    fewer(lambda n: XG.at[me, pl.ds(0, n)], 2, lambda ref: recv(ref, kx + 1))
    y_start(XG, ky[1], sy[1], 1)
    km = new(recvs)
    sm = sender(SM.at[pl.ds(0, 15)])
    for i in range(15):
        send(smix, SM.at[f], sm, km, fs_peers[i])
    SM[f] = smix[...]
    last0, lastn, wide = layout[-1]
    for W in (WGU[-1], WVU[-1], WDN[-1]):
        for k in range(4):
            W[k, lastn:, :] = jnp.zeros((wide - lastn, 256), BF16)
    z_own(9)
    z_own(11)
    z_fwd(0)
    z_fwd(1)
    z_own(2)
    z_own(3)
    y_mid(XG, ky[0], sy[0], 0)
    y_mid(XG, ky[1], sy[1], 1)
    loads[1].wait()
    loads[2].wait()
    for w, kern, off in ((0, gkv, go), (1, vkv, vo)):
        CV[w, :, last0:] = jnp.zeros((4, wide), F32)
        CV[w, 0:3, 0:units] = kern[...]
        CV[w, 3:4, 0:units] = off[...].reshape(1, units)
    y_end(XG, ky[0], sy[0], 0)
    y_end(XG, ky[1], sy[1], 1)
    y_last(XG, ky[0])
    y_last(XG, ky[1])
    scaled(XG, mgain, False, 0, 4)
    z_fin(0)
    z_fin(1)
    for w, W in ((0, WGP), (1, WVP)):
        prod = jnp.dot(XS[...], W[...].reshape(1024, 256), preferred_element_type=F32)
        P1[:, :, w * 256 : w * 256 + 256] = prod.reshape(4, 128, 256)

    def row_loop(first, n, fn):
        def step(i, _):
            fn(pl.ds(pl.multiple_of(first + i * 16, 16), 16))
            return 0

        lax.fori_loop(0, n // 16, step, 0)

    ra, rb = pl.ds(0, 64), pl.ds(64, 64)

    def rounded_rows(p, i, S, k, first, n, cols):
        def fn(rows):
            S[k, rows, cols] = p[i, rows, cols].astype(BF16)

        row_loop(first, n, fn)

    def rs_far(p, S, H, F, k, s, cols=slice(None)):
        rounded_rows(p, 3, S, 0, 0, 128, cols)
        send(S.at[0, ra, cols], H.at[0, :, cols], s, k, x_up)
        send(S.at[0, rb, cols], H.at[1, :, cols], s, k + 1, x_dn)

    def rs_first(p, S, H, F, k, s, cols=slice(None)):
        rounded_rows(p, 0, S, 1, 64, 64, cols)
        send(S.at[1, rb, cols], F.at[0, rb, cols], s, k + 2, x_up)
        rounded_rows(p, 1, S, 2, 0, 64, cols)
        send(S.at[2, ra, cols], F.at[1, ra, cols], s, k + 2, x_dn)

    def rs_second(p, S, H, F, k, s):
        def left(rows):
            S[1, rows, :] = (p[0, rows, :] + H[0, rows, :].astype(F32)).astype(BF16)

        def right(rows):
            low = pl.ds(pl.multiple_of(rows.start + 64, 16), 16)
            S[2, low, :] = (p[1, low, :] + H[1, rows, :].astype(F32)).astype(BF16)

        recv(H.at[0], k)
        row_loop(0, 64, left)
        send(S.at[1, ra], F.at[0, ra], s, k + 2, x_up)
        recv(H.at[1], k + 1)
        row_loop(0, 64, right)
        send(S.at[2, rb], F.at[1, rb], s, k + 2, x_dn)

    def rs_wait(F, k):
        recv(F, k + 2)

    kr = [new(recvs, 3) for _ in layout]
    set1 = (P1, S1, H1, F1, kr[0], sender(S1))
    rs_far(*set1)
    rs_first(*set1)
    z_fwd(2)
    z_own(4)
    rs_second(*set1)
    z_fwd(3)
    z_own(5)
    recv(SM.at[pl.ds(0, 15)], km)
    recv(SSB.at[pl.ds(0, 7)], kss)
    rs_wait(F1, kr[0])

    total = P1[2] + F1[0].astype(F32) + F1[1].astype(F32)
    rs = scale_of(jnp.sum(SSB[...], axis=0)[0:1, :])
    eye = lax.broadcasted_iota(jnp.int32, (128, 128), 0) == lanes_of(128)
    for h in range(2):
        cols = slice(h * 128, h * 128 + 128)
        gated = gelu((rs * total[:, cols]).astype(BF16).astype(F32))
        spread = gelu((rs * total[:, 256 + h * 128 : 384 + h * 128]).astype(BF16).astype(F32))
        spread = spread * lax.rsqrt(jnp.mean(spread * spread, axis=-1, keepdims=True) + EPS)
        spread = (spread * vgain[h : h + 1, :]).astype(BF16)
        matrix = SM[:, h].astype(F32).reshape(128, 128).astype(BF16)
        mixed = jnp.dot(matrix, spread, preferred_element_type=F32)
        bias = jnp.broadcast_to(sbias[h : h + 1, :], (128, 128))
        mixed = mixed + jnp.sum(jnp.where(eye, bias, 0.0), axis=-1, keepdims=True)
        joined = gated * mixed
        joined = joined * lax.rsqrt(jnp.mean(joined * joined, axis=-1, keepdims=True) + EPS)
        MG[2, :, cols] = (joined * hgain[h : h + 1, :]).astype(BF16)

    k2 = new(recvs, 3)
    s2 = sender(MG.at[pl.ds(0, 3)])
    send(MG.at[2], MG.at[1], s2, k2 + 1, x_up)
    send(MG.at[2], MG.at[0], s2, k2 + 2, x_dn)
    send(MG.at[2], MG.at[3], s2, k2, x_far)
    z_fin(2)

    y_order = (far(y), up(y), down(y), y)

    def cy_first(g, product, CS, CR, k, s):
        for n, yt in enumerate(y_order):
            prod = product(yt)
            size = prod.shape[0] // 128
            rows = pl.ds(2 * g, size)
            T[n, rows] = jnp.where(c == 0, prod[:, :128], prod[:, 128:]).reshape(size, 128, 128)
            give = jnp.where(c == 0, prod[:, 128:], prod[:, :128]).astype(BF16)
            CS[n, rows] = give.reshape(size, 128, 128)
            send(CS.at[n, rows], CR.at[n, rows], s, k + n, mate)

    def joined_at(n, b, CR):
        return T[n, b] + CR[n, b].astype(F32)

    def cy_second(g, CR, YS, YH, YF, k, kc, s):
        a, b = 2 * g, 2 * g + 1
        recv(CR.at[0, pl.ds(a, 2)], kc)
        YS[0, a] = joined_at(0, a, CR).astype(BF16)
        YS[0, b] = joined_at(0, b, CR).astype(BF16)
        send(YS.at[0, a], YH.at[a], s, k, y_up)
        send(YS.at[0, b], YH.at[b], s, k + 1, y_dn)
        recv(CR.at[1, pl.ds(a, 2)], kc + 1)
        YS[1, b] = joined_at(1, b, CR).astype(BF16)
        send(YS.at[1, b], YF.at[g, 0, 1], s, k + 2, y_up)
        recv(CR.at[2, pl.ds(a, 2)], kc + 2)
        YS[2, a] = joined_at(2, a, CR).astype(BF16)
        send(YS.at[2, a], YF.at[g, 1, 0], s, k + 2, y_dn)

    def cy_third(g, CR, YS, YH, YF, k, kc, s):
        a, b = 2 * g, 2 * g + 1
        recv(YH.at[a], k)
        YS[1, a] = (joined_at(1, a, CR) + YH[a].astype(F32)).astype(BF16)
        send(YS.at[1, a], YF.at[g, 0, 0], s, k + 2, y_up)
        recv(YH.at[b], k + 1)
        YS[2, b] = (joined_at(2, b, CR) + YH[b].astype(F32)).astype(BF16)
        send(YS.at[2, b], YF.at[g, 1, 1], s, k + 2, y_dn)
        recv(CR.at[3, pl.ds(a, 2)], kc + 3)

    def cy_last(g, CR, YF, k):
        recv(YF.at[g], k + 2)
        return [
            joined_at(3, 2 * g + i, CR) + YF[g, 0, i].astype(F32) + YF[g, 1, i].astype(F32)
            for i in range(2)
        ]

    def merge(g):
        rows = MG[2 * g : 2 * g + 2].reshape(256, 256)
        return lambda yt: jnp.dot(rows, WMP[yt], preferred_element_type=F32)

    kc = [new(recvs, 4) for _ in range(2)]
    k3 = [new(recvs, 3) for _ in range(2)]
    sc, s3 = sender(CS4), sender(YS4)
    recv(MG.at[0], k2 + 2)
    recv(MG.at[1], k2 + 1)
    cy_first(0, merge(0), CS4, CR4, kc[0], sc)
    cy_second(0, CR4, YS4, YH4, YF4, k3[0], kc[0], s3)
    recv(MG.at[3], k2)
    z_own(10)
    z_fwd(9)
    z_fwd(11)
    cy_first(1, merge(1), CS4, CR4, kc[1], sc)
    cy_second(1, CR4, YS4, YH4, YF4, k3[1], kc[1], s3)
    z_fwd(4)
    z_own(6)
    cy_third(0, CR4, YS4, YH4, YF4, k3[0], kc[0], s3)
    cy_third(1, CR4, YS4, YH4, YF4, k3[1], kc[1], s3)


    ko = new(recvs)
    so = new(sends)
    ends.append(lambda: fewer(lambda n: HG.at[0, pl.ds(0, n)], 4, stay(so)))
    spot = 2 * lax.rem(x, 2) + c
    blocks = (up(x), down(x), x, far(x))
    sh = [sender(buf.at[pl.ds(0, 7), pl.ds(0, 2)]) for buf in (HG, HG)]
    for g in range(2):
        branch = cy_last(g, CR4, YF4, k3[g])
        for i in range(2):
            b = 2 * g + i
            HG[me, b] = (XG[me, b].astype(F32) + branch[i]).astype(BF16)
        y_start(HG, ky[g], sh[g], g)
    for b in range(4):
        if b != 2:
            dst = HRES.at[spot]
            send(HG.at[me, b], dst, so, ko, at(x_=blocks[b], c_=x // 2))
            continue

        @pl.when(to_me)
        def _():
            HRES[spot] = HG[me, 2]

        @pl.when(jnp.logical_not(to_me))
        def _():
            send(HG.at[me, 2], HRES.at[spot], so, ko, mate)

    z_fwd(5)
    y_mid(HG, ky[0], sh[0], 0)
    y_mid(HG, ky[1], sh[1], 1)
    y_end(HG, ky[0], sh[0], 0)
    z_fwd(6)
    z_own(7)
    z_own(8)
    z_fwd(10)
    y_end(HG, ky[1], sh[1], 1)
    z_fin(weight("g", 0))
    z_fin(weight("v", 0))
    y_last(HG, ky[0])
    scaled(HG, fgain, True, 0, 2)

    def project(W, p, n, first, b0, b1):
        def cut(cols, to, size):
            w = jnp.concatenate([W[k, cols, :] for k in range(4)], axis=1)
            prod = lax.dot_general(
                XS[b0 * 128 : b1 * 128, :], w, (((1,), (1,)), ((), ())),
                preferred_element_type=F32,
            )
            p[b0:b1, :, to] = prod.reshape(b1 - b0, 128, size)

        def step(i, _):
            cut(
                pl.ds(pl.multiple_of(i * 256, 256), 256),
                pl.ds(pl.multiple_of(first + i * 256, 128), 256), 256,
            )
            return 0

        lax.fori_loop(0, n // 256, step, 0)
        left = n % 256
        if left:
            cut(pl.ds(n - left, left), pl.ds(first + n - left, left), left)

    def both(j, b0=0, b1=4):
        n = layout[j][2]
        project(WGU[j], PC[j], n, 0, b0, b1)
        project(WVU[j], PC[j], n, n, b0, b1)

    def gates(j):
        n = layout[j][2]
        z_fin(weight("g", j))
        project(WGU[j], PC[j], n, 0, 0, 4)
        return slice(0, n)

    def values(j):
        n = layout[j][2]
        z_fin(weight("v", j))
        project(WVU[j], PC[j], n, n, 0, 4)
        return slice(n, 2 * n)

    row = lax.broadcasted_iota(jnp.int32, (128, 128), 0)

    def activate(j):
        p, F, act = PC[j], FC[j], ACT[j]
        at0, _, n = layout[j]

        def conv_tile(i, _):
            def one(first, w):
                at_ = pl.ds(pl.multiple_of(first + i * 128, 128), 128)
                v = p[2, :, at_] + F[0, :, at_].astype(F32) + F[1, :, at_].astype(F32)
                v = (RS[...] * v).astype(BF16).astype(F32)
                prev = jnp.where(row == 0, 0.0, pltpu.roll(v, 1, axis=0))
                after = jnp.where(row == 127, 0.0, pltpu.roll(v, 127, axis=0))
                k = CV[w, :, pl.ds(pl.multiple_of(at0 + i * 128, 128), 128)]
                return k[3:4] + prev * k[0:1] + v * k[1:2] + after * k[2:3]

            cols = pl.ds(pl.multiple_of(i * 128, 128), 128)
            act[2, :, cols] = (gelu(one(0, 0)) * one(n, 1)).astype(BF16)
            return 0

        lax.fori_loop(0, n // 128, conv_tile, 0)

    sets = [
        (PC[j], SC[j], HC[j], FC[j], kr[j], sender(SC[j])) for j in range(chunks)
    ]
    kg = [new(recvs, 4) for _ in layout]
    sg = [sender(ACT[j].at[pl.ds(0, 3)]) for j in range(chunks)]

    def x_start(j):
        buf, k, s = ACT[j], kg[j], sg[j]
        send(buf.at[2, ra], buf.at[1, ra], s, k, z_up)
        send(buf.at[2, rb], buf.at[0, rb], s, k + 1, z_dn)
        send(buf.at[2, rb], buf.at[1, rb], s, k + 2, z_up)
        send(buf.at[2, ra], buf.at[0, ra], s, k + 2, z_dn)

    def x_mid(j):
        buf, k, s = ACT[j], kg[j], sg[j]
        recv(buf.at[1, ra], k)
        send(buf.at[1, ra], buf.at[3, ra], s, k + 3, z_up)
        recv(buf.at[0, rb], k + 1)
        send(buf.at[0, rb], buf.at[3, rb], s, k + 3, z_dn)

    def x_near(j):
        recv(ACT[j].at[0], kg[j] + 2)

    def x_last(j):
        recv(ACT[j].at[3], kg[j] + 3)

    def down_rows(j, b0, b1):
        n = layout[j][2]
        rows = ACT[j][b0:b1].reshape((b1 - b0) * 128, n)
        return lambda k: jnp.dot(rows, WDN[j][k], preferred_element_type=F32)

    def down_early(j):
        product = down_rows(j, 0, 4)

        def step(k, _):
            prod = product(k).reshape(4, 128, 256)
            ACC[k] = prod if j == 0 else ACC[k] + prod
            return 0

        lax.fori_loop(0, 4, step, 0)

    both(0, 0, 2)
    rs_first(*sets[0])
    y_last(HG, ky[1])
    scaled(HG, fgain, True, 2, 2)
    both(0, 2, 4)
    rs_far(*sets[0])
    kf = new(recvs)
    sf = sender(SSF.at[pl.ds(0, 3)])
    SSF[2] = SQR[2]
    send(SQR.at[0], SSF.at[1], sf, kf, x_up)
    send(SQR.at[1], SSF.at[0], sf, kf, x_dn)
    send(SQR.at[3], SSF.at[3], sf, kf, x_far)
    one1 = gates(1)
    rs_far(*sets[1], one1)
    rs_first(*sets[1], one1)
    two1 = values(1)
    rs_far(*sets[1], two1)
    rs_second(*sets[0])
    rs_first(*sets[1], two1)
    z_fwd(7)
    z_fwd(8)
    rs_second(*sets[1])
    recv(SSF.at[pl.ds(0, 3)], kf)
    RS[...] = scale_of(jnp.sum(SSF[...], axis=0)[0:1, :])
    rs_wait(FC[0], kr[0])
    activate(0)
    x_start(0)
    one2 = gates(2)
    rs_far(*sets[2], one2)
    rs_first(*sets[2], one2)
    two2 = values(2)
    rs_far(*sets[2], two2)
    rs_first(*sets[2], two2)
    rs_wait(FC[1], kr[1])
    activate(1)
    x_start(1)
    x_mid(0)
    rs_second(*sets[2])
    x_mid(1)
    x_near(0)
    x_last(0)
    z_fin(9)
    down_early(0)
    rs_wait(FC[2], kr[2])
    activate(2)
    x_start(2)
    x_near(1)
    x_last(1)
    z_fin(10)
    z_fin(11)
    down_early(1)

    k7 = [new(recvs, 2) for _ in range(3)]
    s7 = sender(CS5)
    kt = new(recvs)
    st = new(sends)
    stays = y == z
    ends.append(lambda: fewer(lambda n: TB.at[pl.ds(0, n)], 4, stay(st), stays))

    def give(b):
        for i in range(2):
            TB[b, :, i * 256 : i * 256 + 256] = (T5[i, b] + CR5[i, b].astype(F32)).astype(BF16)
        if b < 2:
            send(TB.at[b], TI.at[y], st, kt, along(1 - 2 * b, z))
        elif b == 3:
            send(TB.at[b, ra], TI.at[y, ra], st, kt, along(-2, z))
            send(TB.at[b, rb], TI.at[y, rb], st, kt, along(2, z))
        else:

            @pl.when(stays)
            def _():
                TI[y] = TB[b]

            @pl.when(jnp.logical_not(stays))
            def _():
                send(TB.at[b], TI.at[y], st, kt, at(y_=z))

    parts = ((2, 3), (0, 2), (3, 4))

    def finish(g):
        b0, b1 = parts[g]
        rows = pl.ds(b0, b1 - b0)
        product = down_rows(2, b0, b1)

        def final(k):
            return product(k).reshape(b1 - b0, 128, 256) + ACC[k, rows]

        for i in range(2):
            CS5[i, rows] = final(2 * other + i).astype(BF16)
            send(CS5.at[i, rows], CR5.at[i, rows], s7, k7[g] + i, mate)
        for i in range(2):
            T5[i, rows] = final(2 * c + i)

    def hand_over(g):
        b0, b1 = parts[g]
        for i in range(2):
            recv(CR5.at[i, pl.ds(b0, b1 - b0)], k7[g] + i)
        for b in range(b0, b1):
            give(b)

    finish(0)
    x_mid(2)
    x_near(2)
    finish(1)
    hand_over(0)
    hand_over(1)
    x_last(2)
    finish(2)
    hand_over(2)

    fewer(lambda n: HRES.at[pl.ds(0, n)], 4, lambda ref: recv(ref, ko))
    fewer(lambda n: TI.at[pl.ds(0, n)], 4, lambda ref: recv(ref, kt), stays)
    for q in range(4):
        cols = slice(q * 128, q * 128 + 128)
        change = sum(TI[n, :, cols].astype(F32) for n in range(4))
        out[:, cols] = (HRES[q].astype(F32) + change).astype(BF16)
    for wait in ends:
        wait()
    assert sends[0] <= ssem.shape[0] and recvs[0] <= rsem.shape[0], (sends[0], recvs[0])


def body(
    tokens, mixer_gain, gate_proj, value_proj, value_gain, spatial_mix, spatial_bias,
    head_gain, merge_proj, ffn_gain, gate_up, value_up, gate_kernel, value_kernel,
    gate_offset, value_offset, down_proj,
):
    units = gate_up.shape[1]
    layout = []
    for first in range(0, units, CHUNK):
        n = min(CHUNK, units - first)
        layout.append((first, n, -(-n // 128) * 128))
    wide = sum(n for _, _, n in layout)
    widths = [n for _, _, n in layout]
    vm = lambda shape, dtype=BF16: pltpu.VMEM(shape, dtype)
    in_vmem = pl.BlockSpec(memory_space=pltpu.VMEM)
    left = pl.BlockSpec(memory_space=pl.ANY)
    call = pl.pallas_call(
        functools.partial(kernel, layout),
        out_shape=jax.ShapeDtypeStruct(tokens.shape, tokens.dtype),
        in_specs=[
            left, in_vmem, in_vmem, left, left, in_vmem, in_vmem, in_vmem, in_vmem, left,
            left, left, left, left, in_vmem, in_vmem, left,
        ],
        out_specs=in_vmem,
        scratch_shapes=[
            vm(tokens.shape), vm(gate_kernel.shape, F32), vm(gate_kernel.shape, F32),
            vm((2, 4, wide), F32),
            vm((8, 4, 128, 128)), vm((8, 4, 128, 128)), vm((512, 1024)),
            vm((4, 8, 128), F32), vm((128, 128), F32), vm((16, 2, 8, 128)),
            vm((4, 128, 256)), vm((8, 8, 128), F32), vm((4, 8, 128), F32), vm((4, 128, 128)),
            vm((4, 128, 512)), vm((4, 128, 512)),
            *[vm((4, 256, 256))] * 3, vm((4, 4, 128, 128), F32), vm((4, 4, 128, 256), F32),
            vm((4, 128, 512), F32), vm((3, 128, 512)), vm((2, 64, 512)), vm((2, 128, 512)),
            vm((4, 4, 128, 128)), vm((4, 4, 128, 128)), vm((3, 4, 128, 128)),
            vm((4, 128, 128)), vm((2, 2, 2, 128, 128)),
            vm((2, 4, 128, 256)), vm((2, 4, 128, 256)), vm((2, 4, 128, 256), F32),
            *[vm((4, n, 256)) for _ in range(3) for n in widths],
            *[vm((4, 128, n)) for n in widths],
            *[vm((4, 128, 2 * n), F32) for n in widths],
            *[vm((3, 128, 2 * n)) for n in widths],
            *[vm((2, 64, 2 * n)) for n in widths],
            *[vm((2, 128, 2 * n)) for n in widths],
            pltpu.SemaphoreType.DMA((SENDS,)), pltpu.SemaphoreType.DMA((RECVS,)),
            pltpu.SemaphoreType.DMA((6 + 3 * len(layout),)),
        ],
        compiler_params=pltpu.CompilerParams(
            collective_id=0, has_side_effects=True, vmem_limit_bytes=58 << 20
        ),
        name="layer",
    )
    return call(
        tokens, mixer_gain, ffn_gain, gate_proj, value_proj, value_gain, spatial_mix,
        spatial_bias, head_gain, merge_proj, gate_up.T, value_up.T, gate_kernel, value_kernel,
        gate_offset, value_offset, down_proj,
    )


def solution(mesh):
    finer = Mesh(
        mesh.devices.reshape(mesh.shape["rep"], 4, 4, 4, 2), ("rep", "fs_0", "fs_1", "tp_0", "tp_1")
    )
    return jax.shard_map(
        body,
        mesh=finer,
        in_specs=(
            P(REP_FS, TP), P(), P(FS, TP), P(FS, TP), P(TP, None), P(TP, FS, None),
            P(TP, None), P(TP, None), P(TP, FS), P(), P(FS, TP), P(FS, TP), P(None, TP),
            P(None, TP), P(TP), P(TP), P(TP, FS),
        ),
        out_specs=P(REP_FS, TP),
        check_vma=False,
    )
```

```python
import functools

import jax
import jax.numpy as jnp
from jax import lax
from jax.experimental import pallas as pl
from jax.experimental.pallas import tpu as pltpu
from jax.sharding import Mesh
from jax.sharding import PartitionSpec as P

TP = ("tp_0", "tp_1")
FS = ("fs_0", "fs_1")
REP_FS = ("rep", "fs_0", "fs_1")
MESH = pl.DeviceIdType.MESH
EPS = 1e-06
SENDS, RECVS = 33, 105
CHUNK = 512
F32 = jnp.float32
BF16 = jnp.bfloat16


def gelu(v):
    return 0.5 * v * (1.0 + lax.erf(v * 0.7071067811865476))


def lanes_of(n):
    return lax.broadcasted_iota(jnp.int32, (n, 128), 1)


def kernel(layout, tok, mgain, fgain, gp, vp, vgain, smix, sbias, hgain, mp, gu, vu, gk, vk, go, vo,
           dn, out, tokv, gkv, vkv, CV, XG, HG, XS, SQR, RS, SM, MG, SSB, SSF, HRES, TB, TI,
           WGP, WVP, WMP, T, ACC, P1, S1, H1, F1, CS4, CR4, YS4, YH4, YF4, CS5, CR5, T5, *rest):
    chunks = len(layout)
    WGU, WVU, WDN, ACT, PC, SC, HC, FC = (rest[i * chunks : (i + 1) * chunks] for i in range(8))
    ssem, rsem, lsem = rest[8 * chunks :]
    r, z, x, y, c = (lax.axis_index(a) for a in ("rep", "fs_0", "fs_1", "tp_0", "tp_1"))
    other = 1 - c
    f = 4 * z + x
    units = dn.shape[0]
    depth = mgain.shape[0]

    def at(z_=None, x_=None, y_=None, c_=None, r_=None):
        pick = lambda new, old: old if new is None else new
        return (pick(r_, r), pick(z_, z), pick(x_, x), pick(y_, y), pick(c_, c))

    up = lambda v: lax.rem(v + 1, 4)
    down = lambda v: lax.rem(v + 3, 4)
    far = lambda v: lax.rem(v + 2, 4)

    zr = 4 * r + z
    zu, zd = lax.rem(zr + 1, 8), lax.rem(zr + 7, 8)
    z_up = at(r_=zu // 4, z_=lax.rem(zu, 4))
    z_dn = at(r_=zd // 4, z_=lax.rem(zd, 4))
    x_up, x_dn, x_far = at(x_=up(x)), at(x_=down(x)), at(x_=far(x))
    y_up, y_dn = at(y_=up(y)), at(y_=down(y))
    y_up_mate, y_dn_mate = at(y_=up(y), c_=other), at(y_=down(y), c_=other)
    mate = at(c_=other)
    fs_peers = []
    for i in range(1, 16):
        g = lax.rem(f + i, 16)
        fs_peers.append(at(z_=g // 4, x_=lax.rem(g, 4)))
    near = []
    for i in range(1, 4):
        near += [at(x_=lax.rem(x + i, 4), c_=k) for k in (c, other)]
        near += [at(y_=lax.rem(y + i, 4), c_=other)]

    def along(d, y_=None):
        there = lax.rem(zr + 8 + d, 8)
        return at(r_=there // 4, z_=lax.rem(there, 4), y_=y_)

    for i in range(4):
        for d in (-2, -1, 0, 1, 2):
            if i or d:
                near.append(along(d, lax.rem(y + i, 4)))

    barrier = pltpu.get_barrier_semaphore()
    greet = [mate] + near + fs_peers
    for peer in greet:
        pl.semaphore_signal(barrier, inc=1, device_id=peer, device_id_type=MESH)
    loads = [
        pltpu.make_async_copy(src, dst, lsem.at[i])
        for i, (src, dst) in enumerate(((tok, tokv), (gk, gkv), (vk, vkv)))
    ]
    for copy in loads:
        copy.start()
    pl.semaphore_wait(barrier, len(greet))

    sends, recvs, ends = [0], [0], []

    def new(counter, n=1):
        counter[0] += n
        return counter[0] - n

    def remote(src, dst, s, k, peer):
        return pltpu.make_async_remote_copy(
            src_ref=src, dst_ref=dst, send_sem=ssem.at[s], recv_sem=rsem.at[k],
            device_id=peer, device_id_type=MESH,
        )

    def send(src, dst, s, k, peer):
        remote(src, dst, s, k, peer).start()

    def recv(dst, k):
        remote(dst, dst, 0, k, mate).wait_recv()

    def sender(ref):
        s = new(sends)
        ends.append(lambda: remote(ref, ref, s, 0, mate).wait_send())
        return s

    pieces = [(gp, WGP, 0, 256), (vp, WVP, 0, 256), (mp, WMP, 0, 256)]
    for (at0, n, _), G, V in zip(layout, WGU, WVU):
        pieces += [(gu, G, at0, n), (vu, V, at0, n)]
    for (at0, n, _), W in zip(layout, WDN):
        pieces.append((dn, W, at0, n))
    zk = [new(recvs, 3) for _ in pieces]
    zs = [sender(buf.at[pl.ds(0, 3), pl.ds(0, n)]) for _, buf, _, n in pieces]

    def z_local(i):
        src, buf, at0, n = pieces[i]
        own = buf.at[ring(i)[0], pl.ds(0, n)]
        return pltpu.make_async_copy(src.at[pl.ds(at0, n)], own, lsem.at[3 + i])

    def ring(i):
        return (x, x_up, x_dn) if pieces[i][0] is dn else (z, z_up, z_dn)

    def z_own(i):
        src, buf, at0, n = pieces[i]
        a, b = pl.ds(0, n // 2), pl.ds(n // 2, n // 2)
        from_a, from_b = src.at[pl.ds(at0, n // 2)], src.at[pl.ds(at0 + n // 2, n // 2)]
        place, above, below = ring(i)
        send(from_a, buf.at[place, a], zs[i], zk[i], above)
        send(from_b, buf.at[place, b], zs[i], zk[i] + 1, below)
        send(from_b, buf.at[place, b], zs[i], zk[i] + 2, above)
        send(from_a, buf.at[place, a], zs[i], zk[i] + 2, below)
        z_local(i).start()

    def z_fwd(i):
        _, buf, _, n = pieces[i]
        place, above, below = ring(i)
        a, b = buf.at[down(place), pl.ds(0, n // 2)], buf.at[up(place), pl.ds(n // 2, n // 2)]
        recv(a, zk[i])
        send(a, a, zs[i], zk[i] + 2, above)
        recv(b, zk[i] + 1)
        send(b, b, zs[i], zk[i] + 2, below)

    def z_fin(i):
        _, buf, _, n = pieces[i]
        recv(buf.at[pl.ds(0, 2), pl.ds(0, n)], zk[i] + 2)
        z_local(i).wait()

    def weight(kind, j):
        return {"g": 3 + 2 * j, "v": 4 + 2 * j, "d": 3 + 2 * chunks + j}[kind]

    me = 2 * y + c
    to_me = x // 2 == c
    loads[0].wait()
    kx = new(recvs, 2)
    sx = new(sends)
    for j in range(2):
        for h in range(2):
            xt = 2 * c + j
            ahead = lax.rem(x - xt + 4, 4)
            place = jnp.where(ahead == 0, 2, jnp.where(ahead == 2, 3, ahead // 2))
            mine = jnp.logical_and(xt == x, c == h)
            block = tokv.at[:, j * 256 + h * 128 : j * 256 + h * 128 + 128]

            @pl.when(jnp.logical_not(mine))
            def _():
                dst = XG.at[2 * y + h, place]
                send(block, dst, sx, kx + place // 2, at(x_=xt, c_=jnp.int32(h)))

            @pl.when(mine)
            def _():
                XG[2 * y + h, 2] = block[...]

    def fewer(ref_of, n, wait, stays=to_me):
        @pl.when(stays)
        def _():
            wait(ref_of(n - 1))

        @pl.when(jnp.logical_not(stays))
        def _():
            wait(ref_of(n))

    stay = lambda s: lambda ref: remote(ref, ref, s, 0, mate).wait_send()
    ends.append(lambda: fewer(lambda n: XG.at[0, pl.ds(0, n)], 4, stay(sx)))
    z_own(0)
    z_own(1)
    square = tokv[...].astype(F32)
    square = jnp.sum(square * square, axis=-1, keepdims=True)
    SSB[me] = jnp.broadcast_to(square, (128, 128)).T[0:8, :]
    kss = new(recvs)
    sss = sender(SSB.at[pl.ds(0, 7)])
    for i in range(1, 8):
        t = lax.rem(me + i, 8)
        send(SSB.at[me], SSB.at[me], sss, kss, at(y_=t // 2, c_=lax.rem(t, 2)))

    lo_y, hi_y, far_y = 2 * down(y) + c, 2 * up(y) + c, 2 * far(y) + c

    def y_start(buf, k, s, g):
        a, b = buf.at[me, 2 * g], buf.at[me, 2 * g + 1]
        send(a, a, s, k, y_up)
        send(b, b, s, k + 1, y_dn)
        send(b, b, s, k + 2, y_up)
        send(a, a, s, k + 3, y_dn)
        both = buf.at[me, pl.ds(2 * g, 2)]
        send(both, both, s, k + 6, mate)

    def y_mid(buf, k, s, g):
        a, b = buf.at[lo_y, 2 * g], buf.at[hi_y, 2 * g + 1]
        recv(a, k)
        send(a, a, s, k + 4, y_up)
        send(a, a, s, k + 6, y_up_mate)
        send(a, a, s, k + 6, mate)
        recv(b, k + 1)
        send(b, b, s, k + 5, y_dn)
        send(b, b, s, k + 6, y_dn_mate)
        send(b, b, s, k + 6, mate)

    def y_end(buf, k, s, g):
        rows = (buf.at[lo_y, 2 * g + 1], buf.at[hi_y, 2 * g], buf.at[far_y, 2 * g], buf.at[far_y, 2 * g + 1])
        for i, ref in enumerate(rows):
            recv(ref, k + 2 + i)
            if i < 2:
                send(ref, ref, s, k + 6, mate)

    def y_last(buf, k):
        recv(buf.at[pl.ds(0, 4), pl.ds(0, 2)], k + 6)

    def scaled(buf, gains, squares, first, n):
        parts = [gains[pl.ds(pl.multiple_of((4 * k + x) * 256, 256), 256)] for k in range(4)]
        gain = jnp.concatenate([part.reshape(1, 256) for part in parts], axis=1)

        def block(b, _):
            rows = jnp.concatenate([buf[i, b] for i in range(8)], axis=1).astype(F32)
            if squares:
                total = jnp.sum(rows * rows, axis=-1, keepdims=True)
                SQR[b] = jnp.broadcast_to(total, (128, 128)).T[0:8, :]
            XS[pl.ds(pl.multiple_of(b * 128, 128), 128), :] = (rows * gain).astype(BF16)
            return 0

        lax.fori_loop(first, first + n, block, 0)

    def scale_of(rows):
        return lax.rsqrt(jnp.broadcast_to(rows, (128, 128)).T / depth + EPS)

    ky = [new(recvs, 7) for _ in range(2)]
    sy = [sender(buf.at[pl.ds(0, 7), pl.ds(0, 2)]) for buf in (XG, XG)]
    recv(XG.at[me, pl.ds(0, 2)], kx)
    y_start(XG, ky[0], sy[0], 0)
    fewer(lambda n: XG.at[me, pl.ds(0, n)], 2, lambda ref: recv(ref, kx + 1))
    y_start(XG, ky[1], sy[1], 1)
    km = new(recvs)
    sm = sender(SM.at[pl.ds(0, 15)])
    for i in range(15):
        send(smix, SM.at[f], sm, km, fs_peers[i])
    SM[f] = smix[...]
    last0, lastn, wide = layout[-1]
    for W in (WGU[-1], WVU[-1], WDN[-1]):
        for k in range(4):
            W[k, lastn:, :] = jnp.zeros((wide - lastn, 256), BF16)
    z_own(9)
    z_own(11)
    z_fwd(0)
    z_fwd(1)
    z_own(2)
    z_own(3)
    y_mid(XG, ky[0], sy[0], 0)
    y_mid(XG, ky[1], sy[1], 1)
    loads[1].wait()
    loads[2].wait()
    for w, kern, off in ((0, gkv, go), (1, vkv, vo)):
        CV[w, :, last0:] = jnp.zeros((4, wide), F32)
        CV[w, 0:3, 0:units] = kern[...]
        CV[w, 3:4, 0:units] = off[...].reshape(1, units)
    y_end(XG, ky[0], sy[0], 0)
    y_end(XG, ky[1], sy[1], 1)
    y_last(XG, ky[0])
    y_last(XG, ky[1])
    scaled(XG, mgain, False, 0, 4)
    z_fin(0)
    z_fin(1)
    for w, W in ((0, WGP), (1, WVP)):
        prod = jnp.dot(XS[...], W[...].reshape(1024, 256), preferred_element_type=F32)
        P1[:, :, w * 256 : w * 256 + 256] = prod.reshape(4, 128, 256)

    def row_loop(first, n, fn):
        def step(i, _):
            fn(pl.ds(pl.multiple_of(first + i * 16, 16), 16))
            return 0

        lax.fori_loop(0, n // 16, step, 0)

    ra, rb = pl.ds(0, 64), pl.ds(64, 64)

    def rounded_rows(p, i, S, k, first, n, cols):
        def fn(rows):
            S[k, rows, cols] = p[i, rows, cols].astype(BF16)

        row_loop(first, n, fn)

    def rs_far(p, S, H, F, k, s, cols=slice(None)):
        rounded_rows(p, 3, S, 0, 0, 128, cols)
        send(S.at[0, ra, cols], H.at[0, :, cols], s, k, x_up)
        send(S.at[0, rb, cols], H.at[1, :, cols], s, k + 1, x_dn)

    def rs_first(p, S, H, F, k, s, cols=slice(None)):
        rounded_rows(p, 0, S, 1, 64, 64, cols)
        send(S.at[1, rb, cols], F.at[0, rb, cols], s, k + 2, x_up)
        rounded_rows(p, 1, S, 2, 0, 64, cols)
        send(S.at[2, ra, cols], F.at[1, ra, cols], s, k + 2, x_dn)

    def rs_second(p, S, H, F, k, s):
        def left(rows):
            S[1, rows, :] = (p[0, rows, :] + H[0, rows, :].astype(F32)).astype(BF16)

        def right(rows):
            low = pl.ds(pl.multiple_of(rows.start + 64, 16), 16)
            S[2, low, :] = (p[1, low, :] + H[1, rows, :].astype(F32)).astype(BF16)

        recv(H.at[0], k)
        row_loop(0, 64, left)
        send(S.at[1, ra], F.at[0, ra], s, k + 2, x_up)
        recv(H.at[1], k + 1)
        row_loop(0, 64, right)
        send(S.at[2, rb], F.at[1, rb], s, k + 2, x_dn)

    def rs_wait(F, k):
        recv(F, k + 2)

    kr = [new(recvs, 3) for _ in layout]
    set1 = (P1, S1, H1, F1, kr[0], sender(S1))
    rs_far(*set1)
    rs_first(*set1)
    z_fwd(2)
    z_own(4)
    rs_second(*set1)
    z_fwd(3)
    z_own(5)
    recv(SM.at[pl.ds(0, 15)], km)
    recv(SSB.at[pl.ds(0, 7)], kss)
    rs_wait(F1, kr[0])

    total = P1[2] + F1[0].astype(F32) + F1[1].astype(F32)
    rs = scale_of(jnp.sum(SSB[...], axis=0)[0:1, :])
    eye = lax.broadcasted_iota(jnp.int32, (128, 128), 0) == lanes_of(128)
    for h in range(2):
        cols = slice(h * 128, h * 128 + 128)
        gated = gelu((rs * total[:, cols]).astype(BF16).astype(F32))
        spread = gelu((rs * total[:, 256 + h * 128 : 384 + h * 128]).astype(BF16).astype(F32))
        spread = spread * lax.rsqrt(jnp.mean(spread * spread, axis=-1, keepdims=True) + EPS)
        spread = (spread * vgain[h : h + 1, :]).astype(BF16)
        matrix = SM[:, h].astype(F32).reshape(128, 128).astype(BF16)
        mixed = jnp.dot(matrix, spread, preferred_element_type=F32)
        bias = jnp.broadcast_to(sbias[h : h + 1, :], (128, 128))
        mixed = mixed + jnp.sum(jnp.where(eye, bias, 0.0), axis=-1, keepdims=True)
        joined = gated * mixed
        joined = joined * lax.rsqrt(jnp.mean(joined * joined, axis=-1, keepdims=True) + EPS)
        MG[2, :, cols] = (joined * hgain[h : h + 1, :]).astype(BF16)

    k2 = new(recvs, 3)
    s2 = sender(MG.at[pl.ds(0, 3)])
    send(MG.at[2], MG.at[1], s2, k2 + 1, x_up)
    send(MG.at[2], MG.at[0], s2, k2 + 2, x_dn)
    send(MG.at[2], MG.at[3], s2, k2, x_far)
    z_fin(2)

    y_order = (far(y), up(y), down(y), y)

    def cy_first(g, product, CS, CR, k, s):
        for n, yt in enumerate(y_order):
            prod = product(yt)
            size = prod.shape[0] // 128
            rows = pl.ds(2 * g, size)
            T[n, rows] = jnp.where(c == 0, prod[:, :128], prod[:, 128:]).reshape(size, 128, 128)
            give = jnp.where(c == 0, prod[:, 128:], prod[:, :128]).astype(BF16)
            CS[n, rows] = give.reshape(size, 128, 128)
            send(CS.at[n, rows], CR.at[n, rows], s, k + n, mate)

    def joined_at(n, b, CR):
        return T[n, b] + CR[n, b].astype(F32)

    def cy_second(g, CR, YS, YH, YF, k, kc, s):
        a, b = 2 * g, 2 * g + 1
        recv(CR.at[0, pl.ds(a, 2)], kc)
        YS[0, a] = joined_at(0, a, CR).astype(BF16)
        YS[0, b] = joined_at(0, b, CR).astype(BF16)
        send(YS.at[0, a], YH.at[a], s, k, y_up)
        send(YS.at[0, b], YH.at[b], s, k + 1, y_dn)
        recv(CR.at[1, pl.ds(a, 2)], kc + 1)
        YS[1, b] = joined_at(1, b, CR).astype(BF16)
        send(YS.at[1, b], YF.at[g, 0, 1], s, k + 2, y_up)
        recv(CR.at[2, pl.ds(a, 2)], kc + 2)
        YS[2, a] = joined_at(2, a, CR).astype(BF16)
        send(YS.at[2, a], YF.at[g, 1, 0], s, k + 2, y_dn)

    def cy_third(g, CR, YS, YH, YF, k, kc, s):
        a, b = 2 * g, 2 * g + 1
        recv(YH.at[a], k)
        YS[1, a] = (joined_at(1, a, CR) + YH[a].astype(F32)).astype(BF16)
        send(YS.at[1, a], YF.at[g, 0, 0], s, k + 2, y_up)
        recv(YH.at[b], k + 1)
        YS[2, b] = (joined_at(2, b, CR) + YH[b].astype(F32)).astype(BF16)
        send(YS.at[2, b], YF.at[g, 1, 1], s, k + 2, y_dn)
        recv(CR.at[3, pl.ds(a, 2)], kc + 3)

    def cy_last(g, CR, YF, k):
        recv(YF.at[g], k + 2)
        return [
            joined_at(3, 2 * g + i, CR) + YF[g, 0, i].astype(F32) + YF[g, 1, i].astype(F32)
            for i in range(2)
        ]

    def merge(g):
        rows = MG[2 * g : 2 * g + 2].reshape(256, 256)
        return lambda yt: jnp.dot(rows, WMP[yt], preferred_element_type=F32)

    kc = [new(recvs, 4) for _ in range(2)]
    k3 = [new(recvs, 3) for _ in range(2)]
    sc, s3 = sender(CS4), sender(YS4)
    recv(MG.at[0], k2 + 2)
    recv(MG.at[1], k2 + 1)
    cy_first(0, merge(0), CS4, CR4, kc[0], sc)
    cy_second(0, CR4, YS4, YH4, YF4, k3[0], kc[0], s3)
    recv(MG.at[3], k2)
    z_own(10)
    z_fwd(9)
    z_fwd(11)
    cy_first(1, merge(1), CS4, CR4, kc[1], sc)
    cy_second(1, CR4, YS4, YH4, YF4, k3[1], kc[1], s3)
    z_fwd(4)
    z_own(6)
    cy_third(0, CR4, YS4, YH4, YF4, k3[0], kc[0], s3)
    cy_third(1, CR4, YS4, YH4, YF4, k3[1], kc[1], s3)


    ko = new(recvs)
    so = new(sends)
    ends.append(lambda: fewer(lambda n: HG.at[0, pl.ds(0, n)], 4, stay(so)))
    spot = 2 * lax.rem(x, 2) + c
    blocks = (up(x), down(x), x, far(x))
    sh = [sender(buf.at[pl.ds(0, 7), pl.ds(0, 2)]) for buf in (HG, HG)]
    for g in range(2):
        branch = cy_last(g, CR4, YF4, k3[g])
        for i in range(2):
            b = 2 * g + i
            HG[me, b] = (XG[me, b].astype(F32) + branch[i]).astype(BF16)
        y_start(HG, ky[g], sh[g], g)
    for b in range(4):
        if b != 2:
            dst = HRES.at[spot]
            send(HG.at[me, b], dst, so, ko, at(x_=blocks[b], c_=x // 2))
            continue

        @pl.when(to_me)
        def _():
            HRES[spot] = HG[me, 2]

        @pl.when(jnp.logical_not(to_me))
        def _():
            send(HG.at[me, 2], HRES.at[spot], so, ko, mate)

    z_fwd(5)
    y_mid(HG, ky[0], sh[0], 0)
    y_mid(HG, ky[1], sh[1], 1)
    y_end(HG, ky[0], sh[0], 0)
    z_fwd(6)
    z_own(7)
    z_own(8)
    z_fwd(10)
    y_end(HG, ky[1], sh[1], 1)
    z_fin(weight("g", 0))
    z_fin(weight("v", 0))
    y_last(HG, ky[0])
    scaled(HG, fgain, True, 0, 2)

    def project(W, p, n, first, b0, b1):
        def cut(cols, to, size):
            w = jnp.concatenate([W[k, cols, :] for k in range(4)], axis=1)
            prod = lax.dot_general(
                XS[b0 * 128 : b1 * 128, :], w, (((1,), (1,)), ((), ())),
                preferred_element_type=F32,
            )
            p[b0:b1, :, to] = prod.reshape(b1 - b0, 128, size)

        def step(i, _):
            cut(
                pl.ds(pl.multiple_of(i * 256, 256), 256),
                pl.ds(pl.multiple_of(first + i * 256, 128), 256), 256,
            )
            return 0

        lax.fori_loop(0, n // 256, step, 0)
        left = n % 256
        if left:
            cut(pl.ds(n - left, left), pl.ds(first + n - left, left), left)

    def gates(j):
        n = layout[j][2]
        z_fin(weight("g", j))
        project(WGU[j], PC[j], n, 0, 0, 4)
        return slice(0, n)

    def values(j):
        n = layout[j][2]
        z_fin(weight("v", j))
        project(WVU[j], PC[j], n, n, 0, 4)
        return slice(n, 2 * n)

    row = lax.broadcasted_iota(jnp.int32, (128, 128), 0)

    def activate(j):
        p, F, act = PC[j], FC[j], ACT[j]
        at0, _, n = layout[j]

        def conv_tile(i, _):
            def one(first, w):
                at_ = pl.ds(pl.multiple_of(first + i * 128, 128), 128)
                v = p[2, :, at_] + F[0, :, at_].astype(F32) + F[1, :, at_].astype(F32)
                v = (RS[...] * v).astype(BF16).astype(F32)
                prev = jnp.where(row == 0, 0.0, pltpu.roll(v, 1, axis=0))
                after = jnp.where(row == 127, 0.0, pltpu.roll(v, 127, axis=0))
                k = CV[w, :, pl.ds(pl.multiple_of(at0 + i * 128, 128), 128)]
                return k[3:4] + prev * k[0:1] + v * k[1:2] + after * k[2:3]

            cols = pl.ds(pl.multiple_of(i * 128, 128), 128)
            act[2, :, cols] = (gelu(one(0, 0)) * one(n, 1)).astype(BF16)
            return 0

        lax.fori_loop(0, n // 128, conv_tile, 0)

    sets = [
        (PC[j], SC[j], HC[j], FC[j], kr[j], sender(SC[j])) for j in range(chunks)
    ]
    kg = [new(recvs, 4) for _ in layout]
    sg = [sender(ACT[j].at[pl.ds(0, 3)]) for j in range(chunks)]

    def x_start(j):
        buf, k, s = ACT[j], kg[j], sg[j]
        send(buf.at[2, ra], buf.at[1, ra], s, k, z_up)
        send(buf.at[2, rb], buf.at[0, rb], s, k + 1, z_dn)
        send(buf.at[2, rb], buf.at[1, rb], s, k + 2, z_up)
        send(buf.at[2, ra], buf.at[0, ra], s, k + 2, z_dn)

    def x_mid(j):
        buf, k, s = ACT[j], kg[j], sg[j]
        recv(buf.at[1, ra], k)
        send(buf.at[1, ra], buf.at[3, ra], s, k + 3, z_up)
        recv(buf.at[0, rb], k + 1)
        send(buf.at[0, rb], buf.at[3, rb], s, k + 3, z_dn)

    def x_near(j):
        recv(ACT[j].at[0], kg[j] + 2)

    def x_last(j):
        recv(ACT[j].at[3], kg[j] + 3)

    def down_rows(j, b0, b1):
        n = layout[j][2]
        rows = ACT[j][b0:b1].reshape((b1 - b0) * 128, n)
        return lambda k: jnp.dot(rows, WDN[j][k], preferred_element_type=F32)

    def down_early(j):
        product = down_rows(j, 0, 4)

        def step(k, _):
            prod = product(k).reshape(4, 128, 256)
            ACC[k] = prod if j == 0 else ACC[k] + prod
            return 0

        lax.fori_loop(0, 4, step, 0)

    n0 = layout[0][2]
    one0, two0 = slice(0, n0), slice(n0, 2 * n0)
    project(WGU[0], PC[0], n0, 0, 0, 2)
    rs_first(*sets[0], one0)
    project(WVU[0], PC[0], n0, n0, 0, 2)
    rs_first(*sets[0], two0)
    y_last(HG, ky[1])
    scaled(HG, fgain, True, 2, 2)
    project(WGU[0], PC[0], n0, 0, 2, 4)
    rs_far(*sets[0], one0)
    project(WVU[0], PC[0], n0, n0, 2, 4)
    rs_far(*sets[0], two0)
    kf = new(recvs)
    sf = sender(SSF.at[pl.ds(0, 3)])
    SSF[2] = SQR[2]
    send(SQR.at[0], SSF.at[1], sf, kf, x_up)
    send(SQR.at[1], SSF.at[0], sf, kf, x_dn)
    send(SQR.at[3], SSF.at[3], sf, kf, x_far)
    one1 = gates(1)
    rs_far(*sets[1], one1)
    two1 = values(1)
    rs_far(*sets[1], two1)
    rs_first(*sets[1], one1)
    rs_second(*sets[0])
    rs_first(*sets[1], two1)
    z_fwd(7)
    z_fwd(8)
    rs_second(*sets[1])
    recv(SSF.at[pl.ds(0, 3)], kf)
    RS[...] = scale_of(jnp.sum(SSF[...], axis=0)[0:1, :])
    rs_wait(FC[0], kr[0])
    activate(0)
    x_start(0)
    one2 = gates(2)
    rs_far(*sets[2], one2)
    two2 = values(2)
    rs_far(*sets[2], two2)
    rs_first(*sets[2])
    rs_wait(FC[1], kr[1])
    activate(1)
    x_start(1)
    x_mid(0)
    rs_second(*sets[2])
    x_mid(1)
    x_near(0)
    x_last(0)
    z_fin(9)
    down_early(0)
    rs_wait(FC[2], kr[2])
    activate(2)
    x_start(2)
    x_near(1)
    x_last(1)
    z_fin(10)
    z_fin(11)
    down_early(1)

    k7 = [new(recvs, 2) for _ in range(3)]
    s7 = sender(CS5)
    kt = new(recvs)
    st = new(sends)
    stays = y == z
    ends.append(lambda: fewer(lambda n: TB.at[pl.ds(0, n)], 4, stay(st), stays))

    def give(b):
        for i in range(2):
            TB[b, :, i * 256 : i * 256 + 256] = (T5[i, b] + CR5[i, b].astype(F32)).astype(BF16)
        if b < 2:
            send(TB.at[b], TI.at[y], st, kt, along(1 - 2 * b, z))
        elif b == 3:
            send(TB.at[b, ra], TI.at[y, ra], st, kt, along(-2, z))
            send(TB.at[b, rb], TI.at[y, rb], st, kt, along(2, z))
        else:

            @pl.when(stays)
            def _():
                TI[y] = TB[b]

            @pl.when(jnp.logical_not(stays))
            def _():
                send(TB.at[b], TI.at[y], st, kt, at(y_=z))

    parts = ((2, 3), (0, 2), (3, 4))

    def finish(g):
        b0, b1 = parts[g]
        rows = pl.ds(b0, b1 - b0)
        product = down_rows(2, b0, b1)

        def final(k):
            return product(k).reshape(b1 - b0, 128, 256) + ACC[k, rows]

        for i in range(2):
            CS5[i, rows] = final(2 * other + i).astype(BF16)
            send(CS5.at[i, rows], CR5.at[i, rows], s7, k7[g] + i, mate)
        for i in range(2):
            T5[i, rows] = final(2 * c + i)

    def hand_over(g):
        b0, b1 = parts[g]
        for i in range(2):
            recv(CR5.at[i, pl.ds(b0, b1 - b0)], k7[g] + i)
        for b in range(b0, b1):
            give(b)

    finish(0)
    x_mid(2)
    hand_over(0)
    x_near(2)
    finish(1)
    hand_over(1)
    x_last(2)
    finish(2)
    hand_over(2)

    fewer(lambda n: HRES.at[pl.ds(0, n)], 4, lambda ref: recv(ref, ko))
    fewer(lambda n: TI.at[pl.ds(0, n)], 4, lambda ref: recv(ref, kt), stays)
    for q in range(4):
        cols = slice(q * 128, q * 128 + 128)
        change = sum(TI[n, :, cols].astype(F32) for n in range(4))
        out[:, cols] = (HRES[q].astype(F32) + change).astype(BF16)
    for wait in ends:
        wait()
    assert sends[0] <= ssem.shape[0] and recvs[0] <= rsem.shape[0], (sends[0], recvs[0])


def body(
    tokens, mixer_gain, gate_proj, value_proj, value_gain, spatial_mix, spatial_bias,
    head_gain, merge_proj, ffn_gain, gate_up, value_up, gate_kernel, value_kernel,
    gate_offset, value_offset, down_proj,
):
    units = gate_up.shape[1]
    layout = []
    for first in range(0, units, CHUNK):
        n = min(CHUNK, units - first)
        layout.append((first, n, -(-n // 128) * 128))
    wide = sum(n for _, _, n in layout)
    widths = [n for _, _, n in layout]
    vm = lambda shape, dtype=BF16: pltpu.VMEM(shape, dtype)
    in_vmem = pl.BlockSpec(memory_space=pltpu.VMEM)
    left = pl.BlockSpec(memory_space=pl.ANY)
    call = pl.pallas_call(
        functools.partial(kernel, layout),
        out_shape=jax.ShapeDtypeStruct(tokens.shape, tokens.dtype),
        in_specs=[
            left, in_vmem, in_vmem, left, left, in_vmem, in_vmem, in_vmem, in_vmem, left,
            left, left, left, left, in_vmem, in_vmem, left,
        ],
        out_specs=in_vmem,
        scratch_shapes=[
            vm(tokens.shape), vm(gate_kernel.shape, F32), vm(gate_kernel.shape, F32),
            vm((2, 4, wide), F32),
            vm((8, 4, 128, 128)), vm((8, 4, 128, 128)), vm((512, 1024)),
            vm((4, 8, 128), F32), vm((128, 128), F32), vm((16, 2, 8, 128)),
            vm((4, 128, 256)), vm((8, 8, 128), F32), vm((4, 8, 128), F32), vm((4, 128, 128)),
            vm((4, 128, 512)), vm((4, 128, 512)),
            *[vm((4, 256, 256))] * 3, vm((4, 4, 128, 128), F32), vm((4, 4, 128, 256), F32),
            vm((4, 128, 512), F32), vm((3, 128, 512)), vm((2, 64, 512)), vm((2, 128, 512)),
            vm((4, 4, 128, 128)), vm((4, 4, 128, 128)), vm((3, 4, 128, 128)),
            vm((4, 128, 128)), vm((2, 2, 2, 128, 128)),
            vm((2, 4, 128, 256)), vm((2, 4, 128, 256)), vm((2, 4, 128, 256), F32),
            *[vm((4, n, 256)) for _ in range(3) for n in widths],
            *[vm((4, 128, n)) for n in widths],
            *[vm((4, 128, 2 * n), F32) for n in widths],
            *[vm((3, 128, 2 * n)) for n in widths],
            *[vm((2, 64, 2 * n)) for n in widths],
            *[vm((2, 128, 2 * n)) for n in widths],
            pltpu.SemaphoreType.DMA((SENDS,)), pltpu.SemaphoreType.DMA((RECVS,)),
            pltpu.SemaphoreType.DMA((6 + 3 * len(layout),)),
        ],
        compiler_params=pltpu.CompilerParams(
            collective_id=0, has_side_effects=True, vmem_limit_bytes=58 << 20
        ),
        name="layer",
    )
    return call(
        tokens, mixer_gain, ffn_gain, gate_proj, value_proj, value_gain, spatial_mix,
        spatial_bias, head_gain, merge_proj, gate_up.T, value_up.T, gate_kernel, value_kernel,
        gate_offset, value_offset, down_proj,
    )


def solution(mesh):
    finer = Mesh(
        mesh.devices.reshape(mesh.shape["rep"], 4, 4, 4, 2), ("rep", "fs_0", "fs_1", "tp_0", "tp_1")
    )
    return jax.shard_map(
        body,
        mesh=finer,
        in_specs=(
            P(REP_FS, TP), P(), P(FS, TP), P(FS, TP), P(TP, None), P(TP, FS, None),
            P(TP, None), P(TP, None), P(TP, FS), P(), P(FS, TP), P(FS, TP), P(None, TP),
            P(None, TP), P(TP), P(TP), P(TP, FS),
        ),
        out_specs=P(REP_FS, TP),
        check_vma=False,
    )
```

```python
import functools

import jax
import jax.numpy as jnp
from jax import lax
from jax.experimental import pallas as pl
from jax.experimental.pallas import tpu as pltpu
from jax.sharding import Mesh
from jax.sharding import PartitionSpec as P

TP = ("tp_0", "tp_1")
FS = ("fs_0", "fs_1")
REP_FS = ("rep", "fs_0", "fs_1")
MESH = pl.DeviceIdType.MESH
EPS = 1e-06
SENDS, RECVS = 33, 105
CHUNK = 512
F32 = jnp.float32
BF16 = jnp.bfloat16


def gelu(v):
    return 0.5 * v * (1.0 + lax.erf(v * 0.7071067811865476))


def lanes_of(n):
    return lax.broadcasted_iota(jnp.int32, (n, 128), 1)


def kernel(layout, tok, mgain, fgain, gp, vp, vgain, smix, sbias, hgain, mp, gu, vu, gk, vk, go, vo,
           dn, out, tokv, gkv, vkv, CV, XG, HG, XS, SQR, RS, SM, MG, SSB, SSF, HRES, TB, TI,
           WGP, WVP, WMP, T, ACC, P1, S1, H1, F1, CS4, CR4, YS4, YH4, YF4, CS5, CR5, T5, *rest):
    chunks = len(layout)
    WGU, WVU, WDN, ACT, PC, SC, HC, FC = (rest[i * chunks : (i + 1) * chunks] for i in range(8))
    ssem, rsem, lsem = rest[8 * chunks :]
    r, z, x, y, c = (lax.axis_index(a) for a in ("rep", "fs_0", "fs_1", "tp_0", "tp_1"))
    other = 1 - c
    f = 4 * z + x
    units = dn.shape[0]
    depth = mgain.shape[0]

    def at(z_=None, x_=None, y_=None, c_=None, r_=None):
        pick = lambda new, old: old if new is None else new
        return (pick(r_, r), pick(z_, z), pick(x_, x), pick(y_, y), pick(c_, c))

    up = lambda v: lax.rem(v + 1, 4)
    down = lambda v: lax.rem(v + 3, 4)
    far = lambda v: lax.rem(v + 2, 4)

    zr = 4 * r + z
    zu, zd = lax.rem(zr + 1, 8), lax.rem(zr + 7, 8)
    z_up = at(r_=zu // 4, z_=lax.rem(zu, 4))
    z_dn = at(r_=zd // 4, z_=lax.rem(zd, 4))
    x_up, x_dn, x_far = at(x_=up(x)), at(x_=down(x)), at(x_=far(x))
    y_up, y_dn = at(y_=up(y)), at(y_=down(y))
    y_up_mate, y_dn_mate = at(y_=up(y), c_=other), at(y_=down(y), c_=other)
    mate = at(c_=other)
    fs_peers = []
    for i in range(1, 16):
        g = lax.rem(f + i, 16)
        fs_peers.append(at(z_=g // 4, x_=lax.rem(g, 4)))
    near = []
    for i in range(1, 4):
        near += [at(x_=lax.rem(x + i, 4), c_=k) for k in (c, other)]
        near += [at(y_=lax.rem(y + i, 4), c_=other)]

    def along(d, y_=None):
        there = lax.rem(zr + 8 + d, 8)
        return at(r_=there // 4, z_=lax.rem(there, 4), y_=y_)

    for i in range(4):
        for d in (-2, -1, 0, 1, 2):
            if i or d:
                near.append(along(d, lax.rem(y + i, 4)))

    barrier = pltpu.get_barrier_semaphore()
    greet = [mate] + near + fs_peers
    for peer in greet:
        pl.semaphore_signal(barrier, inc=1, device_id=peer, device_id_type=MESH)
    loads = [
        pltpu.make_async_copy(src, dst, lsem.at[i])
        for i, (src, dst) in enumerate(((tok, tokv), (gk, gkv), (vk, vkv)))
    ]
    for copy in loads:
        copy.start()
    pl.semaphore_wait(barrier, len(greet))

    sends, recvs, ends = [0], [0], []

    def new(counter, n=1):
        counter[0] += n
        return counter[0] - n

    def remote(src, dst, s, k, peer):
        return pltpu.make_async_remote_copy(
            src_ref=src, dst_ref=dst, send_sem=ssem.at[s], recv_sem=rsem.at[k],
            device_id=peer, device_id_type=MESH,
        )

    def send(src, dst, s, k, peer):
        remote(src, dst, s, k, peer).start()

    def recv(dst, k):
        remote(dst, dst, 0, k, mate).wait_recv()

    def sender(ref):
        s = new(sends)
        ends.append(lambda: remote(ref, ref, s, 0, mate).wait_send())
        return s

    pieces = [(gp, WGP, 0, 256), (vp, WVP, 0, 256), (mp, WMP, 0, 256)]
    for (at0, n, _), G, V in zip(layout, WGU, WVU):
        pieces += [(gu, G, at0, n), (vu, V, at0, n)]
    for (at0, n, _), W in zip(layout, WDN):
        pieces.append((dn, W, at0, n))
    zk = [new(recvs, 3) for _ in pieces]
    zs = [sender(buf.at[pl.ds(0, 3), pl.ds(0, n)]) for _, buf, _, n in pieces]

    def z_local(i):
        src, buf, at0, n = pieces[i]
        own = buf.at[ring(i)[0], pl.ds(0, n)]
        return pltpu.make_async_copy(src.at[pl.ds(at0, n)], own, lsem.at[3 + i])

    def ring(i):
        return (x, x_up, x_dn) if pieces[i][0] is dn else (z, z_up, z_dn)

    def z_own(i):
        src, buf, at0, n = pieces[i]
        a, b = pl.ds(0, n // 2), pl.ds(n // 2, n // 2)
        from_a, from_b = src.at[pl.ds(at0, n // 2)], src.at[pl.ds(at0 + n // 2, n // 2)]
        place, above, below = ring(i)
        send(from_a, buf.at[place, a], zs[i], zk[i], above)
        send(from_b, buf.at[place, b], zs[i], zk[i] + 1, below)
        send(from_b, buf.at[place, b], zs[i], zk[i] + 2, above)
        send(from_a, buf.at[place, a], zs[i], zk[i] + 2, below)
        z_local(i).start()

    def z_fwd(i):
        _, buf, _, n = pieces[i]
        place, above, below = ring(i)
        a, b = buf.at[down(place), pl.ds(0, n // 2)], buf.at[up(place), pl.ds(n // 2, n // 2)]
        recv(a, zk[i])
        send(a, a, zs[i], zk[i] + 2, above)
        recv(b, zk[i] + 1)
        send(b, b, zs[i], zk[i] + 2, below)

    def z_fin(i):
        _, buf, _, n = pieces[i]
        recv(buf.at[pl.ds(0, 2), pl.ds(0, n)], zk[i] + 2)
        z_local(i).wait()

    def weight(kind, j):
        return {"g": 3 + 2 * j, "v": 4 + 2 * j, "d": 3 + 2 * chunks + j}[kind]

    me = 2 * y + c
    to_me = x // 2 == c
    loads[0].wait()
    kx = new(recvs, 2)
    sx = new(sends)
    for j in range(2):
        for h in range(2):
            xt = 2 * c + j
            ahead = lax.rem(x - xt + 4, 4)
            place = jnp.where(ahead == 0, 2, jnp.where(ahead == 2, 3, ahead // 2))
            mine = jnp.logical_and(xt == x, c == h)
            block = tokv.at[:, j * 256 + h * 128 : j * 256 + h * 128 + 128]

            @pl.when(jnp.logical_not(mine))
            def _():
                dst = XG.at[2 * y + h, place]
                send(block, dst, sx, kx + place // 2, at(x_=xt, c_=jnp.int32(h)))

            @pl.when(mine)
            def _():
                XG[2 * y + h, 2] = block[...]

    def fewer(ref_of, n, wait, stays=to_me):
        @pl.when(stays)
        def _():
            wait(ref_of(n - 1))

        @pl.when(jnp.logical_not(stays))
        def _():
            wait(ref_of(n))

    stay = lambda s: lambda ref: remote(ref, ref, s, 0, mate).wait_send()
    ends.append(lambda: fewer(lambda n: XG.at[0, pl.ds(0, n)], 4, stay(sx)))
    z_own(0)
    z_own(1)
    square = tokv[...].astype(F32)
    square = jnp.sum(square * square, axis=-1, keepdims=True)
    SSB[me] = jnp.broadcast_to(square, (128, 128)).T[0:8, :]
    kss = new(recvs)
    sss = sender(SSB.at[pl.ds(0, 7)])
    for i in range(1, 8):
        t = lax.rem(me + i, 8)
        send(SSB.at[me], SSB.at[me], sss, kss, at(y_=t // 2, c_=lax.rem(t, 2)))

    lo_y, hi_y, far_y = 2 * down(y) + c, 2 * up(y) + c, 2 * far(y) + c

    def y_start(buf, k, s, g):
        a, b = buf.at[me, 2 * g], buf.at[me, 2 * g + 1]
        send(a, a, s, k, y_up)
        send(b, b, s, k + 1, y_dn)
        send(b, b, s, k + 2, y_up)
        send(a, a, s, k + 3, y_dn)
        both = buf.at[me, pl.ds(2 * g, 2)]
        send(both, both, s, k + 6, mate)

    def y_mid(buf, k, s, g):
        a, b = buf.at[lo_y, 2 * g], buf.at[hi_y, 2 * g + 1]
        recv(a, k)
        send(a, a, s, k + 4, y_up)
        send(a, a, s, k + 6, y_up_mate)
        send(a, a, s, k + 6, mate)
        recv(b, k + 1)
        send(b, b, s, k + 5, y_dn)
        send(b, b, s, k + 6, y_dn_mate)
        send(b, b, s, k + 6, mate)

    def y_end(buf, k, s, g):
        rows = (buf.at[lo_y, 2 * g + 1], buf.at[hi_y, 2 * g], buf.at[far_y, 2 * g], buf.at[far_y, 2 * g + 1])
        for i, ref in enumerate(rows):
            recv(ref, k + 2 + i)
            if i < 2:
                send(ref, ref, s, k + 6, mate)

    def y_last(buf, k):
        recv(buf.at[pl.ds(0, 4), pl.ds(0, 2)], k + 6)

    def scaled(buf, gains, squares, first, n):
        parts = [gains[pl.ds(pl.multiple_of((4 * k + x) * 256, 256), 256)] for k in range(4)]
        gain = jnp.concatenate([part.reshape(1, 256) for part in parts], axis=1)

        def block(b, _):
            rows = jnp.concatenate([buf[i, b] for i in range(8)], axis=1).astype(F32)
            if squares:
                total = jnp.sum(rows * rows, axis=-1, keepdims=True)
                SQR[b] = jnp.broadcast_to(total, (128, 128)).T[0:8, :]
            XS[pl.ds(pl.multiple_of(b * 128, 128), 128), :] = (rows * gain).astype(BF16)
            return 0

        lax.fori_loop(first, first + n, block, 0)

    def scale_of(rows):
        return lax.rsqrt(jnp.broadcast_to(rows, (128, 128)).T / depth + EPS)

    ky = [new(recvs, 7) for _ in range(2)]
    sy = [sender(buf.at[pl.ds(0, 7), pl.ds(0, 2)]) for buf in (XG, XG)]
    recv(XG.at[me, pl.ds(0, 2)], kx)
    y_start(XG, ky[0], sy[0], 0)
    fewer(lambda n: XG.at[me, pl.ds(0, n)], 2, lambda ref: recv(ref, kx + 1))
    y_start(XG, ky[1], sy[1], 1)
    km = new(recvs)
    sm = sender(SM.at[pl.ds(0, 15)])
    for i in range(15):
        send(smix, SM.at[f], sm, km, fs_peers[i])
    SM[f] = smix[...]
    last0, lastn, wide = layout[-1]
    for W in (WGU[-1], WVU[-1], WDN[-1]):
        for k in range(4):
            W[k, lastn:, :] = jnp.zeros((wide - lastn, 256), BF16)
    z_own(9)
    z_own(11)
    z_fwd(0)
    z_fwd(1)
    z_own(2)
    z_own(3)
    y_mid(XG, ky[0], sy[0], 0)
    y_mid(XG, ky[1], sy[1], 1)
    loads[1].wait()
    loads[2].wait()
    for w, kern, off in ((0, gkv, go), (1, vkv, vo)):
        CV[w, :, last0:] = jnp.zeros((4, wide), F32)
        CV[w, 0:3, 0:units] = kern[...]
        CV[w, 3:4, 0:units] = off[...].reshape(1, units)
    y_end(XG, ky[0], sy[0], 0)
    y_end(XG, ky[1], sy[1], 1)
    y_last(XG, ky[0])
    y_last(XG, ky[1])
    scaled(XG, mgain, False, 0, 4)
    z_fin(0)
    z_fin(1)
    for w, W in ((0, WGP), (1, WVP)):
        prod = jnp.dot(XS[...], W[...].reshape(1024, 256), preferred_element_type=F32)
        P1[:, :, w * 256 : w * 256 + 256] = prod.reshape(4, 128, 256)

    def row_loop(first, n, fn):
        def step(i, _):
            fn(pl.ds(pl.multiple_of(first + i * 16, 16), 16))
            return 0

        lax.fori_loop(0, n // 16, step, 0)

    ra, rb = pl.ds(0, 64), pl.ds(64, 64)

    def rounded_rows(p, i, S, k, first, n, cols):
        def fn(rows):
            S[k, rows, cols] = p[i, rows, cols].astype(BF16)

        row_loop(first, n, fn)

    def rs_far(p, S, H, F, k, s, cols=slice(None)):
        rounded_rows(p, 3, S, 0, 0, 128, cols)
        send(S.at[0, ra, cols], H.at[0, :, cols], s, k, x_up)
        send(S.at[0, rb, cols], H.at[1, :, cols], s, k + 1, x_dn)

    def rs_first(p, S, H, F, k, s, cols=slice(None)):
        rounded_rows(p, 0, S, 1, 64, 64, cols)
        send(S.at[1, rb, cols], F.at[0, rb, cols], s, k + 2, x_up)
        rounded_rows(p, 1, S, 2, 0, 64, cols)
        send(S.at[2, ra, cols], F.at[1, ra, cols], s, k + 2, x_dn)

    def rs_second(p, S, H, F, k, s):
        def left(rows):
            S[1, rows, :] = (p[0, rows, :] + H[0, rows, :].astype(F32)).astype(BF16)

        def right(rows):
            low = pl.ds(pl.multiple_of(rows.start + 64, 16), 16)
            S[2, low, :] = (p[1, low, :] + H[1, rows, :].astype(F32)).astype(BF16)

        recv(H.at[0], k)
        row_loop(0, 64, left)
        send(S.at[1, ra], F.at[0, ra], s, k + 2, x_up)
        recv(H.at[1], k + 1)
        row_loop(0, 64, right)
        send(S.at[2, rb], F.at[1, rb], s, k + 2, x_dn)

    def rs_wait(F, k):
        recv(F, k + 2)

    kr = [new(recvs, 3) for _ in layout]
    set1 = (P1, S1, H1, F1, kr[0], sender(S1))
    rs_far(*set1)
    rs_first(*set1)
    z_fwd(2)
    z_own(4)
    rs_second(*set1)
    z_fwd(3)
    z_own(5)
    recv(SM.at[pl.ds(0, 15)], km)
    recv(SSB.at[pl.ds(0, 7)], kss)
    rs_wait(F1, kr[0])

    total = P1[2] + F1[0].astype(F32) + F1[1].astype(F32)
    rs = scale_of(jnp.sum(SSB[...], axis=0)[0:1, :])
    eye = lax.broadcasted_iota(jnp.int32, (128, 128), 0) == lanes_of(128)
    for h in range(2):
        cols = slice(h * 128, h * 128 + 128)
        gated = gelu((rs * total[:, cols]).astype(BF16).astype(F32))
        spread = gelu((rs * total[:, 256 + h * 128 : 384 + h * 128]).astype(BF16).astype(F32))
        spread = spread * lax.rsqrt(jnp.mean(spread * spread, axis=-1, keepdims=True) + EPS)
        spread = (spread * vgain[h : h + 1, :]).astype(BF16)
        matrix = SM[:, h].astype(F32).reshape(128, 128).astype(BF16)
        mixed = jnp.dot(matrix, spread, preferred_element_type=F32)
        bias = jnp.broadcast_to(sbias[h : h + 1, :], (128, 128))
        mixed = mixed + jnp.sum(jnp.where(eye, bias, 0.0), axis=-1, keepdims=True)
        joined = gated * mixed
        joined = joined * lax.rsqrt(jnp.mean(joined * joined, axis=-1, keepdims=True) + EPS)
        MG[2, :, cols] = (joined * hgain[h : h + 1, :]).astype(BF16)

    k2 = new(recvs, 3)
    s2 = sender(MG.at[pl.ds(0, 3)])
    send(MG.at[2], MG.at[1], s2, k2 + 1, x_up)
    send(MG.at[2], MG.at[0], s2, k2 + 2, x_dn)
    send(MG.at[2], MG.at[3], s2, k2, x_far)
    z_fin(2)

    y_order = (far(y), up(y), down(y), y)

    def cy_first(g, product, CS, CR, k, s):
        for n, yt in enumerate(y_order):
            prod = product(yt)
            size = prod.shape[0] // 128
            rows = pl.ds(2 * g, size)
            T[n, rows] = jnp.where(c == 0, prod[:, :128], prod[:, 128:]).reshape(size, 128, 128)
            give = jnp.where(c == 0, prod[:, 128:], prod[:, :128]).astype(BF16)
            CS[n, rows] = give.reshape(size, 128, 128)
            send(CS.at[n, rows], CR.at[n, rows], s, k + n, mate)

    def joined_at(n, b, CR):
        return T[n, b] + CR[n, b].astype(F32)

    def cy_second(g, CR, YS, YH, YF, k, kc, s):
        a, b = 2 * g, 2 * g + 1
        recv(CR.at[0, pl.ds(a, 2)], kc)
        YS[0, a] = joined_at(0, a, CR).astype(BF16)
        YS[0, b] = joined_at(0, b, CR).astype(BF16)
        send(YS.at[0, a], YH.at[a], s, k, y_up)
        send(YS.at[0, b], YH.at[b], s, k + 1, y_dn)
        recv(CR.at[1, pl.ds(a, 2)], kc + 1)
        YS[1, b] = joined_at(1, b, CR).astype(BF16)
        send(YS.at[1, b], YF.at[g, 0, 1], s, k + 2, y_up)
        recv(CR.at[2, pl.ds(a, 2)], kc + 2)
        YS[2, a] = joined_at(2, a, CR).astype(BF16)
        send(YS.at[2, a], YF.at[g, 1, 0], s, k + 2, y_dn)

    def cy_third(g, CR, YS, YH, YF, k, kc, s):
        a, b = 2 * g, 2 * g + 1
        recv(YH.at[a], k)
        YS[1, a] = (joined_at(1, a, CR) + YH[a].astype(F32)).astype(BF16)
        send(YS.at[1, a], YF.at[g, 0, 0], s, k + 2, y_up)
        recv(YH.at[b], k + 1)
        YS[2, b] = (joined_at(2, b, CR) + YH[b].astype(F32)).astype(BF16)
        send(YS.at[2, b], YF.at[g, 1, 1], s, k + 2, y_dn)
        recv(CR.at[3, pl.ds(a, 2)], kc + 3)

    def cy_last(g, CR, YF, k):
        recv(YF.at[g], k + 2)
        return [
            joined_at(3, 2 * g + i, CR) + YF[g, 0, i].astype(F32) + YF[g, 1, i].astype(F32)
            for i in range(2)
        ]

    def merge(g):
        rows = MG[2 * g : 2 * g + 2].reshape(256, 256)
        return lambda yt: jnp.dot(rows, WMP[yt], preferred_element_type=F32)

    kc = [new(recvs, 4) for _ in range(2)]
    k3 = [new(recvs, 3) for _ in range(2)]
    sc, s3 = sender(CS4), sender(YS4)
    recv(MG.at[0], k2 + 2)
    recv(MG.at[1], k2 + 1)
    cy_first(0, merge(0), CS4, CR4, kc[0], sc)
    cy_second(0, CR4, YS4, YH4, YF4, k3[0], kc[0], s3)
    recv(MG.at[3], k2)
    z_own(10)
    z_fwd(9)
    z_fwd(11)
    cy_first(1, merge(1), CS4, CR4, kc[1], sc)
    cy_second(1, CR4, YS4, YH4, YF4, k3[1], kc[1], s3)
    z_fwd(4)
    z_own(6)
    cy_third(0, CR4, YS4, YH4, YF4, k3[0], kc[0], s3)
    cy_third(1, CR4, YS4, YH4, YF4, k3[1], kc[1], s3)


    ko = new(recvs)
    so = new(sends)
    ends.append(lambda: fewer(lambda n: HG.at[0, pl.ds(0, n)], 4, stay(so)))
    spot = 2 * lax.rem(x, 2) + c
    blocks = (up(x), down(x), x, far(x))
    sh = [sender(buf.at[pl.ds(0, 7), pl.ds(0, 2)]) for buf in (HG, HG)]
    for g in range(2):
        branch = cy_last(g, CR4, YF4, k3[g])
        for i in range(2):
            b = 2 * g + i
            HG[me, b] = (XG[me, b].astype(F32) + branch[i]).astype(BF16)
        y_start(HG, ky[g], sh[g], g)
    for b in range(4):
        if b != 2:
            dst = HRES.at[spot]
            send(HG.at[me, b], dst, so, ko, at(x_=blocks[b], c_=x // 2))
            continue

        @pl.when(to_me)
        def _():
            HRES[spot] = HG[me, 2]

        @pl.when(jnp.logical_not(to_me))
        def _():
            send(HG.at[me, 2], HRES.at[spot], so, ko, mate)

    z_fwd(5)
    y_mid(HG, ky[0], sh[0], 0)
    y_mid(HG, ky[1], sh[1], 1)
    y_end(HG, ky[0], sh[0], 0)
    z_fwd(6)
    z_own(7)
    z_own(8)
    z_fwd(10)
    y_end(HG, ky[1], sh[1], 1)
    z_fin(weight("g", 0))
    z_fin(weight("v", 0))
    y_last(HG, ky[0])
    scaled(HG, fgain, True, 0, 2)

    def project(W, p, n, first, b0, b1):
        def cut(cols, to, size):
            w = jnp.concatenate([W[k, cols, :] for k in range(4)], axis=1)
            prod = lax.dot_general(
                XS[b0 * 128 : b1 * 128, :], w, (((1,), (1,)), ((), ())),
                preferred_element_type=F32,
            )
            p[b0:b1, :, to] = prod.reshape(b1 - b0, 128, size)

        def step(i, _):
            cut(
                pl.ds(pl.multiple_of(i * 256, 256), 256),
                pl.ds(pl.multiple_of(first + i * 256, 128), 256), 256,
            )
            return 0

        lax.fori_loop(0, n // 256, step, 0)
        left = n % 256
        if left:
            cut(pl.ds(n - left, left), pl.ds(first + n - left, left), left)

    def gates(j):
        n = layout[j][2]
        z_fin(weight("g", j))
        project(WGU[j], PC[j], n, 0, 0, 4)
        return slice(0, n)

    def values(j):
        n = layout[j][2]
        z_fin(weight("v", j))
        project(WVU[j], PC[j], n, n, 0, 4)
        return slice(n, 2 * n)

    row = lax.broadcasted_iota(jnp.int32, (128, 128), 0)

    def activate(j):
        p, F, act = PC[j], FC[j], ACT[j]
        at0, _, n = layout[j]

        def conv_tile(i, _):
            def one(first, w):
                at_ = pl.ds(pl.multiple_of(first + i * 128, 128), 128)
                v = p[2, :, at_] + F[0, :, at_].astype(F32) + F[1, :, at_].astype(F32)
                v = (RS[...] * v).astype(BF16).astype(F32)
                prev = jnp.where(row == 0, 0.0, pltpu.roll(v, 1, axis=0))
                after = jnp.where(row == 127, 0.0, pltpu.roll(v, 127, axis=0))
                k = CV[w, :, pl.ds(pl.multiple_of(at0 + i * 128, 128), 128)]
                return k[3:4] + prev * k[0:1] + v * k[1:2] + after * k[2:3]

            cols = pl.ds(pl.multiple_of(i * 128, 128), 128)
            act[2, :, cols] = (gelu(one(0, 0)) * one(n, 1)).astype(BF16)
            return 0

        lax.fori_loop(0, n // 128, conv_tile, 0)

    sets = [
        (PC[j], SC[j], HC[j], FC[j], kr[j], sender(SC[j])) for j in range(chunks)
    ]
    kg = [new(recvs, 4) for _ in layout]
    sg = [sender(ACT[j].at[pl.ds(0, 3)]) for j in range(chunks)]

    def x_start(j):
        buf, k, s = ACT[j], kg[j], sg[j]
        send(buf.at[2, ra], buf.at[1, ra], s, k, z_up)
        send(buf.at[2, rb], buf.at[0, rb], s, k + 1, z_dn)
        send(buf.at[2, rb], buf.at[1, rb], s, k + 2, z_up)
        send(buf.at[2, ra], buf.at[0, ra], s, k + 2, z_dn)

    def x_mid(j):
        buf, k, s = ACT[j], kg[j], sg[j]
        recv(buf.at[1, ra], k)
        send(buf.at[1, ra], buf.at[3, ra], s, k + 3, z_up)
        recv(buf.at[0, rb], k + 1)
        send(buf.at[0, rb], buf.at[3, rb], s, k + 3, z_dn)

    def x_near(j):
        recv(ACT[j].at[0], kg[j] + 2)

    def x_last(j):
        recv(ACT[j].at[3], kg[j] + 3)

    def down_rows(j, b0, b1):
        n = layout[j][2]
        rows = ACT[j][b0:b1].reshape((b1 - b0) * 128, n)
        return lambda k: jnp.dot(rows, WDN[j][k], preferred_element_type=F32)

    def down_early(j):
        product = down_rows(j, 0, 4)

        def step(k, _):
            prod = product(k).reshape(4, 128, 256)
            ACC[k] = prod if j == 0 else ACC[k] + prod
            return 0

        lax.fori_loop(0, 4, step, 0)

    n0 = layout[0][2]
    one0, two0 = slice(0, n0), slice(n0, 2 * n0)
    project(WGU[0], PC[0], n0, 0, 0, 2)
    rs_first(*sets[0], one0)
    project(WVU[0], PC[0], n0, n0, 0, 2)
    rs_first(*sets[0], two0)
    y_last(HG, ky[1])
    scaled(HG, fgain, True, 2, 2)
    project(WGU[0], PC[0], n0, 0, 2, 4)
    rs_far(*sets[0], one0)
    project(WVU[0], PC[0], n0, n0, 2, 4)
    rs_far(*sets[0], two0)
    kf = new(recvs)
    sf = sender(SSF.at[pl.ds(0, 3)])
    SSF[2] = SQR[2]
    send(SQR.at[0], SSF.at[1], sf, kf, x_up)
    send(SQR.at[1], SSF.at[0], sf, kf, x_dn)
    send(SQR.at[3], SSF.at[3], sf, kf, x_far)
    one1 = gates(1)
    rs_far(*sets[1], one1)
    two1 = values(1)
    rs_far(*sets[1], two1)
    rs_first(*sets[1], one1)
    rs_second(*sets[0])
    rs_first(*sets[1], two1)
    z_fwd(7)
    z_fwd(8)
    rs_second(*sets[1])
    recv(SSF.at[pl.ds(0, 3)], kf)
    RS[...] = scale_of(jnp.sum(SSF[...], axis=0)[0:1, :])
    rs_wait(FC[0], kr[0])
    activate(0)
    x_start(0)
    one2 = gates(2)
    rs_far(*sets[2], one2)
    two2 = values(2)
    rs_far(*sets[2], two2)
    rs_first(*sets[2])
    rs_wait(FC[1], kr[1])
    activate(1)
    x_start(1)
    x_mid(0)
    rs_second(*sets[2])
    x_mid(1)
    rs_wait(FC[2], kr[2])
    activate(2)
    x_start(2)
    x_near(0)
    x_last(0)
    z_fin(9)
    down_early(0)
    x_near(1)
    x_last(1)
    z_fin(10)
    z_fin(11)
    down_early(1)

    k7 = [new(recvs, 2) for _ in range(3)]
    s7 = sender(CS5)
    kt = new(recvs)
    st = new(sends)
    stays = y == z
    ends.append(lambda: fewer(lambda n: TB.at[pl.ds(0, n)], 4, stay(st), stays))

    def give(b):
        for i in range(2):
            TB[b, :, i * 256 : i * 256 + 256] = (T5[i, b] + CR5[i, b].astype(F32)).astype(BF16)
        if b < 2:
            send(TB.at[b], TI.at[y], st, kt, along(1 - 2 * b, z))
        elif b == 3:
            send(TB.at[b, ra], TI.at[y, ra], st, kt, along(-2, z))
            send(TB.at[b, rb], TI.at[y, rb], st, kt, along(2, z))
        else:

            @pl.when(stays)
            def _():
                TI[y] = TB[b]

            @pl.when(jnp.logical_not(stays))
            def _():
                send(TB.at[b], TI.at[y], st, kt, at(y_=z))

    parts = ((2, 3), (0, 2), (3, 4))

    def finish(g):
        b0, b1 = parts[g]
        rows = pl.ds(b0, b1 - b0)
        product = down_rows(2, b0, b1)

        def final(k):
            return product(k).reshape(b1 - b0, 128, 256) + ACC[k, rows]

        for i in range(2):
            CS5[i, rows] = final(2 * other + i).astype(BF16)
            send(CS5.at[i, rows], CR5.at[i, rows], s7, k7[g] + i, mate)
        for i in range(2):
            T5[i, rows] = final(2 * c + i)

    def hand_over(g):
        b0, b1 = parts[g]
        for i in range(2):
            recv(CR5.at[i, pl.ds(b0, b1 - b0)], k7[g] + i)
        for b in range(b0, b1):
            give(b)

    x_mid(2)
    finish(0)
    x_near(2)
    finish(1)
    hand_over(0)
    hand_over(1)
    x_last(2)
    finish(2)
    hand_over(2)

    fewer(lambda n: HRES.at[pl.ds(0, n)], 4, lambda ref: recv(ref, ko))
    fewer(lambda n: TI.at[pl.ds(0, n)], 4, lambda ref: recv(ref, kt), stays)
    for q in range(4):
        cols = slice(q * 128, q * 128 + 128)
        change = sum(TI[n, :, cols].astype(F32) for n in range(4))
        out[:, cols] = (HRES[q].astype(F32) + change).astype(BF16)
    for wait in ends:
        wait()
    assert sends[0] <= ssem.shape[0] and recvs[0] <= rsem.shape[0], (sends[0], recvs[0])


def body(
    tokens, mixer_gain, gate_proj, value_proj, value_gain, spatial_mix, spatial_bias,
    head_gain, merge_proj, ffn_gain, gate_up, value_up, gate_kernel, value_kernel,
    gate_offset, value_offset, down_proj,
):
    units = gate_up.shape[1]
    layout = []
    for first in range(0, units, CHUNK):
        n = min(CHUNK, units - first)
        layout.append((first, n, -(-n // 128) * 128))
    wide = sum(n for _, _, n in layout)
    widths = [n for _, _, n in layout]
    vm = lambda shape, dtype=BF16: pltpu.VMEM(shape, dtype)
    in_vmem = pl.BlockSpec(memory_space=pltpu.VMEM)
    left = pl.BlockSpec(memory_space=pl.ANY)
    call = pl.pallas_call(
        functools.partial(kernel, layout),
        out_shape=jax.ShapeDtypeStruct(tokens.shape, tokens.dtype),
        in_specs=[
            left, in_vmem, in_vmem, left, left, in_vmem, in_vmem, in_vmem, in_vmem, left,
            left, left, left, left, in_vmem, in_vmem, left,
        ],
        out_specs=in_vmem,
        scratch_shapes=[
            vm(tokens.shape), vm(gate_kernel.shape, F32), vm(gate_kernel.shape, F32),
            vm((2, 4, wide), F32),
            vm((8, 4, 128, 128)), vm((8, 4, 128, 128)), vm((512, 1024)),
            vm((4, 8, 128), F32), vm((128, 128), F32), vm((16, 2, 8, 128)),
            vm((4, 128, 256)), vm((8, 8, 128), F32), vm((4, 8, 128), F32), vm((4, 128, 128)),
            vm((4, 128, 512)), vm((4, 128, 512)),
            *[vm((4, 256, 256))] * 3, vm((4, 4, 128, 128), F32), vm((4, 4, 128, 256), F32),
            vm((4, 128, 512), F32), vm((3, 128, 512)), vm((2, 64, 512)), vm((2, 128, 512)),
            vm((4, 4, 128, 128)), vm((4, 4, 128, 128)), vm((3, 4, 128, 128)),
            vm((4, 128, 128)), vm((2, 2, 2, 128, 128)),
            vm((2, 4, 128, 256)), vm((2, 4, 128, 256)), vm((2, 4, 128, 256), F32),
            *[vm((4, n, 256)) for _ in range(3) for n in widths],
            *[vm((4, 128, n)) for n in widths],
            *[vm((4, 128, 2 * n), F32) for n in widths],
            *[vm((3, 128, 2 * n)) for n in widths],
            *[vm((2, 64, 2 * n)) for n in widths],
            *[vm((2, 128, 2 * n)) for n in widths],
            pltpu.SemaphoreType.DMA((SENDS,)), pltpu.SemaphoreType.DMA((RECVS,)),
            pltpu.SemaphoreType.DMA((6 + 3 * len(layout),)),
        ],
        compiler_params=pltpu.CompilerParams(
            collective_id=0, has_side_effects=True, vmem_limit_bytes=58 << 20
        ),
        name="layer",
    )
    return call(
        tokens, mixer_gain, ffn_gain, gate_proj, value_proj, value_gain, spatial_mix,
        spatial_bias, head_gain, merge_proj, gate_up.T, value_up.T, gate_kernel, value_kernel,
        gate_offset, value_offset, down_proj,
    )


def solution(mesh):
    finer = Mesh(
        mesh.devices.reshape(mesh.shape["rep"], 4, 4, 4, 2), ("rep", "fs_0", "fs_1", "tp_0", "tp_1")
    )
    return jax.shard_map(
        body,
        mesh=finer,
        in_specs=(
            P(REP_FS, TP), P(), P(FS, TP), P(FS, TP), P(TP, None), P(TP, FS, None),
            P(TP, None), P(TP, None), P(TP, FS), P(), P(FS, TP), P(FS, TP), P(None, TP),
            P(None, TP), P(TP), P(TP), P(TP, FS),
        ),
        out_specs=P(REP_FS, TP),
        check_vma=False,
    )
```

```python
import functools

import jax
import jax.numpy as jnp
from jax import lax
from jax.experimental import pallas as pl
from jax.experimental.pallas import tpu as pltpu
from jax.sharding import Mesh
from jax.sharding import PartitionSpec as P

TP = ("tp_0", "tp_1")
FS = ("fs_0", "fs_1")
REP_FS = ("rep", "fs_0", "fs_1")
MESH = pl.DeviceIdType.MESH
EPS = 1e-06
SENDS, RECVS = 33, 105
CHUNK = 512
F32 = jnp.float32
BF16 = jnp.bfloat16


def gelu(v):
    return 0.5 * v * (1.0 + lax.erf(v * 0.7071067811865476))


def lanes_of(n):
    return lax.broadcasted_iota(jnp.int32, (n, 128), 1)


def kernel(layout, tok, mgain, fgain, gp, vp, vgain, smix, sbias, hgain, mp, gu, vu, gk, vk, go, vo,
           dn, out, tokv, gkv, vkv, CV, XG, HG, XS, SQR, RS, SM, MG, SSB, SSF, HRES, TB, TI,
           WGP, WVP, WMP, T, ACC, P1, S1, H1, F1, CS4, CR4, YS4, YH4, YF4, CS5, CR5, T5, *rest):
    chunks = len(layout)
    WGU, WVU, WDN, ACT, PC, SC, HC, FC = (rest[i * chunks : (i + 1) * chunks] for i in range(8))
    ssem, rsem, lsem = rest[8 * chunks :]
    r, z, x, y, c = (lax.axis_index(a) for a in ("rep", "fs_0", "fs_1", "tp_0", "tp_1"))
    other = 1 - c
    f = 4 * z + x
    units = dn.shape[0]
    depth = mgain.shape[0]

    def at(z_=None, x_=None, y_=None, c_=None, r_=None):
        pick = lambda new, old: old if new is None else new
        return (pick(r_, r), pick(z_, z), pick(x_, x), pick(y_, y), pick(c_, c))

    up = lambda v: lax.rem(v + 1, 4)
    down = lambda v: lax.rem(v + 3, 4)
    far = lambda v: lax.rem(v + 2, 4)

    zr = 4 * r + z
    zu, zd = lax.rem(zr + 1, 8), lax.rem(zr + 7, 8)
    z_up = at(r_=zu // 4, z_=lax.rem(zu, 4))
    z_dn = at(r_=zd // 4, z_=lax.rem(zd, 4))
    x_up, x_dn, x_far = at(x_=up(x)), at(x_=down(x)), at(x_=far(x))
    y_up, y_dn = at(y_=up(y)), at(y_=down(y))
    y_up_mate, y_dn_mate = at(y_=up(y), c_=other), at(y_=down(y), c_=other)
    mate = at(c_=other)
    fs_peers = []
    for i in range(1, 16):
        g = lax.rem(f + i, 16)
        fs_peers.append(at(z_=g // 4, x_=lax.rem(g, 4)))
    near = []
    for i in range(1, 4):
        near += [at(x_=lax.rem(x + i, 4), c_=k) for k in (c, other)]
        near += [at(y_=lax.rem(y + i, 4), c_=other)]

    def along(d, y_=None):
        there = lax.rem(zr + 8 + d, 8)
        return at(r_=there // 4, z_=lax.rem(there, 4), y_=y_)

    for i in range(4):
        for d in (-2, -1, 0, 1, 2):
            if i or d:
                near.append(along(d, lax.rem(y + i, 4)))

    barrier = pltpu.get_barrier_semaphore()
    greet = [mate] + near + fs_peers
    for peer in greet:
        pl.semaphore_signal(barrier, inc=1, device_id=peer, device_id_type=MESH)
    loads = [
        pltpu.make_async_copy(src, dst, lsem.at[i])
        for i, (src, dst) in enumerate(((tok, tokv), (gk, gkv), (vk, vkv)))
    ]
    for copy in loads:
        copy.start()
    pl.semaphore_wait(barrier, len(greet))

    sends, recvs, ends = [0], [0], []

    def new(counter, n=1):
        counter[0] += n
        return counter[0] - n

    def remote(src, dst, s, k, peer):
        return pltpu.make_async_remote_copy(
            src_ref=src, dst_ref=dst, send_sem=ssem.at[s], recv_sem=rsem.at[k],
            device_id=peer, device_id_type=MESH,
        )

    def send(src, dst, s, k, peer):
        remote(src, dst, s, k, peer).start()

    def recv(dst, k):
        remote(dst, dst, 0, k, mate).wait_recv()

    def sender(ref):
        s = new(sends)
        ends.append(lambda: remote(ref, ref, s, 0, mate).wait_send())
        return s

    pieces = [(gp, WGP, 0, 256), (vp, WVP, 0, 256), (mp, WMP, 0, 256)]
    for (at0, n, _), G, V in zip(layout, WGU, WVU):
        pieces += [(gu, G, at0, n), (vu, V, at0, n)]
    for (at0, n, _), W in zip(layout, WDN):
        pieces.append((dn, W, at0, n))
    zk = [new(recvs, 3) for _ in pieces]
    zs = [sender(buf.at[pl.ds(0, 3), pl.ds(0, n)]) for _, buf, _, n in pieces]

    def z_local(i):
        src, buf, at0, n = pieces[i]
        own = buf.at[ring(i)[0], pl.ds(0, n)]
        return pltpu.make_async_copy(src.at[pl.ds(at0, n)], own, lsem.at[3 + i])

    def ring(i):
        return (x, x_up, x_dn) if pieces[i][0] is dn else (z, z_up, z_dn)

    def z_own(i):
        src, buf, at0, n = pieces[i]
        a, b = pl.ds(0, n // 2), pl.ds(n // 2, n // 2)
        from_a, from_b = src.at[pl.ds(at0, n // 2)], src.at[pl.ds(at0 + n // 2, n // 2)]
        place, above, below = ring(i)
        send(from_a, buf.at[place, a], zs[i], zk[i], above)
        send(from_b, buf.at[place, b], zs[i], zk[i] + 1, below)
        send(from_b, buf.at[place, b], zs[i], zk[i] + 2, above)
        send(from_a, buf.at[place, a], zs[i], zk[i] + 2, below)
        z_local(i).start()

    def z_fwd(i):
        _, buf, _, n = pieces[i]
        place, above, below = ring(i)
        a, b = buf.at[down(place), pl.ds(0, n // 2)], buf.at[up(place), pl.ds(n // 2, n // 2)]
        recv(a, zk[i])
        send(a, a, zs[i], zk[i] + 2, above)
        recv(b, zk[i] + 1)
        send(b, b, zs[i], zk[i] + 2, below)

    def z_fin(i):
        _, buf, _, n = pieces[i]
        recv(buf.at[pl.ds(0, 2), pl.ds(0, n)], zk[i] + 2)
        z_local(i).wait()

    def weight(kind, j):
        return {"g": 3 + 2 * j, "v": 4 + 2 * j, "d": 3 + 2 * chunks + j}[kind]

    me = 2 * y + c
    to_me = x // 2 == c
    loads[0].wait()
    kx = new(recvs, 2)
    sx = new(sends)
    for j in range(2):
        for h in range(2):
            xt = 2 * c + j
            ahead = lax.rem(x - xt + 4, 4)
            place = jnp.where(ahead == 0, 2, jnp.where(ahead == 2, 3, ahead // 2))
            mine = jnp.logical_and(xt == x, c == h)
            block = tokv.at[:, j * 256 + h * 128 : j * 256 + h * 128 + 128]

            @pl.when(jnp.logical_not(mine))
            def _():
                dst = XG.at[2 * y + h, place]
                send(block, dst, sx, kx + place // 2, at(x_=xt, c_=jnp.int32(h)))

            @pl.when(mine)
            def _():
                XG[2 * y + h, 2] = block[...]

    def fewer(ref_of, n, wait, stays=to_me):
        @pl.when(stays)
        def _():
            wait(ref_of(n - 1))

        @pl.when(jnp.logical_not(stays))
        def _():
            wait(ref_of(n))

    stay = lambda s: lambda ref: remote(ref, ref, s, 0, mate).wait_send()
    ends.append(lambda: fewer(lambda n: XG.at[0, pl.ds(0, n)], 4, stay(sx)))
    z_own(0)
    z_own(1)
    square = tokv[...].astype(F32)
    square = jnp.sum(square * square, axis=-1, keepdims=True)
    SSB[me] = jnp.broadcast_to(square, (128, 128)).T[0:8, :]
    kss = new(recvs)
    sss = sender(SSB.at[pl.ds(0, 7)])
    for i in range(1, 8):
        t = lax.rem(me + i, 8)
        send(SSB.at[me], SSB.at[me], sss, kss, at(y_=t // 2, c_=lax.rem(t, 2)))

    lo_y, hi_y, far_y = 2 * down(y) + c, 2 * up(y) + c, 2 * far(y) + c

    def y_start(buf, k, s, g, direct=False):
        a, b = buf.at[me, 2 * g], buf.at[me, 2 * g + 1]
        send(a, a, s, k, y_up)
        send(b, b, s, k + 1, y_dn)
        send(b, b, s, k + 2, y_up)
        send(a, a, s, k + 3, y_dn)
        both = buf.at[me, pl.ds(2 * g, 2)]
        if direct:
            send(both, both, s, k + 4, at(y_=far(y)))
        send(both, both, s, k + 6, mate)

    def y_mid(buf, k, s, g, direct=False):
        a, b = buf.at[lo_y, 2 * g], buf.at[hi_y, 2 * g + 1]
        for ref, i, there, there_mate in ((a, 0, y_up, y_up_mate), (b, 1, y_dn, y_dn_mate)):
            recv(ref, k + i)
            if not direct:
                send(ref, ref, s, k + 4 + i, there)
                send(ref, ref, s, k + 6, there_mate)
            send(ref, ref, s, k + 6, mate)

    def y_end(buf, k, s, g, direct=False):
        for i, ref in enumerate((buf.at[lo_y, 2 * g + 1], buf.at[hi_y, 2 * g])):
            recv(ref, k + 2 + i)
            send(ref, ref, s, k + 6, mate)
        if direct:
            ref = buf.at[far_y, pl.ds(2 * g, 2)]
            recv(ref, k + 4)
            send(ref, ref, s, k + 6, mate)
        else:
            recv(buf.at[far_y, 2 * g], k + 4)
            recv(buf.at[far_y, 2 * g + 1], k + 5)

    def y_last(buf, k):
        recv(buf.at[pl.ds(0, 4), pl.ds(0, 2)], k + 6)

    def scaled(buf, gains, squares, first, n):
        parts = [gains[pl.ds(pl.multiple_of((4 * k + x) * 256, 256), 256)] for k in range(4)]
        gain = jnp.concatenate([part.reshape(1, 256) for part in parts], axis=1)

        def block(b, _):
            rows = jnp.concatenate([buf[i, b] for i in range(8)], axis=1).astype(F32)
            if squares:
                total = jnp.sum(rows * rows, axis=-1, keepdims=True)
                SQR[b] = jnp.broadcast_to(total, (128, 128)).T[0:8, :]
            XS[pl.ds(pl.multiple_of(b * 128, 128), 128), :] = (rows * gain).astype(BF16)
            return 0

        lax.fori_loop(first, first + n, block, 0)

    def scale_of(rows):
        return lax.rsqrt(jnp.broadcast_to(rows, (128, 128)).T / depth + EPS)

    ky = [new(recvs, 7) for _ in range(2)]
    sy = [sender(buf.at[pl.ds(0, 7), pl.ds(0, 2)]) for buf in (XG, XG)]
    recv(XG.at[me, pl.ds(0, 2)], kx)
    y_start(XG, ky[0], sy[0], 0)
    fewer(lambda n: XG.at[me, pl.ds(0, n)], 2, lambda ref: recv(ref, kx + 1))
    y_start(XG, ky[1], sy[1], 1)
    km = new(recvs)
    sm = sender(SM.at[pl.ds(0, 15)])
    for i in range(15):
        send(smix, SM.at[f], sm, km, fs_peers[i])
    SM[f] = smix[...]
    last0, lastn, wide = layout[-1]
    for W in (WGU[-1], WVU[-1], WDN[-1]):
        for k in range(4):
            W[k, lastn:, :] = jnp.zeros((wide - lastn, 256), BF16)
    z_own(9)
    z_own(11)
    z_fwd(0)
    z_fwd(1)
    z_own(2)
    z_own(3)
    y_mid(XG, ky[0], sy[0], 0)
    y_mid(XG, ky[1], sy[1], 1)
    loads[1].wait()
    loads[2].wait()
    for w, kern, off in ((0, gkv, go), (1, vkv, vo)):
        CV[w, :, last0:] = jnp.zeros((4, wide), F32)
        CV[w, 0:3, 0:units] = kern[...]
        CV[w, 3:4, 0:units] = off[...].reshape(1, units)
    y_end(XG, ky[0], sy[0], 0)
    y_end(XG, ky[1], sy[1], 1)
    y_last(XG, ky[0])
    y_last(XG, ky[1])
    scaled(XG, mgain, False, 0, 4)
    z_fin(0)
    z_fin(1)
    for w, W in ((0, WGP), (1, WVP)):
        prod = jnp.dot(XS[...], W[...].reshape(1024, 256), preferred_element_type=F32)
        P1[:, :, w * 256 : w * 256 + 256] = prod.reshape(4, 128, 256)

    def row_loop(first, n, fn):
        def step(i, _):
            fn(pl.ds(pl.multiple_of(first + i * 16, 16), 16))
            return 0

        lax.fori_loop(0, n // 16, step, 0)

    ra, rb = pl.ds(0, 64), pl.ds(64, 64)

    def rounded_rows(p, i, S, k, first, n, cols):
        def fn(rows):
            S[k, rows, cols] = p[i, rows, cols].astype(BF16)

        row_loop(first, n, fn)

    def rs_far(p, S, H, F, k, s, cols=slice(None)):
        rounded_rows(p, 3, S, 0, 0, 128, cols)
        send(S.at[0, ra, cols], H.at[0, :, cols], s, k, x_up)
        send(S.at[0, rb, cols], H.at[1, :, cols], s, k + 1, x_dn)

    def rs_first(p, S, H, F, k, s, cols=slice(None)):
        rounded_rows(p, 0, S, 1, 64, 64, cols)
        send(S.at[1, rb, cols], F.at[0, rb, cols], s, k + 2, x_up)
        rounded_rows(p, 1, S, 2, 0, 64, cols)
        send(S.at[2, ra, cols], F.at[1, ra, cols], s, k + 2, x_dn)

    def rs_second(p, S, H, F, k, s):
        def left(rows):
            S[1, rows, :] = (p[0, rows, :] + H[0, rows, :].astype(F32)).astype(BF16)

        def right(rows):
            low = pl.ds(pl.multiple_of(rows.start + 64, 16), 16)
            S[2, low, :] = (p[1, low, :] + H[1, rows, :].astype(F32)).astype(BF16)

        recv(H.at[0], k)
        row_loop(0, 64, left)
        send(S.at[1, ra], F.at[0, ra], s, k + 2, x_up)
        recv(H.at[1], k + 1)
        row_loop(0, 64, right)
        send(S.at[2, rb], F.at[1, rb], s, k + 2, x_dn)

    def rs_wait(F, k):
        recv(F, k + 2)

    kr = [new(recvs, 3) for _ in layout]
    set1 = (P1, S1, H1, F1, kr[0], sender(S1))
    rs_far(*set1)
    rs_first(*set1)
    z_fwd(2)
    z_own(4)
    rs_second(*set1)
    z_fwd(3)
    z_own(5)
    recv(SM.at[pl.ds(0, 15)], km)
    recv(SSB.at[pl.ds(0, 7)], kss)
    rs_wait(F1, kr[0])

    total = P1[2] + F1[0].astype(F32) + F1[1].astype(F32)
    rs = scale_of(jnp.sum(SSB[...], axis=0)[0:1, :])
    eye = lax.broadcasted_iota(jnp.int32, (128, 128), 0) == lanes_of(128)
    for h in range(2):
        cols = slice(h * 128, h * 128 + 128)
        gated = gelu((rs * total[:, cols]).astype(BF16).astype(F32))
        spread = gelu((rs * total[:, 256 + h * 128 : 384 + h * 128]).astype(BF16).astype(F32))
        spread = spread * lax.rsqrt(jnp.mean(spread * spread, axis=-1, keepdims=True) + EPS)
        spread = (spread * vgain[h : h + 1, :]).astype(BF16)
        matrix = SM[:, h].astype(F32).reshape(128, 128).astype(BF16)
        mixed = jnp.dot(matrix, spread, preferred_element_type=F32)
        bias = jnp.broadcast_to(sbias[h : h + 1, :], (128, 128))
        mixed = mixed + jnp.sum(jnp.where(eye, bias, 0.0), axis=-1, keepdims=True)
        joined = gated * mixed
        joined = joined * lax.rsqrt(jnp.mean(joined * joined, axis=-1, keepdims=True) + EPS)
        MG[2, :, cols] = (joined * hgain[h : h + 1, :]).astype(BF16)

    k2 = new(recvs, 3)
    s2 = sender(MG.at[pl.ds(0, 3)])
    send(MG.at[2], MG.at[1], s2, k2 + 1, x_up)
    send(MG.at[2], MG.at[0], s2, k2 + 2, x_dn)
    send(MG.at[2], MG.at[3], s2, k2, x_far)
    z_fin(2)

    y_order = (far(y), up(y), down(y), y)

    def cy_first(g, product, CS, CR, k, s):
        for n, yt in enumerate(y_order):
            prod = product(yt)
            size = prod.shape[0] // 128
            rows = pl.ds(2 * g, size)
            T[n, rows] = jnp.where(c == 0, prod[:, :128], prod[:, 128:]).reshape(size, 128, 128)
            give = jnp.where(c == 0, prod[:, 128:], prod[:, :128]).astype(BF16)
            CS[n, rows] = give.reshape(size, 128, 128)
            send(CS.at[n, rows], CR.at[n, rows], s, k + n, mate)

    def joined_at(n, b, CR):
        return T[n, b] + CR[n, b].astype(F32)

    def cy_second(g, CR, YS, YH, YF, k, kc, s):
        a, b = 2 * g, 2 * g + 1
        recv(CR.at[0, pl.ds(a, 2)], kc)
        YS[0, a] = joined_at(0, a, CR).astype(BF16)
        YS[0, b] = joined_at(0, b, CR).astype(BF16)
        send(YS.at[0, a], YH.at[a], s, k, y_up)
        send(YS.at[0, b], YH.at[b], s, k + 1, y_dn)
        recv(CR.at[1, pl.ds(a, 2)], kc + 1)
        YS[1, b] = joined_at(1, b, CR).astype(BF16)
        send(YS.at[1, b], YF.at[g, 0, 1], s, k + 2, y_up)
        recv(CR.at[2, pl.ds(a, 2)], kc + 2)
        YS[2, a] = joined_at(2, a, CR).astype(BF16)
        send(YS.at[2, a], YF.at[g, 1, 0], s, k + 2, y_dn)

    def cy_third(g, CR, YS, YH, YF, k, kc, s):
        a, b = 2 * g, 2 * g + 1
        recv(YH.at[a], k)
        YS[1, a] = (joined_at(1, a, CR) + YH[a].astype(F32)).astype(BF16)
        send(YS.at[1, a], YF.at[g, 0, 0], s, k + 2, y_up)
        recv(YH.at[b], k + 1)
        YS[2, b] = (joined_at(2, b, CR) + YH[b].astype(F32)).astype(BF16)
        send(YS.at[2, b], YF.at[g, 1, 1], s, k + 2, y_dn)
        recv(CR.at[3, pl.ds(a, 2)], kc + 3)

    def cy_last(g, CR, YF, k):
        recv(YF.at[g], k + 2)
        return [
            joined_at(3, 2 * g + i, CR) + YF[g, 0, i].astype(F32) + YF[g, 1, i].astype(F32)
            for i in range(2)
        ]

    def merge(g):
        rows = MG[2 * g : 2 * g + 2].reshape(256, 256)
        return lambda yt: jnp.dot(rows, WMP[yt], preferred_element_type=F32)

    kc = [new(recvs, 4) for _ in range(2)]
    k3 = [new(recvs, 3) for _ in range(2)]
    sc, s3 = sender(CS4), sender(YS4)
    recv(MG.at[0], k2 + 2)
    recv(MG.at[1], k2 + 1)
    cy_first(0, merge(0), CS4, CR4, kc[0], sc)
    cy_second(0, CR4, YS4, YH4, YF4, k3[0], kc[0], s3)
    recv(MG.at[3], k2)
    z_own(10)
    z_fwd(9)
    z_fwd(11)
    cy_first(1, merge(1), CS4, CR4, kc[1], sc)
    cy_second(1, CR4, YS4, YH4, YF4, k3[1], kc[1], s3)
    z_fwd(4)
    z_own(6)
    cy_third(0, CR4, YS4, YH4, YF4, k3[0], kc[0], s3)
    cy_third(1, CR4, YS4, YH4, YF4, k3[1], kc[1], s3)


    ko = new(recvs)
    so = new(sends)
    ends.append(lambda: fewer(lambda n: HG.at[0, pl.ds(0, n)], 4, stay(so)))
    spot = 2 * lax.rem(x, 2) + c
    blocks = (up(x), down(x), x, far(x))
    sh = [sender(buf.at[pl.ds(0, 7), pl.ds(0, 2)]) for buf in (HG, HG)]
    for g in range(2):
        branch = cy_last(g, CR4, YF4, k3[g])
        for i in range(2):
            b = 2 * g + i
            HG[me, b] = (XG[me, b].astype(F32) + branch[i]).astype(BF16)
        y_start(HG, ky[g], sh[g], g, g == 0)
    for b in range(4):
        if b != 2:
            dst = HRES.at[spot]
            send(HG.at[me, b], dst, so, ko, at(x_=blocks[b], c_=x // 2))
            continue

        @pl.when(to_me)
        def _():
            HRES[spot] = HG[me, 2]

        @pl.when(jnp.logical_not(to_me))
        def _():
            send(HG.at[me, 2], HRES.at[spot], so, ko, mate)

    z_fwd(5)
    y_mid(HG, ky[0], sh[0], 0, True)
    y_mid(HG, ky[1], sh[1], 1)
    y_end(HG, ky[0], sh[0], 0, True)
    z_fwd(6)
    z_own(7)
    z_own(8)
    z_fwd(10)
    y_end(HG, ky[1], sh[1], 1)
    z_fin(weight("g", 0))
    z_fin(weight("v", 0))
    y_last(HG, ky[0])
    scaled(HG, fgain, True, 0, 2)

    def project(W, p, n, first, b0, b1):
        def cut(cols, to, size):
            w = jnp.concatenate([W[k, cols, :] for k in range(4)], axis=1)
            prod = lax.dot_general(
                XS[b0 * 128 : b1 * 128, :], w, (((1,), (1,)), ((), ())),
                preferred_element_type=F32,
            )
            p[b0:b1, :, to] = prod.reshape(b1 - b0, 128, size)

        def step(i, _):
            cut(
                pl.ds(pl.multiple_of(i * 256, 256), 256),
                pl.ds(pl.multiple_of(first + i * 256, 128), 256), 256,
            )
            return 0

        lax.fori_loop(0, n // 256, step, 0)
        left = n % 256
        if left:
            cut(pl.ds(n - left, left), pl.ds(first + n - left, left), left)

    def gates(j):
        n = layout[j][2]
        z_fin(weight("g", j))
        project(WGU[j], PC[j], n, 0, 0, 4)
        return slice(0, n)

    def values(j):
        n = layout[j][2]
        z_fin(weight("v", j))
        project(WVU[j], PC[j], n, n, 0, 4)
        return slice(n, 2 * n)

    row = lax.broadcasted_iota(jnp.int32, (128, 128), 0)

    def activate(j):
        p, F, act = PC[j], FC[j], ACT[j]
        at0, _, n = layout[j]

        def conv_tile(i, _):
            def one(first, w):
                at_ = pl.ds(pl.multiple_of(first + i * 128, 128), 128)
                v = p[2, :, at_] + F[0, :, at_].astype(F32) + F[1, :, at_].astype(F32)
                v = (RS[...] * v).astype(BF16).astype(F32)
                prev = jnp.where(row == 0, 0.0, pltpu.roll(v, 1, axis=0))
                after = jnp.where(row == 127, 0.0, pltpu.roll(v, 127, axis=0))
                k = CV[w, :, pl.ds(pl.multiple_of(at0 + i * 128, 128), 128)]
                return k[3:4] + prev * k[0:1] + v * k[1:2] + after * k[2:3]

            cols = pl.ds(pl.multiple_of(i * 128, 128), 128)
            act[2, :, cols] = (gelu(one(0, 0)) * one(n, 1)).astype(BF16)
            return 0

        lax.fori_loop(0, n // 128, conv_tile, 0)

    sets = [
        (PC[j], SC[j], HC[j], FC[j], kr[j], sender(SC[j])) for j in range(chunks)
    ]
    kg = [new(recvs, 4) for _ in layout]
    sg = [sender(ACT[j].at[pl.ds(0, 3)]) for j in range(chunks)]

    def x_start(j, direct=False):
        buf, k, s = ACT[j], kg[j], sg[j]
        send(buf.at[2, ra], buf.at[1, ra], s, k, z_up)
        send(buf.at[2, rb], buf.at[0, rb], s, k + 1, z_dn)
        send(buf.at[2, rb], buf.at[1, rb], s, k + 2, z_up)
        send(buf.at[2, ra], buf.at[0, ra], s, k + 2, z_dn)

        if direct:
            send(buf.at[2, ra], buf.at[3, ra], s, k + 3, along(2))
            send(buf.at[2, rb], buf.at[3, rb], s, k + 3, along(-2))

    def x_mid(j, direct=False):
        buf, k, s = ACT[j], kg[j], sg[j]
        recv(buf.at[1, ra], k)
        if not direct:
            send(buf.at[1, ra], buf.at[3, ra], s, k + 3, z_up)
        recv(buf.at[0, rb], k + 1)
        if not direct:
            send(buf.at[0, rb], buf.at[3, rb], s, k + 3, z_dn)

    def x_near(j):
        recv(ACT[j].at[0], kg[j] + 2)

    def x_last(j):
        recv(ACT[j].at[3], kg[j] + 3)

    def down_rows(j, b0, b1):
        n = layout[j][2]
        rows = ACT[j][b0:b1].reshape((b1 - b0) * 128, n)
        return lambda k: jnp.dot(rows, WDN[j][k], preferred_element_type=F32)

    def down_early(j):
        product = down_rows(j, 0, 4)

        def step(k, _):
            prod = product(k).reshape(4, 128, 256)
            ACC[k] = prod if j == 0 else ACC[k] + prod
            return 0

        lax.fori_loop(0, 4, step, 0)

    n0 = layout[0][2]
    one0, two0 = slice(0, n0), slice(n0, 2 * n0)
    project(WGU[0], PC[0], n0, 0, 0, 2)
    rs_first(*sets[0], one0)
    project(WVU[0], PC[0], n0, n0, 0, 2)
    rs_first(*sets[0], two0)
    y_last(HG, ky[1])
    scaled(HG, fgain, True, 2, 2)
    project(WGU[0], PC[0], n0, 0, 2, 4)
    rs_far(*sets[0], one0)
    project(WVU[0], PC[0], n0, n0, 2, 4)
    rs_far(*sets[0], two0)
    kf = new(recvs)
    sf = sender(SSF.at[pl.ds(0, 3)])
    SSF[2] = SQR[2]
    send(SQR.at[0], SSF.at[1], sf, kf, x_up)
    send(SQR.at[1], SSF.at[0], sf, kf, x_dn)
    send(SQR.at[3], SSF.at[3], sf, kf, x_far)
    one1 = gates(1)
    rs_far(*sets[1], one1)
    rs_first(*sets[1], one1)
    two1 = values(1)
    rs_far(*sets[1], two1)
    rs_second(*sets[0])
    rs_first(*sets[1], two1)
    z_fwd(7)
    z_fwd(8)
    rs_second(*sets[1])
    recv(SSF.at[pl.ds(0, 3)], kf)
    RS[...] = scale_of(jnp.sum(SSF[...], axis=0)[0:1, :])
    rs_wait(FC[0], kr[0])
    activate(0)
    x_start(0)
    one2 = gates(2)
    rs_far(*sets[2], one2)
    two2 = values(2)
    rs_far(*sets[2], two2)
    rs_first(*sets[2])
    rs_wait(FC[1], kr[1])
    activate(1)
    x_start(1)
    x_mid(0)
    rs_second(*sets[2])
    x_mid(1)
    rs_wait(FC[2], kr[2])
    activate(2)
    x_start(2, True)
    x_near(0)
    x_last(0)
    z_fin(9)
    down_early(0)
    x_near(1)
    x_last(1)
    z_fin(10)
    z_fin(11)
    down_early(1)

    k7 = [new(recvs, 2) for _ in range(3)]
    s7 = sender(CS5)
    kt = new(recvs)
    st = new(sends)
    stays = y == z
    ends.append(lambda: fewer(lambda n: TB.at[pl.ds(0, n)], 4, stay(st), stays))

    def give(b):
        for i in range(2):
            TB[b, :, i * 256 : i * 256 + 256] = (T5[i, b] + CR5[i, b].astype(F32)).astype(BF16)
        if b < 2:
            send(TB.at[b], TI.at[y], st, kt, along(1 - 2 * b, z))
        elif b == 3:
            send(TB.at[b, ra], TI.at[y, ra], st, kt, along(-2, z))
            send(TB.at[b, rb], TI.at[y, rb], st, kt, along(2, z))
        else:

            @pl.when(stays)
            def _():
                TI[y] = TB[b]

            @pl.when(jnp.logical_not(stays))
            def _():
                send(TB.at[b], TI.at[y], st, kt, at(y_=z))

    parts = ((2, 3), (0, 2), (3, 4))

    def finish(g):
        b0, b1 = parts[g]
        rows = pl.ds(b0, b1 - b0)
        product = down_rows(2, b0, b1)

        def final(k):
            return product(k).reshape(b1 - b0, 128, 256) + ACC[k, rows]

        for i in range(2):
            CS5[i, rows] = final(2 * other + i).astype(BF16)
            send(CS5.at[i, rows], CR5.at[i, rows], s7, k7[g] + i, mate)
        for i in range(2):
            T5[i, rows] = final(2 * c + i)

    def hand_over(g):
        b0, b1 = parts[g]
        for i in range(2):
            recv(CR5.at[i, pl.ds(b0, b1 - b0)], k7[g] + i)
        for b in range(b0, b1):
            give(b)

    finish(0)
    x_mid(2, True)
    x_near(2)
    finish(1)
    hand_over(0)
    hand_over(1)
    x_last(2)
    finish(2)
    hand_over(2)

    fewer(lambda n: HRES.at[pl.ds(0, n)], 4, lambda ref: recv(ref, ko))
    fewer(lambda n: TI.at[pl.ds(0, n)], 4, lambda ref: recv(ref, kt), stays)
    for q in range(4):
        cols = slice(q * 128, q * 128 + 128)
        change = sum(TI[n, :, cols].astype(F32) for n in range(4))
        out[:, cols] = (HRES[q].astype(F32) + change).astype(BF16)
    for wait in ends:
        wait()
    assert sends[0] <= ssem.shape[0] and recvs[0] <= rsem.shape[0], (sends[0], recvs[0])


def body(
    tokens, mixer_gain, gate_proj, value_proj, value_gain, spatial_mix, spatial_bias,
    head_gain, merge_proj, ffn_gain, gate_up, value_up, gate_kernel, value_kernel,
    gate_offset, value_offset, down_proj,
):
    units = gate_up.shape[1]
    layout = []
    for first in range(0, units, CHUNK):
        n = min(CHUNK, units - first)
        layout.append((first, n, -(-n // 128) * 128))
    wide = sum(n for _, _, n in layout)
    widths = [n for _, _, n in layout]
    vm = lambda shape, dtype=BF16: pltpu.VMEM(shape, dtype)
    in_vmem = pl.BlockSpec(memory_space=pltpu.VMEM)
    left = pl.BlockSpec(memory_space=pl.ANY)
    call = pl.pallas_call(
        functools.partial(kernel, layout),
        out_shape=jax.ShapeDtypeStruct(tokens.shape, tokens.dtype),
        in_specs=[
            left, in_vmem, in_vmem, left, left, in_vmem, in_vmem, in_vmem, in_vmem, left,
            left, left, left, left, in_vmem, in_vmem, left,
        ],
        out_specs=in_vmem,
        scratch_shapes=[
            vm(tokens.shape), vm(gate_kernel.shape, F32), vm(gate_kernel.shape, F32),
            vm((2, 4, wide), F32),
            vm((8, 4, 128, 128)), vm((8, 4, 128, 128)), vm((512, 1024)),
            vm((4, 8, 128), F32), vm((128, 128), F32), vm((16, 2, 8, 128)),
            vm((4, 128, 256)), vm((8, 8, 128), F32), vm((4, 8, 128), F32), vm((4, 128, 128)),
            vm((4, 128, 512)), vm((4, 128, 512)),
            *[vm((4, 256, 256))] * 3, vm((4, 4, 128, 128), F32), vm((4, 4, 128, 256), F32),
            vm((4, 128, 512), F32), vm((3, 128, 512)), vm((2, 64, 512)), vm((2, 128, 512)),
            vm((4, 4, 128, 128)), vm((4, 4, 128, 128)), vm((3, 4, 128, 128)),
            vm((4, 128, 128)), vm((2, 2, 2, 128, 128)),
            vm((2, 4, 128, 256)), vm((2, 4, 128, 256)), vm((2, 4, 128, 256), F32),
            *[vm((4, n, 256)) for _ in range(3) for n in widths],
            *[vm((4, 128, n)) for n in widths],
            *[vm((4, 128, 2 * n), F32) for n in widths],
            *[vm((3, 128, 2 * n)) for n in widths],
            *[vm((2, 64, 2 * n)) for n in widths],
            *[vm((2, 128, 2 * n)) for n in widths],
            pltpu.SemaphoreType.DMA((SENDS,)), pltpu.SemaphoreType.DMA((RECVS,)),
            pltpu.SemaphoreType.DMA((6 + 3 * len(layout),)),
        ],
        compiler_params=pltpu.CompilerParams(
            collective_id=0, has_side_effects=True, vmem_limit_bytes=58 << 20
        ),
        name="layer",
    )
    return call(
        tokens, mixer_gain, ffn_gain, gate_proj, value_proj, value_gain, spatial_mix,
        spatial_bias, head_gain, merge_proj, gate_up.T, value_up.T, gate_kernel, value_kernel,
        gate_offset, value_offset, down_proj,
    )


def solution(mesh):
    finer = Mesh(
        mesh.devices.reshape(mesh.shape["rep"], 4, 4, 4, 2), ("rep", "fs_0", "fs_1", "tp_0", "tp_1")
    )
    return jax.shard_map(
        body,
        mesh=finer,
        in_specs=(
            P(REP_FS, TP), P(), P(FS, TP), P(FS, TP), P(TP, None), P(TP, FS, None),
            P(TP, None), P(TP, None), P(TP, FS), P(), P(FS, TP), P(FS, TP), P(None, TP),
            P(None, TP), P(TP), P(TP), P(TP, FS),
        ),
        out_specs=P(REP_FS, TP),
        check_vma=False,
    )
```

```python
import functools

import jax
import jax.numpy as jnp
from jax import lax
from jax.experimental import pallas as pl
from jax.experimental.pallas import tpu as pltpu
from jax.sharding import Mesh
from jax.sharding import PartitionSpec as P

TP = ("tp_0", "tp_1")
FS = ("fs_0", "fs_1")
REP_FS = ("rep", "fs_0", "fs_1")
MESH = pl.DeviceIdType.MESH
EPS = 1e-06
SENDS, RECVS = 33, 105
CHUNK = 512
F32 = jnp.float32
BF16 = jnp.bfloat16


def gelu(v):
    return 0.5 * v * (1.0 + lax.erf(v * 0.7071067811865476))


def lanes_of(n):
    return lax.broadcasted_iota(jnp.int32, (n, 128), 1)


def kernel(layout, tok, mgain, fgain, gp, vp, vgain, smix, sbias, hgain, mp, gu, vu, gk, vk, go, vo,
           dn, out, tokv, gkv, vkv, CV, XG, HG, XS, SQR, RS, SM, MG, SSB, SSF, HRES, TB, TI,
           WGP, WVP, WMP, T, ACC, P1, S1, H1, F1, CS4, CR4, YS4, YH4, YF4, CS5, CR5, T5, *rest):
    chunks = len(layout)
    WGU, WVU, WDN, ACT, PC, SC, HC, FC = (rest[i * chunks : (i + 1) * chunks] for i in range(8))
    ssem, rsem, lsem = rest[8 * chunks :]
    r, z, x, y, c = (lax.axis_index(a) for a in ("rep", "fs_0", "fs_1", "tp_0", "tp_1"))
    other = 1 - c
    f = 4 * z + x
    units = dn.shape[0]
    depth = mgain.shape[0]

    def at(z_=None, x_=None, y_=None, c_=None, r_=None):
        pick = lambda new, old: old if new is None else new
        return (pick(r_, r), pick(z_, z), pick(x_, x), pick(y_, y), pick(c_, c))

    up = lambda v: lax.rem(v + 1, 4)
    down = lambda v: lax.rem(v + 3, 4)
    far = lambda v: lax.rem(v + 2, 4)

    zr = 4 * r + z
    zu, zd = lax.rem(zr + 1, 8), lax.rem(zr + 7, 8)
    z_up = at(r_=zu // 4, z_=lax.rem(zu, 4))
    z_dn = at(r_=zd // 4, z_=lax.rem(zd, 4))
    x_up, x_dn, x_far = at(x_=up(x)), at(x_=down(x)), at(x_=far(x))
    y_up, y_dn = at(y_=up(y)), at(y_=down(y))
    y_up_mate, y_dn_mate = at(y_=up(y), c_=other), at(y_=down(y), c_=other)
    mate = at(c_=other)
    fs_peers = []
    for i in range(1, 16):
        g = lax.rem(f + i, 16)
        fs_peers.append(at(z_=g // 4, x_=lax.rem(g, 4)))
    near = []
    for i in range(1, 4):
        near += [at(x_=lax.rem(x + i, 4), c_=k) for k in (c, other)]
        near += [at(y_=lax.rem(y + i, 4), c_=other)]

    def along(d, y_=None):
        there = lax.rem(zr + 8 + d, 8)
        return at(r_=there // 4, z_=lax.rem(there, 4), y_=y_)

    for i in range(4):
        for d in (-2, -1, 0, 1, 2):
            if i or d:
                near.append(along(d, lax.rem(y + i, 4)))

    barrier = pltpu.get_barrier_semaphore()
    greet = [mate] + near + fs_peers
    for peer in greet:
        pl.semaphore_signal(barrier, inc=1, device_id=peer, device_id_type=MESH)
    loads = [
        pltpu.make_async_copy(src, dst, lsem.at[i])
        for i, (src, dst) in enumerate(((tok, tokv), (gk, gkv), (vk, vkv)))
    ]
    for copy in loads:
        copy.start()
    pl.semaphore_wait(barrier, len(greet))

    sends, recvs, ends = [0], [0], []

    def new(counter, n=1):
        counter[0] += n
        return counter[0] - n

    def remote(src, dst, s, k, peer):
        return pltpu.make_async_remote_copy(
            src_ref=src, dst_ref=dst, send_sem=ssem.at[s], recv_sem=rsem.at[k],
            device_id=peer, device_id_type=MESH,
        )

    def send(src, dst, s, k, peer):
        remote(src, dst, s, k, peer).start()

    def recv(dst, k):
        remote(dst, dst, 0, k, mate).wait_recv()

    def sender(ref):
        s = new(sends)
        ends.append(lambda: remote(ref, ref, s, 0, mate).wait_send())
        return s

    pieces = [(gp, WGP, 0, 256), (vp, WVP, 0, 256), (mp, WMP, 0, 256)]
    for (at0, n, _), G, V in zip(layout, WGU, WVU):
        pieces += [(gu, G, at0, n), (vu, V, at0, n)]
    for (at0, n, _), W in zip(layout, WDN):
        pieces.append((dn, W, at0, n))
    zk = [new(recvs, 3) for _ in pieces]
    zs = [sender(buf.at[pl.ds(0, 3), pl.ds(0, n)]) for _, buf, _, n in pieces]

    def z_local(i):
        src, buf, at0, n = pieces[i]
        own = buf.at[ring(i)[0], pl.ds(0, n)]
        return pltpu.make_async_copy(src.at[pl.ds(at0, n)], own, lsem.at[3 + i])

    def ring(i):
        return (x, x_up, x_dn) if pieces[i][0] is dn else (z, z_up, z_dn)

    def z_own(i):
        src, buf, at0, n = pieces[i]
        a, b = pl.ds(0, n // 2), pl.ds(n // 2, n // 2)
        from_a, from_b = src.at[pl.ds(at0, n // 2)], src.at[pl.ds(at0 + n // 2, n // 2)]
        place, above, below = ring(i)
        send(from_a, buf.at[place, a], zs[i], zk[i], above)
        send(from_b, buf.at[place, b], zs[i], zk[i] + 1, below)
        send(from_b, buf.at[place, b], zs[i], zk[i] + 2, above)
        send(from_a, buf.at[place, a], zs[i], zk[i] + 2, below)
        z_local(i).start()

    def z_fwd(i):
        _, buf, _, n = pieces[i]
        place, above, below = ring(i)
        a, b = buf.at[down(place), pl.ds(0, n // 2)], buf.at[up(place), pl.ds(n // 2, n // 2)]
        recv(a, zk[i])
        send(a, a, zs[i], zk[i] + 2, above)
        recv(b, zk[i] + 1)
        send(b, b, zs[i], zk[i] + 2, below)

    def z_fin(i):
        _, buf, _, n = pieces[i]
        recv(buf.at[pl.ds(0, 2), pl.ds(0, n)], zk[i] + 2)
        z_local(i).wait()

    def weight(kind, j):
        return {"g": 3 + 2 * j, "v": 4 + 2 * j, "d": 3 + 2 * chunks + j}[kind]

    me = 2 * y + c
    to_me = x // 2 == c
    loads[0].wait()
    kx = new(recvs, 2)
    sx = new(sends)
    for j in range(2):
        for h in range(2):
            xt = 2 * c + j
            ahead = lax.rem(x - xt + 4, 4)
            place = jnp.where(ahead == 0, 2, jnp.where(ahead == 2, 3, ahead // 2))
            mine = jnp.logical_and(xt == x, c == h)
            block = tokv.at[:, j * 256 + h * 128 : j * 256 + h * 128 + 128]

            @pl.when(jnp.logical_not(mine))
            def _():
                dst = XG.at[2 * y + h, place]
                send(block, dst, sx, kx + place // 2, at(x_=xt, c_=jnp.int32(h)))

            @pl.when(mine)
            def _():
                XG[2 * y + h, 2] = block[...]

    def fewer(ref_of, n, wait, stays=to_me):
        @pl.when(stays)
        def _():
            wait(ref_of(n - 1))

        @pl.when(jnp.logical_not(stays))
        def _():
            wait(ref_of(n))

    stay = lambda s: lambda ref: remote(ref, ref, s, 0, mate).wait_send()
    ends.append(lambda: fewer(lambda n: XG.at[0, pl.ds(0, n)], 4, stay(sx)))
    z_own(0)
    z_own(1)
    square = tokv[...].astype(F32)
    square = jnp.sum(square * square, axis=-1, keepdims=True)
    SSB[me] = jnp.broadcast_to(square, (128, 128)).T[0:8, :]
    kss = new(recvs)
    sss = sender(SSB.at[pl.ds(0, 7)])
    for i in range(1, 8):
        t = lax.rem(me + i, 8)
        send(SSB.at[me], SSB.at[me], sss, kss, at(y_=t // 2, c_=lax.rem(t, 2)))

    lo_y, hi_y, far_y = 2 * down(y) + c, 2 * up(y) + c, 2 * far(y) + c

    def y_start(buf, k, s, g, direct=False):
        a, b = buf.at[me, 2 * g], buf.at[me, 2 * g + 1]
        send(a, a, s, k, y_up)
        send(b, b, s, k + 1, y_dn)
        send(b, b, s, k + 2, y_up)
        send(a, a, s, k + 3, y_dn)
        both = buf.at[me, pl.ds(2 * g, 2)]
        if direct:
            send(both, both, s, k + 4, at(y_=far(y)))
        send(both, both, s, k + 6, mate)

    def y_mid(buf, k, s, g, direct=False):
        a, b = buf.at[lo_y, 2 * g], buf.at[hi_y, 2 * g + 1]
        for ref, i, there, there_mate in ((a, 0, y_up, y_up_mate), (b, 1, y_dn, y_dn_mate)):
            recv(ref, k + i)
            if not direct:
                send(ref, ref, s, k + 4 + i, there)
                send(ref, ref, s, k + 6, there_mate)
            send(ref, ref, s, k + 6, mate)

    def y_end(buf, k, s, g, direct=False):
        for i, ref in enumerate((buf.at[lo_y, 2 * g + 1], buf.at[hi_y, 2 * g])):
            recv(ref, k + 2 + i)
            send(ref, ref, s, k + 6, mate)
        if direct:
            ref = buf.at[far_y, pl.ds(2 * g, 2)]
            recv(ref, k + 4)
            send(ref, ref, s, k + 6, mate)
        else:
            recv(buf.at[far_y, 2 * g], k + 4)
            recv(buf.at[far_y, 2 * g + 1], k + 5)

    def y_last(buf, k):
        recv(buf.at[pl.ds(0, 4), pl.ds(0, 2)], k + 6)

    def scaled(buf, gains, squares, first, n):
        parts = [gains[pl.ds(pl.multiple_of((4 * k + x) * 256, 256), 256)] for k in range(4)]
        gain = jnp.concatenate([part.reshape(1, 256) for part in parts], axis=1)

        def block(b, _):
            rows = jnp.concatenate([buf[i, b] for i in range(8)], axis=1).astype(F32)
            if squares:
                total = jnp.sum(rows * rows, axis=-1, keepdims=True)
                SQR[b] = jnp.broadcast_to(total, (128, 128)).T[0:8, :]
            XS[pl.ds(pl.multiple_of(b * 128, 128), 128), :] = (rows * gain).astype(BF16)
            return 0

        lax.fori_loop(first, first + n, block, 0)

    def scale_of(rows):
        return lax.rsqrt(jnp.broadcast_to(rows, (128, 128)).T / depth + EPS)

    ky = [new(recvs, 7) for _ in range(2)]
    sy = [sender(buf.at[pl.ds(0, 7), pl.ds(0, 2)]) for buf in (XG, XG)]
    recv(XG.at[me, pl.ds(0, 2)], kx)
    y_start(XG, ky[0], sy[0], 0)
    fewer(lambda n: XG.at[me, pl.ds(0, n)], 2, lambda ref: recv(ref, kx + 1))
    y_start(XG, ky[1], sy[1], 1)
    km = new(recvs)
    sm = sender(SM.at[pl.ds(0, 15)])
    for i in range(15):
        send(smix, SM.at[f], sm, km, fs_peers[i])
    SM[f] = smix[...]
    last0, lastn, wide = layout[-1]
    for W in (WGU[-1], WVU[-1], WDN[-1]):
        for k in range(4):
            W[k, lastn:, :] = jnp.zeros((wide - lastn, 256), BF16)
    z_own(9)
    z_own(11)
    z_fwd(0)
    z_fwd(1)
    z_own(2)
    z_own(3)
    y_mid(XG, ky[0], sy[0], 0)
    y_mid(XG, ky[1], sy[1], 1)
    loads[1].wait()
    loads[2].wait()
    for w, kern, off in ((0, gkv, go), (1, vkv, vo)):
        CV[w, :, last0:] = jnp.zeros((4, wide), F32)
        CV[w, 0:3, 0:units] = kern[...]
        CV[w, 3:4, 0:units] = off[...].reshape(1, units)
    y_end(XG, ky[0], sy[0], 0)
    y_end(XG, ky[1], sy[1], 1)
    y_last(XG, ky[0])
    y_last(XG, ky[1])
    scaled(XG, mgain, False, 0, 4)
    z_fin(0)
    z_fin(1)
    for w, W in ((0, WGP), (1, WVP)):
        prod = jnp.dot(XS[...], W[...].reshape(1024, 256), preferred_element_type=F32)
        P1[:, :, w * 256 : w * 256 + 256] = prod.reshape(4, 128, 256)

    def row_loop(first, n, fn):
        def step(i, _):
            fn(pl.ds(pl.multiple_of(first + i * 16, 16), 16))
            return 0

        lax.fori_loop(0, n // 16, step, 0)

    ra, rb = pl.ds(0, 64), pl.ds(64, 64)

    def rounded_rows(p, i, S, k, first, n, cols):
        def fn(rows):
            S[k, rows, cols] = p[i, rows, cols].astype(BF16)

        row_loop(first, n, fn)

    def rs_far(p, S, H, F, k, s, cols=slice(None)):
        rounded_rows(p, 3, S, 0, 0, 128, cols)
        send(S.at[0, ra, cols], H.at[0, :, cols], s, k, x_up)
        send(S.at[0, rb, cols], H.at[1, :, cols], s, k + 1, x_dn)

    def rs_first(p, S, H, F, k, s, cols=slice(None)):
        rounded_rows(p, 0, S, 1, 64, 64, cols)
        send(S.at[1, rb, cols], F.at[0, rb, cols], s, k + 2, x_up)
        rounded_rows(p, 1, S, 2, 0, 64, cols)
        send(S.at[2, ra, cols], F.at[1, ra, cols], s, k + 2, x_dn)

    def rs_second(p, S, H, F, k, s):
        def left(rows):
            S[1, rows, :] = (p[0, rows, :] + H[0, rows, :].astype(F32)).astype(BF16)

        def right(rows):
            low = pl.ds(pl.multiple_of(rows.start + 64, 16), 16)
            S[2, low, :] = (p[1, low, :] + H[1, rows, :].astype(F32)).astype(BF16)

        recv(H.at[0], k)
        row_loop(0, 64, left)
        send(S.at[1, ra], F.at[0, ra], s, k + 2, x_up)
        recv(H.at[1], k + 1)
        row_loop(0, 64, right)
        send(S.at[2, rb], F.at[1, rb], s, k + 2, x_dn)

    def rs_wait(F, k):
        recv(F, k + 2)

    kr = [new(recvs, 3) for _ in layout]
    set1 = (P1, S1, H1, F1, kr[0], sender(S1))
    rs_far(*set1)
    rs_first(*set1)
    z_fwd(2)
    z_own(4)
    rs_second(*set1)
    z_fwd(3)
    z_own(5)
    recv(SM.at[pl.ds(0, 15)], km)
    recv(SSB.at[pl.ds(0, 7)], kss)
    rs_wait(F1, kr[0])

    total = P1[2] + F1[0].astype(F32) + F1[1].astype(F32)
    rs = scale_of(jnp.sum(SSB[...], axis=0)[0:1, :])
    eye = lax.broadcasted_iota(jnp.int32, (128, 128), 0) == lanes_of(128)
    for h in range(2):
        cols = slice(h * 128, h * 128 + 128)
        gated = gelu((rs * total[:, cols]).astype(BF16).astype(F32))
        spread = gelu((rs * total[:, 256 + h * 128 : 384 + h * 128]).astype(BF16).astype(F32))
        spread = spread * lax.rsqrt(jnp.mean(spread * spread, axis=-1, keepdims=True) + EPS)
        spread = (spread * vgain[h : h + 1, :]).astype(BF16)
        matrix = SM[:, h].astype(F32).reshape(128, 128).astype(BF16)
        mixed = jnp.dot(matrix, spread, preferred_element_type=F32)
        bias = jnp.broadcast_to(sbias[h : h + 1, :], (128, 128))
        mixed = mixed + jnp.sum(jnp.where(eye, bias, 0.0), axis=-1, keepdims=True)
        joined = gated * mixed
        joined = joined * lax.rsqrt(jnp.mean(joined * joined, axis=-1, keepdims=True) + EPS)
        MG[2, :, cols] = (joined * hgain[h : h + 1, :]).astype(BF16)

    k2 = new(recvs, 3)
    s2 = sender(MG.at[pl.ds(0, 3)])
    send(MG.at[2], MG.at[1], s2, k2 + 1, x_up)
    send(MG.at[2], MG.at[0], s2, k2 + 2, x_dn)
    send(MG.at[2], MG.at[3], s2, k2, x_far)
    z_fin(2)

    y_order = (far(y), up(y), down(y), y)

    def cy_first(g, product, CS, CR, k, s):
        for n, yt in enumerate(y_order):
            prod = product(yt)
            size = prod.shape[0] // 128
            rows = pl.ds(2 * g, size)
            T[n, rows] = jnp.where(c == 0, prod[:, :128], prod[:, 128:]).reshape(size, 128, 128)
            give = jnp.where(c == 0, prod[:, 128:], prod[:, :128]).astype(BF16)
            CS[n, rows] = give.reshape(size, 128, 128)
            send(CS.at[n, rows], CR.at[n, rows], s, k + n, mate)

    def joined_at(n, b, CR):
        return T[n, b] + CR[n, b].astype(F32)

    def cy_second(g, CR, YS, YH, YF, k, kc, s):
        a, b = 2 * g, 2 * g + 1
        recv(CR.at[0, pl.ds(a, 2)], kc)
        YS[0, a] = joined_at(0, a, CR).astype(BF16)
        YS[0, b] = joined_at(0, b, CR).astype(BF16)
        send(YS.at[0, a], YH.at[a], s, k, y_up)
        send(YS.at[0, b], YH.at[b], s, k + 1, y_dn)
        recv(CR.at[1, pl.ds(a, 2)], kc + 1)
        YS[1, b] = joined_at(1, b, CR).astype(BF16)
        send(YS.at[1, b], YF.at[g, 0, 1], s, k + 2, y_up)
        recv(CR.at[2, pl.ds(a, 2)], kc + 2)
        YS[2, a] = joined_at(2, a, CR).astype(BF16)
        send(YS.at[2, a], YF.at[g, 1, 0], s, k + 2, y_dn)

    def cy_third(g, CR, YS, YH, YF, k, kc, s):
        a, b = 2 * g, 2 * g + 1
        recv(YH.at[a], k)
        YS[1, a] = (joined_at(1, a, CR) + YH[a].astype(F32)).astype(BF16)
        send(YS.at[1, a], YF.at[g, 0, 0], s, k + 2, y_up)
        recv(YH.at[b], k + 1)
        YS[2, b] = (joined_at(2, b, CR) + YH[b].astype(F32)).astype(BF16)
        send(YS.at[2, b], YF.at[g, 1, 1], s, k + 2, y_dn)
        recv(CR.at[3, pl.ds(a, 2)], kc + 3)

    def cy_last(g, CR, YF, k):
        recv(YF.at[g], k + 2)
        return [
            joined_at(3, 2 * g + i, CR) + YF[g, 0, i].astype(F32) + YF[g, 1, i].astype(F32)
            for i in range(2)
        ]

    def merge(g):
        rows = MG[2 * g : 2 * g + 2].reshape(256, 256)
        return lambda yt: jnp.dot(rows, WMP[yt], preferred_element_type=F32)

    kc = [new(recvs, 4) for _ in range(2)]
    k3 = [new(recvs, 3) for _ in range(2)]
    sc, s3 = sender(CS4), sender(YS4)
    recv(MG.at[0], k2 + 2)
    recv(MG.at[1], k2 + 1)
    cy_first(0, merge(0), CS4, CR4, kc[0], sc)
    cy_second(0, CR4, YS4, YH4, YF4, k3[0], kc[0], s3)
    recv(MG.at[3], k2)
    z_own(10)
    z_fwd(9)
    z_fwd(11)
    cy_first(1, merge(1), CS4, CR4, kc[1], sc)
    cy_second(1, CR4, YS4, YH4, YF4, k3[1], kc[1], s3)
    z_fwd(4)
    z_own(6)
    cy_third(0, CR4, YS4, YH4, YF4, k3[0], kc[0], s3)
    cy_third(1, CR4, YS4, YH4, YF4, k3[1], kc[1], s3)


    ko = new(recvs)
    so = new(sends)
    ends.append(lambda: fewer(lambda n: HG.at[0, pl.ds(0, n)], 4, stay(so)))
    spot = 2 * lax.rem(x, 2) + c
    blocks = (up(x), down(x), x, far(x))
    sh = [sender(buf.at[pl.ds(0, 7), pl.ds(0, 2)]) for buf in (HG, HG)]
    for g in range(2):
        branch = cy_last(g, CR4, YF4, k3[g])
        for i in range(2):
            b = 2 * g + i
            HG[me, b] = (XG[me, b].astype(F32) + branch[i]).astype(BF16)
        y_start(HG, ky[g], sh[g], g, g == 0)
    for b in range(4):
        if b != 2:
            dst = HRES.at[spot]
            send(HG.at[me, b], dst, so, ko, at(x_=blocks[b], c_=x // 2))
            continue

        @pl.when(to_me)
        def _():
            HRES[spot] = HG[me, 2]

        @pl.when(jnp.logical_not(to_me))
        def _():
            send(HG.at[me, 2], HRES.at[spot], so, ko, mate)

    z_fwd(5)
    y_mid(HG, ky[0], sh[0], 0, True)
    y_mid(HG, ky[1], sh[1], 1)
    y_end(HG, ky[0], sh[0], 0, True)
    z_fin(weight("g", 0))
    z_fin(weight("v", 0))
    y_last(HG, ky[0])
    scaled(HG, fgain, True, 0, 2)

    def project(W, p, n, first, b0, b1):
        def cut(cols, to, size):
            w = jnp.concatenate([W[k, cols, :] for k in range(4)], axis=1)
            prod = lax.dot_general(
                XS[b0 * 128 : b1 * 128, :], w, (((1,), (1,)), ((), ())),
                preferred_element_type=F32,
            )
            p[b0:b1, :, to] = prod.reshape(b1 - b0, 128, size)

        def step(i, _):
            cut(
                pl.ds(pl.multiple_of(i * 256, 256), 256),
                pl.ds(pl.multiple_of(first + i * 256, 128), 256), 256,
            )
            return 0

        lax.fori_loop(0, n // 256, step, 0)
        left = n % 256
        if left:
            cut(pl.ds(n - left, left), pl.ds(first + n - left, left), left)

    def gates(j):
        n = layout[j][2]
        z_fin(weight("g", j))
        project(WGU[j], PC[j], n, 0, 0, 4)
        return slice(0, n)

    def values(j):
        n = layout[j][2]
        z_fin(weight("v", j))
        project(WVU[j], PC[j], n, n, 0, 4)
        return slice(n, 2 * n)

    row = lax.broadcasted_iota(jnp.int32, (128, 128), 0)

    def activate(j):
        p, F, act = PC[j], FC[j], ACT[j]
        at0, _, n = layout[j]

        def conv_tile(i, _):
            def one(first, w):
                at_ = pl.ds(pl.multiple_of(first + i * 128, 128), 128)
                v = p[2, :, at_] + F[0, :, at_].astype(F32) + F[1, :, at_].astype(F32)
                v = (RS[...] * v).astype(BF16).astype(F32)
                prev = jnp.where(row == 0, 0.0, pltpu.roll(v, 1, axis=0))
                after = jnp.where(row == 127, 0.0, pltpu.roll(v, 127, axis=0))
                k = CV[w, :, pl.ds(pl.multiple_of(at0 + i * 128, 128), 128)]
                return k[3:4] + prev * k[0:1] + v * k[1:2] + after * k[2:3]

            cols = pl.ds(pl.multiple_of(i * 128, 128), 128)
            act[2, :, cols] = (gelu(one(0, 0)) * one(n, 1)).astype(BF16)
            return 0

        lax.fori_loop(0, n // 128, conv_tile, 0)

    sets = [
        (PC[j], SC[j], HC[j], FC[j], kr[j], sender(SC[j])) for j in range(chunks)
    ]
    kg = [new(recvs, 4) for _ in layout]
    sg = [sender(ACT[j].at[pl.ds(0, 3)]) for j in range(chunks)]

    def x_start(j, direct=False):
        buf, k, s = ACT[j], kg[j], sg[j]
        send(buf.at[2, ra], buf.at[1, ra], s, k, z_up)
        send(buf.at[2, rb], buf.at[0, rb], s, k + 1, z_dn)
        send(buf.at[2, rb], buf.at[1, rb], s, k + 2, z_up)
        send(buf.at[2, ra], buf.at[0, ra], s, k + 2, z_dn)

        if direct:
            send(buf.at[2, ra], buf.at[3, ra], s, k + 3, along(2))
            send(buf.at[2, rb], buf.at[3, rb], s, k + 3, along(-2))

    def x_mid(j, direct=False):
        buf, k, s = ACT[j], kg[j], sg[j]
        recv(buf.at[1, ra], k)
        if not direct:
            send(buf.at[1, ra], buf.at[3, ra], s, k + 3, z_up)
        recv(buf.at[0, rb], k + 1)
        if not direct:
            send(buf.at[0, rb], buf.at[3, rb], s, k + 3, z_dn)

    def x_near(j):
        recv(ACT[j].at[0], kg[j] + 2)

    def x_last(j):
        recv(ACT[j].at[3], kg[j] + 3)

    def down_rows(j, b0, b1):
        n = layout[j][2]
        rows = ACT[j][b0:b1].reshape((b1 - b0) * 128, n)
        return lambda k: jnp.dot(rows, WDN[j][k], preferred_element_type=F32)

    def down_early(j):
        product = down_rows(j, 0, 4)

        def step(k, _):
            prod = product(k).reshape(4, 128, 256)
            ACC[k] = prod if j == 0 else ACC[k] + prod
            return 0

        lax.fori_loop(0, 4, step, 0)

    n0 = layout[0][2]
    one0, two0 = slice(0, n0), slice(n0, 2 * n0)
    project(WGU[0], PC[0], n0, 0, 0, 2)
    rs_first(*sets[0], one0)
    z_fwd(6)
    z_own(7)
    z_own(8)
    z_fwd(10)
    project(WVU[0], PC[0], n0, n0, 0, 2)
    rs_first(*sets[0], two0)
    y_end(HG, ky[1], sh[1], 1)
    y_last(HG, ky[1])
    scaled(HG, fgain, True, 2, 2)
    project(WGU[0], PC[0], n0, 0, 2, 4)
    rs_far(*sets[0], one0)
    project(WVU[0], PC[0], n0, n0, 2, 4)
    rs_far(*sets[0], two0)
    kf = new(recvs)
    sf = sender(SSF.at[pl.ds(0, 3)])
    SSF[2] = SQR[2]
    send(SQR.at[0], SSF.at[1], sf, kf, x_up)
    send(SQR.at[1], SSF.at[0], sf, kf, x_dn)
    send(SQR.at[3], SSF.at[3], sf, kf, x_far)
    one1 = gates(1)
    rs_far(*sets[1], one1)
    rs_first(*sets[1], one1)
    two1 = values(1)
    rs_far(*sets[1], two1)
    rs_second(*sets[0])
    rs_first(*sets[1], two1)
    z_fwd(7)
    z_fwd(8)
    rs_second(*sets[1])
    recv(SSF.at[pl.ds(0, 3)], kf)
    RS[...] = scale_of(jnp.sum(SSF[...], axis=0)[0:1, :])
    one2 = gates(2)
    rs_far(*sets[2], one2)
    rs_wait(FC[0], kr[0])
    activate(0)
    x_start(0)
    two2 = values(2)
    rs_far(*sets[2], two2)
    rs_first(*sets[2])
    rs_wait(FC[1], kr[1])
    activate(1)
    x_start(1)
    x_mid(0)
    rs_second(*sets[2])
    x_mid(1)
    rs_wait(FC[2], kr[2])
    activate(2)
    x_start(2, True)
    x_near(0)
    x_last(0)
    z_fin(9)
    down_early(0)
    x_near(1)
    x_last(1)
    z_fin(10)
    z_fin(11)
    down_early(1)

    k7 = [new(recvs, 2) for _ in range(3)]
    s7 = sender(CS5)
    kt = new(recvs)
    st = new(sends)
    stays = y == z
    ends.append(lambda: fewer(lambda n: TB.at[pl.ds(0, n)], 4, stay(st), stays))

    def give(b):
        for i in range(2):
            TB[b, :, i * 256 : i * 256 + 256] = (T5[i, b] + CR5[i, b].astype(F32)).astype(BF16)
        if b < 2:
            send(TB.at[b], TI.at[y], st, kt, along(1 - 2 * b, z))
        elif b == 3:
            send(TB.at[b, ra], TI.at[y, ra], st, kt, along(-2, z))
            send(TB.at[b, rb], TI.at[y, rb], st, kt, along(2, z))
        else:

            @pl.when(stays)
            def _():
                TI[y] = TB[b]

            @pl.when(jnp.logical_not(stays))
            def _():
                send(TB.at[b], TI.at[y], st, kt, at(y_=z))

    parts = ((2, 3), (0, 2), (3, 4))

    def finish(g):
        b0, b1 = parts[g]
        rows = pl.ds(b0, b1 - b0)
        product = down_rows(2, b0, b1)

        def final(k):
            return product(k).reshape(b1 - b0, 128, 256) + ACC[k, rows]

        for i in range(2):
            CS5[i, rows] = final(2 * other + i).astype(BF16)
            send(CS5.at[i, rows], CR5.at[i, rows], s7, k7[g] + i, mate)
        for i in range(2):
            T5[i, rows] = final(2 * c + i)

    def hand_over(g):
        b0, b1 = parts[g]
        for i in range(2):
            recv(CR5.at[i, pl.ds(b0, b1 - b0)], k7[g] + i)
        for b in range(b0, b1):
            give(b)

    finish(0)
    x_mid(2, True)
    hand_over(0)
    x_near(2)
    finish(1)
    hand_over(1)
    x_last(2)
    finish(2)
    hand_over(2)

    fewer(lambda n: HRES.at[pl.ds(0, n)], 4, lambda ref: recv(ref, ko))
    fewer(lambda n: TI.at[pl.ds(0, n)], 4, lambda ref: recv(ref, kt), stays)
    for q in range(4):
        cols = slice(q * 128, q * 128 + 128)
        change = sum(TI[n, :, cols].astype(F32) for n in range(4))
        out[:, cols] = (HRES[q].astype(F32) + change).astype(BF16)
    for wait in ends:
        wait()
    assert sends[0] <= ssem.shape[0] and recvs[0] <= rsem.shape[0], (sends[0], recvs[0])


def body(
    tokens, mixer_gain, gate_proj, value_proj, value_gain, spatial_mix, spatial_bias,
    head_gain, merge_proj, ffn_gain, gate_up, value_up, gate_kernel, value_kernel,
    gate_offset, value_offset, down_proj,
):
    units = gate_up.shape[1]
    layout = []
    for first in range(0, units, CHUNK):
        n = min(CHUNK, units - first)
        layout.append((first, n, -(-n // 128) * 128))
    wide = sum(n for _, _, n in layout)
    widths = [n for _, _, n in layout]
    vm = lambda shape, dtype=BF16: pltpu.VMEM(shape, dtype)
    in_vmem = pl.BlockSpec(memory_space=pltpu.VMEM)
    left = pl.BlockSpec(memory_space=pl.ANY)
    call = pl.pallas_call(
        functools.partial(kernel, layout),
        out_shape=jax.ShapeDtypeStruct(tokens.shape, tokens.dtype),
        in_specs=[
            left, in_vmem, in_vmem, left, left, in_vmem, in_vmem, in_vmem, in_vmem, left,
            left, left, left, left, in_vmem, in_vmem, left,
        ],
        out_specs=in_vmem,
        scratch_shapes=[
            vm(tokens.shape), vm(gate_kernel.shape, F32), vm(gate_kernel.shape, F32),
            vm((2, 4, wide), F32),
            vm((8, 4, 128, 128)), vm((8, 4, 128, 128)), vm((512, 1024)),
            vm((4, 8, 128), F32), vm((128, 128), F32), vm((16, 2, 8, 128)),
            vm((4, 128, 256)), vm((8, 8, 128), F32), vm((4, 8, 128), F32), vm((4, 128, 128)),
            vm((4, 128, 512)), vm((4, 128, 512)),
            *[vm((4, 256, 256))] * 3, vm((4, 4, 128, 128), F32), vm((4, 4, 128, 256), F32),
            vm((4, 128, 512), F32), vm((3, 128, 512)), vm((2, 64, 512)), vm((2, 128, 512)),
            vm((4, 4, 128, 128)), vm((4, 4, 128, 128)), vm((3, 4, 128, 128)),
            vm((4, 128, 128)), vm((2, 2, 2, 128, 128)),
            vm((2, 4, 128, 256)), vm((2, 4, 128, 256)), vm((2, 4, 128, 256), F32),
            *[vm((4, n, 256)) for _ in range(3) for n in widths],
            *[vm((4, 128, n)) for n in widths],
            *[vm((4, 128, 2 * n), F32) for n in widths],
            *[vm((3, 128, 2 * n)) for n in widths],
            *[vm((2, 64, 2 * n)) for n in widths],
            *[vm((2, 128, 2 * n)) for n in widths],
            pltpu.SemaphoreType.DMA((SENDS,)), pltpu.SemaphoreType.DMA((RECVS,)),
            pltpu.SemaphoreType.DMA((6 + 3 * len(layout),)),
        ],
        compiler_params=pltpu.CompilerParams(
            collective_id=0, has_side_effects=True, vmem_limit_bytes=58 << 20
        ),
        name="layer",
    )
    return call(
        tokens, mixer_gain, ffn_gain, gate_proj, value_proj, value_gain, spatial_mix,
        spatial_bias, head_gain, merge_proj, gate_up.T, value_up.T, gate_kernel, value_kernel,
        gate_offset, value_offset, down_proj,
    )


def solution(mesh):
    finer = Mesh(
        mesh.devices.reshape(mesh.shape["rep"], 4, 4, 4, 2), ("rep", "fs_0", "fs_1", "tp_0", "tp_1")
    )
    return jax.shard_map(
        body,
        mesh=finer,
        in_specs=(
            P(REP_FS, TP), P(), P(FS, TP), P(FS, TP), P(TP, None), P(TP, FS, None),
            P(TP, None), P(TP, None), P(TP, FS), P(), P(FS, TP), P(FS, TP), P(None, TP),
            P(None, TP), P(TP), P(TP), P(TP, FS),
        ),
        out_specs=P(REP_FS, TP),
        check_vma=False,
    )
```

```python
import functools

import jax
import jax.numpy as jnp
from jax import lax
from jax.experimental import pallas as pl
from jax.experimental.pallas import tpu as pltpu
from jax.sharding import Mesh
from jax.sharding import PartitionSpec as P

TP = ("tp_0", "tp_1")
FS = ("fs_0", "fs_1")
REP_FS = ("rep", "fs_0", "fs_1")
MESH = pl.DeviceIdType.MESH
EPS = 1e-06
SENDS, RECVS = 33, 105
CHUNK = 512
F32 = jnp.float32
BF16 = jnp.bfloat16


def gelu(v):
    return 0.5 * v * (1.0 + lax.erf(v * 0.7071067811865476))


def lanes_of(n):
    return lax.broadcasted_iota(jnp.int32, (n, 128), 1)


def kernel(layout, tok, mgain, fgain, gp, vp, vgain, smix, sbias, hgain, mp, gu, vu, gk, vk, go, vo,
           dn, out, tokv, gkv, vkv, CV, XG, HG, XS, SQR, RS, SM, MG, SSB, SSF, HRES, TB, TI,
           WGP, WVP, WMP, T, ACC, P1, S1, H1, F1, CS4, CR4, YS4, YH4, YF4, CS5, CR5, T5, *rest):
    chunks = len(layout)
    WGU, WVU, WDN, ACT, PC, SC, HC, FC = (rest[i * chunks : (i + 1) * chunks] for i in range(8))
    ssem, rsem, lsem = rest[8 * chunks :]
    r, z, x, y, c = (lax.axis_index(a) for a in ("rep", "fs_0", "fs_1", "tp_0", "tp_1"))
    other = 1 - c
    f = 4 * z + x
    units = dn.shape[0]
    depth = mgain.shape[0]

    def at(z_=None, x_=None, y_=None, c_=None, r_=None):
        pick = lambda new, old: old if new is None else new
        return (pick(r_, r), pick(z_, z), pick(x_, x), pick(y_, y), pick(c_, c))

    up = lambda v: lax.rem(v + 1, 4)
    down = lambda v: lax.rem(v + 3, 4)
    far = lambda v: lax.rem(v + 2, 4)

    zr = 4 * r + z
    zu, zd = lax.rem(zr + 1, 8), lax.rem(zr + 7, 8)
    z_up = at(r_=zu // 4, z_=lax.rem(zu, 4))
    z_dn = at(r_=zd // 4, z_=lax.rem(zd, 4))
    x_up, x_dn, x_far = at(x_=up(x)), at(x_=down(x)), at(x_=far(x))
    y_up, y_dn = at(y_=up(y)), at(y_=down(y))
    y_up_mate, y_dn_mate = at(y_=up(y), c_=other), at(y_=down(y), c_=other)
    mate = at(c_=other)
    fs_peers = []
    for i in range(1, 16):
        g = lax.rem(f + i, 16)
        fs_peers.append(at(z_=g // 4, x_=lax.rem(g, 4)))
    near = []
    for i in range(1, 4):
        near += [at(x_=lax.rem(x + i, 4), c_=k) for k in (c, other)]
        near += [at(y_=lax.rem(y + i, 4), c_=other)]

    def along(d, y_=None):
        there = lax.rem(zr + 8 + d, 8)
        return at(r_=there // 4, z_=lax.rem(there, 4), y_=y_)

    for i in range(4):
        for d in (-2, -1, 0, 1, 2):
            if i or d:
                near.append(along(d, lax.rem(y + i, 4)))

    barrier = pltpu.get_barrier_semaphore()
    greet = [mate] + near + fs_peers
    for peer in greet:
        pl.semaphore_signal(barrier, inc=1, device_id=peer, device_id_type=MESH)
    loads = [
        pltpu.make_async_copy(src, dst, lsem.at[i])
        for i, (src, dst) in enumerate(((tok, tokv), (gk, gkv), (vk, vkv)))
    ]
    for copy in loads:
        copy.start()
    pl.semaphore_wait(barrier, len(greet))

    sends, recvs, ends = [0], [0], []

    def new(counter, n=1):
        counter[0] += n
        return counter[0] - n

    def remote(src, dst, s, k, peer):
        return pltpu.make_async_remote_copy(
            src_ref=src, dst_ref=dst, send_sem=ssem.at[s], recv_sem=rsem.at[k],
            device_id=peer, device_id_type=MESH,
        )

    def send(src, dst, s, k, peer):
        remote(src, dst, s, k, peer).start()

    def recv(dst, k):
        remote(dst, dst, 0, k, mate).wait_recv()

    def sender(ref):
        s = new(sends)
        ends.append(lambda: remote(ref, ref, s, 0, mate).wait_send())
        return s

    pieces = [(gp, WGP, 0, 256), (vp, WVP, 0, 256), (mp, WMP, 0, 256)]
    for (at0, n, _), G, V in zip(layout, WGU, WVU):
        pieces += [(gu, G, at0, n), (vu, V, at0, n)]
    for (at0, n, _), W in zip(layout, WDN):
        pieces.append((dn, W, at0, n))
    zk = [new(recvs, 3) for _ in pieces]
    zs = [sender(buf.at[pl.ds(0, 3), pl.ds(0, n)]) for _, buf, _, n in pieces]

    def z_local(i):
        src, buf, at0, n = pieces[i]
        own = buf.at[ring(i)[0], pl.ds(0, n)]
        return pltpu.make_async_copy(src.at[pl.ds(at0, n)], own, lsem.at[3 + i])

    def ring(i):
        return (x, x_up, x_dn) if pieces[i][0] is dn else (z, z_up, z_dn)

    def z_own(i):
        src, buf, at0, n = pieces[i]
        a, b = pl.ds(0, n // 2), pl.ds(n // 2, n // 2)
        from_a, from_b = src.at[pl.ds(at0, n // 2)], src.at[pl.ds(at0 + n // 2, n // 2)]
        place, above, below = ring(i)
        send(from_a, buf.at[place, a], zs[i], zk[i], above)
        send(from_b, buf.at[place, b], zs[i], zk[i] + 1, below)
        send(from_b, buf.at[place, b], zs[i], zk[i] + 2, above)
        send(from_a, buf.at[place, a], zs[i], zk[i] + 2, below)
        z_local(i).start()

    def z_fwd(i):
        _, buf, _, n = pieces[i]
        place, above, below = ring(i)
        a, b = buf.at[down(place), pl.ds(0, n // 2)], buf.at[up(place), pl.ds(n // 2, n // 2)]
        recv(a, zk[i])
        send(a, a, zs[i], zk[i] + 2, above)
        recv(b, zk[i] + 1)
        send(b, b, zs[i], zk[i] + 2, below)

    def z_fin(i):
        _, buf, _, n = pieces[i]
        recv(buf.at[pl.ds(0, 2), pl.ds(0, n)], zk[i] + 2)
        z_local(i).wait()

    def weight(kind, j):
        return {"g": 3 + 2 * j, "v": 4 + 2 * j, "d": 3 + 2 * chunks + j}[kind]

    me = 2 * y + c
    to_me = x // 2 == c
    loads[0].wait()
    kx = new(recvs, 2)
    sx = new(sends)
    for j in range(2):
        for h in range(2):
            xt = 2 * c + j
            ahead = lax.rem(x - xt + 4, 4)
            place = jnp.where(ahead == 0, 2, jnp.where(ahead == 2, 3, ahead // 2))
            mine = jnp.logical_and(xt == x, c == h)
            block = tokv.at[:, j * 256 + h * 128 : j * 256 + h * 128 + 128]

            @pl.when(jnp.logical_not(mine))
            def _():
                dst = XG.at[2 * y + h, place]
                send(block, dst, sx, kx + place // 2, at(x_=xt, c_=jnp.int32(h)))

            @pl.when(mine)
            def _():
                XG[2 * y + h, 2] = block[...]

    def fewer(ref_of, n, wait, stays=to_me):
        @pl.when(stays)
        def _():
            wait(ref_of(n - 1))

        @pl.when(jnp.logical_not(stays))
        def _():
            wait(ref_of(n))

    stay = lambda s: lambda ref: remote(ref, ref, s, 0, mate).wait_send()
    ends.append(lambda: fewer(lambda n: XG.at[0, pl.ds(0, n)], 4, stay(sx)))
    z_own(0)
    z_own(1)
    square = tokv[...].astype(F32)
    square = jnp.sum(square * square, axis=-1, keepdims=True)
    SSB[me] = jnp.broadcast_to(square, (128, 128)).T[0:8, :]
    kss = new(recvs)
    sss = sender(SSB.at[pl.ds(0, 7)])
    for i in range(1, 8):
        t = lax.rem(me + i, 8)
        send(SSB.at[me], SSB.at[me], sss, kss, at(y_=t // 2, c_=lax.rem(t, 2)))

    lo_y, hi_y, far_y = 2 * down(y) + c, 2 * up(y) + c, 2 * far(y) + c

    def y_start(buf, k, s, g):
        a, b = buf.at[me, 2 * g], buf.at[me, 2 * g + 1]
        send(a, a, s, k, y_up)
        send(b, b, s, k + 1, y_dn)
        send(b, b, s, k + 2, y_up)
        send(a, a, s, k + 3, y_dn)
        both = buf.at[me, pl.ds(2 * g, 2)]
        send(both, both, s, k + 6, mate)

    def y_mid(buf, k, s, g):
        a, b = buf.at[lo_y, 2 * g], buf.at[hi_y, 2 * g + 1]
        recv(a, k)
        send(a, a, s, k + 4, y_up)
        send(a, a, s, k + 6, y_up_mate)
        send(a, a, s, k + 6, mate)
        recv(b, k + 1)
        send(b, b, s, k + 5, y_dn)
        send(b, b, s, k + 6, y_dn_mate)
        send(b, b, s, k + 6, mate)

    def y_end(buf, k, s, g):
        rows = (buf.at[lo_y, 2 * g + 1], buf.at[hi_y, 2 * g], buf.at[far_y, 2 * g], buf.at[far_y, 2 * g + 1])
        for i, ref in enumerate(rows):
            recv(ref, k + 2 + i)
            if i < 2:
                send(ref, ref, s, k + 6, mate)

    def y_last(buf, k):
        recv(buf.at[pl.ds(0, 4), pl.ds(0, 2)], k + 6)

    def scaled(buf, gains, squares, first, n):
        parts = [gains[pl.ds(pl.multiple_of((4 * k + x) * 256, 256), 256)] for k in range(4)]
        gain = jnp.concatenate([part.reshape(1, 256) for part in parts], axis=1)

        def block(b, _):
            rows = jnp.concatenate([buf[i, b] for i in range(8)], axis=1).astype(F32)
            if squares:
                total = jnp.sum(rows * rows, axis=-1, keepdims=True)
                SQR[b] = jnp.broadcast_to(total, (128, 128)).T[0:8, :]
            XS[pl.ds(pl.multiple_of(b * 128, 128), 128), :] = (rows * gain).astype(BF16)
            return 0

        lax.fori_loop(first, first + n, block, 0)

    def scale_of(rows):
        return lax.rsqrt(jnp.broadcast_to(rows, (128, 128)).T / depth + EPS)

    ky = [new(recvs, 7) for _ in range(2)]
    sy = [sender(buf.at[pl.ds(0, 7), pl.ds(0, 2)]) for buf in (XG, XG)]
    recv(XG.at[me, pl.ds(0, 2)], kx)
    y_start(XG, ky[0], sy[0], 0)
    fewer(lambda n: XG.at[me, pl.ds(0, n)], 2, lambda ref: recv(ref, kx + 1))
    y_start(XG, ky[1], sy[1], 1)
    km = new(recvs)
    sm = sender(SM.at[pl.ds(0, 15)])
    for i in range(15):
        send(smix, SM.at[f], sm, km, fs_peers[i])
    SM[f] = smix[...]
    last0, lastn, wide = layout[-1]
    for W in (WGU[-1], WVU[-1], WDN[-1]):
        for k in range(4):
            W[k, lastn:, :] = jnp.zeros((wide - lastn, 256), BF16)
    z_own(9)
    z_own(11)
    z_fwd(0)
    z_fwd(1)
    z_own(2)
    z_own(3)
    y_mid(XG, ky[0], sy[0], 0)
    y_mid(XG, ky[1], sy[1], 1)
    loads[1].wait()
    loads[2].wait()
    for w, kern, off in ((0, gkv, go), (1, vkv, vo)):
        CV[w, :, last0:] = jnp.zeros((4, wide), F32)
        CV[w, 0:3, 0:units] = kern[...]
        CV[w, 3:4, 0:units] = off[...].reshape(1, units)
    y_end(XG, ky[0], sy[0], 0)
    y_end(XG, ky[1], sy[1], 1)
    y_last(XG, ky[0])
    y_last(XG, ky[1])
    scaled(XG, mgain, False, 0, 4)
    z_fin(0)
    z_fin(1)
    for w, W in ((0, WGP), (1, WVP)):
        prod = jnp.dot(XS[...], W[...].reshape(1024, 256), preferred_element_type=F32)
        P1[:, :, w * 256 : w * 256 + 256] = prod.reshape(4, 128, 256)

    def row_loop(first, n, fn):
        def step(i, _):
            fn(pl.ds(pl.multiple_of(first + i * 16, 16), 16))
            return 0

        lax.fori_loop(0, n // 16, step, 0)

    ra, rb = pl.ds(0, 64), pl.ds(64, 64)

    def rounded_rows(p, i, S, k, first, n, cols):
        def fn(rows):
            S[k, rows, cols] = p[i, rows, cols].astype(BF16)

        row_loop(first, n, fn)

    def rs_far(p, S, H, F, k, s, cols=slice(None)):
        rounded_rows(p, 3, S, 0, 0, 128, cols)
        send(S.at[0, ra, cols], H.at[0, :, cols], s, k, x_up)
        send(S.at[0, rb, cols], H.at[1, :, cols], s, k + 1, x_dn)

    def rs_first(p, S, H, F, k, s, cols=slice(None)):
        rounded_rows(p, 0, S, 1, 64, 64, cols)
        send(S.at[1, rb, cols], F.at[0, rb, cols], s, k + 2, x_up)
        rounded_rows(p, 1, S, 2, 0, 64, cols)
        send(S.at[2, ra, cols], F.at[1, ra, cols], s, k + 2, x_dn)

    def rs_second(p, S, H, F, k, s):
        def left(rows):
            S[1, rows, :] = (p[0, rows, :] + H[0, rows, :].astype(F32)).astype(BF16)

        def right(rows):
            low = pl.ds(pl.multiple_of(rows.start + 64, 16), 16)
            S[2, low, :] = (p[1, low, :] + H[1, rows, :].astype(F32)).astype(BF16)

        recv(H.at[0], k)
        row_loop(0, 64, left)
        send(S.at[1, ra], F.at[0, ra], s, k + 2, x_up)
        recv(H.at[1], k + 1)
        row_loop(0, 64, right)
        send(S.at[2, rb], F.at[1, rb], s, k + 2, x_dn)

    def rs_wait(F, k):
        recv(F, k + 2)

    kr = [new(recvs, 3) for _ in layout]
    set1 = (P1, S1, H1, F1, kr[0], sender(S1))
    rs_far(*set1)
    rs_first(*set1)
    z_fwd(2)
    z_own(4)
    rs_second(*set1)
    z_fwd(3)
    z_own(5)
    recv(SM.at[pl.ds(0, 15)], km)
    recv(SSB.at[pl.ds(0, 7)], kss)
    rs_wait(F1, kr[0])

    total = P1[2] + F1[0].astype(F32) + F1[1].astype(F32)
    rs = scale_of(jnp.sum(SSB[...], axis=0)[0:1, :])
    eye = lax.broadcasted_iota(jnp.int32, (128, 128), 0) == lanes_of(128)
    for h in range(2):
        cols = slice(h * 128, h * 128 + 128)
        gated = gelu((rs * total[:, cols]).astype(BF16).astype(F32))
        spread = gelu((rs * total[:, 256 + h * 128 : 384 + h * 128]).astype(BF16).astype(F32))
        spread = spread * lax.rsqrt(jnp.mean(spread * spread, axis=-1, keepdims=True) + EPS)
        spread = (spread * vgain[h : h + 1, :]).astype(BF16)
        matrix = SM[:, h].astype(F32).reshape(128, 128).astype(BF16)
        mixed = jnp.dot(matrix, spread, preferred_element_type=F32)
        bias = jnp.broadcast_to(sbias[h : h + 1, :], (128, 128))
        mixed = mixed + jnp.sum(jnp.where(eye, bias, 0.0), axis=-1, keepdims=True)
        joined = gated * mixed
        joined = joined * lax.rsqrt(jnp.mean(joined * joined, axis=-1, keepdims=True) + EPS)
        MG[2, :, cols] = (joined * hgain[h : h + 1, :]).astype(BF16)

    k2 = new(recvs, 3)
    s2 = sender(MG.at[pl.ds(0, 3)])
    send(MG.at[2], MG.at[1], s2, k2 + 1, x_up)
    send(MG.at[2], MG.at[0], s2, k2 + 2, x_dn)
    send(MG.at[2], MG.at[3], s2, k2, x_far)
    z_fin(2)

    y_order = (far(y), up(y), down(y), y)

    def cy_first(g, product, CS, CR, k, s):
        for n, yt in enumerate(y_order):
            prod = product(yt)
            size = prod.shape[0] // 128
            rows = pl.ds(2 * g, size)
            T[n, rows] = jnp.where(c == 0, prod[:, :128], prod[:, 128:]).reshape(size, 128, 128)
            give = jnp.where(c == 0, prod[:, 128:], prod[:, :128]).astype(BF16)
            CS[n, rows] = give.reshape(size, 128, 128)
            send(CS.at[n, rows], CR.at[n, rows], s, k + n, mate)

    def joined_at(n, b, CR):
        return T[n, b] + CR[n, b].astype(F32)

    def cy_second(g, CR, YS, YH, YF, k, kc, s):
        a, b = 2 * g, 2 * g + 1
        recv(CR.at[0, pl.ds(a, 2)], kc)
        YS[0, a] = joined_at(0, a, CR).astype(BF16)
        YS[0, b] = joined_at(0, b, CR).astype(BF16)
        send(YS.at[0, a], YH.at[a], s, k, y_up)
        send(YS.at[0, b], YH.at[b], s, k + 1, y_dn)
        recv(CR.at[1, pl.ds(a, 2)], kc + 1)
        YS[1, b] = joined_at(1, b, CR).astype(BF16)
        send(YS.at[1, b], YF.at[g, 0, 1], s, k + 2, y_up)
        recv(CR.at[2, pl.ds(a, 2)], kc + 2)
        YS[2, a] = joined_at(2, a, CR).astype(BF16)
        send(YS.at[2, a], YF.at[g, 1, 0], s, k + 2, y_dn)

    def cy_third(g, CR, YS, YH, YF, k, kc, s):
        a, b = 2 * g, 2 * g + 1
        recv(YH.at[a], k)
        YS[1, a] = (joined_at(1, a, CR) + YH[a].astype(F32)).astype(BF16)
        send(YS.at[1, a], YF.at[g, 0, 0], s, k + 2, y_up)
        recv(YH.at[b], k + 1)
        YS[2, b] = (joined_at(2, b, CR) + YH[b].astype(F32)).astype(BF16)
        send(YS.at[2, b], YF.at[g, 1, 1], s, k + 2, y_dn)
        recv(CR.at[3, pl.ds(a, 2)], kc + 3)

    def cy_last(g, CR, YF, k):
        recv(YF.at[g], k + 2)
        return [
            joined_at(3, 2 * g + i, CR) + YF[g, 0, i].astype(F32) + YF[g, 1, i].astype(F32)
            for i in range(2)
        ]

    def merge(g):
        rows = MG[2 * g : 2 * g + 2].reshape(256, 256)
        return lambda yt: jnp.dot(rows, WMP[yt], preferred_element_type=F32)

    kc = [new(recvs, 4) for _ in range(2)]
    k3 = [new(recvs, 3) for _ in range(2)]
    sc, s3 = sender(CS4), sender(YS4)
    recv(MG.at[0], k2 + 2)
    recv(MG.at[1], k2 + 1)
    cy_first(0, merge(0), CS4, CR4, kc[0], sc)
    cy_second(0, CR4, YS4, YH4, YF4, k3[0], kc[0], s3)
    recv(MG.at[3], k2)
    z_own(10)
    z_fwd(9)
    z_fwd(11)
    cy_first(1, merge(1), CS4, CR4, kc[1], sc)
    cy_second(1, CR4, YS4, YH4, YF4, k3[1], kc[1], s3)
    z_fwd(4)
    z_own(6)
    cy_third(0, CR4, YS4, YH4, YF4, k3[0], kc[0], s3)
    cy_third(1, CR4, YS4, YH4, YF4, k3[1], kc[1], s3)


    ko = new(recvs)
    so = new(sends)
    ends.append(lambda: fewer(lambda n: HG.at[0, pl.ds(0, n)], 4, stay(so)))
    spot = 2 * lax.rem(x, 2) + c
    blocks = (up(x), down(x), x, far(x))
    sh = [sender(buf.at[pl.ds(0, 7), pl.ds(0, 2)]) for buf in (HG, HG)]
    for g in range(2):
        branch = cy_last(g, CR4, YF4, k3[g])
        for i in range(2):
            b = 2 * g + i
            HG[me, b] = (XG[me, b].astype(F32) + branch[i]).astype(BF16)
        y_start(HG, ky[g], sh[g], g)
    for b in range(4):
        if b != 2:
            dst = HRES.at[spot]
            send(HG.at[me, b], dst, so, ko, at(x_=blocks[b], c_=x // 2))
            continue

        @pl.when(to_me)
        def _():
            HRES[spot] = HG[me, 2]

        @pl.when(jnp.logical_not(to_me))
        def _():
            send(HG.at[me, 2], HRES.at[spot], so, ko, mate)

    z_fwd(5)
    y_mid(HG, ky[0], sh[0], 0)
    y_mid(HG, ky[1], sh[1], 1)
    y_end(HG, ky[0], sh[0], 0)
    z_fwd(6)
    z_own(7)
    z_own(8)
    z_fwd(10)
    y_end(HG, ky[1], sh[1], 1)
    z_fin(weight("g", 0))
    z_fin(weight("v", 0))
    y_last(HG, ky[0])
    scaled(HG, fgain, True, 0, 2)

    def project(W, p, n, first, b0, b1):
        def cut(cols, to, size):
            w = jnp.concatenate([W[k, cols, :] for k in range(4)], axis=1)
            prod = lax.dot_general(
                XS[b0 * 128 : b1 * 128, :], w, (((1,), (1,)), ((), ())),
                preferred_element_type=F32,
            )
            p[b0:b1, :, to] = prod.reshape(b1 - b0, 128, size)

        def step(i, _):
            cut(
                pl.ds(pl.multiple_of(i * 256, 256), 256),
                pl.ds(pl.multiple_of(first + i * 256, 128), 256), 256,
            )
            return 0

        lax.fori_loop(0, n // 256, step, 0)
        left = n % 256
        if left:
            cut(pl.ds(n - left, left), pl.ds(first + n - left, left), left)

    def gates(j):
        n = layout[j][2]
        z_fin(weight("g", j))
        project(WGU[j], PC[j], n, 0, 0, 4)
        return slice(0, n)

    def values(j):
        n = layout[j][2]
        z_fin(weight("v", j))
        project(WVU[j], PC[j], n, n, 0, 4)
        return slice(n, 2 * n)

    row = lax.broadcasted_iota(jnp.int32, (128, 128), 0)

    def activate(j):
        p, F, act = PC[j], FC[j], ACT[j]
        at0, _, n = layout[j]

        def conv_tile(i, _):
            def one(first, w):
                at_ = pl.ds(pl.multiple_of(first + i * 128, 128), 128)
                v = p[2, :, at_] + F[0, :, at_].astype(F32) + F[1, :, at_].astype(F32)
                v = (RS[...] * v).astype(BF16).astype(F32)
                prev = jnp.where(row == 0, 0.0, pltpu.roll(v, 1, axis=0))
                after = jnp.where(row == 127, 0.0, pltpu.roll(v, 127, axis=0))
                k = CV[w, :, pl.ds(pl.multiple_of(at0 + i * 128, 128), 128)]
                return k[3:4] + prev * k[0:1] + v * k[1:2] + after * k[2:3]

            cols = pl.ds(pl.multiple_of(i * 128, 128), 128)
            act[2, :, cols] = (gelu(one(0, 0)) * one(n, 1)).astype(BF16)
            return 0

        lax.fori_loop(0, n // 128, conv_tile, 0)

    sets = [
        (PC[j], SC[j], HC[j], FC[j], kr[j], sender(SC[j])) for j in range(chunks)
    ]
    kg = [new(recvs, 4) for _ in layout]
    sg = [sender(ACT[j].at[pl.ds(0, 3)]) for j in range(chunks)]

    def x_start(j):
        buf, k, s = ACT[j], kg[j], sg[j]
        send(buf.at[2, ra], buf.at[1, ra], s, k, z_up)
        send(buf.at[2, rb], buf.at[0, rb], s, k + 1, z_dn)
        send(buf.at[2, rb], buf.at[1, rb], s, k + 2, z_up)
        send(buf.at[2, ra], buf.at[0, ra], s, k + 2, z_dn)

    def x_mid(j):
        buf, k, s = ACT[j], kg[j], sg[j]
        recv(buf.at[1, ra], k)
        send(buf.at[1, ra], buf.at[3, ra], s, k + 3, z_up)
        recv(buf.at[0, rb], k + 1)
        send(buf.at[0, rb], buf.at[3, rb], s, k + 3, z_dn)

    def x_near(j):
        recv(ACT[j].at[0], kg[j] + 2)

    def x_last(j):
        recv(ACT[j].at[3], kg[j] + 3)

    def down_rows(j, b0, b1):
        n = layout[j][2]
        rows = ACT[j][b0:b1].reshape((b1 - b0) * 128, n)
        return lambda k: jnp.dot(rows, WDN[j][k], preferred_element_type=F32)

    def down_early(j):
        product = down_rows(j, 0, 4)

        def step(k, _):
            prod = product(k).reshape(4, 128, 256)
            ACC[k] = prod if j == 0 else ACC[k] + prod
            return 0

        lax.fori_loop(0, 4, step, 0)

    n0 = layout[0][2]
    one0, two0 = slice(0, n0), slice(n0, 2 * n0)
    project(WGU[0], PC[0], n0, 0, 0, 2)
    rs_first(*sets[0], one0)
    project(WVU[0], PC[0], n0, n0, 0, 2)
    rs_first(*sets[0], two0)
    y_last(HG, ky[1])
    scaled(HG, fgain, True, 2, 2)
    project(WGU[0], PC[0], n0, 0, 2, 4)
    rs_far(*sets[0], one0)
    project(WVU[0], PC[0], n0, n0, 2, 4)
    rs_far(*sets[0], two0)
    kf = new(recvs)
    sf = sender(SSF.at[pl.ds(0, 3)])
    SSF[2] = SQR[2]
    send(SQR.at[0], SSF.at[1], sf, kf, x_up)
    send(SQR.at[1], SSF.at[0], sf, kf, x_dn)
    send(SQR.at[3], SSF.at[3], sf, kf, x_far)
    one1 = gates(1)
    rs_far(*sets[1], one1)
    two1 = values(1)
    rs_far(*sets[1], two1)
    rs_second(*sets[0])
    rs_first(*sets[1])
    z_fwd(7)
    rs_second(*sets[1])
    z_fwd(8)
    recv(SSF.at[pl.ds(0, 3)], kf)
    RS[...] = scale_of(jnp.sum(SSF[...], axis=0)[0:1, :])
    rs_wait(FC[0], kr[0])
    activate(0)
    x_start(0)
    one2 = gates(2)
    rs_far(*sets[2], one2)
    two2 = values(2)
    rs_far(*sets[2], two2)
    rs_first(*sets[2])
    rs_wait(FC[1], kr[1])
    activate(1)
    x_start(1)
    x_mid(0)
    rs_second(*sets[2])
    x_mid(1)
    rs_wait(FC[2], kr[2])
    activate(2)
    x_start(2)
    x_near(0)
    x_last(0)
    z_fin(9)
    down_early(0)
    x_near(1)
    x_last(1)
    z_fin(10)
    z_fin(11)
    down_early(1)

    k7 = [new(recvs, 2) for _ in range(3)]
    s7 = sender(CS5)
    kt = new(recvs)
    st = new(sends)
    stays = y == z
    ends.append(lambda: fewer(lambda n: TB.at[pl.ds(0, n)], 4, stay(st), stays))

    def give(b):
        for i in range(2):
            TB[b, :, i * 256 : i * 256 + 256] = (T5[i, b] + CR5[i, b].astype(F32)).astype(BF16)
        if b < 2:
            send(TB.at[b], TI.at[y], st, kt, along(1 - 2 * b, z))
        elif b == 3:
            send(TB.at[b, ra], TI.at[y, ra], st, kt, along(-2, z))
            send(TB.at[b, rb], TI.at[y, rb], st, kt, along(2, z))
        else:

            @pl.when(stays)
            def _():
                TI[y] = TB[b]

            @pl.when(jnp.logical_not(stays))
            def _():
                send(TB.at[b], TI.at[y], st, kt, at(y_=z))

    parts = ((2, 3), (0, 2), (3, 4))

    def finish(g):
        b0, b1 = parts[g]
        rows = pl.ds(b0, b1 - b0)
        product = down_rows(2, b0, b1)

        def final(k):
            return product(k).reshape(b1 - b0, 128, 256) + ACC[k, rows]

        for i in range(2):
            CS5[i, rows] = final(2 * other + i).astype(BF16)
            send(CS5.at[i, rows], CR5.at[i, rows], s7, k7[g] + i, mate)
        for i in range(2):
            T5[i, rows] = final(2 * c + i)

    def hand_over(g):
        b0, b1 = parts[g]
        for i in range(2):
            recv(CR5.at[i, pl.ds(b0, b1 - b0)], k7[g] + i)
        for b in range(b0, b1):
            give(b)

    x_mid(2)
    finish(0)
    x_near(2)
    finish(1)
    hand_over(0)
    hand_over(1)
    x_last(2)
    finish(2)
    hand_over(2)

    fewer(lambda n: HRES.at[pl.ds(0, n)], 4, lambda ref: recv(ref, ko))
    fewer(lambda n: TI.at[pl.ds(0, n)], 4, lambda ref: recv(ref, kt), stays)
    for q in range(4):
        cols = slice(q * 128, q * 128 + 128)
        change = sum(TI[n, :, cols].astype(F32) for n in range(4))
        out[:, cols] = (HRES[q].astype(F32) + change).astype(BF16)
    for wait in ends:
        wait()
    assert sends[0] <= ssem.shape[0] and recvs[0] <= rsem.shape[0], (sends[0], recvs[0])


def body(
    tokens, mixer_gain, gate_proj, value_proj, value_gain, spatial_mix, spatial_bias,
    head_gain, merge_proj, ffn_gain, gate_up, value_up, gate_kernel, value_kernel,
    gate_offset, value_offset, down_proj,
):
    units = gate_up.shape[1]
    layout = []
    for first in range(0, units, CHUNK):
        n = min(CHUNK, units - first)
        layout.append((first, n, -(-n // 128) * 128))
    wide = sum(n for _, _, n in layout)
    widths = [n for _, _, n in layout]
    vm = lambda shape, dtype=BF16: pltpu.VMEM(shape, dtype)
    in_vmem = pl.BlockSpec(memory_space=pltpu.VMEM)
    left = pl.BlockSpec(memory_space=pl.ANY)
    call = pl.pallas_call(
        functools.partial(kernel, layout),
        out_shape=jax.ShapeDtypeStruct(tokens.shape, tokens.dtype),
        in_specs=[
            left, in_vmem, in_vmem, left, left, in_vmem, in_vmem, in_vmem, in_vmem, left,
            left, left, left, left, in_vmem, in_vmem, left,
        ],
        out_specs=in_vmem,
        scratch_shapes=[
            vm(tokens.shape), vm(gate_kernel.shape, F32), vm(gate_kernel.shape, F32),
            vm((2, 4, wide), F32),
            vm((8, 4, 128, 128)), vm((8, 4, 128, 128)), vm((512, 1024)),
            vm((4, 8, 128), F32), vm((128, 128), F32), vm((16, 2, 8, 128)),
            vm((4, 128, 256)), vm((8, 8, 128), F32), vm((4, 8, 128), F32), vm((4, 128, 128)),
            vm((4, 128, 512)), vm((4, 128, 512)),
            *[vm((4, 256, 256))] * 3, vm((4, 4, 128, 128), F32), vm((4, 4, 128, 256), F32),
            vm((4, 128, 512), F32), vm((3, 128, 512)), vm((2, 64, 512)), vm((2, 128, 512)),
            vm((4, 4, 128, 128)), vm((4, 4, 128, 128)), vm((3, 4, 128, 128)),
            vm((4, 128, 128)), vm((2, 2, 2, 128, 128)),
            vm((2, 4, 128, 256)), vm((2, 4, 128, 256)), vm((2, 4, 128, 256), F32),
            *[vm((4, n, 256)) for _ in range(3) for n in widths],
            *[vm((4, 128, n)) for n in widths],
            *[vm((4, 128, 2 * n), F32) for n in widths],
            *[vm((3, 128, 2 * n)) for n in widths],
            *[vm((2, 64, 2 * n)) for n in widths],
            *[vm((2, 128, 2 * n)) for n in widths],
            pltpu.SemaphoreType.DMA((SENDS,)), pltpu.SemaphoreType.DMA((RECVS,)),
            pltpu.SemaphoreType.DMA((6 + 3 * len(layout),)),
        ],
        compiler_params=pltpu.CompilerParams(
            collective_id=0, has_side_effects=True, vmem_limit_bytes=58 << 20
        ),
        name="layer",
    )
    return call(
        tokens, mixer_gain, ffn_gain, gate_proj, value_proj, value_gain, spatial_mix,
        spatial_bias, head_gain, merge_proj, gate_up.T, value_up.T, gate_kernel, value_kernel,
        gate_offset, value_offset, down_proj,
    )


def solution(mesh):
    finer = Mesh(
        mesh.devices.reshape(mesh.shape["rep"], 4, 4, 4, 2), ("rep", "fs_0", "fs_1", "tp_0", "tp_1")
    )
    return jax.shard_map(
        body,
        mesh=finer,
        in_specs=(
            P(REP_FS, TP), P(), P(FS, TP), P(FS, TP), P(TP, None), P(TP, FS, None),
            P(TP, None), P(TP, None), P(TP, FS), P(), P(FS, TP), P(FS, TP), P(None, TP),
            P(None, TP), P(TP), P(TP), P(TP, FS),
        ),
        out_specs=P(REP_FS, TP),
        check_vma=False,
    )
```

```python
import functools

import jax
import jax.numpy as jnp
from jax import lax
from jax.experimental import pallas as pl
from jax.experimental.pallas import tpu as pltpu
from jax.sharding import Mesh
from jax.sharding import PartitionSpec as P

TP = ("tp_0", "tp_1")
FS = ("fs_0", "fs_1")
REP_FS = ("rep", "fs_0", "fs_1")
MESH = pl.DeviceIdType.MESH
EPS = 1e-06
SENDS, RECVS = 33, 105
CHUNK = 512
F32 = jnp.float32
BF16 = jnp.bfloat16


def gelu(v):
    return 0.5 * v * (1.0 + lax.erf(v * 0.7071067811865476))


def lanes_of(n):
    return lax.broadcasted_iota(jnp.int32, (n, 128), 1)


def kernel(layout, tok, mgain, fgain, gp, vp, vgain, smix, sbias, hgain, mp, gu, vu, gk, vk, go, vo,
           dn, out, tokv, gkv, vkv, CV, XG, HG, XS, SQR, RS, SM, MG, SSB, SSF, HRES, TB, TI,
           WGP, WVP, WMP, T, ACC, P1, S1, H1, F1, CS4, CR4, YS4, YH4, YF4, CS5, CR5, T5, *rest):
    chunks = len(layout)
    WGU, WVU, WDN, ACT, PC, SC, HC, FC = (rest[i * chunks : (i + 1) * chunks] for i in range(8))
    ssem, rsem, lsem = rest[8 * chunks :]
    r, z, x, y, c = (lax.axis_index(a) for a in ("rep", "fs_0", "fs_1", "tp_0", "tp_1"))
    other = 1 - c
    f = 4 * z + x
    units = dn.shape[0]
    depth = mgain.shape[0]

    def at(z_=None, x_=None, y_=None, c_=None, r_=None):
        pick = lambda new, old: old if new is None else new
        return (pick(r_, r), pick(z_, z), pick(x_, x), pick(y_, y), pick(c_, c))

    up = lambda v: lax.rem(v + 1, 4)
    down = lambda v: lax.rem(v + 3, 4)
    far = lambda v: lax.rem(v + 2, 4)

    zr = 4 * r + z
    zu, zd = lax.rem(zr + 1, 8), lax.rem(zr + 7, 8)
    z_up = at(r_=zu // 4, z_=lax.rem(zu, 4))
    z_dn = at(r_=zd // 4, z_=lax.rem(zd, 4))
    x_up, x_dn, x_far = at(x_=up(x)), at(x_=down(x)), at(x_=far(x))
    y_up, y_dn = at(y_=up(y)), at(y_=down(y))
    y_up_mate, y_dn_mate = at(y_=up(y), c_=other), at(y_=down(y), c_=other)
    mate = at(c_=other)
    fs_peers = []
    for i in range(1, 16):
        g = lax.rem(f + i, 16)
        fs_peers.append(at(z_=g // 4, x_=lax.rem(g, 4)))
    near = []
    for i in range(1, 4):
        near += [at(x_=lax.rem(x + i, 4), c_=k) for k in (c, other)]
        near += [at(y_=lax.rem(y + i, 4), c_=other)]

    def along(d, y_=None):
        there = lax.rem(zr + 8 + d, 8)
        return at(r_=there // 4, z_=lax.rem(there, 4), y_=y_)

    for i in range(4):
        for d in (-2, -1, 0, 1, 2):
            if i or d:
                near.append(along(d, lax.rem(y + i, 4)))

    barrier = pltpu.get_barrier_semaphore()
    greet = [mate] + near + fs_peers
    for peer in greet:
        pl.semaphore_signal(barrier, inc=1, device_id=peer, device_id_type=MESH)
    loads = [
        pltpu.make_async_copy(src, dst, lsem.at[i])
        for i, (src, dst) in enumerate(((tok, tokv), (gk, gkv), (vk, vkv)))
    ]
    for copy in loads:
        copy.start()
    pl.semaphore_wait(barrier, len(greet))

    sends, recvs, ends = [0], [0], []

    def new(counter, n=1):
        counter[0] += n
        return counter[0] - n

    def remote(src, dst, s, k, peer):
        return pltpu.make_async_remote_copy(
            src_ref=src, dst_ref=dst, send_sem=ssem.at[s], recv_sem=rsem.at[k],
            device_id=peer, device_id_type=MESH,
        )

    def send(src, dst, s, k, peer):
        remote(src, dst, s, k, peer).start()

    def recv(dst, k):
        remote(dst, dst, 0, k, mate).wait_recv()

    def sender(ref):
        s = new(sends)
        ends.append(lambda: remote(ref, ref, s, 0, mate).wait_send())
        return s

    pieces = [(gp, WGP, 0, 256), (vp, WVP, 0, 256), (mp, WMP, 0, 256)]
    for (at0, n, _), G, V in zip(layout, WGU, WVU):
        pieces += [(gu, G, at0, n), (vu, V, at0, n)]
    for (at0, n, _), W in zip(layout, WDN):
        pieces.append((dn, W, at0, n))
    zk = [new(recvs, 3) for _ in pieces]
    zs = [sender(buf.at[pl.ds(0, 3), pl.ds(0, n)]) for _, buf, _, n in pieces]

    def z_local(i):
        src, buf, at0, n = pieces[i]
        own = buf.at[ring(i)[0], pl.ds(0, n)]
        return pltpu.make_async_copy(src.at[pl.ds(at0, n)], own, lsem.at[3 + i])

    def ring(i):
        return (x, x_up, x_dn) if pieces[i][0] is dn else (z, z_up, z_dn)

    def z_own(i):
        src, buf, at0, n = pieces[i]
        a, b = pl.ds(0, n // 2), pl.ds(n // 2, n // 2)
        from_a, from_b = src.at[pl.ds(at0, n // 2)], src.at[pl.ds(at0 + n // 2, n // 2)]
        place, above, below = ring(i)
        send(from_a, buf.at[place, a], zs[i], zk[i], above)
        send(from_b, buf.at[place, b], zs[i], zk[i] + 1, below)
        send(from_b, buf.at[place, b], zs[i], zk[i] + 2, above)
        send(from_a, buf.at[place, a], zs[i], zk[i] + 2, below)
        z_local(i).start()

    def z_fwd(i):
        _, buf, _, n = pieces[i]
        place, above, below = ring(i)
        a, b = buf.at[down(place), pl.ds(0, n // 2)], buf.at[up(place), pl.ds(n // 2, n // 2)]
        recv(a, zk[i])
        send(a, a, zs[i], zk[i] + 2, above)
        recv(b, zk[i] + 1)
        send(b, b, zs[i], zk[i] + 2, below)

    def z_fin(i):
        _, buf, _, n = pieces[i]
        recv(buf.at[pl.ds(0, 2), pl.ds(0, n)], zk[i] + 2)
        z_local(i).wait()

    def weight(kind, j):
        return {"g": 3 + 2 * j, "v": 4 + 2 * j, "d": 3 + 2 * chunks + j}[kind]

    me = 2 * y + c
    to_me = x // 2 == c
    loads[0].wait()
    kx = new(recvs, 2)
    sx = new(sends)
    for j in range(2):
        for h in range(2):
            xt = 2 * c + j
            ahead = lax.rem(x - xt + 4, 4)
            place = jnp.where(ahead == 0, 2, jnp.where(ahead == 2, 3, ahead // 2))
            mine = jnp.logical_and(xt == x, c == h)
            block = tokv.at[:, j * 256 + h * 128 : j * 256 + h * 128 + 128]

            @pl.when(jnp.logical_not(mine))
            def _():
                dst = XG.at[2 * y + h, place]
                send(block, dst, sx, kx + place // 2, at(x_=xt, c_=jnp.int32(h)))

            @pl.when(mine)
            def _():
                XG[2 * y + h, 2] = block[...]

    def fewer(ref_of, n, wait, stays=to_me):
        @pl.when(stays)
        def _():
            wait(ref_of(n - 1))

        @pl.when(jnp.logical_not(stays))
        def _():
            wait(ref_of(n))

    stay = lambda s: lambda ref: remote(ref, ref, s, 0, mate).wait_send()
    ends.append(lambda: fewer(lambda n: XG.at[0, pl.ds(0, n)], 4, stay(sx)))
    z_own(0)
    z_own(1)
    square = tokv[...].astype(F32)
    square = jnp.sum(square * square, axis=-1, keepdims=True)
    SSB[me] = jnp.broadcast_to(square, (128, 128)).T[0:8, :]
    kss = new(recvs)
    sss = sender(SSB.at[pl.ds(0, 7)])
    for i in range(1, 8):
        t = lax.rem(me + i, 8)
        send(SSB.at[me], SSB.at[me], sss, kss, at(y_=t // 2, c_=lax.rem(t, 2)))

    lo_y, hi_y, far_y = 2 * down(y) + c, 2 * up(y) + c, 2 * far(y) + c

    def y_start(buf, k, s, g):
        a, b = buf.at[me, 2 * g], buf.at[me, 2 * g + 1]
        send(a, a, s, k, y_up)
        send(b, b, s, k + 1, y_dn)
        send(b, b, s, k + 2, y_up)
        send(a, a, s, k + 3, y_dn)
        both = buf.at[me, pl.ds(2 * g, 2)]
        send(both, both, s, k + 6, mate)

    def y_mid(buf, k, s, g):
        a, b = buf.at[lo_y, 2 * g], buf.at[hi_y, 2 * g + 1]
        recv(a, k)
        send(a, a, s, k + 4, y_up)
        send(a, a, s, k + 6, y_up_mate)
        send(a, a, s, k + 6, mate)
        recv(b, k + 1)
        send(b, b, s, k + 5, y_dn)
        send(b, b, s, k + 6, y_dn_mate)
        send(b, b, s, k + 6, mate)

    def y_end(buf, k, s, g):
        rows = (buf.at[lo_y, 2 * g + 1], buf.at[hi_y, 2 * g], buf.at[far_y, 2 * g], buf.at[far_y, 2 * g + 1])
        for i, ref in enumerate(rows):
            recv(ref, k + 2 + i)
            if i < 2:
                send(ref, ref, s, k + 6, mate)

    def y_last(buf, k):
        recv(buf.at[pl.ds(0, 4), pl.ds(0, 2)], k + 6)

    def scaled(buf, gains, squares, first, n):
        parts = [gains[pl.ds(pl.multiple_of((4 * k + x) * 256, 256), 256)] for k in range(4)]
        gain = jnp.concatenate([part.reshape(1, 256) for part in parts], axis=1)

        def block(b, _):
            rows = jnp.concatenate([buf[i, b] for i in range(8)], axis=1).astype(F32)
            if squares:
                total = jnp.sum(rows * rows, axis=-1, keepdims=True)
                SQR[b] = jnp.broadcast_to(total, (128, 128)).T[0:8, :]
            XS[pl.ds(pl.multiple_of(b * 128, 128), 128), :] = (rows * gain).astype(BF16)
            return 0

        lax.fori_loop(first, first + n, block, 0)

    def scale_of(rows):
        return lax.rsqrt(jnp.broadcast_to(rows, (128, 128)).T / depth + EPS)

    ky = [new(recvs, 7) for _ in range(2)]
    sy = [sender(buf.at[pl.ds(0, 7), pl.ds(0, 2)]) for buf in (XG, XG)]
    recv(XG.at[me, pl.ds(0, 2)], kx)
    y_start(XG, ky[0], sy[0], 0)
    fewer(lambda n: XG.at[me, pl.ds(0, n)], 2, lambda ref: recv(ref, kx + 1))
    y_start(XG, ky[1], sy[1], 1)
    km = new(recvs)
    sm = sender(SM.at[pl.ds(0, 15)])
    for i in range(15):
        send(smix, SM.at[f], sm, km, fs_peers[i])
    SM[f] = smix[...]
    last0, lastn, wide = layout[-1]
    for W in (WGU[-1], WVU[-1], WDN[-1]):
        for k in range(4):
            W[k, lastn:, :] = jnp.zeros((wide - lastn, 256), BF16)
    z_own(9)
    z_own(11)
    z_fwd(0)
    z_fwd(1)
    z_own(2)
    z_own(3)
    y_mid(XG, ky[0], sy[0], 0)
    y_mid(XG, ky[1], sy[1], 1)
    loads[1].wait()
    loads[2].wait()
    for w, kern, off in ((0, gkv, go), (1, vkv, vo)):
        CV[w, :, last0:] = jnp.zeros((4, wide), F32)
        CV[w, 0:3, 0:units] = kern[...]
        CV[w, 3:4, 0:units] = off[...].reshape(1, units)
    y_end(XG, ky[0], sy[0], 0)
    y_end(XG, ky[1], sy[1], 1)
    y_last(XG, ky[0])
    y_last(XG, ky[1])
    scaled(XG, mgain, False, 0, 4)
    z_fin(0)
    z_fin(1)
    for w, W in ((0, WGP), (1, WVP)):
        prod = jnp.dot(XS[...], W[...].reshape(1024, 256), preferred_element_type=F32)
        P1[:, :, w * 256 : w * 256 + 256] = prod.reshape(4, 128, 256)

    def row_loop(first, n, fn):
        def step(i, _):
            fn(pl.ds(pl.multiple_of(first + i * 16, 16), 16))
            return 0

        lax.fori_loop(0, n // 16, step, 0)

    ra, rb = pl.ds(0, 64), pl.ds(64, 64)

    def rounded_rows(p, i, S, k, first, n, cols):
        def fn(rows):
            S[k, rows, cols] = p[i, rows, cols].astype(BF16)

        row_loop(first, n, fn)

    def rs_far(p, S, H, F, k, s, cols=slice(None)):
        rounded_rows(p, 3, S, 0, 0, 128, cols)
        send(S.at[0, ra, cols], H.at[0, :, cols], s, k, x_up)
        send(S.at[0, rb, cols], H.at[1, :, cols], s, k + 1, x_dn)

    def rs_first(p, S, H, F, k, s, cols=slice(None)):
        rounded_rows(p, 0, S, 1, 64, 64, cols)
        send(S.at[1, rb, cols], F.at[0, rb, cols], s, k + 2, x_up)
        rounded_rows(p, 1, S, 2, 0, 64, cols)
        send(S.at[2, ra, cols], F.at[1, ra, cols], s, k + 2, x_dn)

    def rs_second(p, S, H, F, k, s):
        def left(rows):
            S[1, rows, :] = (p[0, rows, :] + H[0, rows, :].astype(F32)).astype(BF16)

        def right(rows):
            low = pl.ds(pl.multiple_of(rows.start + 64, 16), 16)
            S[2, low, :] = (p[1, low, :] + H[1, rows, :].astype(F32)).astype(BF16)

        recv(H.at[0], k)
        row_loop(0, 64, left)
        send(S.at[1, ra], F.at[0, ra], s, k + 2, x_up)
        recv(H.at[1], k + 1)
        row_loop(0, 64, right)
        send(S.at[2, rb], F.at[1, rb], s, k + 2, x_dn)

    def rs_wait(F, k):
        recv(F, k + 2)

    kr = [new(recvs, 3) for _ in layout]
    set1 = (P1, S1, H1, F1, kr[0], sender(S1))
    rs_far(*set1)
    rs_first(*set1)
    z_fwd(2)
    z_own(4)
    rs_second(*set1)
    z_fwd(3)
    z_own(5)
    recv(SM.at[pl.ds(0, 15)], km)
    recv(SSB.at[pl.ds(0, 7)], kss)
    rs_wait(F1, kr[0])

    total = P1[2] + F1[0].astype(F32) + F1[1].astype(F32)
    rs = scale_of(jnp.sum(SSB[...], axis=0)[0:1, :])
    eye = lax.broadcasted_iota(jnp.int32, (128, 128), 0) == lanes_of(128)
    for h in range(2):
        cols = slice(h * 128, h * 128 + 128)
        gated = gelu((rs * total[:, cols]).astype(BF16).astype(F32))
        spread = gelu((rs * total[:, 256 + h * 128 : 384 + h * 128]).astype(BF16).astype(F32))
        spread = spread * lax.rsqrt(jnp.mean(spread * spread, axis=-1, keepdims=True) + EPS)
        spread = (spread * vgain[h : h + 1, :]).astype(BF16)
        matrix = SM[:, h].astype(F32).reshape(128, 128).astype(BF16)
        mixed = jnp.dot(matrix, spread, preferred_element_type=F32)
        bias = jnp.broadcast_to(sbias[h : h + 1, :], (128, 128))
        mixed = mixed + jnp.sum(jnp.where(eye, bias, 0.0), axis=-1, keepdims=True)
        joined = gated * mixed
        joined = joined * lax.rsqrt(jnp.mean(joined * joined, axis=-1, keepdims=True) + EPS)
        MG[2, :, cols] = (joined * hgain[h : h + 1, :]).astype(BF16)

    k2 = new(recvs, 3)
    s2 = sender(MG.at[pl.ds(0, 3)])
    send(MG.at[2], MG.at[1], s2, k2 + 1, x_up)
    send(MG.at[2], MG.at[0], s2, k2 + 2, x_dn)
    send(MG.at[2], MG.at[3], s2, k2, x_far)
    z_fin(2)

    y_order = (far(y), up(y), down(y), y)

    def cy_first(g, product, CS, CR, k, s):
        for n, yt in enumerate(y_order):
            prod = product(yt)
            size = prod.shape[0] // 128
            rows = pl.ds(2 * g, size)
            T[n, rows] = jnp.where(c == 0, prod[:, :128], prod[:, 128:]).reshape(size, 128, 128)
            give = jnp.where(c == 0, prod[:, 128:], prod[:, :128]).astype(BF16)
            CS[n, rows] = give.reshape(size, 128, 128)
            send(CS.at[n, rows], CR.at[n, rows], s, k + n, mate)

    def joined_at(n, b, CR):
        return T[n, b] + CR[n, b].astype(F32)

    def cy_second(g, CR, YS, YH, YF, k, kc, s):
        a, b = 2 * g, 2 * g + 1
        recv(CR.at[0, pl.ds(a, 2)], kc)
        YS[0, a] = joined_at(0, a, CR).astype(BF16)
        YS[0, b] = joined_at(0, b, CR).astype(BF16)
        send(YS.at[0, a], YH.at[a], s, k, y_up)
        send(YS.at[0, b], YH.at[b], s, k + 1, y_dn)
        recv(CR.at[1, pl.ds(a, 2)], kc + 1)
        YS[1, b] = joined_at(1, b, CR).astype(BF16)
        send(YS.at[1, b], YF.at[g, 0, 1], s, k + 2, y_up)
        recv(CR.at[2, pl.ds(a, 2)], kc + 2)
        YS[2, a] = joined_at(2, a, CR).astype(BF16)
        send(YS.at[2, a], YF.at[g, 1, 0], s, k + 2, y_dn)

    def cy_third(g, CR, YS, YH, YF, k, kc, s):
        a, b = 2 * g, 2 * g + 1
        recv(YH.at[a], k)
        YS[1, a] = (joined_at(1, a, CR) + YH[a].astype(F32)).astype(BF16)
        send(YS.at[1, a], YF.at[g, 0, 0], s, k + 2, y_up)
        recv(YH.at[b], k + 1)
        YS[2, b] = (joined_at(2, b, CR) + YH[b].astype(F32)).astype(BF16)
        send(YS.at[2, b], YF.at[g, 1, 1], s, k + 2, y_dn)
        recv(CR.at[3, pl.ds(a, 2)], kc + 3)

    def cy_last(g, CR, YF, k):
        recv(YF.at[g], k + 2)
        return [
            joined_at(3, 2 * g + i, CR) + YF[g, 0, i].astype(F32) + YF[g, 1, i].astype(F32)
            for i in range(2)
        ]

    def merge(g):
        rows = MG[2 * g : 2 * g + 2].reshape(256, 256)
        return lambda yt: jnp.dot(rows, WMP[yt], preferred_element_type=F32)

    kc = [new(recvs, 4) for _ in range(2)]
    k3 = [new(recvs, 3) for _ in range(2)]
    sc, s3 = sender(CS4), sender(YS4)
    recv(MG.at[0], k2 + 2)
    recv(MG.at[1], k2 + 1)
    cy_first(0, merge(0), CS4, CR4, kc[0], sc)
    cy_second(0, CR4, YS4, YH4, YF4, k3[0], kc[0], s3)
    recv(MG.at[3], k2)
    z_own(10)
    z_fwd(9)
    z_fwd(11)
    cy_first(1, merge(1), CS4, CR4, kc[1], sc)
    cy_second(1, CR4, YS4, YH4, YF4, k3[1], kc[1], s3)
    z_fwd(4)
    z_own(6)
    cy_third(0, CR4, YS4, YH4, YF4, k3[0], kc[0], s3)
    cy_third(1, CR4, YS4, YH4, YF4, k3[1], kc[1], s3)


    ko = new(recvs)
    so = new(sends)
    ends.append(lambda: fewer(lambda n: HG.at[0, pl.ds(0, n)], 4, stay(so)))
    spot = 2 * lax.rem(x, 2) + c
    blocks = (up(x), down(x), x, far(x))
    sh = [sender(buf.at[pl.ds(0, 7), pl.ds(0, 2)]) for buf in (HG, HG)]
    for g in range(2):
        branch = cy_last(g, CR4, YF4, k3[g])
        for i in range(2):
            b = 2 * g + i
            HG[me, b] = (XG[me, b].astype(F32) + branch[i]).astype(BF16)
        y_start(HG, ky[g], sh[g], g)
    for b in range(4):
        if b != 2:
            dst = HRES.at[spot]
            send(HG.at[me, b], dst, so, ko, at(x_=blocks[b], c_=x // 2))
            continue

        @pl.when(to_me)
        def _():
            HRES[spot] = HG[me, 2]

        @pl.when(jnp.logical_not(to_me))
        def _():
            send(HG.at[me, 2], HRES.at[spot], so, ko, mate)

    z_fwd(5)
    y_mid(HG, ky[0], sh[0], 0)
    y_mid(HG, ky[1], sh[1], 1)
    y_end(HG, ky[0], sh[0], 0)
    z_fwd(6)
    z_own(7)
    z_own(8)
    z_fwd(10)
    y_end(HG, ky[1], sh[1], 1)
    z_fin(weight("g", 0))
    z_fin(weight("v", 0))
    y_last(HG, ky[0])
    scaled(HG, fgain, True, 0, 2)

    def project(W, p, n, first, b0, b1):
        def cut(cols, to, size):
            w = jnp.concatenate([W[k, cols, :] for k in range(4)], axis=1)
            prod = lax.dot_general(
                XS[b0 * 128 : b1 * 128, :], w, (((1,), (1,)), ((), ())),
                preferred_element_type=F32,
            )
            p[b0:b1, :, to] = prod.reshape(b1 - b0, 128, size)

        def step(i, _):
            cut(
                pl.ds(pl.multiple_of(i * 256, 256), 256),
                pl.ds(pl.multiple_of(first + i * 256, 128), 256), 256,
            )
            return 0

        lax.fori_loop(0, n // 256, step, 0)
        left = n % 256
        if left:
            cut(pl.ds(n - left, left), pl.ds(first + n - left, left), left)

    def gates(j):
        n = layout[j][2]
        z_fin(weight("g", j))
        project(WGU[j], PC[j], n, 0, 0, 4)
        return slice(0, n)

    def values(j):
        n = layout[j][2]
        z_fin(weight("v", j))
        project(WVU[j], PC[j], n, n, 0, 4)
        return slice(n, 2 * n)

    row = lax.broadcasted_iota(jnp.int32, (128, 128), 0)

    def activate(j):
        p, F, act = PC[j], FC[j], ACT[j]
        at0, _, n = layout[j]

        def conv_tile(i, _):
            def one(first, w):
                at_ = pl.ds(pl.multiple_of(first + i * 128, 128), 128)
                v = p[2, :, at_] + F[0, :, at_].astype(F32) + F[1, :, at_].astype(F32)
                v = (RS[...] * v).astype(BF16).astype(F32)
                prev = jnp.where(row == 0, 0.0, pltpu.roll(v, 1, axis=0))
                after = jnp.where(row == 127, 0.0, pltpu.roll(v, 127, axis=0))
                k = CV[w, :, pl.ds(pl.multiple_of(at0 + i * 128, 128), 128)]
                return k[3:4] + prev * k[0:1] + v * k[1:2] + after * k[2:3]

            cols = pl.ds(pl.multiple_of(i * 128, 128), 128)
            act[2, :, cols] = (gelu(one(0, 0)) * one(n, 1)).astype(BF16)
            return 0

        lax.fori_loop(0, n // 128, conv_tile, 0)

    sets = [
        (PC[j], SC[j], HC[j], FC[j], kr[j], sender(SC[j])) for j in range(chunks)
    ]
    kg = [new(recvs, 4) for _ in layout]
    sg = [sender(ACT[j].at[pl.ds(0, 3)]) for j in range(chunks)]

    def x_start(j):
        buf, k, s = ACT[j], kg[j], sg[j]
        send(buf.at[2, ra], buf.at[1, ra], s, k, z_up)
        send(buf.at[2, rb], buf.at[0, rb], s, k + 1, z_dn)
        send(buf.at[2, rb], buf.at[1, rb], s, k + 2, z_up)
        send(buf.at[2, ra], buf.at[0, ra], s, k + 2, z_dn)

    def x_mid(j):
        buf, k, s = ACT[j], kg[j], sg[j]
        recv(buf.at[1, ra], k)
        send(buf.at[1, ra], buf.at[3, ra], s, k + 3, z_up)
        recv(buf.at[0, rb], k + 1)
        send(buf.at[0, rb], buf.at[3, rb], s, k + 3, z_dn)

    def x_near(j):
        recv(ACT[j].at[0], kg[j] + 2)

    def x_last(j):
        recv(ACT[j].at[3], kg[j] + 3)

    def down_rows(j, b0, b1):
        n = layout[j][2]
        rows = ACT[j][b0:b1].reshape((b1 - b0) * 128, n)
        return lambda k: jnp.dot(rows, WDN[j][k], preferred_element_type=F32)

    def down_early(j):
        product = down_rows(j, 0, 4)

        def step(k, _):
            prod = product(k).reshape(4, 128, 256)
            ACC[k] = prod if j == 0 else ACC[k] + prod
            return 0

        lax.fori_loop(0, 4, step, 0)

    n0 = layout[0][2]
    one0, two0 = slice(0, n0), slice(n0, 2 * n0)
    project(WGU[0], PC[0], n0, 0, 0, 2)
    rs_first(*sets[0], one0)
    project(WVU[0], PC[0], n0, n0, 0, 2)
    rs_first(*sets[0], two0)
    y_last(HG, ky[1])
    scaled(HG, fgain, True, 2, 2)
    project(WGU[0], PC[0], n0, 0, 2, 4)
    rs_far(*sets[0], one0)
    project(WVU[0], PC[0], n0, n0, 2, 4)
    rs_far(*sets[0], two0)
    kf = new(recvs)
    sf = sender(SSF.at[pl.ds(0, 3)])
    SSF[2] = SQR[2]
    send(SQR.at[0], SSF.at[1], sf, kf, x_up)
    send(SQR.at[1], SSF.at[0], sf, kf, x_dn)
    send(SQR.at[3], SSF.at[3], sf, kf, x_far)
    one1 = gates(1)
    rs_far(*sets[1], one1)
    two1 = values(1)
    rs_far(*sets[1], two1)
    rs_second(*sets[0])
    rs_first(*sets[1])
    z_fwd(7)
    rs_second(*sets[1])
    z_fwd(8)
    recv(SSF.at[pl.ds(0, 3)], kf)
    RS[...] = scale_of(jnp.sum(SSF[...], axis=0)[0:1, :])
    rs_wait(FC[0], kr[0])
    activate(0)
    x_start(0)
    one2 = gates(2)
    rs_far(*sets[2], one2)
    two2 = values(2)
    rs_far(*sets[2], two2)
    rs_first(*sets[2])
    rs_wait(FC[1], kr[1])
    activate(1)
    x_start(1)
    x_mid(0)
    rs_second(*sets[2])
    x_mid(1)
    rs_wait(FC[2], kr[2])
    activate(2)
    x_start(2)
    x_near(0)
    x_last(0)
    z_fin(9)
    down_early(0)
    x_near(1)
    x_last(1)
    z_fin(10)
    z_fin(11)
    down_early(1)

    k7 = [new(recvs, 2) for _ in range(3)]
    s7 = sender(CS5)
    kt = new(recvs)
    st = new(sends)
    stays = y == z
    ends.append(lambda: fewer(lambda n: TB.at[pl.ds(0, n)], 4, stay(st), stays))

    def give(b):
        for i in range(2):
            TB[b, :, i * 256 : i * 256 + 256] = (T5[i, b] + CR5[i, b].astype(F32)).astype(BF16)
        if b < 2:
            send(TB.at[b], TI.at[y], st, kt, along(1 - 2 * b, z))
        elif b == 3:
            send(TB.at[b, ra], TI.at[y, ra], st, kt, along(-2, z))
            send(TB.at[b, rb], TI.at[y, rb], st, kt, along(2, z))
        else:

            @pl.when(stays)
            def _():
                TI[y] = TB[b]

            @pl.when(jnp.logical_not(stays))
            def _():
                send(TB.at[b], TI.at[y], st, kt, at(y_=z))

    parts = ((2, 3), (0, 2), (3, 4))

    def finish(g):
        b0, b1 = parts[g]
        rows = pl.ds(b0, b1 - b0)
        product = down_rows(2, b0, b1)

        def final(k):
            return product(k).reshape(b1 - b0, 128, 256) + ACC[k, rows]

        for i in range(2):
            CS5[i, rows] = final(2 * other + i).astype(BF16)
            send(CS5.at[i, rows], CR5.at[i, rows], s7, k7[g] + i, mate)
        for i in range(2):
            T5[i, rows] = final(2 * c + i)

    def hand_over(g):
        b0, b1 = parts[g]
        for i in range(2):
            recv(CR5.at[i, pl.ds(b0, b1 - b0)], k7[g] + i)
        for b in range(b0, b1):
            give(b)

    x_mid(2)
    finish(0)
    x_near(2)
    hand_over(0)
    finish(1)
    hand_over(1)
    x_last(2)
    finish(2)
    hand_over(2)

    fewer(lambda n: HRES.at[pl.ds(0, n)], 4, lambda ref: recv(ref, ko))
    fewer(lambda n: TI.at[pl.ds(0, n)], 4, lambda ref: recv(ref, kt), stays)
    for q in range(4):
        cols = slice(q * 128, q * 128 + 128)
        change = sum(TI[n, :, cols].astype(F32) for n in range(4))
        out[:, cols] = (HRES[q].astype(F32) + change).astype(BF16)
    for wait in ends:
        wait()
    assert sends[0] <= ssem.shape[0] and recvs[0] <= rsem.shape[0], (sends[0], recvs[0])


def body(
    tokens, mixer_gain, gate_proj, value_proj, value_gain, spatial_mix, spatial_bias,
    head_gain, merge_proj, ffn_gain, gate_up, value_up, gate_kernel, value_kernel,
    gate_offset, value_offset, down_proj,
):
    units = gate_up.shape[1]
    layout = []
    for first in range(0, units, CHUNK):
        n = min(CHUNK, units - first)
        layout.append((first, n, -(-n // 128) * 128))
    wide = sum(n for _, _, n in layout)
    widths = [n for _, _, n in layout]
    vm = lambda shape, dtype=BF16: pltpu.VMEM(shape, dtype)
    in_vmem = pl.BlockSpec(memory_space=pltpu.VMEM)
    left = pl.BlockSpec(memory_space=pl.ANY)
    call = pl.pallas_call(
        functools.partial(kernel, layout),
        out_shape=jax.ShapeDtypeStruct(tokens.shape, tokens.dtype),
        in_specs=[
            left, in_vmem, in_vmem, left, left, in_vmem, in_vmem, in_vmem, in_vmem, left,
            left, left, left, left, in_vmem, in_vmem, left,
        ],
        out_specs=in_vmem,
        scratch_shapes=[
            vm(tokens.shape), vm(gate_kernel.shape, F32), vm(gate_kernel.shape, F32),
            vm((2, 4, wide), F32),
            vm((8, 4, 128, 128)), vm((8, 4, 128, 128)), vm((512, 1024)),
            vm((4, 8, 128), F32), vm((128, 128), F32), vm((16, 2, 8, 128)),
            vm((4, 128, 256)), vm((8, 8, 128), F32), vm((4, 8, 128), F32), vm((4, 128, 128)),
            vm((4, 128, 512)), vm((4, 128, 512)),
            *[vm((4, 256, 256))] * 3, vm((4, 4, 128, 128), F32), vm((4, 4, 128, 256), F32),
            vm((4, 128, 512), F32), vm((3, 128, 512)), vm((2, 64, 512)), vm((2, 128, 512)),
            vm((4, 4, 128, 128)), vm((4, 4, 128, 128)), vm((3, 4, 128, 128)),
            vm((4, 128, 128)), vm((2, 2, 2, 128, 128)),
            vm((2, 4, 128, 256)), vm((2, 4, 128, 256)), vm((2, 4, 128, 256), F32),
            *[vm((4, n, 256)) for _ in range(3) for n in widths],
            *[vm((4, 128, n)) for n in widths],
            *[vm((4, 128, 2 * n), F32) for n in widths],
            *[vm((3, 128, 2 * n)) for n in widths],
            *[vm((2, 64, 2 * n)) for n in widths],
            *[vm((2, 128, 2 * n)) for n in widths],
            pltpu.SemaphoreType.DMA((SENDS,)), pltpu.SemaphoreType.DMA((RECVS,)),
            pltpu.SemaphoreType.DMA((6 + 3 * len(layout),)),
        ],
        compiler_params=pltpu.CompilerParams(
            collective_id=0, has_side_effects=True, vmem_limit_bytes=58 << 20
        ),
        name="layer",
    )
    return call(
        tokens, mixer_gain, ffn_gain, gate_proj, value_proj, value_gain, spatial_mix,
        spatial_bias, head_gain, merge_proj, gate_up.T, value_up.T, gate_kernel, value_kernel,
        gate_offset, value_offset, down_proj,
    )


def solution(mesh):
    finer = Mesh(
        mesh.devices.reshape(mesh.shape["rep"], 4, 4, 4, 2), ("rep", "fs_0", "fs_1", "tp_0", "tp_1")
    )
    return jax.shard_map(
        body,
        mesh=finer,
        in_specs=(
            P(REP_FS, TP), P(), P(FS, TP), P(FS, TP), P(TP, None), P(TP, FS, None),
            P(TP, None), P(TP, None), P(TP, FS), P(), P(FS, TP), P(FS, TP), P(None, TP),
            P(None, TP), P(TP), P(TP), P(TP, FS),
        ),
        out_specs=P(REP_FS, TP),
        check_vma=False,
    )
```
